256 devices in a mesh: kv: 32 (over z, y), tp: 8 (over x, core).
Axes of the slice: x: 4, y: 4, z: 8, core: 2. Of those that a mesh axis runs over, the one named last changes fastest.
Arguments:
- tokens: bfloat16 [32768, 1024], P('kv', 'tp'), may hold values from -6 to 6
- query_weight: bfloat16 [1024, 2048], P(None, 'tp'), may hold values from -0.1875 to 0.1875
- latent_weight: bfloat16 [1024, 128], replicated, may hold values from -0.1875 to 0.1875
- query_gain: float32 [128], replicated, may hold values from 0.5 to 1.5
- key_gain: float32 [128], replicated, may hold values from 0.5 to 1.5
- value_up: bfloat16 [16, 128, 64], P('tp'), may hold values from -0.5 to 0.5
- out_weight: bfloat16 [1024, 1024], P('tp'), may hold values from -0.25 to 0.25
- out_gain: float32 [1024], replicated, may hold values from 0.5 to 1.5
- chosen: int32 [256, 32], P('kv'), may hold values from -1 to 255, as said below
Outputs:
- mixed_out: bfloat16 [32768, 1024], P('kv', 'tp')
The draws below stay inside these ranges and needn't reach their ends.
Inputs may be any that keep to these rules, and one draw needn't show every extreme that they name: Row b lists the key blocks chosen for query block b: entry 0 is b itself, then distinct blocks before b, then -1 in every unused place. Block j is held by index j // 8 of kv. All query blocks of one index of kv together choose at most 2 distinct blocks held by any one other index, and some pair of indices reaches that bound; blocks held by the same index are chosen freely.
All inputs are finite; a program needn't handle non-finite values.
Results may differ from the reference program's by a relative error of at most 0.02.
Values may be sent and summed in bfloat16 or wider, within the bound.
A program may use at most 64 MiB of HBM per device.

```python
import jax
import jax.numpy as jnp
from jax import lax

D = 1024
HEADS = 16
LATENT = 128
VDIM = 64
BLOCK = 128
PICKS = 32
PER_OWNER = 2
TOKENS = 32768
BLOCKS_DEV = 8
BLOCKS = 256


def draw_chosen(key, part):
    per_dev = BLOCKS_DEV
    block_count = BLOCKS
    devices = block_count // per_dev
    level_key = jax.random.fold_in(key, 11)
    order_key = jax.random.fold_in(key, 12)
    pick_key = jax.random.fold_in(key, 13)
    classes = jax.random.randint(level_key, (devices,), 0, 4)
    levels = jnp.where(classes == 0, PER_OWNER, jnp.where(classes == 1, 1, 0)).astype(jnp.int32)
    levels = jnp.minimum(levels, PER_OWNER)
    levels = levels.at[0].set(PER_OWNER)
    block_ids = jnp.arange(block_count, dtype=jnp.int32)
    owner_ids = block_ids // per_dev
    local_ids = block_ids % per_dev
    raw_order = jax.random.randint(order_key, (devices, block_count), 0, 1 << 16)
    distinct = raw_order * per_dev + local_ids[None, :]
    grouped = distinct.reshape(devices, devices, per_dev)
    ranking = jnp.argsort(jnp.argsort(grouped, axis=2), axis=2).reshape(devices, block_count)
    requester = jnp.arange(devices, dtype=jnp.int32)
    allowed = (ranking < levels[owner_ids][None, :]) & (owner_ids[None, :] < requester[:, None])
    local_before = (owner_ids[None, :] == owner_ids[:, None]) & (block_ids[None, :] < block_ids[:, None])
    candidate = allowed[owner_ids] | local_before
    raw_pick = jax.random.randint(pick_key, (block_count, block_count), 0, 1 << 16)
    scores = jnp.where(candidate, raw_pick * block_count + block_ids[None, :], -1)
    best_scores, where_best = lax.top_k(scores, PICKS - 1)
    others = jnp.where(best_scores >= 0, where_best, -1).astype(jnp.int32)
    return jnp.concatenate([block_ids[:, None], others], axis=1).astype(jnp.int32)


def with_spikes(result, rng, source, target, shards_of, factor):
    def block_of(dim):
        return (jnp.arange(result.shape[dim]) // (result.shape[dim] // shards_of)).reshape((-1,) + (1,) * (result.ndim - 1 - dim))

    one_side = jax.random.permutation(rng, shards_of)[block_of(target)]
    far = (block_of(target) + shards_of // 2) % shards_of
    return jnp.where((block_of(source) == one_side) | (block_of(source) == far), factor * result, result)


def block_scale(stream_key, dims, cuts, smallest, high):
    gain = 1.0
    for position, shards_of in cuts:
        draws = jax.random.uniform(jax.random.fold_in(jax.random.fold_in(stream_key, 6), position), (shards_of,), jnp.float32, smallest / len(cuts), high / len(cuts))
        gain = gain * jnp.repeat(jnp.exp(draws), dims[position] // shards_of).reshape((-1,) + (1,) * (len(dims) - 1 - position))
    return gain


def bell_draw(own_key, dims, width, most, shards=(), kind=jnp.bfloat16):
    array = width * jax.random.normal(own_key, dims, jnp.float32)
    if shards:
        array = array * block_scale(own_key, dims, shards, -0.22, 0.18)
    return jnp.clip(array, -most, most).astype(kind)


def bell_draw_with(key, extent, width, limit, pieces, heavy, kind=jnp.bfloat16):
    drawn = width * jax.random.normal(key, extent, jnp.float32)
    if pieces:
        drawn = drawn * block_scale(key, extent, pieces, -0.22, 0.18)
    return jnp.clip(with_spikes(drawn, jax.random.fold_in(key, 3), *heavy), -limit, limit).astype(kind)


def setup_inputs(seed: int = 0) -> dict:
    splits = jax.random.split(jax.random.key(seed), 10)
    tokens = bell_draw(splits[0], (TOKENS, D), 1.0, 6.0, ((0, 32), (1, 8)))
    query_weight = bell_draw(splits[1], (D, HEADS * LATENT), D ** -0.5, 0.1875, ((1, 8),))
    latent_weight = bell_draw(splits[2], (D, LATENT), D ** -0.5, 0.1875)
    query_gain = jnp.clip(1.0 + 0.1 * jax.random.normal(splits[3], (LATENT,), jnp.float32), 0.5, 1.5)
    key_gain = jnp.clip(1.0 + 0.1 * jax.random.normal(splits[4], (LATENT,), jnp.float32), 0.5, 1.5)
    value_up = bell_draw(splits[5], (HEADS, LATENT, VDIM), LATENT ** -0.5, 0.5, ((0, 8),))
    out_weight = bell_draw_with(splits[6], (HEADS * VDIM, D), (HEADS * VDIM) ** -0.5, 0.25, ((0, 8),), (0, 1, 8, 2.0))
    out_gain = jnp.clip(1.0 + 0.1 * jax.random.normal(splits[7], (D,), jnp.float32), 0.5, 1.5)
    chosen = draw_chosen(jax.random.fold_in(splits[9], 71), 0)
    return {"tokens": tokens, "query_weight": query_weight, "latent_weight": latent_weight, "query_gain": query_gain, "key_gain": key_gain, "value_up": value_up, "out_weight": out_weight, "out_gain": out_gain, "chosen": chosen}


epsilon = 1e-06
masked_score = -1e+30

def rms_scale(values, gain_row):
    widened = values.astype(jnp.float32)
    mean_sq = lax.optimization_barrier(jnp.mean(widened * widened, axis=-1, keepdims=True))
    return (widened * lax.rsqrt(mean_sq + epsilon) * gain_row).astype(jnp.bfloat16)

def reference(tokens, query_weight, latent_weight, query_gain, key_gain, value_up, out_weight, out_gain, chosen):
    queries = jnp.dot(tokens, query_weight, preferred_element_type=jnp.float32).astype(jnp.bfloat16)
    queries = rms_scale(queries.reshape(TOKENS, HEADS, LATENT), query_gain)
    latent = jnp.dot(tokens, latent_weight, preferred_element_type=jnp.float32).astype(jnp.bfloat16)
    normed_keys = rms_scale(latent, key_gain)
    key_blocks = normed_keys.reshape(BLOCKS, BLOCK, LATENT)
    value_blocks = latent.reshape(BLOCKS, BLOCK, LATENT)
    query_blocks = queries.reshape(BLOCKS, BLOCK, HEADS, LATENT)
    offsets = jnp.arange(BLOCK, dtype=jnp.int32)

    def attend(packed):
        query_block, chosen_row, start_pos = packed
        clamped = jnp.maximum(chosen_row, 0).astype(jnp.int32)
        picked_keys = key_blocks[clamped].astype(jnp.float32)
        picked_values = value_blocks[clamped].astype(jnp.float32)
        scores = jnp.einsum('qhl,ckl->qhck', query_block.astype(jnp.float32), picked_keys) * LATENT ** (-0.5)
        key_pos = clamped[:, None] * BLOCK + offsets[None, :]
        query_pos = start_pos + offsets
        allowed = (chosen_row[:, None] >= 0)[None] & (key_pos[None] <= query_pos[:, None, None])
        allowed = allowed[:, None]
        scores = jnp.where(allowed, scores, masked_score)
        row_max = lax.optimization_barrier(jnp.max(scores, axis=(2, 3), keepdims=True))
        exp_scores = jnp.where(allowed, jnp.exp(scores - row_max), 0.0)
        weights = (exp_scores / lax.optimization_barrier(jnp.sum(exp_scores, axis=(2, 3), keepdims=True))).astype(jnp.bfloat16)
        attended = jnp.einsum('qhck,ckl->qhl', weights.astype(jnp.float32), picked_values)
        return attended.astype(jnp.bfloat16)
    block_starts = jnp.arange(BLOCKS, dtype=jnp.int32) * BLOCK
    attended = lax.map(attend, (query_blocks, chosen, block_starts))
    attended = attended.reshape(TOKENS, HEADS, LATENT)
    heads_out = jnp.einsum('thl,hlv->thv', attended.astype(jnp.float32), value_up.astype(jnp.float32))
    heads_out = heads_out.astype(jnp.bfloat16).reshape(TOKENS, HEADS * VDIM)
    projected = jnp.dot(heads_out, out_weight, preferred_element_type=jnp.float32)
    return rms_scale(projected, out_gain)
```

```python
import jax
import jax.numpy as jnp
from jax import lax
from jax.experimental import pallas as pl
from jax.experimental.pallas import tpu as pltpu
from jax.sharding import Mesh
from jax.sharding import PartitionSpec as P

BLOCK = 128
PER_OWNER = 2
KV = ("kv_0", "kv_1")
GROUP = 8
LOG2E = 1.4426950408889634


epsilon = 1e-06
masked_score = -1e30


def taken_in(shard, axis, dim, absorb, carry):
    whole = jax.tree.map(lambda part: lax.all_gather(part, axis, axis=dim, tiled=True), shard)
    return absorb(carry, whole, jnp.int32(0))


def split_up(shard, dim, length):
    return jnp.stack(jnp.split(shard, length, axis=dim))


def laid_out(parts, dim):
    lengths = list(parts.shape[1:])
    lengths[dim] *= parts.shape[0]
    return jnp.moveaxis(parts, 0, dim).reshape(lengths)


def exchange_in_order(parts, axes, turns):
    inside = parts.shape[1:]
    result = parts.reshape(*(lax.axis_size(a) for a in axes), *inside)
    for k in turns:
        result = lax.all_to_all(result, axes[k], k, k, tiled=True)
    return result.reshape(-1, *inside)


def one_axis_at_a_time(shard, axes, turns, split_dim, concat_dim):
    parts = split_up(shard, split_dim, lax.axis_size(axes))
    return laid_out(exchange_in_order(parts, axes, turns), concat_dim)


def attend_block(slots_ref, query_ref, pool_ref, query_gain_ref, key_gain_ref, up_ref, out_ref, keys, values):
    step = pl.program_id(0)
    width = pool_ref.shape[1]
    heads = up_ref.shape[0]
    picks = slots_ref.shape[1]
    pool_rows = pool_ref.shape[0]

    @pl.when(step == 0)
    def _():
        def prepare(j, carry):
            rows = pl.ds(pl.multiple_of(j * 2 * BLOCK, 2 * BLOCK), 2 * BLOCK)
            latent = pool_ref[rows, :]
            wide = latent.astype(jnp.float32)
            mean_sq = jnp.mean(wide * wide, axis=-1, keepdims=True)
            keys[rows, :] = (wide * lax.rsqrt(mean_sq + epsilon) * key_gain_ref[...]).astype(jnp.bfloat16)
            values[rows, :width] = latent
            values[rows, width:] = jnp.ones((2 * BLOCK, width), jnp.bfloat16)
            return carry

        lax.fori_loop(0, pool_rows // (2 * BLOCK), prepare, 0)
        keys[pool_rows:, :] = jnp.zeros((BLOCK, width), jnp.bfloat16)
        values[pool_rows:, :] = jnp.zeros((BLOCK, 2 * width), jnp.bfloat16)

    scale = width ** (-0.5) * LOG2E
    parts = []
    for h in range(heads):
        wide = query_ref[:, h * width : (h + 1) * width].astype(jnp.float32)
        mean_sq = jnp.mean(wide * wide, axis=-1, keepdims=True)
        parts.append((wide * lax.rsqrt(mean_sq + epsilon) * (query_gain_ref[...] * scale)).astype(jnp.bfloat16))
    queries = jnp.concatenate(parts, axis=0)

    def rows_of(c):
        return pl.ds(pl.multiple_of(slots_ref[step, c] * BLOCK, BLOCK), BLOCK)

    def group(first, masked):
        places = [rows_of(first + i) for i in range(GROUP)]
        picked = jnp.concatenate([keys[r, :] for r in places], axis=0)
        scores = lax.dot_general(
            queries, picked, (((1,), (1,)), ((), ())), preferred_element_type=jnp.float32
        )
        if masked:
            row = lax.broadcasted_iota(jnp.int32, scores.shape, 0) % BLOCK
            col = lax.broadcasted_iota(jnp.int32, scores.shape, 1)
            scores = jnp.where((col <= row) | (col >= BLOCK), scores, masked_score)
        weights = jnp.exp2(scores).astype(jnp.bfloat16)
        held = jnp.concatenate([values[r, :] for r in places], axis=0)
        return jnp.dot(weights, held, preferred_element_type=jnp.float32)

    total = group(0, True)
    total = lax.fori_loop(1, picks // GROUP, lambda g, t: t + group(g * GROUP, False), total)
    attended = (total[:, :width] / total[:, width:]).astype(jnp.bfloat16)
    outs = [
        jnp.dot(attended[h * BLOCK : (h + 1) * BLOCK], up_ref[h], preferred_element_type=jnp.float32)
        for h in range(heads)
    ]
    out_ref[...] = jnp.concatenate(outs, axis=1).astype(jnp.bfloat16)


def attention(slots, queries, pool, query_gain, key_gain, value_up):
    rows, cols = queries.shape
    pool_rows, width = pool.shape
    heads, _, vdim = value_up.shape
    whole = pl.BlockSpec(memory_space=pltpu.VMEM)
    return pl.pallas_call(
        attend_block,
        grid=(rows // BLOCK,),
        out_shape=jax.ShapeDtypeStruct((rows, heads * vdim), jnp.bfloat16),
        in_specs=[
            pl.BlockSpec(memory_space=pltpu.SMEM),
            pl.BlockSpec((BLOCK, cols), lambda b: (b, 0)),
            whole,
            whole,
            whole,
            whole,
        ],
        out_specs=pl.BlockSpec((BLOCK, heads * vdim), lambda b: (b, 0)),
        scratch_shapes=[
            pltpu.VMEM((pool_rows + BLOCK, width), jnp.bfloat16),
            pltpu.VMEM((pool_rows + BLOCK, 2 * width), jnp.bfloat16),
        ],
    )(slots, queries, pool, query_gain, key_gain, value_up)


def shards(
    tokens,
    query_weight,
    latent_weight,
    query_gain,
    key_gain,
    value_up,
    out_weight,
    out_gain,
    chosen,
):
    tok_rows = tokens.shape[0]
    head_cols = query_weight.shape[1]
    lat_width = latent_weight.shape[1]
    local_heads = head_cols // lat_width
    block_size = BLOCK
    blocks_dev = tok_rows // block_size
    owners = lax.axis_size(KV)
    my_owner = lax.axis_index(KV)

    def project(totals, shard_piece, offset):
        query_rows = lax.dynamic_slice_in_dim(query_weight, offset, shard_piece.shape[1], 0)
        latent_rows = lax.dynamic_slice_in_dim(latent_weight, offset, shard_piece.shape[1], 0)
        return (
            totals[0] + jnp.dot(shard_piece, query_rows, preferred_element_type=jnp.float32),
            totals[1] + jnp.dot(shard_piece, latent_rows, preferred_element_type=jnp.float32),
        )

    query_zero = jnp.zeros((tok_rows, head_cols), jnp.float32)
    latent_zero = jnp.zeros((tok_rows, lat_width), jnp.float32)
    query_acc, latent_acc = taken_in(tokens, "tp", 1, project, (query_zero, latent_zero))
    latent = latent_acc.astype(jnp.bfloat16)
    latent_blocks = latent.reshape(blocks_dev, block_size, lat_width)
    clamped = jnp.maximum(chosen, 0)
    owner_of = clamped // blocks_dev
    index_in = clamped % blocks_dev
    flat_owner = owner_of.reshape(-1)
    flat_index = index_in.reshape(-1)
    remote = (chosen.reshape(-1) >= 0) & (flat_owner != my_owner)
    owner_ids = jnp.arange(owners, dtype=jnp.int32)
    local_ids = jnp.arange(blocks_dev, dtype=jnp.int32)
    matches = (
        remote[:, None, None]
        & (flat_owner[:, None, None] == owner_ids[None, :, None])
        & (flat_index[:, None, None] == local_ids[None, None, :])
    )
    needed = jnp.any(matches, axis=0)
    ranking = jnp.cumsum(needed.astype(jnp.int32), axis=1) - 1
    slot_ids = jnp.arange(PER_OWNER, dtype=jnp.int32)
    placed = needed[:, None, :] & (ranking[:, None, :] == slot_ids[None, :, None])
    wanted = jnp.where(
        jnp.any(placed, axis=2), jnp.sum(jnp.where(placed, local_ids[None, None, :], 0), axis=2), -1
    )
    requested = one_axis_at_a_time(wanted, KV, (0, 1), 0, 0)
    served = latent_blocks[jnp.maximum(requested, 0)]
    served = jnp.where((requested >= 0)[:, :, None, None], served, jnp.zeros_like(served))
    arrived = lax.all_to_all(served, KV, split_axis=0, concat_axis=0, tiled=True)
    block_pool = jnp.concatenate(
        [latent_blocks, arrived.reshape(owners * PER_OWNER, block_size, lat_width)], axis=0
    )
    slot_of = jnp.sum(jnp.where(wanted[owner_of] == index_in[:, :, None], slot_ids, 0), axis=2)
    where_from = jnp.where(
        owner_of == my_owner, index_in, blocks_dev + owner_of * PER_OWNER + slot_of
    )
    pool_count = block_pool.shape[0]
    slots = jnp.where(chosen >= 0, where_from, pool_count).astype(jnp.int32)
    heads_out = attention(
        slots,
        query_acc.astype(jnp.bfloat16),
        block_pool.reshape(pool_count * block_size, lat_width),
        query_gain.reshape(1, lat_width),
        key_gain.reshape(1, lat_width),
        value_up,
    )
    model_width = out_weight.shape[1]
    tp_count = lax.axis_size("tp")
    feature_rows = model_width // tp_count
    gain_part = lax.dynamic_slice_in_dim(
        out_gain, lax.axis_index("tp") * feature_rows, feature_rows, 0
    )
    column_block = lax.all_to_all(out_weight, "tp", split_axis=1, concat_axis=0, tiled=True)

    def contract(total, head_piece, offset):
        weight_rows = lax.dynamic_slice_in_dim(column_block, offset, head_piece.shape[1], 0)
        return total + jnp.dot(head_piece, weight_rows, preferred_element_type=jnp.float32)

    empty_cols = jnp.zeros((tok_rows, feature_rows), jnp.float32)
    summed = taken_in(heads_out, "tp", 1, contract, empty_cols)
    squares = lax.psum(jnp.sum(summed * summed, axis=1), "tp")
    mixed_out = (summed * lax.rsqrt(squares / model_width + epsilon)[:, None] * gain_part).astype(
        jnp.bfloat16
    )
    return mixed_out


def solution(mesh):
    torus = Mesh(mesh.devices.reshape(8, 4, mesh.shape["tp"]), ("kv_0", "kv_1", "tp"))
    in_specs = (
        P(KV, "tp"),
        P(None, "tp"),
        P(),
        P(),
        P(),
        P("tp", None, None),
        P("tp", None),
        P(),
        P(KV, None),
    )
    out_specs = P(KV, "tp")
    return jax.shard_map(
        shards, mesh=torus, in_specs=in_specs, out_specs=out_specs, check_vma=False
    )
```

```python
import jax
import jax.numpy as jnp
from jax import lax
from jax.experimental import pallas as pl
from jax.experimental.pallas import tpu as pltpu
from jax.sharding import PartitionSpec as P

BLOCK = 128
PER_OWNER = 2
MESH = pl.DeviceIdType.MESH
GROUP = 8
LOG2E = 1.4426950408889634


epsilon = 1e-06
masked_score = -1e30


def taken_in(shard, axis, dim, absorb, carry):
    whole = jax.tree.map(lambda part: lax.all_gather(part, axis, axis=dim, tiled=True), shard)
    return absorb(carry, whole, jnp.int32(0))


def neighbours(tp):
    side = lax.rem(tp, 2)
    right = lax.rem(tp + 2, 8)
    left = lax.rem(tp + 6, 8)
    far = lax.rem(tp + 4, 8)
    return right, left, far, tp + 1 - 2 * side


class Spread:
    def __init__(self, full, first, size, send_sem, recv_sem):
        self.full, self.send_sem, self.recv_sem = full, send_sem, recv_sem
        half = size // 2
        self.ranges = ((first, half), (first + half, size - half))
        self.tp = lax.axis_index("tp")
        self.right, self.left, self.far, self.other = neighbours(self.tp)

    def copy(self, slot, part, dest, kind):
        first, size = self.ranges[part]
        piece = self.full.at[slot, pl.ds(first, size)]
        return pltpu.make_async_remote_copy(
            src_ref=piece,
            dst_ref=piece,
            send_sem=self.send_sem.at[kind],
            recv_sem=self.recv_sem.at[slot, part],
            device_id={"tp": dest},
            device_id_type=MESH,
        )

    def sends(self):
        me, right, left, far, other = self.tp, self.right, self.left, self.far, self.other
        return (
            (me, 0, right), (me, 1, left), (me, 1, right), (me, 0, left), (me, 0, other), (me, 1, other),
            (left, 0, right), (right, 1, left), (left, 0, other), (right, 1, other), (left, 1, other),
            (right, 0, other), (far, 0, other), (far, 1, other),
        )

    def start(self, *kinds):
        every = self.sends()
        for kind in kinds:
            self.copy(*every[kind], kind).start()

    def arrived(self, slot, part):
        self.copy(slot, part, self.other, 0).wait_recv()

    def own(self):
        self.start(0, 1, 2, 3, 4, 5)

    def relay_first(self):
        self.arrived(self.left, 0)
        self.start(6, 8)
        self.arrived(self.right, 1)
        self.start(7, 9)

    def relay_rest(self):
        self.arrived(self.left, 1)
        self.start(10)
        self.arrived(self.right, 0)
        self.start(11)
        self.arrived(self.far, 0)
        self.start(12)
        self.arrived(self.far, 1)
        self.start(13)

    def finish(self):
        side = 1 - 2 * lax.rem(self.tp, 2)
        for slot in (self.other, self.left + side, self.right + side, self.far + side):
            for part in (0, 1):
                self.arrived(slot, part)
        for kind, (slot, part, dest) in enumerate(self.sends()):
            self.copy(slot, part, dest, kind).wait_send()


def collect_kernel(
    chosen, tokens, latent_weight,
    full, pool, table,
    weight, rows, asked, asks, served,
    local_sem, rows_send, rows_recv, ask_send, ask_recv, serve_send, serve_recv,
    tok_send, tok_recv, here_send, here_recv, low_send, low_recv, high_send, high_recv,
):
    kv, tp = lax.axis_index("kv"), lax.axis_index("tp")
    owners = asked.shape[0]
    peers = full.shape[0]
    blocks, groups = rows.shape[1], peers
    group = rows.shape[2]

    own_tokens = pltpu.make_async_copy(tokens, full.at[tp], local_sem.at[0])
    own_tokens.start()
    own_weight = pltpu.make_async_copy(latent_weight, weight, local_sem.at[1])
    own_weight.start()

    barrier = pltpu.get_barrier_semaphore()

    def greet_tp(step, carry):
        pl.semaphore_signal(barrier, inc=1, device_id={"tp": lax.rem(tp + step, peers)}, device_id_type=MESH)
        return carry

    def greet_kv(step, carry):
        pl.semaphore_signal(barrier, inc=1, device_id={"kv": lax.rem(kv + step, owners)}, device_id_type=MESH)
        return carry

    lax.fori_loop(1, owners, greet_kv, 0)
    lax.fori_loop(1, peers, greet_tp, 0)

    tile = (blocks, 128)
    lane = lax.broadcasted_iota(jnp.int32, tile, 1)
    ids = lane * blocks + lax.broadcasted_iota(jnp.int32, tile, 0)

    def mark(b, needed):
        for c in range(chosen.shape[1]):
            needed = jnp.where(ids == chosen[b, c], 1, needed)
        return needed

    needed = lax.fori_loop(0, blocks, mark, jnp.zeros(tile, jnp.int32))
    first = jnp.full((1, 128), -1, jnp.int32)
    second = first
    for j in reversed(range(blocks)):
        hit = needed[j : j + 1, :] > 0
        second = jnp.where(hit, first, second)
        first = jnp.where(hit, j, first)
    sub = lax.broadcasted_iota(jnp.int32, tile, 0)
    listed = jnp.where(sub == 0, first, jnp.where(sub == 1, second, 0))
    table[...] = listed
    wide = listed.astype(jnp.float32)

    def write_ask(o, carry):
        asks[o] = jnp.broadcast_to(jnp.sum(jnp.where(lane == o, wide, 0.0), axis=1, keepdims=True), tile)
        return carry

    lax.fori_loop(0, owners, write_ask, 0)
    own_tokens.wait()
    pl.semaphore_wait(barrier, owners + peers - 2)

    def rows_copy(to):
        return pltpu.make_async_remote_copy(
            src_ref=full.at[tp, :, to],
            dst_ref=rows.at[tp],
            send_sem=rows_send.at[to],
            recv_sem=rows_recv.at[tp],
            device_id={"tp": to},
            device_id_type=MESH,
        )

    def rows_arrival(source):
        return pltpu.make_async_remote_copy(
            src_ref=rows.at[source],
            dst_ref=rows.at[source],
            send_sem=rows_send.at[source],
            recv_sem=rows_recv.at[source],
            device_id={"tp": source},
            device_id_type=MESH,
        )

    def ask_copy(owner, slot):
        return pltpu.make_async_remote_copy(
            src_ref=asks.at[owner],
            dst_ref=asked.at[slot],
            send_sem=ask_send.at[owner],
            recv_sem=ask_recv.at[slot],
            device_id={"kv": owner},
            device_id_type=MESH,
        )

    def serve_copy(to, slot):
        return pltpu.make_async_remote_copy(
            src_ref=served.at[to],
            dst_ref=pool.at[tp, pl.ds(blocks + slot * PER_OWNER, PER_OWNER)],
            send_sem=serve_send.at[to],
            recv_sem=serve_recv.at[slot],
            device_id={"kv": to},
            device_id_type=MESH,
        )

    def each(low, high, act):
        def step(i, carry):
            act(i)
            return carry

        lax.fori_loop(low, high, step, 0)

    each(1, peers, lambda i: rows_copy(lax.rem(tp + i, peers)).start())
    each(0, kv, lambda o: ask_copy(o, kv).start())
    flat = full.reshape(peers, blocks * groups, group, 128)
    token_spread = Spread(flat, 0, blocks * groups, tok_send, tok_recv)
    token_spread.own()

    rows[tp] = full[tp, :, tp]
    own_weight.wait()
    each(1, peers, lambda i: rows_arrival(lax.rem(tp + i, peers)).wait_recv())
    lines = blocks * group
    latent = jnp.zeros((lines, 128), jnp.float32)
    for p in range(peers):
        latent += jnp.dot(
            rows[p].reshape(lines, 128), weight[p * 128 : (p + 1) * 128, :], preferred_element_type=jnp.float32
        )
    latent = latent.astype(jnp.bfloat16).reshape(blocks, group, 128)
    pool[tp, 0:blocks] = latent
    latent = latent.astype(jnp.float32)

    def serve(r):
        ask_copy(r, r).wait_recv()
        for k in range(PER_OWNER):
            want = asked[r, k : k + 1, :]
            picked = jnp.zeros((group, 128), jnp.float32)
            for j in range(blocks):
                picked = jnp.where(want == float(j), latent[j], picked)
            served[r, k] = picked.astype(jnp.bfloat16)
        serve_copy(r, kv).start()

    each(kv + 1, owners, serve)
    half = owners * PER_OWNER // 2
    here = Spread(pool, 0, blocks, here_send, here_recv)
    low = Spread(pool, blocks, half, low_send, low_recv)
    high = Spread(pool, blocks + half, half, high_send, high_recv)
    here.own()
    token_spread.relay_first()

    each(0, jnp.minimum(kv, owners // 2), lambda o: serve_copy(o, o).wait_recv())
    low.own()
    each(owners // 2, jnp.maximum(kv, owners // 2), lambda o: serve_copy(o, o).wait_recv())
    high.own()
    token_spread.relay_rest()
    here.relay_first()
    low.relay_first()
    high.relay_first()
    here.relay_rest()
    low.relay_rest()
    high.relay_rest()
    each(1, peers, lambda i: rows_copy(lax.rem(tp + i, peers)).wait_send())
    each(0, kv, lambda o: ask_copy(o, kv).wait_send())
    each(kv + 1, owners, lambda r: serve_copy(r, kv).wait_send())
    for spread in (token_spread, here, low, high):
        spread.finish()


def collect(chosen, tokens, latent_weight):
    peers, owners = lax.axis_size("tp"), lax.axis_size("kv")
    blocks = chosen.shape[0]
    rows, width = tokens.shape
    group = BLOCK // peers
    slots = blocks + owners * PER_OWNER
    vmem = pl.BlockSpec(memory_space=pltpu.VMEM)
    dma = pltpu.SemaphoreType.DMA
    full, pool, table = pl.pallas_call(
        collect_kernel,
        out_shape=(
            jax.ShapeDtypeStruct((peers, blocks, peers, group, width), jnp.bfloat16),
            jax.ShapeDtypeStruct((peers, slots, group, 128), jnp.bfloat16),
            jax.ShapeDtypeStruct((blocks, 128), jnp.int32),
        ),
        in_specs=[
            pl.BlockSpec(memory_space=pltpu.SMEM),
            pl.BlockSpec(memory_space=pl.ANY),
            pl.BlockSpec(memory_space=pl.ANY),
        ],
        out_specs=(vmem, vmem, vmem),
        scratch_shapes=[
            pltpu.VMEM(latent_weight.shape, jnp.bfloat16),
            pltpu.VMEM((peers, blocks, group, width), jnp.bfloat16),
            pltpu.VMEM((owners, blocks, 128), jnp.float32),
            pltpu.VMEM((owners, blocks, 128), jnp.float32),
            pltpu.VMEM((owners, PER_OWNER, group, 128), jnp.bfloat16),
            dma((2,)),
            dma((peers,)), dma((peers,)),
            dma((owners,)), dma((owners,)),
            dma((owners,)), dma((owners,)),
            dma((14,)), dma((peers, 2)),
            dma((14,)), dma((peers, 2)),
            dma((14,)), dma((peers, 2)),
            dma((14,)), dma((peers, 2)),
        ],
        compiler_params=pltpu.CompilerParams(collective_id=0, has_side_effects=True),
    )(chosen, tokens.reshape(blocks, peers, group, width), latent_weight)
    return full.reshape(peers, rows, width), pool, table


def attend_block(
    chosen_ref, table_ref, tokens_ref, weight_ref, pool_ref, query_gain_ref, key_gain_ref, up_ref, out_ref, keys, values
):
    step = pl.program_id(0)
    kv = lax.axis_index("kv")
    peers, slots, group, width = pool_ref.shape
    heads = up_ref.shape[0]
    blocks, picks = chosen_ref.shape

    @pl.when(step == 0)
    def _():
        def prepare(j, carry):
            rows = pl.ds(pl.multiple_of(j * 2 * BLOCK, 2 * BLOCK), 2 * BLOCK)
            latent = jnp.concatenate(
                [pool_ref[:, 2 * j + i].reshape(BLOCK, width) for i in range(2)], axis=0
            )
            wide = latent.astype(jnp.float32)
            mean_sq = jnp.mean(wide * wide, axis=-1, keepdims=True)
            keys[rows, :] = (wide * lax.rsqrt(mean_sq + epsilon) * key_gain_ref[...]).astype(jnp.bfloat16)
            values[rows, :width] = latent
            values[rows, width:] = jnp.ones((2 * BLOCK, width), jnp.bfloat16)
            return carry

        lax.fori_loop(0, slots // 2, prepare, 0)
        keys[slots * BLOCK :, :] = jnp.zeros((BLOCK, width), jnp.bfloat16)
        values[slots * BLOCK :, :] = jnp.zeros((BLOCK, 2 * width), jnp.bfloat16)

    scale = width ** (-0.5) * LOG2E
    lines = pl.ds(pl.multiple_of(step * BLOCK, BLOCK), BLOCK)
    features = jnp.concatenate([tokens_ref[p, lines, :] for p in range(peers)], axis=1)
    projected = jnp.dot(features, weight_ref[...], preferred_element_type=jnp.float32).astype(jnp.bfloat16)
    parts = []
    for h in range(heads):
        wide = projected[:, h * width : (h + 1) * width].astype(jnp.float32)
        mean_sq = jnp.mean(wide * wide, axis=-1, keepdims=True)
        parts.append((wide * lax.rsqrt(mean_sq + epsilon) * (query_gain_ref[...] * scale)).astype(jnp.bfloat16))
    queries = jnp.concatenate(parts, axis=0)

    def rows_of(c):
        block = chosen_ref[step, c]
        held = jnp.maximum(block, 0)
        owner = lax.shift_right_logical(held, 3)
        inside = lax.bitwise_and(held, 7)
        remote = blocks + owner * PER_OWNER + jnp.where(table_ref[1, owner] == inside, 1, 0)
        slot = jnp.where(block < 0, slots, jnp.where(owner == kv, inside, remote))
        return pl.ds(pl.multiple_of(slot * BLOCK, BLOCK), BLOCK)

    def group(first, masked):
        places = [rows_of(first + i) for i in range(GROUP)]
        picked = jnp.concatenate([keys[r, :] for r in places], axis=0)
        scores = lax.dot_general(
            queries, picked, (((1,), (1,)), ((), ())), preferred_element_type=jnp.float32
        )
        if masked:
            row = lax.broadcasted_iota(jnp.int32, scores.shape, 0) % BLOCK
            col = lax.broadcasted_iota(jnp.int32, scores.shape, 1)
            scores = jnp.where((col <= row) | (col >= BLOCK), scores, masked_score)
        weights = jnp.exp2(scores).astype(jnp.bfloat16)
        held = jnp.concatenate([values[r, :] for r in places], axis=0)
        return jnp.dot(weights, held, preferred_element_type=jnp.float32)

    total = group(0, True)
    total = lax.fori_loop(1, picks // GROUP, lambda g, t: t + group(g * GROUP, False), total)
    attended = (total[:, :width] / total[:, width:]).astype(jnp.bfloat16)
    outs = [
        jnp.dot(attended[h * BLOCK : (h + 1) * BLOCK], up_ref[h], preferred_element_type=jnp.float32)
        for h in range(heads)
    ]
    out_ref[...] = jnp.concatenate(outs, axis=1).astype(jnp.bfloat16)


def attention(chosen, table, tokens, query_weight, pool, query_gain, key_gain, value_up):
    peers, rows, _ = tokens.shape
    _, slots, _, width = pool.shape
    heads, _, vdim = value_up.shape
    whole = pl.BlockSpec(memory_space=pltpu.VMEM)
    smem = pl.BlockSpec(memory_space=pltpu.SMEM)
    return pl.pallas_call(
        attend_block,
        grid=(rows // BLOCK,),
        out_shape=jax.ShapeDtypeStruct((rows, heads * vdim), jnp.bfloat16),
        in_specs=[smem, smem, whole, whole, whole, whole, whole, whole],
        out_specs=pl.BlockSpec((BLOCK, heads * vdim), lambda b: (b, 0)),
        scratch_shapes=[
            pltpu.VMEM(((slots + 1) * BLOCK, width), jnp.bfloat16),
            pltpu.VMEM(((slots + 1) * BLOCK, 2 * width), jnp.bfloat16),
        ],
    )(chosen, table, tokens, query_weight, pool, query_gain, key_gain, value_up)


def shards(
    tokens,
    query_weight,
    latent_weight,
    query_gain,
    key_gain,
    value_up,
    out_weight,
    out_gain,
    chosen,
):
    tok_rows = tokens.shape[0]
    lat_width = latent_weight.shape[1]
    full, pool, table = collect(chosen, tokens, latent_weight)
    heads_out = attention(
        chosen, table, full, query_weight, pool,
        query_gain.reshape(1, lat_width), key_gain.reshape(1, lat_width), value_up,
    )
    model_width = out_weight.shape[1]
    tp_count = lax.axis_size("tp")
    feature_rows = model_width // tp_count
    gain_part = lax.dynamic_slice_in_dim(
        out_gain, lax.axis_index("tp") * feature_rows, feature_rows, 0
    )
    column_block = lax.all_to_all(out_weight, "tp", split_axis=1, concat_axis=0, tiled=True)

    def contract(total, head_piece, offset):
        weight_rows = lax.dynamic_slice_in_dim(column_block, offset, head_piece.shape[1], 0)
        return total + jnp.dot(head_piece, weight_rows, preferred_element_type=jnp.float32)

    empty_cols = jnp.zeros((tok_rows, feature_rows), jnp.float32)
    summed = taken_in(heads_out, "tp", 1, contract, empty_cols)
    squares = lax.psum(jnp.sum(summed * summed, axis=1), "tp")
    mixed_out = (summed * lax.rsqrt(squares / model_width + epsilon)[:, None] * gain_part).astype(
        jnp.bfloat16
    )
    return mixed_out


def solution(mesh):
    in_specs = (
        P("kv", "tp"),
        P(None, "tp"),
        P(),
        P(),
        P(),
        P("tp", None, None),
        P("tp", None),
        P(),
        P("kv", None),
    )
    out_specs = P("kv", "tp")
    return jax.shard_map(
        shards, mesh=mesh, in_specs=in_specs, out_specs=out_specs, check_vma=False
    )
```

```python
import jax
import jax.numpy as jnp
from jax import lax
from jax.experimental import pallas as pl
from jax.experimental.pallas import tpu as pltpu
from jax.sharding import PartitionSpec as P

BLOCK = 128
PER_OWNER = 2
MESH = pl.DeviceIdType.MESH
GROUP = 8
PIECES = 4
ONES = 16
HALF = 4
LOG2E = 1.4426950408889634


epsilon = 1e-06
masked_score = -1e30


def neighbours(tp):
    side = lax.rem(tp, 2)
    right = lax.rem(tp + 2, 8)
    left = lax.rem(tp + 6, 8)
    far = lax.rem(tp + 4, 8)
    return right, left, far, tp + 1 - 2 * side


class Spread:
    def __init__(self, full, first, size, send_sem, recv_sem):
        self.full, self.send_sem, self.recv_sem = full, send_sem, recv_sem
        half = size // 2
        self.ranges = ((first, half), (first + half, size - half))
        self.tp = lax.axis_index("tp")
        self.right, self.left, self.far, self.other = neighbours(self.tp)

    def copy(self, slot, part, dest, kind):
        first, size = self.ranges[part]
        piece = self.full.at[slot, pl.ds(first, size)]
        return pltpu.make_async_remote_copy(
            src_ref=piece,
            dst_ref=piece,
            send_sem=self.send_sem.at[kind],
            recv_sem=self.recv_sem.at[slot, part],
            device_id={"tp": dest},
            device_id_type=MESH,
        )

    def sends(self):
        me, right, left, far, other = self.tp, self.right, self.left, self.far, self.other
        return (
            (me, 0, right), (me, 1, left), (me, 1, right), (me, 0, left), (me, 0, other), (me, 1, other),
            (left, 0, right), (right, 1, left), (left, 0, other), (right, 1, other), (left, 1, other),
            (right, 0, other), (far, 0, other), (far, 1, other),
        )

    def start(self, *kinds):
        every = self.sends()
        for kind in kinds:
            self.copy(*every[kind], kind).start()

    def arrived(self, slot, part):
        self.copy(slot, part, self.other, 0).wait_recv()

    def own(self):
        self.start(0, 1, 2, 3, 4, 5)

    def relay_first(self):
        self.arrived(self.left, 0)
        self.start(6, 8)
        self.arrived(self.right, 1)
        self.start(7, 9)

    def relay_rest(self):
        self.arrived(self.left, 1)
        self.start(10)
        self.arrived(self.right, 0)
        self.start(11)
        self.arrived(self.far, 0)
        self.start(12)
        self.arrived(self.far, 1)
        self.start(13)

    def finish(self):
        side = 1 - 2 * lax.rem(self.tp, 2)
        for slot in (self.other, self.left + side, self.right + side, self.far + side):
            for part in (0, 1):
                self.arrived(slot, part)

    def drain(self):
        for kind, (slot, part, dest) in enumerate(self.sends()):
            self.copy(slot, part, dest, kind).wait_send()


def each(low, high, act):
    def step(i, carry):
        act(i)
        return carry

    lax.fori_loop(low, high, step, 0)


def remote(source, target, send_sem, recv_sem, axis, to):
    return pltpu.make_async_remote_copy(
        src_ref=source,
        dst_ref=target,
        send_sem=send_sem,
        recv_sem=recv_sem,
        device_id={axis: to},
        device_id_type=MESH,
    )


def unit(values, gain_row):
    mean_sq = jnp.mean(values * values, axis=-1, keepdims=True)
    return (values * lax.rsqrt(mean_sq + epsilon) * gain_row).astype(jnp.bfloat16)


def kernel(
    chosen, tokens, latent_weight, query_weight, out_weight, query_gain, key_gain, up, out_gain,
    out,
    full, pool, wide_weight, weight, projection, rows, asked, asks, served, listed, table,
    queries, keys, values, staged, heads, finished,
    local_sem, rows_send, rows_recv, ask_send, ask_recv, serve_send, serve_recv,
    heads_send, heads_recv, out_send, out_recv, spread_send, spread_recv,
):
    kv, tp = lax.axis_index("kv"), lax.axis_index("tp")
    owners, peers = asked.shape[0], full.shape[0]
    blocks, group, width = rows.shape[1:]
    picks = chosen.shape[1]
    slots = pool.shape[1]
    lines = blocks * group

    own_tokens = pltpu.make_async_copy(tokens, full.at[tp], local_sem.at[0])
    own_latent = pltpu.make_async_copy(latent_weight, weight, local_sem.at[1])
    own_query = pltpu.make_async_copy(query_weight, projection, local_sem.at[2])
    own_out = pltpu.make_async_copy(out_weight, wide_weight.at[tp], local_sem.at[3])
    for copy in (own_tokens, own_latent, own_query, own_out):
        copy.start()

    barrier = pltpu.get_barrier_semaphore()

    def greet(axis, index, size):
        def signal(step):
            pl.semaphore_signal(barrier, inc=1, device_id={axis: lax.rem(index + step, size)}, device_id_type=MESH)

        each(1, size, signal)

    greet("kv", kv, owners)
    greet("tp", tp, peers)

    tile = (blocks, 128)
    lane = lax.broadcasted_iota(jnp.int32, tile, 1)
    sub = lax.broadcasted_iota(jnp.int32, tile, 0)
    ids = lane * blocks + sub

    def mark(b, needed):
        for c in range(picks):
            needed = jnp.where(ids == chosen[b, c], 1, needed)
        return needed

    needed = lax.fori_loop(0, blocks, mark, jnp.zeros(tile, jnp.int32))
    first = jnp.full((1, 128), -1, jnp.int32)
    second = first
    for j in reversed(range(blocks)):
        hit = needed[j : j + 1, :] > 0
        second = jnp.where(hit, first, second)
        first = jnp.where(hit, j, first)
    both = jnp.where(sub == 0, first, jnp.where(sub == 1, second, 0))
    listed[...] = both
    to_scalars = pltpu.make_async_copy(listed, table, local_sem.at[4])
    to_scalars.start()
    both = both.astype(jnp.float32)

    def write_ask(o):
        asks[o] = jnp.broadcast_to(jnp.sum(jnp.where(lane == o, both, 0.0), axis=1, keepdims=True), tile)

    each(0, owners, write_ask)
    own_tokens.wait()
    pl.semaphore_wait(barrier, owners + peers - 2)

    def rows_copy(to, slot):
        return remote(full.at[tp, :, to], rows.at[slot], rows_send.at[to], rows_recv.at[slot], "tp", to)

    def ask_copy(to, slot):
        return remote(asks.at[to], asked.at[slot], ask_send.at[to], ask_recv.at[slot], "kv", to)

    def serve_copy(to, slot):
        target = pool.at[tp, pl.ds(blocks + slot * PER_OWNER, PER_OWNER)]
        return remote(served.at[to], target, serve_send.at[to], serve_recv.at[slot], "kv", to)

    def peer(i):
        return lax.rem(tp + i, peers)

    each(1, peers, lambda i: rows_copy(peer(i), tp).start())
    each(0, kv, lambda o: ask_copy(o, kv).start())
    token_spread = Spread(
        full.reshape(peers, blocks * peers, group, width), 0, blocks * peers, spread_send.at[0], spread_recv.at[0]
    )
    token_spread.own()

    rows[tp] = full[tp, :, tp]
    own_latent.wait()
    each(1, peers, lambda i: rows_copy(peer(i), peer(i)).wait_recv())
    features = jnp.concatenate([rows[p].reshape(lines, width) for p in range(peers)], axis=1)
    latent = jnp.dot(features, weight[...], preferred_element_type=jnp.float32)
    latent = latent.astype(jnp.bfloat16).reshape(blocks, group, 128)
    pool[tp, 0:blocks] = latent
    latent = latent.astype(jnp.float32)

    def serve(i):
        r = owners - 1 - i
        ask_copy(r, r).wait_recv()
        for k in range(PER_OWNER):
            want = asked[r, k : k + 1, :]
            picked = jnp.zeros((group, 128), jnp.float32)
            for j in range(blocks):
                picked = jnp.where(want == float(j), latent[j], picked)
            served[r, k] = picked.astype(jnp.bfloat16)
        serve_copy(r, kv).start()

    each(0, owners - 1 - kv, serve)
    here = Spread(pool, 0, blocks, spread_send.at[1], spread_recv.at[1])
    here.own()

    share = owners // PIECES
    spreads = [
        Spread(pool, blocks + i * share * PER_OWNER, share * PER_OWNER, spread_send.at[2 + i], spread_recv.at[2 + i])
        for i in range(PIECES)
    ]

    def gathered(i):
        low = i * share
        each(low, jnp.clip(kv, low, low + share), lambda o: serve_copy(o, o).wait_recv())
        spreads[i].own()

    scale = width ** (-0.5) * LOG2E
    query_row = query_gain[...] * scale

    def project(b):
        features = jnp.concatenate([full[p, b].reshape(BLOCK, width) for p in range(peers)], axis=1)
        projected = jnp.dot(features, projection[...], preferred_element_type=jnp.float32)
        projected = projected.astype(jnp.bfloat16).astype(jnp.float32)
        for h in range(up.shape[0]):
            queries[b, h * BLOCK : (h + 1) * BLOCK, :] = unit(projected[:, h * 128 : (h + 1) * 128], query_row)

    def prepare(low, high):
        def pair(j):
            for i in range(2):
                slot = low + 2 * j + i
                block = pool[:, slot].reshape(BLOCK, width).astype(jnp.float32)
                keys[slot] = unit(block, key_gain[...])
                values[slot, :BLOCK, :] = jnp.transpose(block).astype(jnp.bfloat16)

        each(0, (high - low) // 2, pair)

    token_spread.relay_first()
    gathered(0)
    token_spread.relay_rest()
    here.relay_first()
    gathered(1)
    here.relay_rest()
    token_spread.finish()
    own_query.wait()
    each(0, blocks // 2, project)
    spreads[0].relay_first()
    gathered(2)
    spreads[1].relay_first()
    gathered(3)
    spreads[2].relay_first()
    spreads[0].relay_rest()
    spreads[3].relay_first()
    for i in range(1, PIECES):
        spreads[i].relay_rest()
    own_out.wait()
    out_spread = Spread(wide_weight, 0, 128, spread_send.at[2 + PIECES], spread_recv.at[2 + PIECES])
    out_spread.own()
    each(blocks // 2, blocks, project)
    ones = jnp.ones((ONES, BLOCK), jnp.bfloat16)

    def fill(slot):
        values[slot, BLOCK:, :] = ones

    each(0, slots, fill)
    keys[slots] = jnp.zeros((BLOCK, width), jnp.bfloat16)
    values[slots] = jnp.zeros((BLOCK + ONES, BLOCK), jnp.bfloat16)
    here.finish()
    prepare(0, blocks)
    for i in range(PIECES):
        spreads[i].finish()
        prepare(blocks + i * share * PER_OWNER, blocks + (i + 1) * share * PER_OWNER)
    to_scalars.wait()

    def heads_copy(to, b, slot):
        return remote(staged.at[b, to], heads.at[slot, b], heads_send.at[to, b], heads_recv.at[slot, b], "tp", to)

    def attend(b):
        def slot_of(c):
            block = chosen[b, c]
            held = jnp.maximum(block, 0)
            owner = lax.div(held, blocks)
            inside = held - owner * blocks
            away = blocks + owner * PER_OWNER + jnp.where(table[1, owner] == inside, 1, 0)
            return jnp.where(block < 0, slots, jnp.where(owner == kv, inside, away))

        def grouped(start, masked):
            places = [slot_of(start + i) for i in range(GROUP)]
            picked = jnp.concatenate([keys[s] for s in places], axis=0)
            scores = lax.dot_general(
                picked, queries[b], (((1,), (1,)), ((), ())), preferred_element_type=jnp.float32
            )
            if masked:
                key = lax.broadcasted_iota(jnp.int32, (BLOCK, scores.shape[1]), 0)
                query = lax.rem(lax.broadcasted_iota(jnp.int32, (BLOCK, scores.shape[1]), 1), BLOCK)
                diagonal = jnp.where(key <= query, scores[:BLOCK], masked_score)
                scores = jnp.concatenate([diagonal, scores[BLOCK:]], axis=0)
            weights = jnp.exp2(scores).astype(jnp.bfloat16)
            held = jnp.concatenate([values[s] for s in places], axis=1)
            return jnp.dot(held, weights, preferred_element_type=jnp.float32)

        total = grouped(0, True)
        total = lax.fori_loop(1, picks // GROUP, lambda g, t: t + grouped(g * GROUP, False), total)
        attended = (total[:BLOCK] / total[BLOCK : BLOCK + 1]).astype(jnp.bfloat16)
        turned = jnp.concatenate(
            [
                jnp.dot(up[h], attended[:, h * BLOCK : (h + 1) * BLOCK], preferred_element_type=jnp.float32)
                for h in range(up.shape[0])
            ],
            axis=0,
        )
        staged[b] = jnp.transpose(turned).astype(jnp.bfloat16).reshape(peers, group, width)
        each(1, peers, lambda i: heads_copy(peer(i), b, tp).start())

    def out_copy(to, half, slot):
        lower = pl.ds(half * HALF, HALF)
        return remote(
            finished.at[to, lower], out.at[lower, slot], out_send.at[to, half], out_recv.at[slot, half], "tp", to
        )

    def conclude(half):
        lower = pl.ds(half * HALF, HALF)

        def landed(i):
            for b in range(HALF):
                heads_copy(peer(i), half * HALF + b, peer(i)).wait_recv()

        each(1, peers, landed)
        for b in range(HALF):
            heads[tp, half * HALF + b] = staged[half * HALF + b, tp]
        features = jnp.concatenate([heads[p, lower].reshape(HALF * group, width) for p in range(peers)], axis=1)
        summed = jnp.dot(
            features, wide_weight[...].reshape(peers * 128, peers * 128), preferred_element_type=jnp.float32
        )
        mixed = unit(summed, out_gain[...])
        for t in range(peers):
            finished[t, lower] = mixed[:, t * 128 : (t + 1) * 128].reshape(HALF, group, 128)
        each(1, peers, lambda i: out_copy(peer(i), half, tp).start())
        out[lower, tp] = finished[tp, lower]

    def turn(b):
        attend(b)

        @pl.when(b == 1)
        def _():
            out_spread.relay_first()

        @pl.when(b == 3)
        def _():
            out_spread.relay_rest()

        @pl.when(b == 5)
        def _():
            out_spread.finish()
            conclude(0)

    each(0, blocks, turn)
    conclude(1)

    each(1, peers, lambda i: rows_copy(peer(i), tp).wait_send())
    each(0, kv, lambda o: ask_copy(o, kv).wait_send())
    each(kv + 1, owners, lambda r: serve_copy(r, kv).wait_send())
    for spread in (token_spread, here, out_spread, *spreads):
        spread.drain()

    def settle(i):
        for b in range(blocks):
            heads_copy(peer(i), b, tp).wait_send()
        for half in range(2):
            out_copy(peer(i), half, tp).wait_send()
            out_copy(peer(i), half, peer(i)).wait_recv()

    each(1, peers, settle)


def shards(
    tokens, query_weight, latent_weight, query_gain, key_gain, value_up, out_weight, out_gain, chosen
):
    peers, owners = lax.axis_size("tp"), lax.axis_size("kv")
    blocks, picks = chosen.shape
    rows, width = tokens.shape
    group = BLOCK // peers
    slots = blocks + owners * PER_OWNER
    heads = value_up.shape[0]
    vmem = pl.BlockSpec(memory_space=pltpu.VMEM)
    anywhere = pl.BlockSpec(memory_space=pl.ANY)
    dma = pltpu.SemaphoreType.DMA
    bf16 = jnp.bfloat16
    mixed = pl.pallas_call(
        kernel,
        out_shape=jax.ShapeDtypeStruct((blocks, peers, group, width), bf16),
        in_specs=[pl.BlockSpec(memory_space=pltpu.SMEM)] + [anywhere] * 4 + [vmem] * 4,
        out_specs=vmem,
        scratch_shapes=[
            pltpu.VMEM((peers, blocks, peers, group, width), bf16),
            pltpu.VMEM((peers, slots, group, width), bf16),
            pltpu.VMEM((peers, *out_weight.shape), bf16),
            pltpu.VMEM(latent_weight.shape, bf16),
            pltpu.VMEM(query_weight.shape, bf16),
            pltpu.VMEM((peers, blocks, group, width), bf16),
            pltpu.VMEM((owners, blocks, 128), jnp.float32),
            pltpu.VMEM((owners, blocks, 128), jnp.float32),
            pltpu.VMEM((owners, PER_OWNER, group, width), bf16),
            pltpu.VMEM((blocks, 128), jnp.int32),
            pltpu.SMEM((blocks, 128), jnp.int32),
            pltpu.VMEM((blocks, heads * BLOCK, width), bf16),
            pltpu.VMEM((slots + 1, BLOCK, width), bf16),
            pltpu.VMEM((slots + 1, BLOCK + ONES, BLOCK), bf16),
            pltpu.VMEM((blocks, peers, group, width), bf16),
            pltpu.VMEM((peers, blocks, group, width), bf16),
            pltpu.VMEM((peers, blocks, group, width), bf16),
            dma((5,)),
            dma((peers,)), dma((peers,)),
            dma((owners,)), dma((owners,)),
            dma((owners,)), dma((owners,)),
            dma((peers, blocks)), dma((peers, blocks)),
            dma((peers, 2)), dma((peers, 2)),
            dma((3 + PIECES, 14)), dma((3 + PIECES, peers, 2)),
        ],
        compiler_params=pltpu.CompilerParams(collective_id=0, has_side_effects=True),
    )(
        chosen,
        tokens.reshape(blocks, peers, group, width),
        latent_weight,
        query_weight,
        out_weight,
        query_gain.reshape(1, width),
        key_gain.reshape(1, width),
        jnp.swapaxes(value_up, 1, 2),
        out_gain.reshape(1, out_gain.shape[0]),
    )
    return mixed.reshape(rows, width)


def solution(mesh):
    in_specs = (
        P("kv", "tp"),
        P(None, "tp"),
        P(),
        P(),
        P(),
        P("tp", None, None),
        P("tp", None),
        P(),
        P("kv", None),
    )
    return jax.shard_map(shards, mesh=mesh, in_specs=in_specs, out_specs=P("kv", "tp"), check_vma=False)
```

```python
import functools

import jax
import jax.numpy as jnp
from jax import lax
from jax.experimental import pallas as pl
from jax.experimental.pallas import tpu as pltpu
from jax.sharding import PartitionSpec as P

BLOCK = 128
PER_OWNER = 2
MESH = pl.DeviceIdType.MESH
GROUP = 8
PIECES = 4
ONES = 16
HALF = 4
LOG2E = 1.4426950408889634


epsilon = 1e-06
masked_score = -1e30


def neighbours(tp):
    side = lax.rem(tp, 2)
    right = lax.rem(tp + 2, 8)
    left = lax.rem(tp + 6, 8)
    far = lax.rem(tp + 4, 8)
    return right, left, far, tp + 1 - 2 * side


class Spread:
    def __init__(self, full, first, size, send_sem, recv_sem):
        self.full, self.send_sem, self.recv_sem = full, send_sem, recv_sem
        half = size // 2
        self.ranges = ((first, half), (first + half, size - half))
        self.tp = lax.axis_index("tp")
        self.right, self.left, self.far, self.other = neighbours(self.tp)

    def copy(self, slot, part, dest, kind):
        first, size = self.ranges[part]
        piece = self.full.at[slot, pl.ds(first, size)]
        return pltpu.make_async_remote_copy(
            src_ref=piece,
            dst_ref=piece,
            send_sem=self.send_sem.at[kind],
            recv_sem=self.recv_sem.at[slot, part],
            device_id={"tp": dest},
            device_id_type=MESH,
        )

    def sends(self):
        me, right, left, far, other = self.tp, self.right, self.left, self.far, self.other
        return (
            (me, 0, right), (me, 1, left), (me, 1, right), (me, 0, left), (me, 0, other), (me, 1, other),
            (left, 0, right), (right, 1, left), (left, 0, other), (right, 1, other), (left, 1, other),
            (right, 0, other), (far, 0, other), (far, 1, other),
        )

    def start(self, *kinds):
        every = self.sends()
        for kind in kinds:
            self.copy(*every[kind], kind).start()

    def arrived(self, slot, part):
        self.copy(slot, part, self.other, 0).wait_recv()

    def own(self):
        self.start(0, 1, 2, 3, 4, 5)

    def relay_first(self):
        self.arrived(self.left, 0)
        self.start(6, 8)
        self.arrived(self.right, 1)
        self.start(7, 9)

    def relay_rest(self):
        self.arrived(self.left, 1)
        self.start(10)
        self.arrived(self.right, 0)
        self.start(11)
        self.arrived(self.far, 0)
        self.start(12)
        self.arrived(self.far, 1)
        self.start(13)

    def finish(self):
        side = 1 - 2 * lax.rem(self.tp, 2)
        for slot in (self.other, self.left + side, self.right + side, self.far + side):
            for part in (0, 1):
                self.arrived(slot, part)

    def drain(self):
        for kind, (slot, part, dest) in enumerate(self.sends()):
            self.copy(slot, part, dest, kind).wait_send()


def each(low, high, act):
    def step(i, carry):
        act(i)
        return carry

    lax.fori_loop(low, high, step, 0)


def remote(source, target, send_sem, recv_sem, axis, to):
    return pltpu.make_async_remote_copy(
        src_ref=source,
        dst_ref=target,
        send_sem=send_sem,
        recv_sem=recv_sem,
        device_id={axis: to},
        device_id_type=MESH,
    )


def unit(values, gain_row):
    mean_sq = jnp.mean(values * values, axis=-1, keepdims=True)
    return (values * lax.rsqrt(mean_sq + epsilon) * gain_row).astype(jnp.bfloat16)


def kernel(
    chosen, tokens, latent_weight, query_weight, out_weight, query_gain, key_gain, up, out_gain,
    out,
    full, pool, wide_weight, weight, projection, rows, asked, asks, served, listed, table,
    queries, keys, values, places, staged, heads,
    local_sem, rows_send, rows_recv, ask_send, ask_recv, serve_send, serve_recv,
    heads_send, heads_recv, out_send, out_recv, spread_send, spread_recv,
):
    kv, tp = lax.axis_index("kv"), lax.axis_index("tp")
    owners, peers = asked.shape[0], full.shape[0]
    blocks, group, width = rows.shape[1:]
    picks = chosen.shape[1]
    slots = pool.shape[1]
    lines = blocks * group

    own_tokens = pltpu.make_async_copy(tokens, full.at[tp], local_sem.at[0])
    own_latent = pltpu.make_async_copy(latent_weight, weight, local_sem.at[1])
    own_query = pltpu.make_async_copy(query_weight, projection, local_sem.at[2])
    own_out = pltpu.make_async_copy(out_weight, wide_weight.at[tp], local_sem.at[3])
    for copy in (own_tokens, own_latent, own_query, own_out):
        copy.start()

    barrier = pltpu.get_barrier_semaphore()

    def greet(axis, index, size):
        def signal(step):
            pl.semaphore_signal(barrier, inc=1, device_id={axis: lax.rem(index + step, size)}, device_id_type=MESH)

        each(1, size, signal)

    greet("kv", kv, owners)
    greet("tp", tp, peers)

    own_tokens.wait()
    pl.semaphore_wait(barrier, owners + peers - 2)

    def rows_copy(to, slot):
        return remote(full.at[tp, :, to], rows.at[slot], rows_send.at[to], rows_recv.at[slot], "tp", to)

    def ask_copy(to, slot):
        return remote(asks.at[to], asked.at[slot], ask_send.at[to], ask_recv.at[slot], "kv", to)

    def serve_copy(to, slot):
        target = pool.at[tp, pl.ds(blocks + slot * PER_OWNER, PER_OWNER)]
        return remote(served.at[to], target, serve_send.at[to], serve_recv.at[slot], "kv", to)

    def peer(i):
        return lax.rem(tp + i, peers)

    each(1, peers, lambda i: rows_copy(peer(i), tp).start())
    token_spread = Spread(
        full.reshape(peers, blocks * peers, group, width), 0, blocks * peers, spread_send.at[0], spread_recv.at[0]
    )
    token_spread.own()

    tile = (blocks, 128)
    lane = lax.broadcasted_iota(jnp.int32, tile, 1)
    sub = lax.broadcasted_iota(jnp.int32, tile, 0)
    ids = lane * blocks + sub

    def mark(b, needed):
        for c in range(picks):
            needed = jnp.where(ids == chosen[b, c], 1, needed)
        return needed

    needed = lax.fori_loop(0, blocks, mark, jnp.zeros(tile, jnp.int32))
    first = jnp.full((1, 128), -1, jnp.int32)
    second = first
    for j in reversed(range(blocks)):
        hit = needed[j : j + 1, :] > 0
        second = jnp.where(hit, first, second)
        first = jnp.where(hit, j, first)
    both = jnp.where(sub == 0, first, jnp.where(sub == 1, second, 0))
    listed[...] = both
    to_scalars = pltpu.make_async_copy(listed, table, local_sem.at[4])
    to_scalars.start()
    both = both.astype(jnp.float32)

    for o in range(owners - 1):
        asks[o] = jnp.broadcast_to(jnp.sum(jnp.where(lane == o, both, 0.0), axis=1, keepdims=True), tile)
    each(0, kv, lambda o: ask_copy(o, kv).start())

    ones = jnp.ones((ONES, BLOCK), jnp.bfloat16)

    def fill(slot):
        values[slot, BLOCK:, :] = ones

    each(0, slots, fill)
    keys[slots] = jnp.zeros((BLOCK, width), jnp.bfloat16)
    values[slots] = jnp.zeros((BLOCK + ONES, BLOCK), jnp.bfloat16)
    rows[tp] = full[tp, :, tp]
    own_latent.wait()
    each(1, peers, lambda i: rows_copy(peer(i), peer(i)).wait_recv())
    @jax.jit
    def compress():
        features = jnp.concatenate([rows[p].reshape(lines, width) for p in range(peers)], axis=1)
        latent = jnp.dot(features, weight[...], preferred_element_type=jnp.float32)
        return latent.astype(jnp.bfloat16).reshape(blocks, group, 128)

    latent = compress()
    pool[tp, 0:blocks] = latent
    latent = latent.astype(jnp.float32)

    def serve(i):
        r = owners - 1 - i
        ask_copy(r, r).wait_recv()
        for k in range(PER_OWNER):
            want = asked[r, k : k + 1, :]
            picked = jnp.zeros((group, 128), jnp.float32)
            for j in range(blocks):
                picked = jnp.where(want == float(j), latent[j], picked)
            served[r, k] = picked.astype(jnp.bfloat16)
        serve_copy(r, kv).start()

    each(0, owners - 1 - kv, serve)
    here = Spread(pool, 0, blocks, spread_send.at[1], spread_recv.at[1])
    here.own()

    share = owners // PIECES
    spreads = [
        Spread(pool, blocks + i * share * PER_OWNER, share * PER_OWNER, spread_send.at[2 + i], spread_recv.at[2 + i])
        for i in range(PIECES)
    ]

    def gathered(i):
        low = i * share
        each(low, jnp.clip(kv, low, low + share), lambda o: serve_copy(o, o).wait_recv())
        spreads[i].own()

    scale = width ** (-0.5) * LOG2E
    query_row = query_gain[...] * scale

    def project(b):
        features = jnp.concatenate([full[p, b].reshape(BLOCK, width) for p in range(peers)], axis=1)
        projected = jnp.dot(features, projection[...], preferred_element_type=jnp.float32)
        projected = projected.astype(jnp.bfloat16).astype(jnp.float32)
        for h in range(up.shape[0]):
            queries[b, h * BLOCK : (h + 1) * BLOCK, :] = unit(projected[:, h * 128 : (h + 1) * 128], query_row)

    def prepare(low, high):
        def several(j):
            for i in range(4):
                slot = low + 4 * j + i
                block = pool[:, slot].reshape(BLOCK, width).astype(jnp.float32)
                keys[slot] = unit(block, key_gain[...])
                values[slot, :BLOCK, :] = jnp.transpose(block).astype(jnp.bfloat16)

        each(0, (high - low) // 4, several)

    def place(b):
        for c in range(picks):
            block = chosen[b, c]
            held = jnp.maximum(block, 0)
            owner = lax.div(held, blocks)
            inside = held - owner * blocks
            away = blocks + owner * PER_OWNER + jnp.where(table[1, owner] == inside, 1, 0)
            places[b, c] = jnp.where(block < 0, slots, jnp.where(owner == kv, inside, away))

    to_scalars.wait()
    each(1, peers, lambda i: rows_copy(peer(i), tp).wait_send())
    each(0, blocks, place)
    own_query.wait()
    own_out.wait()
    token_spread.relay_first()
    here.relay_first()
    for i in range(PIECES):
        gathered(i)
    here.relay_rest()
    token_spread.relay_rest()
    token_spread.finish()
    token_spread.drain()
    here.finish()
    step = blocks // PIECES
    for i in range(PIECES):
        spreads[i].relay_first()
        each(i * step, (i + 1) * step, project)
        if i == 0:
            prepare(0, blocks)
    out_spread = Spread(wide_weight, 0, 128, spread_send.at[2 + PIECES], spread_recv.at[2 + PIECES])
    for i in range(PIECES):
        spreads[i].relay_rest()
        if i == PIECES - 1:
            out_spread.own()
        spreads[i].finish()
        prepare(blocks + i * share * PER_OWNER, blocks + (i + 1) * share * PER_OWNER)

    def heads_copy(to, b, slot):
        return remote(staged.at[b, to], heads.at[slot, b], heads_send.at[to, b], heads_recv.at[slot, b], "tp", to)

    def attend(b):
        def grouped(start, masked):
            chose = [places[b, start + i] for i in range(GROUP)]
            picked = jnp.concatenate([keys[s] for s in chose], axis=0)
            scores = lax.dot_general(
                picked, queries[b], (((1,), (1,)), ((), ())), preferred_element_type=jnp.float32
            )
            if masked:
                key = lax.broadcasted_iota(jnp.int32, (BLOCK, scores.shape[1]), 0)
                query = lax.rem(lax.broadcasted_iota(jnp.int32, (BLOCK, scores.shape[1]), 1), BLOCK)
                diagonal = jnp.where(key <= query, scores[:BLOCK], masked_score)
                scores = jnp.concatenate([diagonal, scores[BLOCK:]], axis=0)
            weights = jnp.exp2(scores).astype(jnp.bfloat16)
            held = jnp.concatenate([values[s] for s in chose], axis=1)
            return jnp.dot(held, weights, preferred_element_type=jnp.float32)

        total = grouped(0, True)
        total = lax.fori_loop(1, picks // GROUP, lambda g, t: t + grouped(g * GROUP, False), total)
        attended = (total[:BLOCK] / total[BLOCK : BLOCK + 1]).astype(jnp.bfloat16)
        turned = jnp.concatenate(
            [
                jnp.dot(up[h], attended[:, h * BLOCK : (h + 1) * BLOCK], preferred_element_type=jnp.float32)
                for h in range(up.shape[0])
            ],
            axis=0,
        )
        staged[b] = jnp.transpose(turned).astype(jnp.bfloat16).reshape(peers, group, width)
        each(1, peers, lambda i: heads_copy(peer(i), b, tp).start())

    def out_copy(to, half, slot):
        lower = pl.ds(half * HALF, HALF)
        return remote(
            rows.at[to, lower], out.at[lower, slot], out_send.at[to, half], out_recv.at[slot, half], "tp", to
        )

    @functools.partial(jax.jit, static_argnums=0)
    def mix(half):
        lower = pl.ds(half * HALF, HALF)
        features = jnp.concatenate([heads[p, lower].reshape(HALF * group, width) for p in range(peers)], axis=1)
        summed = jnp.dot(
            features, wide_weight[...].reshape(peers * 128, peers * 128), preferred_element_type=jnp.float32
        )
        mixed = unit(summed, out_gain[...])
        for t in range(peers):
            rows[t, lower] = mixed[:, t * 128 : (t + 1) * 128].reshape(HALF, group, 128)

    def conclude(half):
        lower = pl.ds(half * HALF, HALF)

        def landed(i):
            for b in range(HALF):
                heads_copy(peer(i), half * HALF + b, peer(i)).wait_recv()

        each(1, peers, landed)
        for b in range(HALF):
            heads[tp, half * HALF + b] = staged[half * HALF + b, tp]
        mix(half)
        each(1, peers, lambda i: out_copy(peer(i), half, tp).start())
        out[lower, tp] = rows[tp, lower]

    def turn(i):
        attend(i)

        @pl.when(i == 2)
        def _():
            out_spread.relay_first()

        @pl.when(i == 4)
        def _():
            out_spread.relay_rest()

    each(0, blocks, turn)
    out_spread.finish()
    conclude(0)
    conclude(1)

    each(0, kv, lambda o: ask_copy(o, kv).wait_send())
    each(kv + 1, owners, lambda r: serve_copy(r, kv).wait_send())
    for spread in (here, out_spread, *spreads):
        spread.drain()

    def settle(i):
        for b in range(blocks):
            heads_copy(peer(i), b, tp).wait_send()
        for half in range(2):
            out_copy(peer(i), half, tp).wait_send()
            out_copy(peer(i), half, peer(i)).wait_recv()

    each(1, peers, settle)


def shards(
    tokens, query_weight, latent_weight, query_gain, key_gain, value_up, out_weight, out_gain, chosen
):
    peers, owners = lax.axis_size("tp"), lax.axis_size("kv")
    blocks, picks = chosen.shape
    rows, width = tokens.shape
    group = BLOCK // peers
    slots = blocks + owners * PER_OWNER
    heads = value_up.shape[0]
    vmem = pl.BlockSpec(memory_space=pltpu.VMEM)
    anywhere = pl.BlockSpec(memory_space=pl.ANY)
    dma = pltpu.SemaphoreType.DMA
    bf16 = jnp.bfloat16
    mixed = pl.pallas_call(
        kernel,
        out_shape=jax.ShapeDtypeStruct((blocks, peers, group, width), bf16),
        in_specs=[pl.BlockSpec(memory_space=pltpu.SMEM)] + [anywhere] * 4 + [vmem] * 4,
        out_specs=vmem,
        scratch_shapes=[
            pltpu.VMEM((peers, blocks, peers, group, width), bf16),
            pltpu.VMEM((peers, slots, group, width), bf16),
            pltpu.VMEM((peers, *out_weight.shape), bf16),
            pltpu.VMEM(latent_weight.shape, bf16),
            pltpu.VMEM(query_weight.shape, bf16),
            pltpu.VMEM((peers, blocks, group, width), bf16),
            pltpu.VMEM((owners, blocks, 128), jnp.float32),
            pltpu.VMEM((owners, blocks, 128), jnp.float32),
            pltpu.VMEM((owners, PER_OWNER, group, width), bf16),
            pltpu.VMEM((blocks, 128), jnp.int32),
            pltpu.SMEM((blocks, 128), jnp.int32),
            pltpu.VMEM((blocks, heads * BLOCK, width), bf16),
            pltpu.VMEM((slots + 1, BLOCK, width), bf16),
            pltpu.VMEM((slots + 1, BLOCK + ONES, BLOCK), bf16),
            pltpu.SMEM((blocks, picks), jnp.int32),
            pltpu.VMEM((blocks, peers, group, width), bf16),
            pltpu.VMEM((peers, blocks, group, width), bf16),
            dma((5,)),
            dma((peers,)), dma((peers,)),
            dma((owners,)), dma((owners,)),
            dma((owners,)), dma((owners,)),
            dma((peers, blocks)), dma((peers, blocks)),
            dma((peers, 2)), dma((peers, 2)),
            dma((3 + PIECES, 14)), dma((3 + PIECES, peers, 2)),
        ],
        compiler_params=pltpu.CompilerParams(collective_id=0, has_side_effects=True),
    )(
        chosen,
        tokens.reshape(blocks, peers, group, width),
        latent_weight,
        query_weight,
        out_weight,
        query_gain.reshape(1, width),
        key_gain.reshape(1, width),
        jnp.swapaxes(value_up, 1, 2),
        out_gain.reshape(1, out_gain.shape[0]),
    )
    return mixed.reshape(rows, width)


def solution(mesh):
    in_specs = (
        P("kv", "tp"),
        P(None, "tp"),
        P(),
        P(),
        P(),
        P("tp", None, None),
        P("tp", None),
        P(),
        P("kv", None),
    )
    return jax.shard_map(shards, mesh=mesh, in_specs=in_specs, out_specs=P("kv", "tp"), check_vma=False)
```

```python
import functools

import jax
import jax.numpy as jnp
from jax import lax
from jax.experimental import pallas as pl
from jax.experimental.pallas import tpu as pltpu
from jax.sharding import PartitionSpec as P

BLOCK = 128
PER_OWNER = 2
MESH = pl.DeviceIdType.MESH
GROUP = 8
PIECES = 4
ONES = 16
HALF = 4
LOG2E = 1.4426950408889634


epsilon = 1e-06
masked_score = -1e30


def neighbours(tp):
    side = lax.rem(tp, 2)
    right = lax.rem(tp + 2, 8)
    left = lax.rem(tp + 6, 8)
    far = lax.rem(tp + 4, 8)
    return right, left, far, tp + 1 - 2 * side


class Spread:
    def __init__(self, full, first, size, send_sem, recv_sem):
        self.full, self.send_sem, self.recv_sem = full, send_sem, recv_sem
        half = size // 2
        self.ranges = ((first, half), (first + half, size - half))
        self.tp = lax.axis_index("tp")
        self.right, self.left, self.far, self.other = neighbours(self.tp)

    def copy(self, slot, part, dest, kind):
        first, size = self.ranges[part]
        piece = self.full.at[slot, pl.ds(first, size)]
        return pltpu.make_async_remote_copy(
            src_ref=piece,
            dst_ref=piece,
            send_sem=self.send_sem.at[kind],
            recv_sem=self.recv_sem.at[slot, part],
            device_id={"tp": dest},
            device_id_type=MESH,
        )

    def sends(self):
        me, right, left, far, other = self.tp, self.right, self.left, self.far, self.other
        return (
            (me, 0, right), (me, 1, left), (me, 1, right), (me, 0, left), (me, 0, other), (me, 1, other),
            (left, 0, right), (right, 1, left), (left, 0, other), (right, 1, other), (left, 1, other),
            (right, 0, other), (far, 0, other), (far, 1, other),
        )

    def start(self, *kinds):
        every = self.sends()
        for kind in kinds:
            self.copy(*every[kind], kind).start()

    def arrived(self, slot, part):
        self.copy(slot, part, self.other, 0).wait_recv()

    def own(self):
        self.start(0, 1, 2, 3, 4, 5)

    def relay_first(self):
        self.arrived(self.left, 0)
        self.start(6, 8)
        self.arrived(self.right, 1)
        self.start(7, 9)

    def relay_rest(self):
        self.arrived(self.left, 1)
        self.start(10)
        self.arrived(self.right, 0)
        self.start(11)
        self.arrived(self.far, 0)
        self.start(12)
        self.arrived(self.far, 1)
        self.start(13)

    def finish(self):
        side = 1 - 2 * lax.rem(self.tp, 2)
        for slot in (self.other, self.left + side, self.right + side, self.far + side):
            for part in (0, 1):
                self.arrived(slot, part)

    def drain(self):
        for kind, (slot, part, dest) in enumerate(self.sends()):
            self.copy(slot, part, dest, kind).wait_send()


def each(low, high, act):
    def step(i, carry):
        act(i)
        return carry

    lax.fori_loop(low, high, step, 0)


def remote(source, target, send_sem, recv_sem, axis, to):
    return pltpu.make_async_remote_copy(
        src_ref=source,
        dst_ref=target,
        send_sem=send_sem,
        recv_sem=recv_sem,
        device_id={axis: to},
        device_id_type=MESH,
    )


def unit(values, gain_row):
    mean_sq = jnp.mean(values * values, axis=-1, keepdims=True)
    return (values * lax.rsqrt(mean_sq + epsilon) * gain_row).astype(jnp.bfloat16)


def kernel(
    chosen, tokens, latent_weight, query_weight, out_weight, query_gain, key_gain, up, out_gain,
    out,
    full, pool, wide_weight, weight, projection, rows, asked, asks, served, listed, table,
    queries, keys, values, totals, bias, places, staged, heads,
    local_sem, rows_send, rows_recv, ask_send, ask_recv, serve_send, serve_recv,
    heads_send, heads_recv, out_send, out_recv, spread_send, spread_recv,
):
    kv, tp = lax.axis_index("kv"), lax.axis_index("tp")
    owners, peers = asked.shape[0], full.shape[0]
    blocks, group, width = rows.shape[1:]
    picks = chosen.shape[1]
    slots = pool.shape[1]
    lines = blocks * group

    own_tokens = pltpu.make_async_copy(tokens, full.at[tp], local_sem.at[0])
    own_latent = pltpu.make_async_copy(latent_weight, weight, local_sem.at[1])
    own_query = pltpu.make_async_copy(query_weight, projection, local_sem.at[2])
    own_out = pltpu.make_async_copy(out_weight, wide_weight.at[tp], local_sem.at[3])
    for copy in (own_tokens, own_latent, own_query, own_out):
        copy.start()

    barrier = pltpu.get_barrier_semaphore()

    def greet(axis, index, size):
        def signal(step):
            pl.semaphore_signal(barrier, inc=1, device_id={axis: lax.rem(index + step, size)}, device_id_type=MESH)

        each(1, size, signal)

    greet("kv", kv, owners)
    greet("tp", tp, peers)

    own_tokens.wait()
    pl.semaphore_wait(barrier, owners + peers - 2)

    def rows_copy(to, slot):
        return remote(full.at[tp, :, to], rows.at[slot], rows_send.at[to], rows_recv.at[slot], "tp", to)

    def ask_copy(to, slot):
        return remote(asks.at[to], asked.at[slot], ask_send.at[to], ask_recv.at[slot], "kv", to)

    def serve_copy(to, slot):
        target = pool.at[tp, pl.ds(blocks + slot * PER_OWNER, PER_OWNER)]
        return remote(served.at[to], target, serve_send.at[to], serve_recv.at[slot], "kv", to)

    def peer(i):
        return lax.rem(tp + i, peers)

    each(1, peers, lambda i: rows_copy(peer(i), tp).start())
    token_spread = Spread(
        full.reshape(peers, blocks * peers, group, width), 0, blocks * peers, spread_send.at[0], spread_recv.at[0]
    )
    token_spread.own()

    tile = (blocks, 128)
    lane = lax.broadcasted_iota(jnp.int32, tile, 1)
    sub = lax.broadcasted_iota(jnp.int32, tile, 0)
    ids = lane * blocks + sub

    def mark(b, needed):
        for c in range(picks):
            needed = jnp.where(ids == chosen[b, c], 1, needed)
        return needed

    needed = lax.fori_loop(0, blocks, mark, jnp.zeros(tile, jnp.int32))
    first = jnp.full((1, 128), -1, jnp.int32)
    second = first
    for j in reversed(range(blocks)):
        hit = needed[j : j + 1, :] > 0
        second = jnp.where(hit, first, second)
        first = jnp.where(hit, j, first)
    both = jnp.where(sub == 0, first, jnp.where(sub == 1, second, 0))
    listed[...] = both
    to_scalars = pltpu.make_async_copy(listed, table, local_sem.at[4])
    to_scalars.start()
    both = both.astype(jnp.float32)

    for o in range(owners - 1):
        asks[o] = jnp.broadcast_to(jnp.sum(jnp.where(lane == o, both, 0.0), axis=1, keepdims=True), tile)
    each(0, kv, lambda o: ask_copy(o, kv).start())

    ones = jnp.ones((ONES, BLOCK), jnp.bfloat16)

    def fill(slot):
        values[slot, BLOCK:, :] = ones

    each(0, slots, fill)
    key = lax.broadcasted_iota(jnp.int32, bias.shape[1:], 0)
    query = lax.rem(lax.broadcasted_iota(jnp.int32, bias.shape[1:], 1), BLOCK)
    bias[0] = jnp.where(key <= query, 0.0, masked_score)
    bias[1] = jnp.zeros(bias.shape[1:], jnp.float32)
    keys[slots] = jnp.zeros((BLOCK, width), jnp.bfloat16)
    values[slots] = jnp.zeros((BLOCK + ONES, BLOCK), jnp.bfloat16)
    rows[tp] = full[tp, :, tp]
    own_latent.wait()
    each(1, peers, lambda i: rows_copy(peer(i), peer(i)).wait_recv())
    @jax.jit
    def compress():
        features = jnp.concatenate([rows[p].reshape(lines, width) for p in range(peers)], axis=1)
        latent = jnp.dot(features, weight[...], preferred_element_type=jnp.float32)
        return latent.astype(jnp.bfloat16).reshape(blocks, group, 128)

    latent = compress()
    pool[tp, 0:blocks] = latent
    latent = latent.astype(jnp.float32)

    def serve(i):
        r = owners - 1 - i
        ask_copy(r, r).wait_recv()
        for k in range(PER_OWNER):
            want = asked[r, k : k + 1, :]
            picked = jnp.zeros((group, 128), jnp.float32)
            for j in range(blocks):
                picked = jnp.where(want == float(j), latent[j], picked)
            served[r, k] = picked.astype(jnp.bfloat16)
        serve_copy(r, kv).start()

    each(0, owners - 1 - kv, serve)
    here = Spread(pool, 0, blocks, spread_send.at[1], spread_recv.at[1])
    here.own()

    share = owners // PIECES
    spreads = [
        Spread(pool, blocks + i * share * PER_OWNER, share * PER_OWNER, spread_send.at[2 + i], spread_recv.at[2 + i])
        for i in range(PIECES)
    ]

    def gathered(i):
        low = i * share
        each(low, jnp.clip(kv, low, low + share), lambda o: serve_copy(o, o).wait_recv())
        spreads[i].own()

    scale = width ** (-0.5) * LOG2E
    query_row = query_gain[...] * scale

    def project(b):
        features = jnp.concatenate([full[p, b].reshape(BLOCK, width) for p in range(peers)], axis=1)
        projected = jnp.dot(features, projection[...], preferred_element_type=jnp.float32)
        projected = projected.astype(jnp.bfloat16).astype(jnp.float32)
        for h in range(up.shape[0]):
            queries[b, h * BLOCK : (h + 1) * BLOCK, :] = unit(projected[:, h * 128 : (h + 1) * 128], query_row)

    def prepare(low, high):
        def several(j):
            for i in range(4):
                slot = low + 4 * j + i
                block = pool[:, slot].reshape(BLOCK, width).astype(jnp.float32)
                keys[slot] = unit(block, key_gain[...])
                values[slot, :BLOCK, :] = jnp.transpose(block).astype(jnp.bfloat16)

        each(0, (high - low) // 4, several)

    def place(b):
        for c in range(picks):
            block = chosen[b, c]
            held = jnp.maximum(block, 0)
            owner = lax.div(held, blocks)
            inside = held - owner * blocks
            away = blocks + owner * PER_OWNER + jnp.where(table[1, owner] == inside, 1, 0)
            places[b, c] = jnp.where(block < 0, slots, jnp.where(owner == kv, inside, away))

    to_scalars.wait()
    each(1, peers, lambda i: rows_copy(peer(i), tp).wait_send())
    each(0, blocks, place)
    own_query.wait()
    own_out.wait()
    token_spread.relay_first()
    here.relay_first()
    for i in range(PIECES):
        gathered(i)
    here.relay_rest()
    token_spread.relay_rest()
    token_spread.finish()
    token_spread.drain()
    here.finish()
    step = blocks // PIECES
    for i in range(PIECES):
        spreads[i].relay_first()
        each(i * step, (i + 1) * step, project)
        if i == 0:
            prepare(0, blocks)
    out_spread = Spread(wide_weight, 0, 128, spread_send.at[2 + PIECES], spread_recv.at[2 + PIECES])
    for i in range(PIECES):
        spreads[i].relay_rest()
        if i == PIECES - 1:
            out_spread.own()
        spreads[i].finish()
        prepare(blocks + i * share * PER_OWNER, blocks + (i + 1) * share * PER_OWNER)

    def heads_copy(to, b, slot):
        return remote(staged.at[b, to], heads.at[slot, b], heads_send.at[to, b], heads_recv.at[slot, b], "tp", to)

    sides, heads_here = 2, up.shape[0]
    span = GROUP * BLOCK
    weights = full.reshape(sides, heads_here, -1, width)

    def weigh(b, side, g):
        picked = jnp.concatenate([keys[places[b, g * GROUP + i]] for i in range(GROUP)], axis=0)
        scores = lax.dot_general(
            picked, queries[b], (((1,), (1,)), ((), ())), preferred_element_type=jnp.float32
        )
        diagonal = jnp.exp2(scores[:BLOCK] + bias[jnp.minimum(g, 1)]).astype(jnp.bfloat16)
        others = jnp.exp2(scores[BLOCK:]).astype(jnp.bfloat16)
        for h in range(heads_here):
            cols = slice(h * BLOCK, (h + 1) * BLOCK)
            weights[side, h, :BLOCK, :] = diagonal[:, cols]
            weights[side, h, BLOCK:span, :] = others[:, cols]

    def add_up(b, side, g):
        held = jnp.concatenate([values[places[b, g * GROUP + i]] for i in range(GROUP)], axis=1)
        right = jnp.concatenate([weights[side, h, :span, :] for h in range(heads_here)], axis=1)
        return jnp.dot(held, right, preferred_element_type=jnp.float32)

    def hand_over(b, ended):
        shares = []
        for total in ended:
            shares.append((total[:BLOCK] / total[BLOCK : BLOCK + 1]).astype(jnp.bfloat16))
        turned, flipped = [], []
        for side in range(sides):
            for h in range(heads_here):
                share = shares[side][:, h * BLOCK : (h + 1) * BLOCK]
                turned.append(jnp.dot(up[h], share, preferred_element_type=jnp.float32))
        for side in range(sides):
            both = jnp.concatenate(turned[side * heads_here : (side + 1) * heads_here], axis=0)
            flipped.append(jnp.transpose(both).astype(jnp.bfloat16).reshape(peers, group, width))
        for side in range(sides):
            staged[b + side] = flipped[side]

    def attend(i):
        first = sides * i
        for side in range(sides):
            weigh(first + side, side, 0)
            totals[side] = jnp.zeros(totals.shape[1:], jnp.float32)

        def both(g):
            for side in range(sides):
                totals[side] = totals[side] + add_up(first + side, side, g - 1)
            for side in range(sides):
                weigh(first + side, side, g)

        each(1, picks // GROUP, both)
        ended = [totals[side] + add_up(first + side, side, picks // GROUP - 1) for side in range(sides)]
        hand_over(first, ended)
        for side in range(sides):
            each(1, peers, lambda j: heads_copy(peer(j), first + side, tp).start())

    def out_copy(to, half, slot):
        lower = pl.ds(half * HALF, HALF)
        return remote(
            rows.at[to, lower], out.at[lower, slot], out_send.at[to, half], out_recv.at[slot, half], "tp", to
        )

    @functools.partial(jax.jit, static_argnums=0)
    def mix(half):
        lower = pl.ds(half * HALF, HALF)
        features = jnp.concatenate([heads[p, lower].reshape(HALF * group, width) for p in range(peers)], axis=1)
        summed = jnp.dot(
            features, wide_weight[...].reshape(peers * 128, peers * 128), preferred_element_type=jnp.float32
        )
        mixed = unit(summed, out_gain[...])
        for t in range(peers):
            rows[t, lower] = mixed[:, t * 128 : (t + 1) * 128].reshape(HALF, group, 128)

    def conclude(half):
        lower = pl.ds(half * HALF, HALF)

        def landed(i):
            for b in range(HALF):
                heads_copy(peer(i), half * HALF + b, peer(i)).wait_recv()

        each(1, peers, landed)
        for b in range(HALF):
            heads[tp, half * HALF + b] = staged[half * HALF + b, tp]
        mix(half)
        each(1, peers, lambda i: out_copy(peer(i), half, tp).start())
        out[lower, tp] = rows[tp, lower]

    def turn(i):
        attend(i)

        @pl.when(i == 1)
        def _():
            out_spread.relay_first()

        @pl.when(i == 2)
        def _():
            out_spread.relay_rest()

    each(0, blocks // sides, turn)
    out_spread.finish()
    conclude(0)
    conclude(1)

    each(0, kv, lambda o: ask_copy(o, kv).wait_send())
    each(kv + 1, owners, lambda r: serve_copy(r, kv).wait_send())
    for spread in (here, out_spread, *spreads):
        spread.drain()

    def settle(i):
        for b in range(blocks):
            heads_copy(peer(i), b, tp).wait_send()
        for half in range(2):
            out_copy(peer(i), half, tp).wait_send()
            out_copy(peer(i), half, peer(i)).wait_recv()

    each(1, peers, settle)


def shards(
    tokens, query_weight, latent_weight, query_gain, key_gain, value_up, out_weight, out_gain, chosen
):
    peers, owners = lax.axis_size("tp"), lax.axis_size("kv")
    blocks, picks = chosen.shape
    rows, width = tokens.shape
    group = BLOCK // peers
    slots = blocks + owners * PER_OWNER
    heads = value_up.shape[0]
    vmem = pl.BlockSpec(memory_space=pltpu.VMEM)
    anywhere = pl.BlockSpec(memory_space=pl.ANY)
    dma = pltpu.SemaphoreType.DMA
    bf16 = jnp.bfloat16
    mixed = pl.pallas_call(
        kernel,
        out_shape=jax.ShapeDtypeStruct((blocks, peers, group, width), bf16),
        in_specs=[pl.BlockSpec(memory_space=pltpu.SMEM)] + [anywhere] * 4 + [vmem] * 4,
        out_specs=vmem,
        scratch_shapes=[
            pltpu.VMEM((peers, blocks, peers, group, width), bf16),
            pltpu.VMEM((peers, slots, group, width), bf16),
            pltpu.VMEM((peers, *out_weight.shape), bf16),
            pltpu.VMEM(latent_weight.shape, bf16),
            pltpu.VMEM(query_weight.shape, bf16),
            pltpu.VMEM((peers, blocks, group, width), bf16),
            pltpu.VMEM((owners, blocks, 128), jnp.float32),
            pltpu.VMEM((owners, blocks, 128), jnp.float32),
            pltpu.VMEM((owners, PER_OWNER, group, width), bf16),
            pltpu.VMEM((blocks, 128), jnp.int32),
            pltpu.SMEM((blocks, 128), jnp.int32),
            pltpu.VMEM((blocks, heads * BLOCK, width), bf16),
            pltpu.VMEM((slots + 1, BLOCK, width), bf16),
            pltpu.VMEM((slots + 1, BLOCK + ONES, BLOCK), bf16),
            pltpu.VMEM((2, BLOCK + ONES, heads * BLOCK), jnp.float32),
            pltpu.VMEM((2, BLOCK, heads * BLOCK), jnp.float32),
            pltpu.SMEM((blocks, picks), jnp.int32),
            pltpu.VMEM((blocks, peers, group, width), bf16),
            pltpu.VMEM((peers, blocks, group, width), bf16),
            dma((5,)),
            dma((peers,)), dma((peers,)),
            dma((owners,)), dma((owners,)),
            dma((owners,)), dma((owners,)),
            dma((peers, blocks)), dma((peers, blocks)),
            dma((peers, 2)), dma((peers, 2)),
            dma((3 + PIECES, 14)), dma((3 + PIECES, peers, 2)),
        ],
        compiler_params=pltpu.CompilerParams(collective_id=0, has_side_effects=True),
    )(
        chosen,
        tokens.reshape(blocks, peers, group, width),
        latent_weight,
        query_weight,
        out_weight,
        query_gain.reshape(1, width),
        key_gain.reshape(1, width),
        jnp.swapaxes(value_up, 1, 2),
        out_gain.reshape(1, out_gain.shape[0]),
    )
    return mixed.reshape(rows, width)


def solution(mesh):
    in_specs = (
        P("kv", "tp"),
        P(None, "tp"),
        P(),
        P(),
        P(),
        P("tp", None, None),
        P("tp", None),
        P(),
        P("kv", None),
    )
    return jax.shard_map(shards, mesh=mesh, in_specs=in_specs, out_specs=P("kv", "tp"), check_vma=False)
```

```python
import functools

import jax
import jax.numpy as jnp
from jax import lax
from jax.experimental import pallas as pl
from jax.experimental.pallas import tpu as pltpu
from jax.sharding import PartitionSpec as P

BLOCK = 128
PER_OWNER = 2
MESH = pl.DeviceIdType.MESH
GROUP = 8
PIECES = 4
ONES = 16
HALF = 4
LOG2E = 1.4426950408889634


epsilon = 1e-06
masked_score = -1e30


def neighbours(tp):
    side = lax.rem(tp, 2)
    right = lax.rem(tp + 2, 8)
    left = lax.rem(tp + 6, 8)
    far = lax.rem(tp + 4, 8)
    return right, left, far, tp + 1 - 2 * side


class Spread:
    def __init__(self, full, first, size, send_sem, recv_sem):
        self.full, self.send_sem, self.recv_sem = full, send_sem, recv_sem
        half = size // 2
        self.ranges = ((first, half), (first + half, size - half))
        self.tp = lax.axis_index("tp")
        self.right, self.left, self.far, self.other = neighbours(self.tp)

    def sends(self):
        me, right, left, far, other = self.tp, self.right, self.left, self.far, self.other
        return (
            (me, 0, right, 0), (me, 1, left, 0), (me, 1, right, 1), (me, 0, left, 1), (me, 0, other, 2), (me, 1, other, 2),
            (left, 0, right, 1), (right, 1, left, 1), (left, 0, other, 2), (right, 1, other, 2), (left, 1, other, 2),
            (right, 0, other, 2), (far, 0, other, 2), (far, 1, other, 2),
        )

    def start(self, *kinds):
        every = self.sends()
        for kind in kinds:
            slot, part, dest, arrival = every[kind]
            first, size = self.ranges[part]
            piece = self.full.at[slot, pl.ds(first, size)]
            remote(piece, piece, self.send_sem, self.recv_sem.at[arrival], "tp", dest).start()

    def slices(self, count, sem):
        wait_bytes(self.full.at[pl.ds(0, count), pl.ds(self.ranges[0][0], sum(size for _, size in self.ranges))], sem)

    def own(self):
        self.start(0, 1, 2, 3, 4, 5)

    def relay_first(self):
        self.slices(1, self.recv_sem.at[0])
        self.start(6, 7, 8, 9)

    def relay_rest(self):
        self.slices(2, self.recv_sem.at[1])
        self.start(10, 11, 12, 13)

    def finish(self):
        self.slices(4, self.recv_sem.at[2])

    def drain(self):
        self.slices(7, self.send_sem)


def wait_bytes(region, sem):
    pltpu.make_async_copy(region, region, sem).wait()


def each(low, high, act):
    def step(i, carry):
        act(i)
        return carry

    lax.fori_loop(low, high, step, 0)


def remote(source, target, send_sem, recv_sem, axis, to):
    return pltpu.make_async_remote_copy(
        src_ref=source,
        dst_ref=target,
        send_sem=send_sem,
        recv_sem=recv_sem,
        device_id={axis: to},
        device_id_type=MESH,
    )


def unit(values, gain_row):
    mean_sq = jnp.mean(values * values, axis=-1, keepdims=True)
    return (values * lax.rsqrt(mean_sq + epsilon) * gain_row).astype(jnp.bfloat16)


def kernel(
    chosen_in, tokens, latent_weight, query_weight, out_weight, query_gain_in, key_gain_in, up_in, out_gain_in,
    out,
    chosen, query_gain, key_gain, up, out_gain,
    full, pool, wide_weight, weight, projection, rows, asked, asks, served, listed, table,
    queries, keys, values, totals, bias, places, staged, heads,
    local_sem, rows_send, rows_recv, ask_send, ask_recv, serve_send, serve_recv,
    heads_send, heads_recv, out_send, out_recv, spread_send, spread_recv,
):
    kv, tp = lax.axis_index("kv"), lax.axis_index("tp")
    owners, peers = asked.shape[0], full.shape[0]
    blocks, group, width = rows.shape[1:]
    picks = chosen.shape[1]
    slots = pool.shape[1]
    lines = blocks * group

    own_tokens = pltpu.make_async_copy(tokens, full.at[tp], local_sem.at[0])
    own_latent = pltpu.make_async_copy(latent_weight, weight, local_sem.at[1])
    own_query = pltpu.make_async_copy(query_weight, projection, local_sem.at[2])
    own_out = pltpu.make_async_copy(out_weight, wide_weight.at[tp], local_sem.at[3])
    small = [
        pltpu.make_async_copy(source, target, local_sem.at[5 + i])
        for i, (source, target) in enumerate(
            (
                (chosen_in, chosen), (query_gain_in, query_gain), (key_gain_in, key_gain), (up_in, up), (out_gain_in, out_gain)
            )
        )
    ]
    barrier = pltpu.get_barrier_semaphore()

    def greet(axis, index, size):
        def signal(step):
            pl.semaphore_signal(barrier, inc=1, device_id={axis: lax.rem(index + step, size)}, device_id_type=MESH)

        each(1, size, signal)

    greet("kv", kv, owners)
    greet("tp", tp, peers)

    for copy in (own_tokens, *small, own_latent, own_query, own_out):
        copy.start()
    own_tokens.wait()
    pl.semaphore_wait(barrier, owners + peers - 2)

    share = owners // PIECES

    def rows_copy(to, slot):
        return remote(full.at[tp, :, to], rows.at[slot], rows_send, rows_recv, "tp", to)

    def ask_copy(to, slot):
        return remote(asks.at[to], asked.at[slot], ask_send, ask_recv, "kv", to)

    def serve_copy(to, slot):
        target = pool.at[tp, pl.ds(blocks + slot * PER_OWNER, PER_OWNER)]
        return remote(served.at[to], target, serve_send, serve_recv.at[lax.div(slot, share)], "kv", to)

    def peer(i):
        return lax.rem(tp + i, peers)

    each(1, peers, lambda i: rows_copy(peer(i), tp).start())
    token_spread = Spread(
        full.reshape(peers, blocks * peers, group, width), 0, blocks * peers, spread_send.at[0], spread_recv.at[0]
    )
    token_spread.own()

    tile = (blocks, 128)
    lane = lax.broadcasted_iota(jnp.int32, tile, 1)
    sub = lax.broadcasted_iota(jnp.int32, tile, 0)
    ids = lane * blocks + sub

    small[0].wait()

    def mark(b, needed):
        for c in range(picks):
            needed = jnp.where(ids == chosen[b, c], 1, needed)
        return needed

    needed = lax.fori_loop(0, blocks, mark, jnp.zeros(tile, jnp.int32))
    first = jnp.full((1, 128), -1, jnp.int32)
    second = first
    for j in reversed(range(blocks)):
        hit = needed[j : j + 1, :] > 0
        second = jnp.where(hit, first, second)
        first = jnp.where(hit, j, first)
    both = jnp.where(sub == 0, first, jnp.where(sub == 1, second, 0))
    listed[...] = both
    to_scalars = pltpu.make_async_copy(listed, table, local_sem.at[4])
    to_scalars.start()
    both = both.astype(jnp.float32)

    for o in range(owners):
        spread_out = jnp.sum(jnp.where(lane == o, both, 0.0), axis=1, keepdims=True)
        asks[o] = jnp.broadcast_to(spread_out, tile)[:PER_OWNER]
    others = owners - 1

    def owner_at(i):
        return lax.rem(kv + i, owners)

    each(1, owners, lambda i: ask_copy(owner_at(i), kv).start())

    ones = jnp.ones((ONES, BLOCK), jnp.bfloat16)

    def fill(slot):
        values[slot, BLOCK:, :] = ones

    each(0, slots, fill)
    key = lax.broadcasted_iota(jnp.int32, bias.shape[1:], 0)
    query = lax.rem(lax.broadcasted_iota(jnp.int32, bias.shape[1:], 1), BLOCK)
    bias[0] = jnp.where(key <= query, 0.0, masked_score)
    bias[1] = jnp.zeros(bias.shape[1:], jnp.float32)
    keys[slots] = jnp.zeros((BLOCK, width), jnp.bfloat16)
    values[slots] = jnp.zeros((BLOCK + ONES, BLOCK), jnp.bfloat16)
    def place(b):
        for c in range(picks):
            block = chosen[b, c]
            held = jnp.maximum(block, 0)
            owner = lax.div(held, blocks)
            inside = held - owner * blocks
            away = blocks + owner * PER_OWNER + jnp.where(table[1, owner] == inside, 1, 0)
            places[b, c] = jnp.where(block < 0, slots, jnp.where(owner == kv, inside, away))

    to_scalars.wait()
    each(0, blocks, place)
    for copy in small[1:]:
        copy.wait()
    rows[tp] = full[tp, :, tp]
    own_latent.wait()
    wait_bytes(rows.at[pl.ds(0, peers - 1)], rows_recv)

    @jax.jit
    def compress():
        features = jnp.concatenate([rows[p].reshape(lines, width) for p in range(peers)], axis=1)
        latent = jnp.dot(features, weight[...], preferred_element_type=jnp.float32)
        return latent.astype(jnp.bfloat16).reshape(blocks, group, 128)

    latent = compress()
    pool[tp, 0:blocks] = latent
    latent = latent.astype(jnp.float32)

    def serve(i):
        r = owner_at(i)
        for k in range(PER_OWNER):
            want = asked[r, k : k + 1, :]
            picked = jnp.zeros((group, 128), jnp.float32)
            for j in range(blocks):
                picked = jnp.where(want == float(j), latent[j], picked)
            served[r, k] = picked.astype(jnp.bfloat16)
        serve_copy(r, kv).start()

    wait_bytes(asked.at[pl.ds(0, others)], ask_recv)
    each(owners // 2, owners, serve)
    each(1, owners // 2, serve)
    pltpu.make_async_copy(
        pool.at[tp, pl.ds(0, PER_OWNER)],
        pool.at[tp, pl.ds(blocks + kv * PER_OWNER, PER_OWNER)],
        serve_recv.at[lax.div(kv, share)],
    ).start()
    here = Spread(pool, 0, blocks, spread_send.at[1], spread_recv.at[1])
    here.own()

    spreads = [
        Spread(pool, blocks + i * share * PER_OWNER, share * PER_OWNER, spread_send.at[2 + i], spread_recv.at[2 + i])
        for i in range(PIECES)
    ]

    def gathered(i):
        per_piece = share * PER_OWNER
        wait_bytes(pool.at[tp, pl.ds(blocks + i * per_piece, per_piece)], serve_recv.at[i])
        spreads[i].own()

    scale = width ** (-0.5) * LOG2E
    query_row = query_gain[...] * scale

    def project(b):
        features = jnp.concatenate([full[p, b].reshape(BLOCK, width) for p in range(peers)], axis=1)
        projected = jnp.dot(features, projection[...], preferred_element_type=jnp.float32)
        projected = projected.astype(jnp.bfloat16).astype(jnp.float32)
        for h in range(up.shape[0]):
            queries[b, h * BLOCK : (h + 1) * BLOCK, :] = unit(projected[:, h * 128 : (h + 1) * 128], query_row)

    def prepare(low, high):
        def several(j):
            for i in range(4):
                slot = low + 4 * j + i
                block = pool[:, slot].reshape(BLOCK, width).astype(jnp.float32)
                keys[slot] = unit(block, key_gain[...])
                values[slot, :BLOCK, :] = jnp.transpose(block).astype(jnp.bfloat16)

        each(0, (high - low) // 4, several)

    wait_bytes(rows.at[pl.ds(0, peers - 1)], rows_send)
    token_spread.relay_first()
    here.relay_first()
    for i in range(PIECES):
        gathered(i)
    here.relay_rest()
    token_spread.relay_rest()
    token_spread.finish()
    here.finish()
    for spread in spreads:
        spread.relay_first()
    own_query.wait()
    own_out.wait()
    each(0, blocks, project)
    prepare(0, blocks)
    out_spread = Spread(wide_weight, 0, 128, spread_send.at[2 + PIECES], spread_recv.at[2 + PIECES])
    for i in range(PIECES):
        spreads[i].relay_rest()
        if i == PIECES - 1:
            out_spread.own()
        spreads[i].finish()
        prepare(blocks + i * share * PER_OWNER, blocks + (i + 1) * share * PER_OWNER)
    token_spread.drain()

    def heads_copy(to, b, slot):
        return remote(staged.at[b, to], heads.at[slot, b], heads_send, heads_recv.at[lax.div(b, HALF)], "tp", to)

    sides, heads_here = 2, up.shape[0]
    span = GROUP * BLOCK
    weights = full.reshape(sides, heads_here, -1, width)

    def weigh(b, side, g):
        picked = jnp.concatenate([keys[places[b, g * GROUP + i]] for i in range(GROUP)], axis=0)
        scores = lax.dot_general(
            picked, queries[b], (((1,), (1,)), ((), ())), preferred_element_type=jnp.float32
        )
        diagonal = jnp.exp2(scores[:BLOCK] + bias[jnp.minimum(g, 1)]).astype(jnp.bfloat16)
        others = jnp.exp2(scores[BLOCK:]).astype(jnp.bfloat16)
        for h in range(heads_here):
            cols = slice(h * BLOCK, (h + 1) * BLOCK)
            weights[side, h, :BLOCK, :] = diagonal[:, cols]
            weights[side, h, BLOCK:span, :] = others[:, cols]

    def add_up(b, side, g):
        held = jnp.concatenate([values[places[b, g * GROUP + i]] for i in range(GROUP)], axis=1)
        right = jnp.concatenate([weights[side, h, :span, :] for h in range(heads_here)], axis=1)
        return jnp.dot(held, right, preferred_element_type=jnp.float32)

    def hand_over(b, ended):
        shares = []
        for total in ended:
            shares.append((total[:BLOCK] / total[BLOCK : BLOCK + 1]).astype(jnp.bfloat16))
        turned, flipped = [], []
        for side in range(sides):
            for h in range(heads_here):
                share = shares[side][:, h * BLOCK : (h + 1) * BLOCK]
                turned.append(jnp.dot(up[h], share, preferred_element_type=jnp.float32))
        for side in range(sides):
            both = jnp.concatenate(turned[side * heads_here : (side + 1) * heads_here], axis=0)
            flipped.append(jnp.transpose(both).astype(jnp.bfloat16).reshape(peers, group, width))
        for side in range(sides):
            staged[b + side] = flipped[side]

    def attend(i):
        first = sides * i
        for side in range(sides):
            weigh(first + side, side, 0)
            totals[side] = jnp.zeros(totals.shape[1:], jnp.float32)

        def both(g):
            for side in range(sides):
                totals[side] = totals[side] + add_up(first + side, side, g - 1)
            for side in range(sides):
                weigh(first + side, side, g)

        each(1, picks // GROUP, both)
        ended = [totals[side] + add_up(first + side, side, picks // GROUP - 1) for side in range(sides)]
        hand_over(first, ended)
        for side in range(sides):
            each(1, peers, lambda j: heads_copy(peer(j), first + side, tp).start())

    def out_copy(to, half, slot):
        lower = pl.ds(half * HALF, HALF)
        return remote(
            rows.at[to, lower], out.at[lower, slot], out_send, out_recv, "tp", to
        )

    @functools.partial(jax.jit, static_argnums=0)
    def mix(half):
        lower = pl.ds(half * HALF, HALF)
        features = jnp.concatenate([heads[p, lower].reshape(HALF * group, width) for p in range(peers)], axis=1)
        summed = jnp.dot(
            features, wide_weight[...].reshape(peers * 128, peers * 128), preferred_element_type=jnp.float32
        )
        mixed = unit(summed, out_gain[...])
        for t in range(peers):
            rows[t, lower] = mixed[:, t * 128 : (t + 1) * 128].reshape(HALF, group, 128)

    def conclude(half):
        lower = pl.ds(half * HALF, HALF)

        wait_bytes(heads.at[pl.ds(0, peers - 1), lower], heads_recv.at[half])
        for b in range(HALF):
            heads[tp, half * HALF + b] = staged[half * HALF + b, tp]
        mix(half)
        each(1, peers, lambda i: out_copy(peer(i), half, tp).start())
        out[lower, tp] = rows[tp, lower]

    def turn(i):
        attend(i)

        @pl.when(i == 0)
        def _():
            out_spread.relay_first()

        @pl.when(i == 2)
        def _():
            out_spread.relay_rest()

    each(0, blocks // sides, turn)
    out_spread.finish()
    conclude(0)
    conclude(1)

    wait_bytes(asks.at[pl.ds(0, others)], ask_send)
    wait_bytes(served.at[pl.ds(0, others)], serve_send)
    for spread in (here, out_spread, *spreads):
        spread.drain()
    wait_bytes(staged.at[:, pl.ds(0, peers - 1)], heads_send)
    wait_bytes(rows.at[pl.ds(0, peers - 1)], out_send)
    wait_bytes(out.at[:, pl.ds(0, peers - 1)], out_recv)


def shards(
    tokens, query_weight, latent_weight, query_gain, key_gain, value_up, out_weight, out_gain, chosen
):
    peers, owners = lax.axis_size("tp"), lax.axis_size("kv")
    blocks, picks = chosen.shape
    rows, width = tokens.shape
    group = BLOCK // peers
    slots = blocks + owners * PER_OWNER
    heads = value_up.shape[0]
    vmem = pl.BlockSpec(memory_space=pltpu.VMEM)
    anywhere = pl.BlockSpec(memory_space=pl.ANY)
    dma = pltpu.SemaphoreType.DMA
    bf16 = jnp.bfloat16
    mixed = pl.pallas_call(
        kernel,
        out_shape=jax.ShapeDtypeStruct((blocks, peers, group, width), bf16),
        in_specs=[anywhere] * 9,
        out_specs=vmem,
        scratch_shapes=[
            pltpu.SMEM((blocks, picks), jnp.int32),
            pltpu.VMEM((1, width), jnp.float32),
            pltpu.VMEM((1, width), jnp.float32),
            pltpu.VMEM((heads, value_up.shape[2], width), bf16),
            pltpu.VMEM((1, out_gain.shape[0]), jnp.float32),
            pltpu.VMEM((peers, blocks, peers, group, width), bf16),
            pltpu.VMEM((peers, slots, group, width), bf16),
            pltpu.VMEM((peers, *out_weight.shape), bf16),
            pltpu.VMEM(latent_weight.shape, bf16),
            pltpu.VMEM(query_weight.shape, bf16),
            pltpu.VMEM((peers, blocks, group, width), bf16),
            pltpu.VMEM((owners, PER_OWNER, 128), jnp.float32),
            pltpu.VMEM((owners, PER_OWNER, 128), jnp.float32),
            pltpu.VMEM((owners, PER_OWNER, group, width), bf16),
            pltpu.VMEM((blocks, 128), jnp.int32),
            pltpu.SMEM((blocks, 128), jnp.int32),
            pltpu.VMEM((blocks, heads * BLOCK, width), bf16),
            pltpu.VMEM((slots + 1, BLOCK, width), bf16),
            pltpu.VMEM((slots + 1, BLOCK + ONES, BLOCK), bf16),
            pltpu.VMEM((2, BLOCK + ONES, heads * BLOCK), jnp.float32),
            pltpu.VMEM((2, BLOCK, heads * BLOCK), jnp.float32),
            pltpu.SMEM((blocks, picks), jnp.int32),
            pltpu.VMEM((blocks, peers, group, width), bf16),
            pltpu.VMEM((peers, blocks, group, width), bf16),
            dma((10,)),
            dma, dma,
            dma, dma,
            dma, dma((PIECES,)),
            dma, dma((2,)),
            dma, dma,
            dma((3 + PIECES,)), dma((3 + PIECES, 3)),
        ],
        compiler_params=pltpu.CompilerParams(collective_id=0, has_side_effects=True),
    )(
        chosen,
        tokens.reshape(blocks, peers, group, width),
        latent_weight,
        query_weight,
        out_weight,
        query_gain.reshape(1, width),
        key_gain.reshape(1, width),
        jnp.swapaxes(value_up, 1, 2),
        out_gain.reshape(1, out_gain.shape[0]),
    )
    return mixed.reshape(rows, width)


def solution(mesh):
    in_specs = (
        P("kv", "tp"),
        P(None, "tp"),
        P(),
        P(),
        P(),
        P("tp", None, None),
        P("tp", None),
        P(),
        P("kv", None),
    )
    return jax.shard_map(shards, mesh=mesh, in_specs=in_specs, out_specs=P("kv", "tp"), check_vma=False)
```

```python
import functools

import jax
import jax.numpy as jnp
from jax import lax
from jax.experimental import pallas as pl
from jax.experimental.pallas import tpu as pltpu
from jax.sharding import PartitionSpec as P

BLOCK = 128
PER_OWNER = 2
MESH = pl.DeviceIdType.MESH
GROUP = 8
PIECES = 4
ONES = 16
HALF = 4
LOG2E = 1.4426950408889634


epsilon = 1e-06
masked_score = -1e30


def neighbours(tp):
    side = lax.rem(tp, 2)
    right = lax.rem(tp + 2, 8)
    left = lax.rem(tp + 6, 8)
    far = lax.rem(tp + 4, 8)
    return right, left, far, tp + 1 - 2 * side


class Spread:
    def __init__(self, full, first, size, send_sem, recv_sem):
        self.full, self.send_sem, self.recv_sem = full, send_sem, recv_sem
        half = size // 2
        self.ranges = ((first, half), (first + half, size - half))
        self.tp = lax.axis_index("tp")
        self.right, self.left, self.far, self.other = neighbours(self.tp)

    def sends(self):
        me, right, left, far, other = self.tp, self.right, self.left, self.far, self.other
        return (
            (me, 0, right, 0), (me, 1, left, 0), (me, 1, right, 1), (me, 0, left, 1), (me, 0, other, 2), (me, 1, other, 2),
            (left, 0, right, 1), (right, 1, left, 1), (left, 0, other, 2), (right, 1, other, 2), (left, 1, other, 2),
            (right, 0, other, 2), (far, 0, other, 2), (far, 1, other, 2),
        )

    def start(self, *kinds):
        every = self.sends()
        for kind in kinds:
            slot, part, dest, arrival = every[kind]
            first, size = self.ranges[part]
            piece = self.full.at[slot, pl.ds(first, size)]
            remote(piece, piece, self.send_sem, self.recv_sem.at[arrival], "tp", dest).start()

    def slices(self, count, sem):
        wait_bytes(self.full.at[pl.ds(0, count), pl.ds(self.ranges[0][0], sum(size for _, size in self.ranges))], sem)

    def own(self):
        self.start(0, 1, 2, 3, 4, 5)

    def relay_first(self):
        self.slices(1, self.recv_sem.at[0])
        self.start(6, 7, 8, 9)

    def relay_rest(self):
        self.slices(2, self.recv_sem.at[1])
        self.start(10, 11, 12, 13)

    def finish(self):
        self.slices(4, self.recv_sem.at[2])

    def drain(self):
        self.slices(7, self.send_sem)


def wait_bytes(region, sem):
    pltpu.make_async_copy(region, region, sem).wait()


def each(low, high, act):
    def step(i, carry):
        act(i)
        return carry

    lax.fori_loop(low, high, step, 0)


def remote(source, target, send_sem, recv_sem, axis, to):
    return pltpu.make_async_remote_copy(
        src_ref=source,
        dst_ref=target,
        send_sem=send_sem,
        recv_sem=recv_sem,
        device_id={axis: to},
        device_id_type=MESH,
    )


def unit(values, gain_row):
    mean_sq = jnp.mean(values * values, axis=-1, keepdims=True)
    return (values * lax.rsqrt(mean_sq + epsilon) * gain_row).astype(jnp.bfloat16)


def kernel(
    chosen_in, tokens, latent_weight, query_weight, out_weight, query_gain_in, key_gain_in, up_in, out_gain_in,
    out,
    chosen, query_gain, key_gain, up, out_gain,
    full, pool, wide_weight, weight, projection, rows, asked, asks, served, listed, table,
    queries, keys, values, totals, bias, places, staged, heads,
    local_sem, rows_send, rows_recv, ask_send, ask_recv, serve_send, serve_recv,
    heads_send, heads_recv, out_send, out_recv, spread_send, spread_recv,
):
    kv, tp = lax.axis_index("kv"), lax.axis_index("tp")
    owners, peers = asked.shape[0], full.shape[0]
    blocks, group, width = rows.shape[1:]
    picks = chosen.shape[1]
    slots = pool.shape[1]
    lines = blocks * group

    own_tokens = pltpu.make_async_copy(tokens, full.at[tp], local_sem.at[0])
    own_latent = pltpu.make_async_copy(latent_weight, weight, local_sem.at[1])
    own_query = pltpu.make_async_copy(query_weight, projection, local_sem.at[2])
    own_out = pltpu.make_async_copy(out_weight, wide_weight.at[tp], local_sem.at[3])
    small = [
        pltpu.make_async_copy(source, target, local_sem.at[5 + i])
        for i, (source, target) in enumerate(
            (
                (chosen_in, chosen), (query_gain_in, query_gain), (key_gain_in, key_gain), (up_in, up), (out_gain_in, out_gain)
            )
        )
    ]
    barrier = pltpu.get_barrier_semaphore()

    def greet(axis, index, size):
        def signal(step):
            pl.semaphore_signal(barrier, inc=1, device_id={axis: lax.rem(index + step, size)}, device_id_type=MESH)

        each(1, size, signal)

    greet("kv", kv, owners)
    greet("tp", tp, peers)

    for copy in (own_tokens, *small, own_latent, own_query, own_out):
        copy.start()
    own_tokens.wait()
    pl.semaphore_wait(barrier, owners + peers - 2)

    share = owners // PIECES

    def rows_copy(to, slot):
        return remote(full.at[tp, :, to], rows.at[slot], rows_send, rows_recv, "tp", to)

    def ask_copy(to, slot):
        return remote(asks.at[to], asked.at[slot], ask_send, ask_recv, "kv", to)

    def serve_target(slot):
        return pool.at[tp, pl.ds(blocks + slot * PER_OWNER, PER_OWNER)]

    def serve_copy(to, slot):
        return remote(served.at[to], serve_target(slot), serve_send, serve_recv.at[lax.div(slot, share)], "kv", to)

    def peer(i):
        return lax.rem(tp + i, peers)

    each(1, peers, lambda i: rows_copy(peer(i), tp).start())
    token_spread = Spread(
        full.reshape(peers, blocks * peers, group, width), 0, blocks * peers, spread_send.at[0], spread_recv.at[0]
    )
    token_spread.own()

    tile = (blocks, 128)
    lane = lax.broadcasted_iota(jnp.int32, tile, 1)
    sub = lax.broadcasted_iota(jnp.int32, tile, 0)
    ids = lane * blocks + sub

    small[0].wait()

    def mark(b, needed):
        for c in range(picks):
            needed = jnp.where(ids == chosen[b, c], 1, needed)
        return needed

    needed = lax.fori_loop(0, blocks, mark, jnp.zeros(tile, jnp.int32))
    first = jnp.full((1, 128), -1, jnp.int32)
    second = first
    for j in reversed(range(blocks)):
        hit = needed[j : j + 1, :] > 0
        second = jnp.where(hit, first, second)
        first = jnp.where(hit, j, first)
    both = jnp.where(sub == 0, first, jnp.where(sub == 1, second, 0))
    listed[...] = both
    to_scalars = pltpu.make_async_copy(listed, table, local_sem.at[4])
    to_scalars.start()
    both = both.astype(jnp.float32)

    for o in range(owners):
        spread_out = jnp.sum(jnp.where(lane == o, both, 0.0), axis=1, keepdims=True)
        asks[o] = jnp.broadcast_to(spread_out, tile)[:PER_OWNER]
    others = owners - 1

    def stay(source, target, sem):
        pltpu.make_async_copy(source, target, sem).start()

    each(0, kv, lambda o: ask_copy(o, kv).start())
    each(0, kv, lambda o: stay(asks.at[kv], asked.at[o], ask_recv))
    each(kv + 1, owners, lambda o: stay(asks.at[kv], asks.at[o], ask_send))

    ones = jnp.ones((ONES, BLOCK), jnp.bfloat16)

    def fill(slot):
        values[slot, BLOCK:, :] = ones

    each(0, slots, fill)
    key = lax.broadcasted_iota(jnp.int32, bias.shape[1:], 0)
    query = lax.rem(lax.broadcasted_iota(jnp.int32, bias.shape[1:], 1), BLOCK)
    bias[0] = jnp.where(key <= query, 0.0, masked_score)
    bias[1] = jnp.zeros(bias.shape[1:], jnp.float32)
    keys[slots] = jnp.zeros((BLOCK, width), jnp.bfloat16)
    values[slots] = jnp.zeros((BLOCK + ONES, BLOCK), jnp.bfloat16)
    def place(b):
        for c in range(picks):
            block = chosen[b, c]
            held = jnp.maximum(block, 0)
            owner = lax.div(held, blocks)
            inside = held - owner * blocks
            away = blocks + owner * PER_OWNER + jnp.where(table[1, owner] == inside, 1, 0)
            places[b, c] = jnp.where(block < 0, slots, jnp.where(owner == kv, inside, away))

    to_scalars.wait()
    each(0, blocks, place)
    for copy in small[1:]:
        copy.wait()
    rows[tp] = full[tp, :, tp]
    own_latent.wait()
    wait_bytes(rows.at[pl.ds(0, peers - 1)], rows_recv)

    @jax.jit
    def compress():
        features = jnp.concatenate([rows[p].reshape(lines, width) for p in range(peers)], axis=1)
        latent = jnp.dot(features, weight[...], preferred_element_type=jnp.float32)
        return latent.astype(jnp.bfloat16).reshape(blocks, group, 128)

    latent = compress()
    pool[tp, 0:blocks] = latent
    latent = latent.astype(jnp.float32)

    def serve(i):
        r = others - i
        for k in range(PER_OWNER):
            want = asked[r, k : k + 1, :]
            picked = jnp.zeros((group, 128), jnp.float32)
            for j in range(blocks):
                picked = jnp.where(want == float(j), latent[j], picked)
            served[r, k] = picked.astype(jnp.bfloat16)
        serve_copy(r, kv).start()

    wait_bytes(asked.at[pl.ds(0, others)], ask_recv)
    each(0, others - kv, serve)
    low = pool.at[tp, pl.ds(0, PER_OWNER)]
    each(0, kv, lambda o: stay(low, served.at[o], serve_send))
    each(kv, owners, lambda o: stay(low, serve_target(o), serve_recv.at[lax.div(o, share)]))
    here = Spread(pool, 0, blocks, spread_send.at[1], spread_recv.at[1])
    here.own()

    spreads = [
        Spread(pool, blocks + i * share * PER_OWNER, share * PER_OWNER, spread_send.at[2 + i], spread_recv.at[2 + i])
        for i in range(PIECES)
    ]

    def gathered(i):
        per_piece = share * PER_OWNER
        wait_bytes(pool.at[tp, pl.ds(blocks + i * per_piece, per_piece)], serve_recv.at[i])
        spreads[i].own()

    scale = width ** (-0.5) * LOG2E
    query_row = query_gain[...] * scale

    def project(b):
        features = jnp.concatenate([full[p, b].reshape(BLOCK, width) for p in range(peers)], axis=1)
        projected = jnp.dot(features, projection[...], preferred_element_type=jnp.float32)
        projected = projected.astype(jnp.bfloat16).astype(jnp.float32)
        for h in range(up.shape[0]):
            queries[b, h * BLOCK : (h + 1) * BLOCK, :] = unit(projected[:, h * 128 : (h + 1) * 128], query_row)

    def prepare(low, high):
        def several(j):
            for i in range(4):
                slot = low + 4 * j + i
                block = pool[:, slot].reshape(BLOCK, width).astype(jnp.float32)
                keys[slot] = unit(block, key_gain[...])
                values[slot, :BLOCK, :] = jnp.transpose(block).astype(jnp.bfloat16)

        each(0, (high - low) // 4, several)

    wait_bytes(rows.at[pl.ds(0, peers - 1)], rows_send)
    token_spread.relay_first()
    token_spread.relay_rest()
    for i in range(PIECES):
        gathered(i)
    token_spread.finish()
    own_query.wait()
    own_out.wait()
    here.relay_first()
    each(0, blocks, project)
    here.relay_rest()
    for spread in spreads:
        spread.relay_first()
    here.finish()
    prepare(0, blocks)
    out_spread = Spread(wide_weight, 0, 128, spread_send.at[2 + PIECES], spread_recv.at[2 + PIECES])
    for spread in spreads:
        spread.relay_rest()
    out_spread.own()
    for i in range(PIECES):
        spreads[i].finish()
        prepare(blocks + i * share * PER_OWNER, blocks + (i + 1) * share * PER_OWNER)
    token_spread.drain()

    def heads_copy(to, b, slot):
        return remote(staged.at[b, to], heads.at[slot, b], heads_send, heads_recv.at[lax.div(b, HALF)], "tp", to)

    sides, heads_here = 2, up.shape[0]
    span = GROUP * BLOCK
    weights = full.reshape(sides, heads_here, -1, width)

    def weigh(b, side, g):
        picked = jnp.concatenate([keys[places[b, g * GROUP + i]] for i in range(GROUP)], axis=0)
        scores = lax.dot_general(
            picked, queries[b], (((1,), (1,)), ((), ())), preferred_element_type=jnp.float32
        )
        diagonal = jnp.exp2(scores[:BLOCK] + bias[jnp.minimum(g, 1)]).astype(jnp.bfloat16)
        others = jnp.exp2(scores[BLOCK:]).astype(jnp.bfloat16)
        for h in range(heads_here):
            cols = slice(h * BLOCK, (h + 1) * BLOCK)
            weights[side, h, :BLOCK, :] = diagonal[:, cols]
            weights[side, h, BLOCK:span, :] = others[:, cols]

    def add_up(b, side, g):
        held = jnp.concatenate([values[places[b, g * GROUP + i]] for i in range(GROUP)], axis=1)
        right = jnp.concatenate([weights[side, h, :span, :] for h in range(heads_here)], axis=1)
        return jnp.dot(held, right, preferred_element_type=jnp.float32)

    def hand_over(b, ended):
        shares = []
        for total in ended:
            shares.append((total[:BLOCK] / total[BLOCK : BLOCK + 1]).astype(jnp.bfloat16))
        turned, flipped = [], []
        for side in range(sides):
            for h in range(heads_here):
                share = shares[side][:, h * BLOCK : (h + 1) * BLOCK]
                turned.append(jnp.dot(up[h], share, preferred_element_type=jnp.float32))
        for side in range(sides):
            both = jnp.concatenate(turned[side * heads_here : (side + 1) * heads_here], axis=0)
            flipped.append(jnp.transpose(both).astype(jnp.bfloat16).reshape(peers, group, width))
        for side in range(sides):
            staged[b + side] = flipped[side]

    def attend(i):
        first = sides * i
        for side in range(sides):
            weigh(first + side, side, 0)
            totals[side] = jnp.zeros(totals.shape[1:], jnp.float32)

        def both(g):
            for side in range(sides):
                totals[side] = totals[side] + add_up(first + side, side, g - 1)
            for side in range(sides):
                weigh(first + side, side, g)

        each(1, picks // GROUP, both)
        ended = [totals[side] + add_up(first + side, side, picks // GROUP - 1) for side in range(sides)]
        hand_over(first, ended)
        for side in range(sides):
            each(1, peers, lambda j: heads_copy(peer(j), first + side, tp).start())

    def out_copy(to, half, slot):
        lower = pl.ds(half * HALF, HALF)
        return remote(
            rows.at[to, lower], out.at[lower, slot], out_send, out_recv, "tp", to
        )

    @functools.partial(jax.jit, static_argnums=0)
    def mix(half):
        lower = pl.ds(half * HALF, HALF)
        features = jnp.concatenate([heads[p, lower].reshape(HALF * group, width) for p in range(peers)], axis=1)
        summed = jnp.dot(
            features, wide_weight[...].reshape(peers * 128, peers * 128), preferred_element_type=jnp.float32
        )
        mixed = unit(summed, out_gain[...])
        for t in range(peers):
            rows[t, lower] = mixed[:, t * 128 : (t + 1) * 128].reshape(HALF, group, 128)

    def conclude(half):
        lower = pl.ds(half * HALF, HALF)

        wait_bytes(heads.at[pl.ds(0, peers - 1), lower], heads_recv.at[half])
        for b in range(HALF):
            heads[tp, half * HALF + b] = staged[half * HALF + b, tp]
        mix(half)
        each(1, peers, lambda i: out_copy(peer(i), half, tp).start())
        out[lower, tp] = rows[tp, lower]

    def turn(i):
        attend(i)

        @pl.when(i == 1)
        def _():
            out_spread.relay_first()

        @pl.when(i == 3)
        def _():
            out_spread.relay_rest()

    each(0, blocks // sides, turn)
    out_spread.finish()
    conclude(0)
    conclude(1)

    wait_bytes(asks.at[pl.ds(0, others)], ask_send)
    wait_bytes(served.at[pl.ds(0, others)], serve_send)
    for spread in (here, out_spread, *spreads):
        spread.drain()
    wait_bytes(staged.at[:, pl.ds(0, peers - 1)], heads_send)
    wait_bytes(rows.at[pl.ds(0, peers - 1)], out_send)
    wait_bytes(out.at[:, pl.ds(0, peers - 1)], out_recv)


def shards(
    tokens, query_weight, latent_weight, query_gain, key_gain, value_up, out_weight, out_gain, chosen
):
    peers, owners = lax.axis_size("tp"), lax.axis_size("kv")
    blocks, picks = chosen.shape
    rows, width = tokens.shape
    group = BLOCK // peers
    slots = blocks + owners * PER_OWNER
    heads = value_up.shape[0]
    vmem = pl.BlockSpec(memory_space=pltpu.VMEM)
    anywhere = pl.BlockSpec(memory_space=pl.ANY)
    dma = pltpu.SemaphoreType.DMA
    bf16 = jnp.bfloat16
    mixed = pl.pallas_call(
        kernel,
        out_shape=jax.ShapeDtypeStruct((blocks, peers, group, width), bf16),
        in_specs=[anywhere] * 9,
        out_specs=vmem,
        scratch_shapes=[
            pltpu.SMEM((blocks, picks), jnp.int32),
            pltpu.VMEM((1, width), jnp.float32),
            pltpu.VMEM((1, width), jnp.float32),
            pltpu.VMEM((heads, value_up.shape[2], width), bf16),
            pltpu.VMEM((1, out_gain.shape[0]), jnp.float32),
            pltpu.VMEM((peers, blocks, peers, group, width), bf16),
            pltpu.VMEM((peers, slots, group, width), bf16),
            pltpu.VMEM((peers, *out_weight.shape), bf16),
            pltpu.VMEM(latent_weight.shape, bf16),
            pltpu.VMEM(query_weight.shape, bf16),
            pltpu.VMEM((peers, blocks, group, width), bf16),
            pltpu.VMEM((owners, PER_OWNER, 128), jnp.float32),
            pltpu.VMEM((owners, PER_OWNER, 128), jnp.float32),
            pltpu.VMEM((owners, PER_OWNER, group, width), bf16),
            pltpu.VMEM((blocks, 128), jnp.int32),
            pltpu.SMEM((blocks, 128), jnp.int32),
            pltpu.VMEM((blocks, heads * BLOCK, width), bf16),
            pltpu.VMEM((slots + 1, BLOCK, width), bf16),
            pltpu.VMEM((slots + 1, BLOCK + ONES, BLOCK), bf16),
            pltpu.VMEM((2, BLOCK + ONES, heads * BLOCK), jnp.float32),
            pltpu.VMEM((2, BLOCK, heads * BLOCK), jnp.float32),
            pltpu.SMEM((blocks, picks), jnp.int32),
            pltpu.VMEM((blocks, peers, group, width), bf16),
            pltpu.VMEM((peers, blocks, group, width), bf16),
            dma((10,)),
            dma, dma,
            dma, dma,
            dma, dma((PIECES,)),
            dma, dma((2,)),
            dma, dma,
            dma((3 + PIECES,)), dma((3 + PIECES, 3)),
        ],
        compiler_params=pltpu.CompilerParams(collective_id=0, has_side_effects=True),
    )(
        chosen,
        tokens.reshape(blocks, peers, group, width),
        latent_weight,
        query_weight,
        out_weight,
        query_gain.reshape(1, width),
        key_gain.reshape(1, width),
        jnp.swapaxes(value_up, 1, 2),
        out_gain.reshape(1, out_gain.shape[0]),
    )
    return mixed.reshape(rows, width)


def solution(mesh):
    in_specs = (
        P("kv", "tp"),
        P(None, "tp"),
        P(),
        P(),
        P(),
        P("tp", None, None),
        P("tp", None),
        P(),
        P("kv", None),
    )
    return jax.shard_map(shards, mesh=mesh, in_specs=in_specs, out_specs=P("kv", "tp"), check_vma=False)
```

```python
import functools

import jax
import jax.numpy as jnp
from jax import lax
from jax.experimental import pallas as pl
from jax.experimental.pallas import tpu as pltpu
from jax.sharding import PartitionSpec as P

BLOCK = 128
PER_OWNER = 2
MESH = pl.DeviceIdType.MESH
GROUP = 8
PIECES = 4
ONES = 16
HALF = 4
LOG2E = 1.4426950408889634


epsilon = 1e-06
masked_score = -1e30


def neighbours(tp):
    side = lax.rem(tp, 2)
    right = lax.rem(tp + 2, 8)
    left = lax.rem(tp + 6, 8)
    far = lax.rem(tp + 4, 8)
    return right, left, far, tp + 1 - 2 * side


class Spread:
    def __init__(self, full, first, size, send_sem, recv_sem):
        self.full, self.send_sem, self.recv_sem = full, send_sem, recv_sem
        half = size // 2
        self.ranges = ((first, half), (first + half, size - half))
        self.tp = lax.axis_index("tp")
        self.right, self.left, self.far, self.other = neighbours(self.tp)

    def sends(self):
        me, right, left, far, other = self.tp, self.right, self.left, self.far, self.other
        return (
            (me, 0, right, 0), (me, 1, left, 0), (me, 1, right, 1), (me, 0, left, 1), (me, 0, other, 2), (me, 1, other, 2),
            (left, 0, right, 1), (right, 1, left, 1), (left, 0, other, 2), (right, 1, other, 2), (left, 1, other, 2),
            (right, 0, other, 2), (far, 0, other, 2), (far, 1, other, 2),
        )

    def start(self, *kinds):
        every = self.sends()
        for kind in kinds:
            slot, part, dest, arrival = every[kind]
            first, size = self.ranges[part]
            piece = self.full.at[slot, pl.ds(first, size)]
            remote(piece, piece, self.send_sem, self.recv_sem.at[arrival], "tp", dest).start()

    def slices(self, count, sem):
        wait_bytes(self.full.at[pl.ds(0, count), pl.ds(self.ranges[0][0], sum(size for _, size in self.ranges))], sem)

    def own(self):
        self.start(0, 1, 2, 3, 4, 5)

    def relay_first(self):
        self.slices(1, self.recv_sem.at[0])
        self.start(6, 7, 8, 9)

    def relay_rest(self):
        self.slices(2, self.recv_sem.at[1])
        self.start(10, 11, 12, 13)

    def finish(self):
        self.slices(4, self.recv_sem.at[2])

    def drain(self):
        self.slices(7, self.send_sem)


def wait_bytes(region, sem):
    pltpu.make_async_copy(region, region, sem).wait()


def each(low, high, act):
    def step(i, carry):
        act(i)
        return carry

    lax.fori_loop(low, high, step, 0)


def remote(source, target, send_sem, recv_sem, axis, to):
    return pltpu.make_async_remote_copy(
        src_ref=source,
        dst_ref=target,
        send_sem=send_sem,
        recv_sem=recv_sem,
        device_id={axis: to},
        device_id_type=MESH,
    )


def unit(values, gain_row):
    mean_sq = jnp.mean(values * values, axis=-1, keepdims=True)
    return (values * lax.rsqrt(mean_sq + epsilon) * gain_row).astype(jnp.bfloat16)


def kernel(
    chosen_in, tokens, latent_weight, query_weight, out_weight, query_gain_in, key_gain_in, up_in, out_gain_in,
    out,
    chosen, query_gain, key_gain, up, out_gain,
    full, pool, wide_weight, weight, projection, rows, asked, asks, served, listed, table,
    queries, keys, values, totals, bias, places, staged, heads,
    local_sem, rows_send, rows_recv, ask_send, ask_recv, serve_send, serve_recv,
    heads_send, heads_recv, out_send, out_recv, spread_send, spread_recv,
):
    kv, tp = lax.axis_index("kv"), lax.axis_index("tp")
    owners, peers = asked.shape[0], full.shape[0]
    blocks, group, width = rows.shape[1:]
    picks = chosen.shape[1]
    slots = pool.shape[1]
    lines = blocks * group

    own_tokens = pltpu.make_async_copy(tokens, full.at[tp], local_sem.at[0])
    own_latent = pltpu.make_async_copy(latent_weight, weight, local_sem.at[1])
    own_query = pltpu.make_async_copy(query_weight, projection, local_sem.at[2])
    own_out = pltpu.make_async_copy(out_weight, wide_weight.at[tp], local_sem.at[3])
    small = [
        pltpu.make_async_copy(source, target, local_sem.at[5 + i])
        for i, (source, target) in enumerate(
            (
                (chosen_in, chosen), (query_gain_in, query_gain), (key_gain_in, key_gain), (up_in, up), (out_gain_in, out_gain)
            )
        )
    ]
    barrier = pltpu.get_barrier_semaphore()

    def greet(axis, index, size):
        def signal(step):
            pl.semaphore_signal(barrier, inc=1, device_id={axis: lax.rem(index + step, size)}, device_id_type=MESH)

        each(1, size, signal)

    greet("kv", kv, owners)
    greet("tp", tp, peers)

    for copy in (own_tokens, *small, own_latent, own_query, own_out):
        copy.start()
    own_tokens.wait()
    pl.semaphore_wait(barrier, owners + peers - 2)

    share = owners // PIECES

    def rows_copy(to, slot):
        return remote(full.at[tp, :, to], rows.at[slot], rows_send, rows_recv, "tp", to)

    def ask_copy(to, slot):
        return remote(asks.at[to], asked.at[slot], ask_send, ask_recv, "kv", to)

    def serve_target(slot):
        return pool.at[tp, pl.ds(blocks + slot * PER_OWNER, PER_OWNER)]

    def serve_copy(to, slot):
        return remote(served.at[to], serve_target(slot), serve_send, serve_recv.at[lax.div(slot, share)], "kv", to)

    def peer(i):
        return lax.rem(tp + i, peers)

    each(1, peers, lambda i: rows_copy(peer(i), tp).start())
    token_spread = Spread(
        full.reshape(peers, blocks * peers, group, width), 0, blocks * peers, spread_send.at[0], spread_recv.at[0]
    )
    token_spread.own()

    tile = (blocks, 128)
    lane = lax.broadcasted_iota(jnp.int32, tile, 1)
    sub = lax.broadcasted_iota(jnp.int32, tile, 0)
    ids = lane * blocks + sub

    small[0].wait()

    def mark(b, needed):
        for c in range(picks):
            needed = jnp.where(ids == chosen[b, c], 1, needed)
        return needed

    needed = lax.fori_loop(0, blocks, mark, jnp.zeros(tile, jnp.int32))
    first = jnp.full((1, 128), -1, jnp.int32)
    second = first
    for j in reversed(range(blocks)):
        hit = needed[j : j + 1, :] > 0
        second = jnp.where(hit, first, second)
        first = jnp.where(hit, j, first)
    both = jnp.where(sub == 0, first, jnp.where(sub == 1, second, 0))
    listed[...] = both
    to_scalars = pltpu.make_async_copy(listed, table, local_sem.at[4])
    to_scalars.start()
    both = both.astype(jnp.float32)

    for o in range(owners):
        spread_out = jnp.sum(jnp.where(lane == o, both, 0.0), axis=1, keepdims=True)
        asks[o] = jnp.broadcast_to(spread_out, tile)[:PER_OWNER]
    others = owners - 1

    def stay(source, target, sem):
        pltpu.make_async_copy(source, target, sem).start()

    each(0, kv, lambda o: ask_copy(o, kv).start())
    each(0, kv, lambda o: stay(asks.at[kv], asked.at[o], ask_recv))
    each(kv + 1, owners, lambda o: stay(asks.at[kv], asks.at[o], ask_send))

    ones = jnp.ones((ONES, BLOCK), jnp.bfloat16)

    def fill(slot):
        values[slot, BLOCK:, :] = ones

    each(0, slots, fill)
    key = lax.broadcasted_iota(jnp.int32, bias.shape[1:], 0)
    query = lax.rem(lax.broadcasted_iota(jnp.int32, bias.shape[1:], 1), BLOCK)
    bias[0] = jnp.where(key <= query, 0.0, masked_score)
    bias[1] = jnp.zeros(bias.shape[1:], jnp.float32)
    keys[slots] = jnp.zeros((BLOCK, width), jnp.bfloat16)
    values[slots] = jnp.zeros((BLOCK + ONES, BLOCK), jnp.bfloat16)
    def place(b):
        for c in range(picks):
            block = chosen[b, c]
            held = jnp.maximum(block, 0)
            owner = lax.div(held, blocks)
            inside = held - owner * blocks
            away = blocks + owner * PER_OWNER + jnp.where(table[1, owner] == inside, 1, 0)
            places[b, c] = jnp.where(block < 0, slots, jnp.where(owner == kv, inside, away))

    to_scalars.wait()
    each(0, blocks, place)
    for copy in small[1:]:
        copy.wait()
    rows[tp] = full[tp, :, tp]
    own_latent.wait()
    wait_bytes(rows.at[pl.ds(0, peers - 1)], rows_recv)

    @jax.jit
    def compress():
        features = jnp.concatenate([rows[p].reshape(lines, width) for p in range(peers)], axis=1)
        latent = jnp.dot(features, weight[...], preferred_element_type=jnp.float32)
        return latent.astype(jnp.bfloat16).reshape(blocks, group, 128)

    latent = compress()
    pool[tp, 0:blocks] = latent
    latent = latent.astype(jnp.float32)

    def serve(i):
        r = others - i
        for k in range(PER_OWNER):
            want = asked[r, k : k + 1, :]
            picked = jnp.zeros((group, 128), jnp.float32)
            for j in range(blocks):
                picked = jnp.where(want == float(j), latent[j], picked)
            served[r, k] = picked.astype(jnp.bfloat16)
        serve_copy(r, kv).start()

    wait_bytes(asked.at[pl.ds(0, others)], ask_recv)
    each(0, others - kv, serve)
    low = pool.at[tp, pl.ds(0, PER_OWNER)]
    each(0, kv, lambda o: stay(low, served.at[o], serve_send))
    each(kv, owners, lambda o: stay(low, serve_target(o), serve_recv.at[lax.div(o, share)]))
    here = Spread(pool, 0, blocks, spread_send.at[1], spread_recv.at[1])
    here.own()

    spreads = [
        Spread(pool, blocks + i * share * PER_OWNER, share * PER_OWNER, spread_send.at[2 + i], spread_recv.at[2 + i])
        for i in range(PIECES)
    ]

    def gathered(i):
        per_piece = share * PER_OWNER
        wait_bytes(pool.at[tp, pl.ds(blocks + i * per_piece, per_piece)], serve_recv.at[i])
        spreads[i].own()

    scale = width ** (-0.5) * LOG2E
    query_row = query_gain[...] * scale

    def project(b):
        features = jnp.concatenate([full[p, b].reshape(BLOCK, width) for p in range(peers)], axis=1)
        projected = jnp.dot(features, projection[...], preferred_element_type=jnp.float32)
        projected = projected.astype(jnp.bfloat16).astype(jnp.float32)
        for h in range(up.shape[0]):
            queries[b, h * BLOCK : (h + 1) * BLOCK, :] = unit(projected[:, h * 128 : (h + 1) * 128], query_row)

    def prepare(low, high):
        def several(j):
            for i in range(4):
                slot = low + 4 * j + i
                block = pool[:, slot].reshape(BLOCK, width).astype(jnp.float32)
                keys[slot] = unit(block, key_gain[...])
                values[slot, :BLOCK, :] = jnp.transpose(block).astype(jnp.bfloat16)

        each(0, (high - low) // 4, several)

    wait_bytes(rows.at[pl.ds(0, peers - 1)], rows_send)
    token_spread.relay_first()
    here.relay_first()
    token_spread.relay_rest()
    for i in range(PIECES):
        gathered(i)
    token_spread.finish()
    own_query.wait()
    own_out.wait()
    each(0, blocks, project)
    for spread in spreads:
        spread.relay_first()
    out_spread = Spread(wide_weight, 0, 128, spread_send.at[2 + PIECES], spread_recv.at[2 + PIECES])
    out_spread.own()
    here.relay_rest()
    here.finish()
    prepare(0, blocks)

    def complete(i):
        spreads[i].finish()
        prepare(blocks + i * share * PER_OWNER, blocks + (i + 1) * share * PER_OWNER)

    spreads[0].relay_rest()
    for i in range(1, PIECES):
        spreads[i].relay_rest()
        complete(i - 1)
    complete(PIECES - 1)
    token_spread.drain()

    def heads_copy(to, b, slot):
        return remote(staged.at[b, to], heads.at[slot, b], heads_send, heads_recv.at[lax.div(b, HALF)], "tp", to)

    sides, heads_here = 2, up.shape[0]
    span = GROUP * BLOCK
    weights = full.reshape(sides, heads_here, -1, width)

    def weigh(b, side, g):
        picked = jnp.concatenate([keys[places[b, g * GROUP + i]] for i in range(GROUP)], axis=0)
        scores = lax.dot_general(
            picked, queries[b], (((1,), (1,)), ((), ())), preferred_element_type=jnp.float32
        )
        diagonal = jnp.exp2(scores[:BLOCK] + bias[jnp.minimum(g, 1)]).astype(jnp.bfloat16)
        others = jnp.exp2(scores[BLOCK:]).astype(jnp.bfloat16)
        for h in range(heads_here):
            cols = slice(h * BLOCK, (h + 1) * BLOCK)
            weights[side, h, :BLOCK, :] = diagonal[:, cols]
            weights[side, h, BLOCK:span, :] = others[:, cols]

    def add_up(b, side, g):
        held = jnp.concatenate([values[places[b, g * GROUP + i]] for i in range(GROUP)], axis=1)
        right = jnp.concatenate([weights[side, h, :span, :] for h in range(heads_here)], axis=1)
        return jnp.dot(held, right, preferred_element_type=jnp.float32)

    def hand_over(b, ended):
        shares = []
        for total in ended:
            shares.append((total[:BLOCK] / total[BLOCK : BLOCK + 1]).astype(jnp.bfloat16))
        turned, flipped = [], []
        for side in range(sides):
            for h in range(heads_here):
                share = shares[side][:, h * BLOCK : (h + 1) * BLOCK]
                turned.append(jnp.dot(up[h], share, preferred_element_type=jnp.float32))
        for side in range(sides):
            both = jnp.concatenate(turned[side * heads_here : (side + 1) * heads_here], axis=0)
            flipped.append(jnp.transpose(both).astype(jnp.bfloat16).reshape(peers, group, width))
        for side in range(sides):
            staged[b + side] = flipped[side]

    def start(i):
        for side in range(sides):
            weigh(sides * i + side, side, 0)

    def attend(i, following):
        first = sides * i
        for side in range(sides):
            totals[side] = jnp.zeros(totals.shape[1:], jnp.float32)

        def both(g):
            for side in range(sides):
                totals[side] = totals[side] + add_up(first + side, side, g - 1)
            for side in range(sides):
                weigh(first + side, side, g)

        each(1, picks // GROUP, both)
        ended = [totals[side] + add_up(first + side, side, picks // GROUP - 1) for side in range(sides)]
        if following:
            start(i + 1)
        hand_over(first, ended)
        for side in range(sides):
            each(1, peers, lambda j: heads_copy(peer(j), first + side, tp).start())

    def out_copy(to, half, slot):
        lower = pl.ds(half * HALF, HALF)
        return remote(
            rows.at[to, lower], out.at[lower, slot], out_send, out_recv, "tp", to
        )

    @functools.partial(jax.jit, static_argnums=0)
    def mix(half):
        lower = pl.ds(half * HALF, HALF)
        features = jnp.concatenate([heads[p, lower].reshape(HALF * group, width) for p in range(peers)], axis=1)
        summed = jnp.dot(
            features, wide_weight[...].reshape(peers * 128, peers * 128), preferred_element_type=jnp.float32
        )
        mixed = unit(summed, out_gain[...])
        for t in range(peers):
            rows[t, lower] = mixed[:, t * 128 : (t + 1) * 128].reshape(HALF, group, 128)

    def conclude(half):
        lower = pl.ds(half * HALF, HALF)

        wait_bytes(heads.at[pl.ds(0, peers - 1), lower], heads_recv.at[half])
        for b in range(HALF):
            heads[tp, half * HALF + b] = staged[half * HALF + b, tp]
        mix(half)
        each(1, peers, lambda i: out_copy(peer(i), half, tp).start())
        out[lower, tp] = rows[tp, lower]

    def turn(i):
        attend(i, True)

        @pl.when(i == 0)
        def _():
            out_spread.relay_first()

        @pl.when(i == 2)
        def _():
            out_spread.relay_rest()
            out_spread.finish()
            conclude(0)

    last = blocks // sides - 1
    each(0, 1, start)
    each(0, last, turn)
    each(last, last + 1, lambda i: attend(i, False))
    conclude(1)

    wait_bytes(asks.at[pl.ds(0, others)], ask_send)
    wait_bytes(served.at[pl.ds(0, others)], serve_send)
    for spread in (here, out_spread, *spreads):
        spread.drain()
    wait_bytes(staged.at[:, pl.ds(0, peers - 1)], heads_send)
    wait_bytes(rows.at[pl.ds(0, peers - 1)], out_send)
    wait_bytes(out.at[:, pl.ds(0, peers - 1)], out_recv)


def shards(
    tokens, query_weight, latent_weight, query_gain, key_gain, value_up, out_weight, out_gain, chosen
):
    peers, owners = lax.axis_size("tp"), lax.axis_size("kv")
    blocks, picks = chosen.shape
    rows, width = tokens.shape
    group = BLOCK // peers
    slots = blocks + owners * PER_OWNER
    heads = value_up.shape[0]
    vmem = pl.BlockSpec(memory_space=pltpu.VMEM)
    anywhere = pl.BlockSpec(memory_space=pl.ANY)
    dma = pltpu.SemaphoreType.DMA
    bf16 = jnp.bfloat16
    mixed = pl.pallas_call(
        kernel,
        out_shape=jax.ShapeDtypeStruct((blocks, peers, group, width), bf16),
        in_specs=[anywhere] * 9,
        out_specs=vmem,
        scratch_shapes=[
            pltpu.SMEM((blocks, picks), jnp.int32),
            pltpu.VMEM((1, width), jnp.float32),
            pltpu.VMEM((1, width), jnp.float32),
            pltpu.VMEM((heads, value_up.shape[2], width), bf16),
            pltpu.VMEM((1, out_gain.shape[0]), jnp.float32),
            pltpu.VMEM((peers, blocks, peers, group, width), bf16),
            pltpu.VMEM((peers, slots, group, width), bf16),
            pltpu.VMEM((peers, *out_weight.shape), bf16),
            pltpu.VMEM(latent_weight.shape, bf16),
            pltpu.VMEM(query_weight.shape, bf16),
            pltpu.VMEM((peers, blocks, group, width), bf16),
            pltpu.VMEM((owners, PER_OWNER, 128), jnp.float32),
            pltpu.VMEM((owners, PER_OWNER, 128), jnp.float32),
            pltpu.VMEM((owners, PER_OWNER, group, width), bf16),
            pltpu.VMEM((blocks, 128), jnp.int32),
            pltpu.SMEM((blocks, 128), jnp.int32),
            pltpu.VMEM((blocks, heads * BLOCK, width), bf16),
            pltpu.VMEM((slots + 1, BLOCK, width), bf16),
            pltpu.VMEM((slots + 1, BLOCK + ONES, BLOCK), bf16),
            pltpu.VMEM((2, BLOCK + ONES, heads * BLOCK), jnp.float32),
            pltpu.VMEM((2, BLOCK, heads * BLOCK), jnp.float32),
            pltpu.SMEM((blocks, picks), jnp.int32),
            pltpu.VMEM((blocks, peers, group, width), bf16),
            pltpu.VMEM((peers, blocks, group, width), bf16),
            dma((10,)),
            dma, dma,
            dma, dma,
            dma, dma((PIECES,)),
            dma, dma((2,)),
            dma, dma,
            dma((3 + PIECES,)), dma((3 + PIECES, 3)),
        ],
        compiler_params=pltpu.CompilerParams(collective_id=0, has_side_effects=True),
    )(
        chosen,
        tokens.reshape(blocks, peers, group, width),
        latent_weight,
        query_weight,
        out_weight,
        query_gain.reshape(1, width),
        key_gain.reshape(1, width),
        jnp.swapaxes(value_up, 1, 2),
        out_gain.reshape(1, out_gain.shape[0]),
    )
    return mixed.reshape(rows, width)


def solution(mesh):
    in_specs = (
        P("kv", "tp"),
        P(None, "tp"),
        P(),
        P(),
        P(),
        P("tp", None, None),
        P("tp", None),
        P(),
        P("kv", None),
    )
    return jax.shard_map(shards, mesh=mesh, in_specs=in_specs, out_specs=P("kv", "tp"), check_vma=False)
```

```python
import functools

import jax
import jax.numpy as jnp
from jax import lax
from jax.experimental import pallas as pl
from jax.experimental.pallas import tpu as pltpu
from jax.sharding import PartitionSpec as P

BLOCK = 128
PER_OWNER = 2
MESH = pl.DeviceIdType.MESH
GROUP = 8
PIECES = 4
ONES = 16
HALF = 4
LOG2E = 1.4426950408889634


epsilon = 1e-06
masked_score = -1e30


def neighbours(tp):
    side = lax.rem(tp, 2)
    right = lax.rem(tp + 2, 8)
    left = lax.rem(tp + 6, 8)
    far = lax.rem(tp + 4, 8)
    return right, left, far, tp + 1 - 2 * side


class Spread:
    def __init__(self, full, first, size, send_sem, recv_sem):
        self.full, self.send_sem, self.recv_sem = full, send_sem, recv_sem
        half = size // 2
        self.ranges = ((first, half), (first + half, size - half))
        self.tp = lax.axis_index("tp")
        self.right, self.left, self.far, self.other = neighbours(self.tp)

    def sends(self):
        me, right, left, far, other = self.tp, self.right, self.left, self.far, self.other
        return (
            (me, 0, right, 0), (me, 1, left, 0), (me, 1, right, 1), (me, 0, left, 1), (me, 0, other, 2), (me, 1, other, 2),
            (left, 0, right, 1), (right, 1, left, 1), (left, 0, other, 2), (right, 1, other, 2), (left, 1, other, 2),
            (right, 0, other, 2), (far, 0, other, 2), (far, 1, other, 2),
        )

    def start(self, *kinds):
        every = self.sends()
        for kind in kinds:
            slot, part, dest, arrival = every[kind]
            first, size = self.ranges[part]
            piece = self.full.at[slot, pl.ds(first, size)]
            remote(piece, piece, self.send_sem, self.recv_sem.at[arrival], "tp", dest).start()

    def slices(self, count, sem):
        wait_bytes(self.full.at[pl.ds(0, count), pl.ds(self.ranges[0][0], sum(size for _, size in self.ranges))], sem)

    def own(self):
        self.start(0, 1, 2, 3, 4, 5)

    def relay_first(self):
        self.slices(1, self.recv_sem.at[0])
        self.start(6, 7, 8, 9)

    def relay_rest(self):
        self.slices(2, self.recv_sem.at[1])
        self.start(10, 11, 12, 13)

    def finish(self):
        self.slices(4, self.recv_sem.at[2])

    def drain(self):
        self.slices(7, self.send_sem)


def wait_bytes(region, sem):
    pltpu.make_async_copy(region, region, sem).wait()


def each(low, high, act):
    def step(i, carry):
        act(i)
        return carry

    lax.fori_loop(low, high, step, 0)


def remote(source, target, send_sem, recv_sem, axis, to):
    return pltpu.make_async_remote_copy(
        src_ref=source,
        dst_ref=target,
        send_sem=send_sem,
        recv_sem=recv_sem,
        device_id={axis: to},
        device_id_type=MESH,
    )


def unit(values, gain_row):
    mean_sq = jnp.mean(values * values, axis=-1, keepdims=True)
    return (values * lax.rsqrt(mean_sq + epsilon) * gain_row).astype(jnp.bfloat16)


def kernel(
    chosen_in, tokens, latent_weight, query_weight, out_weight, query_gain_in, key_gain_in, up_in, out_gain_in,
    out,
    chosen, query_gain, key_gain, up, out_gain,
    full, pool, wide_weight, weight, projection, rows, asked, asks, served, listed, table,
    queries, keys, values, totals, bias, places, staged, heads,
    local_sem, rows_send, rows_recv, ask_send, ask_recv, serve_send, serve_recv,
    heads_send, heads_recv, out_send, out_recv, spread_send, spread_recv,
):
    kv, tp = lax.axis_index("kv"), lax.axis_index("tp")
    owners, peers = asked.shape[0], full.shape[0]
    blocks, group, width = rows.shape[1:]
    picks = chosen.shape[1]
    slots = pool.shape[1]
    lines = blocks * group

    own_tokens = pltpu.make_async_copy(tokens, full.at[tp], local_sem.at[0])
    own_latent = pltpu.make_async_copy(latent_weight, weight, local_sem.at[1])
    own_query = pltpu.make_async_copy(query_weight, projection, local_sem.at[2])
    own_out = pltpu.make_async_copy(out_weight, wide_weight.at[tp], local_sem.at[3])
    small = [
        pltpu.make_async_copy(source, target, local_sem.at[5 + i])
        for i, (source, target) in enumerate(
            (
                (chosen_in, chosen), (query_gain_in, query_gain), (key_gain_in, key_gain), (up_in, up), (out_gain_in, out_gain)
            )
        )
    ]
    barrier = pltpu.get_barrier_semaphore()

    def greet(axis, index, size):
        def signal(step):
            pl.semaphore_signal(barrier, inc=1, device_id={axis: lax.rem(index + step, size)}, device_id_type=MESH)

        each(1, size, signal)

    greet("kv", kv, owners)
    greet("tp", tp, peers)

    for copy in (own_tokens, *small, own_latent, own_query, own_out):
        copy.start()
    own_tokens.wait()
    pl.semaphore_wait(barrier, owners + peers - 2)

    share = owners // PIECES

    def rows_copy(to, slot):
        return remote(full.at[tp, :, to], rows.at[slot], rows_send, rows_recv, "tp", to)

    def ask_copy(to, slot):
        return remote(asks.at[to], asked.at[slot], ask_send, ask_recv, "kv", to)

    def serve_target(slot):
        return pool.at[tp, pl.ds(blocks + slot * PER_OWNER, PER_OWNER)]

    def serve_copy(to, slot):
        return remote(served.at[to], serve_target(slot), serve_send, serve_recv.at[lax.div(slot, share)], "kv", to)

    def peer(i):
        return lax.rem(tp + i, peers)

    each(1, peers, lambda i: rows_copy(peer(i), tp).start())
    token_spread = Spread(
        full.reshape(peers, blocks * peers, group, width), 0, blocks * peers, spread_send.at[0], spread_recv.at[0]
    )
    token_spread.own()

    tile = (blocks, 128)
    lane = lax.broadcasted_iota(jnp.int32, tile, 1)
    sub = lax.broadcasted_iota(jnp.int32, tile, 0)
    ids = lane * blocks + sub

    small[0].wait()

    def mark(b, needed):
        for c in range(picks):
            needed = jnp.where(ids == chosen[b, c], 1, needed)
        return needed

    needed = lax.fori_loop(0, blocks, mark, jnp.zeros(tile, jnp.int32))
    first = jnp.full((1, 128), -1, jnp.int32)
    second = first
    for j in reversed(range(blocks)):
        hit = needed[j : j + 1, :] > 0
        second = jnp.where(hit, first, second)
        first = jnp.where(hit, j, first)
    both = jnp.where(sub == 0, first, jnp.where(sub == 1, second, 0))
    listed[...] = both
    to_scalars = pltpu.make_async_copy(listed, table, local_sem.at[4])
    to_scalars.start()
    both = both.astype(jnp.float32)

    for o in range(owners):
        spread_out = jnp.sum(jnp.where(lane == o, both, 0.0), axis=1, keepdims=True)
        asks[o] = jnp.broadcast_to(spread_out, tile)[:PER_OWNER]
    others = owners - 1

    def stay(source, target, sem):
        pltpu.make_async_copy(source, target, sem).start()

    each(0, kv, lambda o: ask_copy(o, kv).start())
    each(0, kv, lambda o: stay(asks.at[kv], asked.at[o], ask_recv))
    each(kv + 1, owners, lambda o: stay(asks.at[kv], asks.at[o], ask_send))

    ones = jnp.ones((ONES, BLOCK), jnp.bfloat16)

    def fill(slot):
        values[slot, BLOCK:, :] = ones

    each(0, slots, fill)
    key = lax.broadcasted_iota(jnp.int32, bias.shape[1:], 0)
    query = lax.rem(lax.broadcasted_iota(jnp.int32, bias.shape[1:], 1), BLOCK)
    bias[0] = jnp.where(key <= query, 0.0, masked_score)
    bias[1] = jnp.zeros(bias.shape[1:], jnp.float32)
    keys[slots] = jnp.zeros((BLOCK, width), jnp.bfloat16)
    values[slots] = jnp.zeros((BLOCK + ONES, BLOCK), jnp.bfloat16)
    def place(b):
        for c in range(picks):
            block = chosen[b, c]
            held = jnp.maximum(block, 0)
            owner = lax.div(held, blocks)
            inside = held - owner * blocks
            away = blocks + owner * PER_OWNER + jnp.where(table[1, owner] == inside, 1, 0)
            places[b, c] = jnp.where(block < 0, slots, jnp.where(owner == kv, inside, away))

    to_scalars.wait()
    each(0, blocks, place)
    for copy in small[1:]:
        copy.wait()
    rows[tp] = full[tp, :, tp]
    own_latent.wait()
    wait_bytes(rows.at[pl.ds(0, peers - 1)], rows_recv)

    @jax.jit
    def compress():
        features = jnp.concatenate([rows[p].reshape(lines, width) for p in range(peers)], axis=1)
        latent = jnp.dot(features, weight[...], preferred_element_type=jnp.float32)
        return latent.astype(jnp.bfloat16).reshape(blocks, group, 128)

    latent = compress()
    pool[tp, 0:blocks] = latent
    latent = latent.astype(jnp.float32)

    def serve(i):
        r = others - i
        for k in range(PER_OWNER):
            want = asked[r, k : k + 1, :]
            picked = jnp.zeros((group, 128), jnp.float32)
            for j in range(blocks):
                picked = jnp.where(want == float(j), latent[j], picked)
            served[r, k] = picked.astype(jnp.bfloat16)
        serve_copy(r, kv).start()

    wait_bytes(asked.at[pl.ds(0, others)], ask_recv)
    each(0, others - kv, serve)
    low = pool.at[tp, pl.ds(0, PER_OWNER)]
    each(0, kv, lambda o: stay(low, served.at[o], serve_send))
    each(kv, owners, lambda o: stay(low, serve_target(o), serve_recv.at[lax.div(o, share)]))
    here = Spread(pool, 0, blocks, spread_send.at[1], spread_recv.at[1])
    here.own()

    spreads = [
        Spread(pool, blocks + i * share * PER_OWNER, share * PER_OWNER, spread_send.at[2 + i], spread_recv.at[2 + i])
        for i in range(PIECES)
    ]

    def gathered(i):
        per_piece = share * PER_OWNER
        wait_bytes(pool.at[tp, pl.ds(blocks + i * per_piece, per_piece)], serve_recv.at[i])
        spreads[i].start(0, 1)

    scale = width ** (-0.5) * LOG2E
    query_row = query_gain[...] * scale

    def project(b):
        features = jnp.concatenate([full[p, b].reshape(BLOCK, width) for p in range(peers)], axis=1)
        projected = jnp.dot(features, projection[...], preferred_element_type=jnp.float32)
        projected = projected.astype(jnp.bfloat16).astype(jnp.float32)
        for h in range(up.shape[0]):
            queries[b, h * BLOCK : (h + 1) * BLOCK, :] = unit(projected[:, h * 128 : (h + 1) * 128], query_row)

    def prepare(low, high):
        def several(j):
            for i in range(4):
                slot = low + 4 * j + i
                block = pool[:, slot].reshape(BLOCK, width).astype(jnp.float32)
                keys[slot] = unit(block, key_gain[...])
                values[slot, :BLOCK, :] = jnp.transpose(block).astype(jnp.bfloat16)

        each(0, (high - low) // 4, several)

    wait_bytes(rows.at[pl.ds(0, peers - 1)], rows_send)
    token_spread.relay_first()
    here.relay_first()
    for i in range(PIECES):
        gathered(i)
    for spread in spreads:
        spread.start(2, 3, 4, 5)
    token_spread.relay_rest()
    token_spread.finish()
    own_query.wait()
    own_out.wait()
    each(0, blocks, project)
    for spread in spreads:
        spread.relay_first()
    out_spread = Spread(wide_weight, 0, 128, spread_send.at[2 + PIECES], spread_recv.at[2 + PIECES])
    out_spread.own()
    here.relay_rest()
    here.finish()
    prepare(0, blocks)

    def complete(i):
        spreads[i].finish()
        prepare(blocks + i * share * PER_OWNER, blocks + (i + 1) * share * PER_OWNER)

    spreads[0].relay_rest()
    for i in range(1, PIECES):
        spreads[i].relay_rest()
        complete(i - 1)
    complete(PIECES - 1)
    token_spread.drain()

    def heads_copy(to, b, slot):
        return remote(staged.at[b, to], heads.at[slot, b], heads_send, heads_recv.at[lax.div(b, HALF)], "tp", to)

    sides, heads_here = 2, up.shape[0]
    span = GROUP * BLOCK
    weights = full.reshape(sides, heads_here, -1, width)

    def weigh(b, side, g):
        picked = jnp.concatenate([keys[places[b, g * GROUP + i]] for i in range(GROUP)], axis=0)
        scores = lax.dot_general(
            picked, queries[b], (((1,), (1,)), ((), ())), preferred_element_type=jnp.float32
        )
        diagonal = jnp.exp2(scores[:BLOCK] + bias[jnp.minimum(g, 1)]).astype(jnp.bfloat16)
        others = jnp.exp2(scores[BLOCK:]).astype(jnp.bfloat16)
        for h in range(heads_here):
            cols = slice(h * BLOCK, (h + 1) * BLOCK)
            weights[side, h, :BLOCK, :] = diagonal[:, cols]
            weights[side, h, BLOCK:span, :] = others[:, cols]

    def add_up(b, side, g):
        held = jnp.concatenate([values[places[b, g * GROUP + i]] for i in range(GROUP)], axis=1)
        right = jnp.concatenate([weights[side, h, :span, :] for h in range(heads_here)], axis=1)
        return jnp.dot(held, right, preferred_element_type=jnp.float32)

    def hand_over(b, ended):
        shares = []
        for total in ended:
            shares.append((total[:BLOCK] / total[BLOCK : BLOCK + 1]).astype(jnp.bfloat16))
        turned, flipped = [], []
        for side in range(sides):
            for h in range(heads_here):
                share = shares[side][:, h * BLOCK : (h + 1) * BLOCK]
                turned.append(jnp.dot(up[h], share, preferred_element_type=jnp.float32))
        for side in range(sides):
            both = jnp.concatenate(turned[side * heads_here : (side + 1) * heads_here], axis=0)
            flipped.append(jnp.transpose(both).astype(jnp.bfloat16).reshape(peers, group, width))
        for side in range(sides):
            staged[b + side] = flipped[side]

    def start(i):
        for side in range(sides):
            weigh(sides * i + side, side, 0)

    def attend(i, following):
        first = sides * i
        for side in range(sides):
            totals[side] = jnp.zeros(totals.shape[1:], jnp.float32)

        def both(g):
            for side in range(sides):
                totals[side] = totals[side] + add_up(first + side, side, g - 1)
            for side in range(sides):
                weigh(first + side, side, g)

        each(1, picks // GROUP, both)
        ended = [totals[side] + add_up(first + side, side, picks // GROUP - 1) for side in range(sides)]
        if following:
            start(i + 1)
        hand_over(first, ended)
        for side in range(sides):
            each(1, peers, lambda j: heads_copy(peer(j), first + side, tp).start())

    def out_copy(to, half, slot):
        lower = pl.ds(half * HALF, HALF)
        return remote(
            rows.at[to, lower], out.at[lower, slot], out_send, out_recv, "tp", to
        )

    @functools.partial(jax.jit, static_argnums=0)
    def mix(half):
        lower = pl.ds(half * HALF, HALF)
        features = jnp.concatenate([heads[p, lower].reshape(HALF * group, width) for p in range(peers)], axis=1)
        summed = jnp.dot(
            features, wide_weight[...].reshape(peers * 128, peers * 128), preferred_element_type=jnp.float32
        )
        mixed = unit(summed, out_gain[...])
        for t in range(peers):
            rows[t, lower] = mixed[:, t * 128 : (t + 1) * 128].reshape(HALF, group, 128)

    def conclude(half):
        lower = pl.ds(half * HALF, HALF)

        wait_bytes(heads.at[pl.ds(0, peers - 1), lower], heads_recv.at[half])
        for b in range(HALF):
            heads[tp, half * HALF + b] = staged[half * HALF + b, tp]
        mix(half)
        each(1, peers, lambda i: out_copy(peer(i), half, tp).start())
        out[lower, tp] = rows[tp, lower]

    def turn(i):
        attend(i, True)

        @pl.when(i == 0)
        def _():
            out_spread.relay_first()

        @pl.when(i == 2)
        def _():
            out_spread.relay_rest()

    last = blocks // sides - 1
    each(0, 1, start)
    each(0, last, turn)
    each(last, last + 1, lambda i: attend(i, False))
    out_spread.finish()
    conclude(0)
    conclude(1)

    wait_bytes(asks.at[pl.ds(0, others)], ask_send)
    wait_bytes(served.at[pl.ds(0, others)], serve_send)
    for spread in (here, out_spread, *spreads):
        spread.drain()
    wait_bytes(staged.at[:, pl.ds(0, peers - 1)], heads_send)
    wait_bytes(rows.at[pl.ds(0, peers - 1)], out_send)
    wait_bytes(out.at[:, pl.ds(0, peers - 1)], out_recv)


def shards(
    tokens, query_weight, latent_weight, query_gain, key_gain, value_up, out_weight, out_gain, chosen
):
    peers, owners = lax.axis_size("tp"), lax.axis_size("kv")
    blocks, picks = chosen.shape
    rows, width = tokens.shape
    group = BLOCK // peers
    slots = blocks + owners * PER_OWNER
    heads = value_up.shape[0]
    vmem = pl.BlockSpec(memory_space=pltpu.VMEM)
    anywhere = pl.BlockSpec(memory_space=pl.ANY)
    dma = pltpu.SemaphoreType.DMA
    bf16 = jnp.bfloat16
    mixed = pl.pallas_call(
        kernel,
        out_shape=pltpu.VMEM((blocks, peers, group, width), bf16),
        in_specs=[anywhere] * 9,
        out_specs=vmem,
        scratch_shapes=[
            pltpu.SMEM((blocks, picks), jnp.int32),
            pltpu.VMEM((1, width), jnp.float32),
            pltpu.VMEM((1, width), jnp.float32),
            pltpu.VMEM((heads, value_up.shape[2], width), bf16),
            pltpu.VMEM((1, out_gain.shape[0]), jnp.float32),
            pltpu.VMEM((peers, blocks, peers, group, width), bf16),
            pltpu.VMEM((peers, slots, group, width), bf16),
            pltpu.VMEM((peers, *out_weight.shape), bf16),
            pltpu.VMEM(latent_weight.shape, bf16),
            pltpu.VMEM(query_weight.shape, bf16),
            pltpu.VMEM((peers, blocks, group, width), bf16),
            pltpu.VMEM((owners, PER_OWNER, 128), jnp.float32),
            pltpu.VMEM((owners, PER_OWNER, 128), jnp.float32),
            pltpu.VMEM((owners, PER_OWNER, group, width), bf16),
            pltpu.VMEM((blocks, 128), jnp.int32),
            pltpu.SMEM((blocks, 128), jnp.int32),
            pltpu.VMEM((blocks, heads * BLOCK, width), bf16),
            pltpu.VMEM((slots + 1, BLOCK, width), bf16),
            pltpu.VMEM((slots + 1, BLOCK + ONES, BLOCK), bf16),
            pltpu.VMEM((2, BLOCK + ONES, heads * BLOCK), jnp.float32),
            pltpu.VMEM((2, BLOCK, heads * BLOCK), jnp.float32),
            pltpu.SMEM((blocks, picks), jnp.int32),
            pltpu.VMEM((blocks, peers, group, width), bf16),
            pltpu.VMEM((peers, blocks, group, width), bf16),
            dma((10,)),
            dma, dma,
            dma, dma,
            dma, dma((PIECES,)),
            dma, dma((2,)),
            dma, dma,
            dma((3 + PIECES,)), dma((3 + PIECES, 3)),
        ],
        compiler_params=pltpu.CompilerParams(collective_id=0, has_side_effects=True),
    )(
        chosen,
        tokens.reshape(blocks, peers, group, width),
        latent_weight,
        query_weight,
        out_weight,
        query_gain.reshape(1, width),
        key_gain.reshape(1, width),
        jnp.swapaxes(value_up, 1, 2),
        out_gain.reshape(1, out_gain.shape[0]),
    )
    return mixed.reshape(rows, width)


def solution(mesh):
    in_specs = (
        P("kv", "tp"),
        P(None, "tp"),
        P(),
        P(),
        P(),
        P("tp", None, None),
        P("tp", None),
        P(),
        P("kv", None),
    )
    return jax.shard_map(shards, mesh=mesh, in_specs=in_specs, out_specs=P("kv", "tp"), check_vma=False)
```

```python
import functools

import jax
import jax.numpy as jnp
from jax import lax
from jax.experimental import pallas as pl
from jax.experimental.pallas import tpu as pltpu
from jax.sharding import PartitionSpec as P

BLOCK = 128
PER_OWNER = 2
MESH = pl.DeviceIdType.MESH
GROUP = 8
PIECES = 4
ONES = 16
HALF = 6
LOG2E = 1.4426950408889634


epsilon = 1e-06
masked_score = -1e30


def neighbours(tp):
    side = lax.rem(tp, 2)
    right = lax.rem(tp + 2, 8)
    left = lax.rem(tp + 6, 8)
    far = lax.rem(tp + 4, 8)
    return right, left, far, tp + 1 - 2 * side


class Spread:
    def __init__(self, full, first, size, send_sem, recv_sem):
        self.full, self.send_sem, self.recv_sem = full, send_sem, recv_sem
        half = size // 2
        self.ranges = ((first, half), (first + half, size - half))
        self.tp = lax.axis_index("tp")
        self.right, self.left, self.far, self.other = neighbours(self.tp)

    def sends(self):
        me, right, left, far, other = self.tp, self.right, self.left, self.far, self.other
        return (
            (me, 0, right, 0), (me, 1, left, 0), (me, 1, right, 1), (me, 0, left, 1), (me, 0, other, 2), (me, 1, other, 2),
            (left, 0, right, 1), (right, 1, left, 1), (left, 0, other, 2), (right, 1, other, 2), (left, 1, other, 2),
            (right, 0, other, 2), (far, 0, other, 2), (far, 1, other, 2),
        )

    def start(self, *kinds):
        every = self.sends()
        for kind in kinds:
            slot, part, dest, arrival = every[kind]
            first, size = self.ranges[part]
            piece = self.full.at[slot, pl.ds(first, size)]
            remote(piece, piece, self.send_sem, self.recv_sem.at[arrival], "tp", dest).start()

    def slices(self, count, sem):
        wait_bytes(self.full.at[pl.ds(0, count), pl.ds(self.ranges[0][0], sum(size for _, size in self.ranges))], sem)

    def own(self):
        self.start(0, 1, 2, 3, 4, 5)

    def relay_first(self):
        self.slices(1, self.recv_sem.at[0])
        self.start(6, 7, 8, 9)

    def relay_rest(self):
        self.slices(2, self.recv_sem.at[1])
        self.start(10, 11, 12, 13)

    def finish(self):
        self.slices(4, self.recv_sem.at[2])

    def drain(self):
        self.slices(7, self.send_sem)


def wait_bytes(region, sem):
    pltpu.make_async_copy(region, region, sem).wait()


def each(low, high, act):
    def step(i, carry):
        act(i)
        return carry

    lax.fori_loop(low, high, step, 0)


def remote(source, target, send_sem, recv_sem, axis, to):
    return pltpu.make_async_remote_copy(
        src_ref=source,
        dst_ref=target,
        send_sem=send_sem,
        recv_sem=recv_sem,
        device_id={axis: to},
        device_id_type=MESH,
    )


def unit(values, gain_row):
    mean_sq = jnp.mean(values * values, axis=-1, keepdims=True)
    return (values * lax.rsqrt(mean_sq + epsilon) * gain_row).astype(jnp.bfloat16)


def kernel(
    chosen_in, tokens, latent_weight, query_weight, out_weight, query_gain_in, key_gain_in, up_in, out_gain_in,
    out,
    chosen, query_gain, key_gain, up, out_gain,
    full, pool, wide_weight, weight, projection, rows, asked, asks, served, listed, table,
    queries, keys, values, totals, bias, places, staged, heads,
    local_sem, rows_send, rows_recv, ask_send, ask_recv, serve_send, serve_recv,
    heads_send, heads_recv, out_send, out_recv, spread_send, spread_recv,
):
    kv, tp = lax.axis_index("kv"), lax.axis_index("tp")
    owners, peers = asked.shape[0], full.shape[0]
    blocks, group, width = rows.shape[1:]
    picks = chosen.shape[1]
    slots = pool.shape[1]
    lines = blocks * group

    own_tokens = pltpu.make_async_copy(tokens, full.at[tp], local_sem.at[0])
    own_latent = pltpu.make_async_copy(latent_weight, weight, local_sem.at[1])
    own_query = pltpu.make_async_copy(query_weight, projection, local_sem.at[2])
    own_out = pltpu.make_async_copy(out_weight, wide_weight.at[tp], local_sem.at[3])
    small = [
        pltpu.make_async_copy(source, target, local_sem.at[5 + i])
        for i, (source, target) in enumerate(
            (
                (chosen_in, chosen), (query_gain_in, query_gain), (key_gain_in, key_gain), (up_in, up), (out_gain_in, out_gain)
            )
        )
    ]
    barrier = pltpu.get_barrier_semaphore()

    def greet(axis, index, size):
        def signal(step):
            pl.semaphore_signal(barrier, inc=1, device_id={axis: lax.rem(index + step, size)}, device_id_type=MESH)

        each(1, size, signal)

    greet("kv", kv, owners)
    greet("tp", tp, peers)

    for copy in (own_tokens, *small, own_latent, own_query, own_out):
        copy.start()
    own_tokens.wait()
    pl.semaphore_wait(barrier, owners + peers - 2)

    share = owners // PIECES

    def rows_copy(to, slot):
        return remote(full.at[tp, :, to], rows.at[slot], rows_send, rows_recv, "tp", to)

    def ask_copy(to, slot):
        return remote(asks.at[to], asked.at[slot], ask_send, ask_recv, "kv", to)

    def serve_target(slot):
        return pool.at[tp, pl.ds(blocks + slot * PER_OWNER, PER_OWNER)]

    def serve_copy(to, slot):
        return remote(served.at[to], serve_target(slot), serve_send, serve_recv.at[lax.div(slot, share)], "kv", to)

    def peer(i):
        return lax.rem(tp + i, peers)

    each(1, peers, lambda i: rows_copy(peer(i), tp).start())
    token_spread = Spread(
        full.reshape(peers, blocks * peers, group, width), 0, blocks * peers, spread_send.at[0], spread_recv.at[0]
    )
    token_spread.own()

    tile = (blocks, 128)
    lane = lax.broadcasted_iota(jnp.int32, tile, 1)
    sub = lax.broadcasted_iota(jnp.int32, tile, 0)
    ids = lane * blocks + sub

    small[0].wait()

    def mark(b, needed):
        for c in range(picks):
            needed = jnp.where(ids == chosen[b, c], 1, needed)
        return needed

    needed = lax.fori_loop(0, blocks, mark, jnp.zeros(tile, jnp.int32))
    first = jnp.full((1, 128), -1, jnp.int32)
    second = first
    for j in reversed(range(blocks)):
        hit = needed[j : j + 1, :] > 0
        second = jnp.where(hit, first, second)
        first = jnp.where(hit, j, first)
    both = jnp.where(sub == 0, first, jnp.where(sub == 1, second, 0))
    listed[...] = both
    to_scalars = pltpu.make_async_copy(listed, table, local_sem.at[4])
    to_scalars.start()
    both = both.astype(jnp.float32)

    for o in range(owners):
        spread_out = jnp.sum(jnp.where(lane == o, both, 0.0), axis=1, keepdims=True)
        asks[o] = jnp.broadcast_to(spread_out, tile)[:PER_OWNER]
    others = owners - 1

    def stay(source, target, sem):
        pltpu.make_async_copy(source, target, sem).start()

    each(0, kv, lambda o: ask_copy(o, kv).start())
    each(0, kv, lambda o: stay(asks.at[kv], asked.at[o], ask_recv))
    each(kv + 1, owners, lambda o: stay(asks.at[kv], asks.at[o], ask_send))

    ones = jnp.ones((ONES, BLOCK), jnp.bfloat16)

    def fill(slot):
        values[slot, BLOCK:, :] = ones

    each(0, slots, fill)
    key = lax.broadcasted_iota(jnp.int32, bias.shape[1:], 0)
    query = lax.rem(lax.broadcasted_iota(jnp.int32, bias.shape[1:], 1), BLOCK)
    bias[0] = jnp.where(key <= query, 0.0, masked_score)
    bias[1] = jnp.zeros(bias.shape[1:], jnp.float32)
    keys[slots] = jnp.zeros((BLOCK, width), jnp.bfloat16)
    values[slots] = jnp.zeros((BLOCK + ONES, BLOCK), jnp.bfloat16)
    def place(b):
        for c in range(picks):
            block = chosen[b, c]
            held = jnp.maximum(block, 0)
            owner = lax.div(held, blocks)
            inside = held - owner * blocks
            away = blocks + owner * PER_OWNER + jnp.where(table[1, owner] == inside, 1, 0)
            places[b, c] = jnp.where(block < 0, slots, jnp.where(owner == kv, inside, away))

    to_scalars.wait()
    each(0, blocks, place)
    for copy in small[1:]:
        copy.wait()
    rows[tp] = full[tp, :, tp]
    own_latent.wait()
    wait_bytes(rows.at[pl.ds(0, peers - 1)], rows_recv)

    @jax.jit
    def compress():
        features = jnp.concatenate([rows[p].reshape(lines, width) for p in range(peers)], axis=1)
        latent = jnp.dot(features, weight[...], preferred_element_type=jnp.float32)
        return latent.astype(jnp.bfloat16).reshape(blocks, group, 128)

    latent = compress()
    pool[tp, 0:blocks] = latent
    latent = latent.astype(jnp.float32)

    def serve(i):
        r = others - i
        for k in range(PER_OWNER):
            want = asked[r, k : k + 1, :]
            picked = jnp.zeros((group, 128), jnp.float32)
            for j in range(blocks):
                picked = jnp.where(want == float(j), latent[j], picked)
            served[r, k] = picked.astype(jnp.bfloat16)
        serve_copy(r, kv).start()

    wait_bytes(asked.at[pl.ds(0, others)], ask_recv)
    each(0, others - kv, serve)
    low = pool.at[tp, pl.ds(0, PER_OWNER)]
    each(0, kv, lambda o: stay(low, served.at[o], serve_send))
    each(kv, owners, lambda o: stay(low, serve_target(o), serve_recv.at[lax.div(o, share)]))
    here = Spread(pool, 0, blocks, spread_send.at[1], spread_recv.at[1])
    here.own()

    spreads = [
        Spread(pool, blocks + i * share * PER_OWNER, share * PER_OWNER, spread_send.at[2 + i], spread_recv.at[2 + i])
        for i in range(PIECES)
    ]

    def gathered(i):
        per_piece = share * PER_OWNER
        wait_bytes(pool.at[tp, pl.ds(blocks + i * per_piece, per_piece)], serve_recv.at[i])
        spreads[i].start(0, 1)

    scale = width ** (-0.5) * LOG2E
    query_row = query_gain[...] * scale

    def project(b):
        features = jnp.concatenate([full[p, b].reshape(BLOCK, width) for p in range(peers)], axis=1)
        projected = jnp.dot(features, projection[...], preferred_element_type=jnp.float32)
        projected = projected.astype(jnp.bfloat16).astype(jnp.float32)
        for h in range(up.shape[0]):
            queries[b, h * BLOCK : (h + 1) * BLOCK, :] = unit(projected[:, h * 128 : (h + 1) * 128], query_row)

    eye_shape = (BLOCK, BLOCK)
    same = lax.broadcasted_iota(jnp.int32, eye_shape, 0) == lax.broadcasted_iota(jnp.int32, eye_shape, 1)
    eye = jnp.where(same, 1.0, 0.0).astype(jnp.bfloat16)

    def prepare(low, high):
        def several(j):
            first = low + 4 * j
            picked = [pool[:, first + i].reshape(BLOCK, width) for i in range(4)]
            turned = lax.dot_general(
                eye, jnp.concatenate(picked, axis=0), (((1,), (1,)), ((), ())), preferred_element_type=jnp.float32
            ).astype(jnp.bfloat16)
            for i in range(4):
                keys[first + i] = unit(picked[i].astype(jnp.float32), key_gain[...])
                values[first + i, :BLOCK, :] = turned[:, i * BLOCK : (i + 1) * BLOCK]

        each(0, (high - low) // 4, several)

    wait_bytes(rows.at[pl.ds(0, peers - 1)], rows_send)
    token_spread.relay_first()
    here.relay_first()
    for i in range(PIECES):
        gathered(i)
    for spread in spreads:
        spread.start(2, 3, 4, 5)
    token_spread.relay_rest()
    token_spread.finish()
    own_query.wait()
    own_out.wait()
    each(0, blocks, project)
    for spread in spreads:
        spread.relay_first()
    out_spread = Spread(wide_weight, 0, 128, spread_send.at[2 + PIECES], spread_recv.at[2 + PIECES])
    out_spread.own()
    here.relay_rest()
    here.finish()
    prepare(0, blocks)

    def complete(i):
        spreads[i].finish()
        prepare(blocks + i * share * PER_OWNER, blocks + (i + 1) * share * PER_OWNER)

    spreads[0].relay_rest()
    for i in range(1, PIECES):
        spreads[i].relay_rest()
        complete(i - 1)
    complete(PIECES - 1)
    token_spread.drain()

    def heads_copy(to, b, slot):
        return remote(staged.at[b, to], heads.at[slot, b], heads_send, heads_recv.at[lax.div(b, HALF)], "tp", to)

    sides, heads_here = 2, up.shape[0]
    span = GROUP * BLOCK
    weights = full.reshape(sides, heads_here, -1, width)

    def weigh(b, side, g):
        picked = jnp.concatenate([keys[places[b, g * GROUP + i]] for i in range(GROUP)], axis=0)
        scores = lax.dot_general(
            picked, queries[b], (((1,), (1,)), ((), ())), preferred_element_type=jnp.float32
        )
        diagonal = jnp.exp2(scores[:BLOCK] + bias[jnp.minimum(g, 1)]).astype(jnp.bfloat16)
        others = jnp.exp2(scores[BLOCK:]).astype(jnp.bfloat16)
        for h in range(heads_here):
            cols = slice(h * BLOCK, (h + 1) * BLOCK)
            weights[side, h, :BLOCK, :] = diagonal[:, cols]
            weights[side, h, BLOCK:span, :] = others[:, cols]

    def add_up(b, side, g):
        held = jnp.concatenate([values[places[b, g * GROUP + i]] for i in range(GROUP)], axis=1)
        right = jnp.concatenate([weights[side, h, :span, :] for h in range(heads_here)], axis=1)
        return jnp.dot(held, right, preferred_element_type=jnp.float32)

    def hand_over(b, ended):
        shares = []
        for total in ended:
            shares.append((total[:BLOCK] / total[BLOCK : BLOCK + 1]).astype(jnp.bfloat16))
        turned, flipped = [], []
        for side in range(sides):
            for h in range(heads_here):
                share = shares[side][:, h * BLOCK : (h + 1) * BLOCK]
                turned.append(jnp.dot(up[h], share, preferred_element_type=jnp.float32))
        for side in range(sides):
            both = jnp.concatenate(turned[side * heads_here : (side + 1) * heads_here], axis=0)
            flipped.append(jnp.transpose(both).astype(jnp.bfloat16).reshape(peers, group, width))
        for side in range(sides):
            staged[b + side] = flipped[side]

    def start(i):
        for side in range(sides):
            weigh(sides * i + side, side, 0)

    def attend(i, following):
        first = sides * i
        for side in range(sides):
            totals[side] = jnp.zeros(totals.shape[1:], jnp.float32)

        def both(g):
            for side in range(sides):
                totals[side] = totals[side] + add_up(first + side, side, g - 1)
            for side in range(sides):
                weigh(first + side, side, g)

        each(1, picks // GROUP, both)
        ended = [totals[side] + add_up(first + side, side, picks // GROUP - 1) for side in range(sides)]
        if following:
            start(i + 1)
        hand_over(first, ended)
        for side in range(sides):
            each(1, peers, lambda j: heads_copy(peer(j), first + side, tp).start())

    def part(half):
        return (0, HALF) if half == 0 else (HALF, blocks - HALF)

    def out_copy(to, half, slot):
        lower = pl.ds(*part(half))
        return remote(rows.at[to, lower], out.at[lower, slot], out_send, out_recv, "tp", to)

    @functools.partial(jax.jit, static_argnums=0)
    def mix(half):
        lower, count = pl.ds(*part(half)), part(half)[1]
        features = jnp.concatenate([heads[p, lower].reshape(count * group, width) for p in range(peers)], axis=1)
        summed = jnp.dot(
            features, wide_weight[...].reshape(peers * 128, peers * 128), preferred_element_type=jnp.float32
        )
        mixed = unit(summed, out_gain[...])
        for t in range(peers):
            rows[t, lower] = mixed[:, t * 128 : (t + 1) * 128].reshape(count, group, 128)

    def conclude(half):
        first, count = part(half)
        lower = pl.ds(first, count)
        wait_bytes(heads.at[pl.ds(0, peers - 1), lower], heads_recv.at[half])
        for b in range(first, first + count):
            heads[tp, b] = staged[b, tp]
        mix(half)
        each(1, peers, lambda i: out_copy(peer(i), half, tp).start())
        out[lower, tp] = rows[tp, lower]

    def turn(i):
        attend(i, True)

        @pl.when(i == 0)
        def _():
            out_spread.relay_first()

        @pl.when(i == 2)
        def _():
            out_spread.relay_rest()

    last = blocks // sides - 1
    each(0, 1, start)
    each(0, last, turn)
    each(last, last + 1, lambda i: attend(i, False))
    out_spread.finish()
    conclude(0)
    conclude(1)

    wait_bytes(asks.at[pl.ds(0, others)], ask_send)
    wait_bytes(served.at[pl.ds(0, others)], serve_send)
    for spread in (here, out_spread, *spreads):
        spread.drain()
    wait_bytes(staged.at[:, pl.ds(0, peers - 1)], heads_send)
    wait_bytes(rows.at[pl.ds(0, peers - 1)], out_send)
    wait_bytes(out.at[:, pl.ds(0, peers - 1)], out_recv)


def shards(
    tokens, query_weight, latent_weight, query_gain, key_gain, value_up, out_weight, out_gain, chosen
):
    peers, owners = lax.axis_size("tp"), lax.axis_size("kv")
    blocks, picks = chosen.shape
    rows, width = tokens.shape
    group = BLOCK // peers
    slots = blocks + owners * PER_OWNER
    heads = value_up.shape[0]
    vmem = pl.BlockSpec(memory_space=pltpu.VMEM)
    anywhere = pl.BlockSpec(memory_space=pl.ANY)
    dma = pltpu.SemaphoreType.DMA
    bf16 = jnp.bfloat16
    mixed = pl.pallas_call(
        kernel,
        out_shape=pltpu.VMEM((blocks, peers, group, width), bf16),
        in_specs=[anywhere] * 9,
        out_specs=vmem,
        scratch_shapes=[
            pltpu.SMEM((blocks, picks), jnp.int32),
            pltpu.VMEM((1, width), jnp.float32),
            pltpu.VMEM((1, width), jnp.float32),
            pltpu.VMEM((heads, value_up.shape[2], width), bf16),
            pltpu.VMEM((1, out_gain.shape[0]), jnp.float32),
            pltpu.VMEM((peers, blocks, peers, group, width), bf16),
            pltpu.VMEM((peers, slots, group, width), bf16),
            pltpu.VMEM((peers, *out_weight.shape), bf16),
            pltpu.VMEM(latent_weight.shape, bf16),
            pltpu.VMEM(query_weight.shape, bf16),
            pltpu.VMEM((peers, blocks, group, width), bf16),
            pltpu.VMEM((owners, PER_OWNER, 128), jnp.float32),
            pltpu.VMEM((owners, PER_OWNER, 128), jnp.float32),
            pltpu.VMEM((owners, PER_OWNER, group, width), bf16),
            pltpu.VMEM((blocks, 128), jnp.int32),
            pltpu.SMEM((blocks, 128), jnp.int32),
            pltpu.VMEM((blocks, heads * BLOCK, width), bf16),
            pltpu.VMEM((slots + 1, BLOCK, width), bf16),
            pltpu.VMEM((slots + 1, BLOCK + ONES, BLOCK), bf16),
            pltpu.VMEM((2, BLOCK + ONES, heads * BLOCK), jnp.float32),
            pltpu.VMEM((2, BLOCK, heads * BLOCK), jnp.float32),
            pltpu.SMEM((blocks, picks), jnp.int32),
            pltpu.VMEM((blocks, peers, group, width), bf16),
            pltpu.VMEM((peers, blocks, group, width), bf16),
            dma((10,)),
            dma, dma,
            dma, dma,
            dma, dma((PIECES,)),
            dma, dma((2,)),
            dma, dma,
            dma((3 + PIECES,)), dma((3 + PIECES, 3)),
        ],
        compiler_params=pltpu.CompilerParams(collective_id=0, has_side_effects=True),
    )(
        chosen,
        tokens.reshape(blocks, peers, group, width),
        latent_weight,
        query_weight,
        out_weight,
        query_gain.reshape(1, width),
        key_gain.reshape(1, width),
        jnp.swapaxes(value_up, 1, 2),
        out_gain.reshape(1, out_gain.shape[0]),
    )
    return mixed.reshape(rows, width)


def solution(mesh):
    in_specs = (
        P("kv", "tp"),
        P(None, "tp"),
        P(),
        P(),
        P(),
        P("tp", None, None),
        P("tp", None),
        P(),
        P("kv", None),
    )
    return jax.shard_map(shards, mesh=mesh, in_specs=in_specs, out_specs=P("kv", "tp"), check_vma=False)
```

```python
import functools

import jax
import jax.numpy as jnp
from jax import lax
from jax.experimental import pallas as pl
from jax.experimental.pallas import tpu as pltpu
from jax.sharding import PartitionSpec as P

BLOCK = 128
PER_OWNER = 2
MESH = pl.DeviceIdType.MESH
GROUP = 8
PIECES = 4
ONES = 16
HALF = 6
LOG2E = 1.4426950408889634


epsilon = 1e-06
masked_score = -1e30


def neighbours(tp):
    side = lax.rem(tp, 2)
    right = lax.rem(tp + 2, 8)
    left = lax.rem(tp + 6, 8)
    far = lax.rem(tp + 4, 8)
    return right, left, far, tp + 1 - 2 * side


class Spread:
    def __init__(self, full, first, size, send_sem, recv_sem):
        self.full, self.send_sem, self.recv_sem = full, send_sem, recv_sem
        half = size // 2
        self.ranges = ((first, half), (first + half, size - half))
        self.tp = lax.axis_index("tp")
        self.right, self.left, self.far, self.other = neighbours(self.tp)

    def sends(self):
        me, right, left, far, other = self.tp, self.right, self.left, self.far, self.other
        return (
            (me, 0, right, 0), (me, 1, left, 0), (me, 1, right, 1), (me, 0, left, 1), (me, 0, other, 2), (me, 1, other, 2),
            (left, 0, right, 1), (right, 1, left, 1), (left, 0, other, 2), (right, 1, other, 2), (left, 1, other, 2),
            (right, 0, other, 2), (far, 0, other, 2), (far, 1, other, 2),
        )

    def start(self, *kinds):
        every = self.sends()
        for kind in kinds:
            slot, part, dest, arrival = every[kind]
            first, size = self.ranges[part]
            piece = self.full.at[slot, pl.ds(first, size)]
            remote(piece, piece, self.send_sem, self.recv_sem.at[arrival], "tp", dest).start()

    def slices(self, count, sem):
        wait_bytes(self.full.at[pl.ds(0, count), pl.ds(self.ranges[0][0], sum(size for _, size in self.ranges))], sem)

    def own(self):
        self.start(0, 1, 2, 3, 4, 5)

    def relay_first(self):
        self.slices(1, self.recv_sem.at[0])
        self.start(6, 7, 8, 9)

    def relay_rest(self):
        self.slices(2, self.recv_sem.at[1])
        self.start(10, 11, 12, 13)

    def finish(self):
        self.slices(4, self.recv_sem.at[2])

    def drain(self):
        self.slices(7, self.send_sem)


def wait_bytes(region, sem):
    pltpu.make_async_copy(region, region, sem).wait()


def each(low, high, act):
    def step(i, carry):
        act(i)
        return carry

    lax.fori_loop(low, high, step, 0)


def remote(source, target, send_sem, recv_sem, axis, to):
    return pltpu.make_async_remote_copy(
        src_ref=source,
        dst_ref=target,
        send_sem=send_sem,
        recv_sem=recv_sem,
        device_id={axis: to},
        device_id_type=MESH,
    )


def unit(values, gain_row):
    mean_sq = jnp.mean(values * values, axis=-1, keepdims=True)
    return (values * lax.rsqrt(mean_sq + epsilon) * gain_row).astype(jnp.bfloat16)


def kernel(
    chosen_in, tokens, latent_weight, query_weight, out_weight, query_gain_in, key_gain_in, up_in, out_gain_in,
    out,
    chosen, query_gain, key_gain, up, out_gain,
    full, pool, wide_weight, weight, projection, rows, asked, asks, served, listed, table,
    queries, keys, values, totals, bias, places, staged, heads,
    local_sem, rows_send, rows_recv, ask_send, ask_recv, serve_send, serve_recv,
    heads_send, heads_recv, out_send, out_recv, spread_send, spread_recv,
):
    kv, tp = lax.axis_index("kv"), lax.axis_index("tp")
    owners, peers = asked.shape[0], full.shape[0]
    blocks, group, width = rows.shape[1:]
    picks = chosen.shape[1]
    slots = pool.shape[1]
    lines = blocks * group

    own_tokens = pltpu.make_async_copy(tokens, full.at[tp], local_sem.at[0])
    own_latent = pltpu.make_async_copy(latent_weight, weight, local_sem.at[1])
    own_query = pltpu.make_async_copy(query_weight, projection, local_sem.at[2])
    own_out = pltpu.make_async_copy(out_weight, wide_weight.at[tp], local_sem.at[3])
    small = [
        pltpu.make_async_copy(source, target, local_sem.at[5 + i])
        for i, (source, target) in enumerate(
            (
                (chosen_in, chosen), (query_gain_in, query_gain), (key_gain_in, key_gain), (up_in, up), (out_gain_in, out_gain)
            )
        )
    ]
    barrier = pltpu.get_barrier_semaphore()

    def greet(axis, index, size):
        def signal(step):
            pl.semaphore_signal(barrier, inc=1, device_id={axis: lax.rem(index + step, size)}, device_id_type=MESH)

        each(1, size, signal)

    greet("kv", kv, owners)
    greet("tp", tp, peers)

    for copy in (own_tokens, *small, own_latent, own_query, own_out):
        copy.start()
    own_tokens.wait()
    pl.semaphore_wait(barrier, owners + peers - 2)

    share = owners // PIECES

    def rows_copy(to, slot):
        return remote(full.at[tp, :, to], rows.at[slot], rows_send, rows_recv, "tp", to)

    def ask_copy(to, slot):
        return remote(asks.at[to], asked.at[slot], ask_send, ask_recv, "kv", to)

    def serve_target(slot):
        return pool.at[tp, pl.ds(blocks + slot * PER_OWNER, PER_OWNER)]

    def serve_copy(to, slot):
        return remote(served.at[to], serve_target(slot), serve_send, serve_recv.at[lax.div(slot, share)], "kv", to)

    def peer(i):
        return lax.rem(tp + i, peers)

    each(1, peers, lambda i: rows_copy(peer(i), tp).start())
    token_spread = Spread(
        full.reshape(peers, blocks * peers, group, width), 0, blocks * peers, spread_send.at[0], spread_recv.at[0]
    )
    token_spread.own()

    tile = (blocks, 128)
    lane = lax.broadcasted_iota(jnp.int32, tile, 1)
    sub = lax.broadcasted_iota(jnp.int32, tile, 0)
    ids = lane * blocks + sub

    small[0].wait()

    def mark(b, needed):
        for c in range(picks):
            needed = jnp.where(ids == chosen[b, c], 1, needed)
        return needed

    needed = lax.fori_loop(0, blocks, mark, jnp.zeros(tile, jnp.int32))
    first = jnp.full((1, 128), -1, jnp.int32)
    second = first
    for j in reversed(range(blocks)):
        hit = needed[j : j + 1, :] > 0
        second = jnp.where(hit, first, second)
        first = jnp.where(hit, j, first)
    both = jnp.where(sub == 0, first, jnp.where(sub == 1, second, 0))
    listed[...] = both
    to_scalars = pltpu.make_async_copy(listed, table, local_sem.at[4])
    to_scalars.start()
    both = both.astype(jnp.float32)

    for o in range(owners):
        spread_out = jnp.sum(jnp.where(lane == o, both, 0.0), axis=1, keepdims=True)
        asks[o] = jnp.broadcast_to(spread_out, tile)[:PER_OWNER]
    others = owners - 1

    def stay(source, target, sem):
        pltpu.make_async_copy(source, target, sem).start()

    each(0, kv, lambda o: ask_copy(o, kv).start())
    each(0, kv, lambda o: stay(asks.at[kv], asked.at[o], ask_recv))
    each(kv + 1, owners, lambda o: stay(asks.at[kv], asks.at[o], ask_send))

    ones = jnp.ones((ONES, BLOCK), jnp.bfloat16)

    def fill(slot):
        values[slot, BLOCK:, :] = ones

    each(0, slots, fill)
    key = lax.broadcasted_iota(jnp.int32, bias.shape[1:], 0)
    query = lax.rem(lax.broadcasted_iota(jnp.int32, bias.shape[1:], 1), BLOCK)
    bias[0] = jnp.where(key <= query, 0.0, masked_score)
    bias[1] = jnp.zeros(bias.shape[1:], jnp.float32)
    keys[slots] = jnp.zeros((BLOCK, width), jnp.bfloat16)
    values[slots] = jnp.zeros((BLOCK + ONES, BLOCK), jnp.bfloat16)
    def place(b):
        for c in range(picks):
            block = chosen[b, c]
            held = jnp.maximum(block, 0)
            owner = lax.div(held, blocks)
            inside = held - owner * blocks
            away = blocks + owner * PER_OWNER + jnp.where(table[1, owner] == inside, 1, 0)
            places[b, c] = jnp.where(block < 0, slots, jnp.where(owner == kv, inside, away))

    to_scalars.wait()
    each(0, blocks, place)
    for copy in small[1:]:
        copy.wait()
    rows[tp] = full[tp, :, tp]
    own_latent.wait()
    wait_bytes(rows.at[pl.ds(0, peers - 1)], rows_recv)

    @jax.jit
    def compress():
        features = jnp.concatenate([rows[p].reshape(lines, width) for p in range(peers)], axis=1)
        latent = jnp.dot(features, weight[...], preferred_element_type=jnp.float32)
        return latent.astype(jnp.bfloat16).reshape(blocks, group, 128)

    latent = compress()
    pool[tp, 0:blocks] = latent
    latent = latent.astype(jnp.float32)

    def serve(i):
        r = others - i
        for k in range(PER_OWNER):
            want = asked[r, k : k + 1, :]
            picked = jnp.zeros((group, 128), jnp.float32)
            for j in range(blocks):
                picked = jnp.where(want == float(j), latent[j], picked)
            served[r, k] = picked.astype(jnp.bfloat16)
        serve_copy(r, kv).start()

    wait_bytes(asked.at[pl.ds(0, others)], ask_recv)
    each(0, others - kv, serve)
    low = pool.at[tp, pl.ds(0, PER_OWNER)]
    each(0, kv, lambda o: stay(low, served.at[o], serve_send))
    each(kv, owners, lambda o: stay(low, serve_target(o), serve_recv.at[lax.div(o, share)]))
    here = Spread(pool, 0, blocks, spread_send.at[1], spread_recv.at[1])
    here.own()

    spreads = [
        Spread(pool, blocks + i * share * PER_OWNER, share * PER_OWNER, spread_send.at[2 + i], spread_recv.at[2 + i])
        for i in range(PIECES)
    ]

    def gathered(i):
        per_piece = share * PER_OWNER
        wait_bytes(pool.at[tp, pl.ds(blocks + i * per_piece, per_piece)], serve_recv.at[i])
        spreads[i].start(0, 1)

    scale = width ** (-0.5) * LOG2E
    query_row = query_gain[...] * scale

    def project(b):
        features = jnp.concatenate([full[p, b].reshape(BLOCK, width) for p in range(peers)], axis=1)
        projected = jnp.dot(features, projection[...], preferred_element_type=jnp.float32)
        projected = projected.astype(jnp.bfloat16).astype(jnp.float32)
        for h in range(up.shape[0]):
            queries[b, h * BLOCK : (h + 1) * BLOCK, :] = unit(projected[:, h * 128 : (h + 1) * 128], query_row)

    eye_shape = (BLOCK, BLOCK)
    same = lax.broadcasted_iota(jnp.int32, eye_shape, 0) == lax.broadcasted_iota(jnp.int32, eye_shape, 1)
    eye = jnp.where(same, 1.0, 0.0).astype(jnp.bfloat16)

    def prepare(low, high):
        def several(j):
            first = low + 8 * j
            picked = [pool[:, first + i].reshape(BLOCK, width) for i in range(8)]
            turned = lax.dot_general(
                eye, jnp.concatenate(picked, axis=0), (((1,), (1,)), ((), ())), preferred_element_type=jnp.float32
            ).astype(jnp.bfloat16)
            for i in range(8):
                keys[first + i] = unit(picked[i].astype(jnp.float32), key_gain[...])
                values[first + i, :BLOCK, :] = turned[:, i * BLOCK : (i + 1) * BLOCK]

        each(0, (high - low) // 8, several)

    wait_bytes(rows.at[pl.ds(0, peers - 1)], rows_send)
    token_spread.relay_first()
    here.relay_first()
    for i in range(PIECES):
        gathered(i)
    for spread in spreads:
        spread.start(2, 3, 4, 5)
    token_spread.relay_rest()
    token_spread.finish()
    own_query.wait()
    own_out.wait()
    def project_two(j):
        project(2 * j)
        project(2 * j + 1)

    each(0, blocks // 2, project_two)
    for spread in spreads:
        spread.relay_first()
    out_spread = Spread(wide_weight, 0, 128, spread_send.at[2 + PIECES], spread_recv.at[2 + PIECES])
    out_spread.own()
    here.relay_rest()
    here.finish()
    prepare(0, blocks)

    def complete(i):
        spreads[i].finish()
        prepare(blocks + i * share * PER_OWNER, blocks + (i + 1) * share * PER_OWNER)

    spreads[0].relay_rest()
    for i in range(1, PIECES):
        spreads[i].relay_rest()
        complete(i - 1)
    complete(PIECES - 1)
    token_spread.drain()

    def heads_copy(to, b, slot):
        return remote(staged.at[b, to], heads.at[slot, b], heads_send, heads_recv.at[lax.div(b, HALF)], "tp", to)

    sides, heads_here = 2, up.shape[0]
    span = GROUP * BLOCK
    weights = full.reshape(sides, heads_here, -1, width)

    def weigh(b, side, g):
        picked = jnp.concatenate([keys[places[b, g * GROUP + i]] for i in range(GROUP)], axis=0)
        scores = lax.dot_general(
            picked, queries[b], (((1,), (1,)), ((), ())), preferred_element_type=jnp.float32
        )
        diagonal = jnp.exp2(scores[:BLOCK] + bias[jnp.minimum(g, 1)]).astype(jnp.bfloat16)
        others = jnp.exp2(scores[BLOCK:]).astype(jnp.bfloat16)
        for h in range(heads_here):
            cols = slice(h * BLOCK, (h + 1) * BLOCK)
            weights[side, h, :BLOCK, :] = diagonal[:, cols]
            weights[side, h, BLOCK:span, :] = others[:, cols]

    def add_up(b, side, g):
        held = jnp.concatenate([values[places[b, g * GROUP + i]] for i in range(GROUP)], axis=1)
        right = jnp.concatenate([weights[side, h, :span, :] for h in range(heads_here)], axis=1)
        return jnp.dot(held, right, preferred_element_type=jnp.float32)

    def hand_over(b, ended):
        shares = []
        for total in ended:
            shares.append((total[:BLOCK] / total[BLOCK : BLOCK + 1]).astype(jnp.bfloat16))
        turned, flipped = [], []
        for side in range(sides):
            for h in range(heads_here):
                share = shares[side][:, h * BLOCK : (h + 1) * BLOCK]
                turned.append(jnp.dot(up[h], share, preferred_element_type=jnp.float32))
        for side in range(sides):
            both = jnp.concatenate(turned[side * heads_here : (side + 1) * heads_here], axis=0)
            flipped.append(jnp.transpose(both).astype(jnp.bfloat16).reshape(peers, group, width))
        for side in range(sides):
            staged[b + side] = flipped[side]

    def start(i):
        for side in range(sides):
            weigh(sides * i + side, side, 0)

    def attend(i, following):
        first = sides * i
        for side in range(sides):
            totals[side] = jnp.zeros(totals.shape[1:], jnp.float32)

        def both(g):
            for side in range(sides):
                totals[side] = totals[side] + add_up(first + side, side, g - 1)
            for side in range(sides):
                weigh(first + side, side, g)

        each(1, picks // GROUP, both)
        ended = [totals[side] + add_up(first + side, side, picks // GROUP - 1) for side in range(sides)]
        if following:
            start(i + 1)
        hand_over(first, ended)
        for side in range(sides):
            each(1, peers, lambda j: heads_copy(peer(j), first + side, tp).start())

    def part(half):
        return (0, HALF) if half == 0 else (HALF, blocks - HALF)

    def out_copy(to, half, slot):
        lower = pl.ds(*part(half))
        return remote(rows.at[to, lower], out.at[lower, slot], out_send, out_recv, "tp", to)

    @functools.partial(jax.jit, static_argnums=0)
    def mix(half):
        lower, count = pl.ds(*part(half)), part(half)[1]
        features = jnp.concatenate([heads[p, lower].reshape(count * group, width) for p in range(peers)], axis=1)
        summed = jnp.dot(
            features, wide_weight[...].reshape(peers * 128, peers * 128), preferred_element_type=jnp.float32
        )
        mixed = unit(summed, out_gain[...])
        for t in range(peers):
            rows[t, lower] = mixed[:, t * 128 : (t + 1) * 128].reshape(count, group, 128)

    def conclude(half):
        first, count = part(half)
        lower = pl.ds(first, count)
        wait_bytes(heads.at[pl.ds(0, peers - 1), lower], heads_recv.at[half])
        for b in range(first, first + count):
            heads[tp, b] = staged[b, tp]
        mix(half)
        each(1, peers, lambda i: out_copy(peer(i), half, tp).start())
        out[lower, tp] = rows[tp, lower]

    def turn(i):
        attend(i, True)

        @pl.when(i == 0)
        def _():
            out_spread.relay_first()

        @pl.when(i == 2)
        def _():
            out_spread.relay_rest()

    last = blocks // sides - 1
    each(0, 1, start)
    each(0, last, turn)
    each(last, last + 1, lambda i: attend(i, False))
    out_spread.finish()
    conclude(0)
    conclude(1)

    wait_bytes(asks.at[pl.ds(0, others)], ask_send)
    wait_bytes(served.at[pl.ds(0, others)], serve_send)
    for spread in (here, out_spread, *spreads):
        spread.drain()
    wait_bytes(staged.at[:, pl.ds(0, peers - 1)], heads_send)
    wait_bytes(rows.at[pl.ds(0, peers - 1)], out_send)
    wait_bytes(out.at[:, pl.ds(0, peers - 1)], out_recv)


def shards(
    tokens, query_weight, latent_weight, query_gain, key_gain, value_up, out_weight, out_gain, chosen
):
    peers, owners = lax.axis_size("tp"), lax.axis_size("kv")
    blocks, picks = chosen.shape
    rows, width = tokens.shape
    group = BLOCK // peers
    slots = blocks + owners * PER_OWNER
    heads = value_up.shape[0]
    vmem = pl.BlockSpec(memory_space=pltpu.VMEM)
    anywhere = pl.BlockSpec(memory_space=pl.ANY)
    dma = pltpu.SemaphoreType.DMA
    bf16 = jnp.bfloat16
    mixed = pl.pallas_call(
        kernel,
        out_shape=pltpu.VMEM((blocks, peers, group, width), bf16),
        in_specs=[anywhere] * 9,
        out_specs=vmem,
        scratch_shapes=[
            pltpu.SMEM((blocks, picks), jnp.int32),
            pltpu.VMEM((1, width), jnp.float32),
            pltpu.VMEM((1, width), jnp.float32),
            pltpu.VMEM((heads, value_up.shape[2], width), bf16),
            pltpu.VMEM((1, out_gain.shape[0]), jnp.float32),
            pltpu.VMEM((peers, blocks, peers, group, width), bf16),
            pltpu.VMEM((peers, slots, group, width), bf16),
            pltpu.VMEM((peers, *out_weight.shape), bf16),
            pltpu.VMEM(latent_weight.shape, bf16),
            pltpu.VMEM(query_weight.shape, bf16),
            pltpu.VMEM((peers, blocks, group, width), bf16),
            pltpu.VMEM((owners, PER_OWNER, 128), jnp.float32),
            pltpu.VMEM((owners, PER_OWNER, 128), jnp.float32),
            pltpu.VMEM((owners, PER_OWNER, group, width), bf16),
            pltpu.VMEM((blocks, 128), jnp.int32),
            pltpu.SMEM((blocks, 128), jnp.int32),
            pltpu.VMEM((blocks, heads * BLOCK, width), bf16),
            pltpu.VMEM((slots + 1, BLOCK, width), bf16),
            pltpu.VMEM((slots + 1, BLOCK + ONES, BLOCK), bf16),
            pltpu.VMEM((2, BLOCK + ONES, heads * BLOCK), jnp.float32),
            pltpu.VMEM((2, BLOCK, heads * BLOCK), jnp.float32),
            pltpu.SMEM((blocks, picks), jnp.int32),
            pltpu.VMEM((blocks, peers, group, width), bf16),
            pltpu.VMEM((peers, blocks, group, width), bf16),
            dma((10,)),
            dma, dma,
            dma, dma,
            dma, dma((PIECES,)),
            dma, dma((2,)),
            dma, dma,
            dma((3 + PIECES,)), dma((3 + PIECES, 3)),
        ],
        compiler_params=pltpu.CompilerParams(collective_id=0, has_side_effects=True),
    )(
        chosen,
        tokens.reshape(blocks, peers, group, width),
        latent_weight,
        query_weight,
        out_weight,
        query_gain.reshape(1, width),
        key_gain.reshape(1, width),
        jnp.swapaxes(value_up, 1, 2),
        out_gain.reshape(1, out_gain.shape[0]),
    )
    return mixed.reshape(rows, width)


def solution(mesh):
    in_specs = (
        P("kv", "tp"),
        P(None, "tp"),
        P(),
        P(),
        P(),
        P("tp", None, None),
        P("tp", None),
        P(),
        P("kv", None),
    )
    return jax.shard_map(shards, mesh=mesh, in_specs=in_specs, out_specs=P("kv", "tp"), check_vma=False)
```

```python
import functools

import jax
import jax.numpy as jnp
from jax import lax
from jax.experimental import pallas as pl
from jax.experimental.pallas import tpu as pltpu
from jax.sharding import PartitionSpec as P

BLOCK = 128
PER_OWNER = 2
MESH = pl.DeviceIdType.MESH
GROUP = 8
PIECES = 4
ONES = 16
HALF = 6
LOG2E = 1.4426950408889634


epsilon = 1e-06
masked_score = -1e30


def neighbours(tp):
    side = lax.rem(tp, 2)
    right = lax.rem(tp + 2, 8)
    left = lax.rem(tp + 6, 8)
    far = lax.rem(tp + 4, 8)
    return right, left, far, tp + 1 - 2 * side


class Spread:
    def __init__(self, full, first, size, send_sem, recv_sem):
        self.full, self.send_sem, self.recv_sem = full, send_sem, recv_sem
        half = size // 2
        self.ranges = ((first, half), (first + half, size - half))
        self.tp = lax.axis_index("tp")
        self.right, self.left, self.far, self.other = neighbours(self.tp)

    def sends(self):
        me, right, left, far, other = self.tp, self.right, self.left, self.far, self.other
        return (
            (me, 0, right, 0), (me, 1, left, 0), (me, 1, right, 1), (me, 0, left, 1), (me, 0, other, 2), (me, 1, other, 2),
            (left, 0, right, 1), (right, 1, left, 1), (left, 0, other, 2), (right, 1, other, 2), (left, 1, other, 2),
            (right, 0, other, 2), (far, 0, other, 2), (far, 1, other, 2),
        )

    def start(self, *kinds):
        every = self.sends()
        for kind in kinds:
            slot, part, dest, arrival = every[kind]
            first, size = self.ranges[part]
            piece = self.full.at[slot, pl.ds(first, size)]
            remote(piece, piece, self.send_sem, self.recv_sem.at[arrival], "tp", dest).start()

    def slices(self, count, sem):
        wait_bytes(self.full.at[pl.ds(0, count), pl.ds(self.ranges[0][0], sum(size for _, size in self.ranges))], sem)

    def own(self):
        self.start(0, 1, 2, 3, 4, 5)

    def relay_first(self):
        self.slices(1, self.recv_sem.at[0])
        self.start(6, 7, 8, 9)

    def relay_rest(self):
        self.slices(2, self.recv_sem.at[1])
        self.start(10, 11, 12, 13)

    def finish(self):
        self.slices(4, self.recv_sem.at[2])

    def drain(self):
        self.slices(7, self.send_sem)


def wait_bytes(region, sem):
    pltpu.make_async_copy(region, region, sem).wait()


def each(low, high, act):
    def step(i, carry):
        act(i)
        return carry

    lax.fori_loop(low, high, step, 0)


def remote(source, target, send_sem, recv_sem, axis, to):
    return pltpu.make_async_remote_copy(
        src_ref=source,
        dst_ref=target,
        send_sem=send_sem,
        recv_sem=recv_sem,
        device_id={axis: to},
        device_id_type=MESH,
    )


def unit(values, gain_row):
    mean_sq = jnp.mean(values * values, axis=-1, keepdims=True)
    return (values * lax.rsqrt(mean_sq + epsilon) * gain_row).astype(jnp.bfloat16)


def kernel(
    chosen_in, tokens, latent_weight, query_weight, out_weight, query_gain_in, key_gain_in, up_in, out_gain_in,
    out,
    chosen, query_gain, key_gain, up, out_gain,
    full, pool, wide_weight, weight, projection, rows, asked, asks, served, listed, table,
    queries, keys, values, totals, bias, places, staged, heads,
    local_sem, rows_send, rows_recv, ask_send, ask_recv, serve_send, serve_recv,
    heads_send, heads_recv, out_send, out_recv, spread_send, spread_recv,
):
    kv, tp = lax.axis_index("kv"), lax.axis_index("tp")
    owners, peers = asked.shape[0], full.shape[0]
    blocks, group, width = rows.shape[1:]
    picks = chosen.shape[1]
    slots = pool.shape[1]
    lines = blocks * group

    own_tokens = pltpu.make_async_copy(tokens, full.at[tp], local_sem.at[0])
    own_latent = pltpu.make_async_copy(latent_weight, weight, local_sem.at[1])
    own_query = pltpu.make_async_copy(query_weight, projection, local_sem.at[2])
    own_out = pltpu.make_async_copy(out_weight, wide_weight.at[tp], local_sem.at[3])
    small = [
        pltpu.make_async_copy(source, target, local_sem.at[5 + i])
        for i, (source, target) in enumerate(
            (
                (chosen_in, chosen), (query_gain_in, query_gain), (key_gain_in, key_gain), (up_in, up), (out_gain_in, out_gain)
            )
        )
    ]
    barrier = pltpu.get_barrier_semaphore()

    def greet(axis, index, size):
        def signal(step):
            pl.semaphore_signal(barrier, inc=1, device_id={axis: lax.rem(index + step, size)}, device_id_type=MESH)

        each(1, size, signal)

    greet("kv", kv, owners)
    greet("tp", tp, peers)

    for copy in (own_tokens, *small, own_latent, own_query, own_out):
        copy.start()
    own_tokens.wait()
    pl.semaphore_wait(barrier, owners + peers - 2)

    share = owners // PIECES

    def rows_copy(to, slot):
        return remote(full.at[tp, :, to], rows.at[slot], rows_send, rows_recv, "tp", to)

    def ask_copy(to, slot):
        return remote(asks.at[to], asked.at[slot], ask_send, ask_recv, "kv", to)

    def serve_target(slot):
        return pool.at[tp, pl.ds(blocks + slot * PER_OWNER, PER_OWNER)]

    def serve_copy(to, slot):
        return remote(served.at[to], serve_target(slot), serve_send, serve_recv.at[lax.div(slot, share)], "kv", to)

    def peer(i):
        return lax.rem(tp + i, peers)

    each(1, peers, lambda i: rows_copy(peer(i), tp).start())
    token_spread = Spread(
        full.reshape(peers, blocks * peers, group, width), 0, blocks * peers, spread_send.at[0], spread_recv.at[0]
    )
    token_spread.own()

    tile = (blocks, 128)
    lane = lax.broadcasted_iota(jnp.int32, tile, 1)
    sub = lax.broadcasted_iota(jnp.int32, tile, 0)
    ids = lane * blocks + sub

    small[0].wait()

    def mark(b, needed):
        for c in range(picks):
            needed = jnp.where(ids == chosen[b, c], 1, needed)
        return needed

    needed = lax.fori_loop(0, blocks, mark, jnp.zeros(tile, jnp.int32))
    first = jnp.full((1, 128), -1, jnp.int32)
    second = first
    for j in reversed(range(blocks)):
        hit = needed[j : j + 1, :] > 0
        second = jnp.where(hit, first, second)
        first = jnp.where(hit, j, first)
    both = jnp.where(sub == 0, first, jnp.where(sub == 1, second, 0))
    listed[...] = both
    to_scalars = pltpu.make_async_copy(listed, table, local_sem.at[4])
    to_scalars.start()
    both = both.astype(jnp.float32)

    for o in range(owners):
        spread_out = jnp.sum(jnp.where(lane == o, both, 0.0), axis=1, keepdims=True)
        asks[o] = jnp.broadcast_to(spread_out, tile)[:PER_OWNER]
    others = owners - 1

    def stay(source, target, sem):
        pltpu.make_async_copy(source, target, sem).start()

    each(0, kv, lambda o: ask_copy(o, kv).start())
    each(0, kv, lambda o: stay(asks.at[kv], asked.at[o], ask_recv))
    each(kv + 1, owners, lambda o: stay(asks.at[kv], asks.at[o], ask_send))

    ones = jnp.ones((ONES, BLOCK), jnp.bfloat16)

    def fill(slot):
        values[slot, BLOCK:, :] = ones

    each(0, slots, fill)
    key = lax.broadcasted_iota(jnp.int32, bias.shape[1:], 0)
    query = lax.rem(lax.broadcasted_iota(jnp.int32, bias.shape[1:], 1), BLOCK)
    bias[0] = jnp.where(key <= query, 0.0, masked_score)
    bias[1] = jnp.zeros(bias.shape[1:], jnp.float32)
    keys[slots] = jnp.zeros((BLOCK, width), jnp.bfloat16)
    values[slots] = jnp.zeros((BLOCK + ONES, BLOCK), jnp.bfloat16)
    def place(b):
        for c in range(picks):
            block = chosen[b, c]
            held = jnp.maximum(block, 0)
            owner = lax.div(held, blocks)
            inside = held - owner * blocks
            away = blocks + owner * PER_OWNER + jnp.where(table[1, owner] == inside, 1, 0)
            places[b, c] = jnp.where(block < 0, slots, jnp.where(owner == kv, inside, away))

    to_scalars.wait()
    each(0, blocks, place)
    for copy in small[1:]:
        copy.wait()
    rows[tp] = full[tp, :, tp]
    own_latent.wait()
    wait_bytes(rows.at[pl.ds(0, peers - 1)], rows_recv)

    @jax.jit
    def compress():
        features = jnp.concatenate([rows[p].reshape(lines, width) for p in range(peers)], axis=1)
        latent = jnp.dot(features, weight[...], preferred_element_type=jnp.float32)
        return latent.astype(jnp.bfloat16).reshape(blocks, group, 128)

    latent = compress()
    pool[tp, 0:blocks] = latent
    latent = latent.astype(jnp.float32)

    def serve(i):
        r = others - i
        for k in range(PER_OWNER):
            want = asked[r, k : k + 1, :]
            picked = jnp.zeros((group, 128), jnp.float32)
            for j in range(blocks):
                picked = jnp.where(want == float(j), latent[j], picked)
            served[r, k] = picked.astype(jnp.bfloat16)
        serve_copy(r, kv).start()

    wait_bytes(asked.at[pl.ds(0, others)], ask_recv)
    each(0, others - kv, serve)
    low = pool.at[tp, pl.ds(0, PER_OWNER)]
    each(0, kv, lambda o: stay(low, served.at[o], serve_send))
    full_share = lax.div(kv + share - 1, share) * share
    each(kv, full_share, lambda o: stay(low, serve_target(o), serve_recv.at[lax.div(o, share)]))
    here = Spread(pool, 0, blocks, spread_send.at[1], spread_recv.at[1])
    here.own()

    per_piece = share * PER_OWNER
    pieces = [lax.rem(lax.div(kv, share) + step, PIECES) for step in (0, 3, 1, 2)]
    firsts = [blocks + piece * per_piece for piece in pieces]
    spreads = [
        Spread(pool, first, per_piece, spread_send.at[2 + k], spread_recv.at[2 + k]) for k, first in enumerate(firsts)
    ]

    def if_needed(k, act):
        pl.when(pieces[k] * share < kv)(act)

    def gathered(k):
        wait_bytes(pool.at[tp, pl.ds(firsts[k], per_piece)], serve_recv.at[pieces[k]])
        spreads[k].start(0, 1)

    scale = width ** (-0.5) * LOG2E
    query_row = query_gain[...] * scale

    def project(j):
        features = jnp.concatenate(
            [full[p, pl.ds(2 * j, 2)].reshape(2 * BLOCK, width) for p in range(peers)], axis=1
        )
        projected = jnp.dot(features, projection[...], preferred_element_type=jnp.float32)
        projected = projected.astype(jnp.bfloat16).astype(jnp.float32)
        for i in range(2):
            for h in range(up.shape[0]):
                head = projected[i * BLOCK : (i + 1) * BLOCK, h * 128 : (h + 1) * 128]
                queries[2 * j + i, h * BLOCK : (h + 1) * BLOCK, :] = unit(head, query_row)

    eye_shape = (BLOCK, BLOCK)
    same = lax.broadcasted_iota(jnp.int32, eye_shape, 0) == lax.broadcasted_iota(jnp.int32, eye_shape, 1)
    eye = jnp.where(same, 1.0, 0.0).astype(jnp.bfloat16)

    def prepare(low, count):
        def several(j):
            first = low + 8 * j
            picked = [pool[:, first + i].reshape(BLOCK, width) for i in range(8)]
            turned = lax.dot_general(
                eye, jnp.concatenate(picked, axis=0), (((1,), (1,)), ((), ())), preferred_element_type=jnp.float32
            ).astype(jnp.bfloat16)
            for i in range(8):
                keys[first + i] = unit(picked[i].astype(jnp.float32), key_gain[...])
                values[first + i, :BLOCK, :] = turned[:, i * BLOCK : (i + 1) * BLOCK]

        each(0, count // 8, several)

    wait_bytes(rows.at[pl.ds(0, peers - 1)], rows_send)
    token_spread.relay_first()
    here.relay_first()
    for k in range(PIECES):
        if_needed(k, functools.partial(gathered, k))
    for k in range(PIECES):
        if_needed(k, functools.partial(spreads[k].start, 2, 3, 4, 5))
    token_spread.relay_rest()
    token_spread.finish()
    own_query.wait()
    own_out.wait()
    each(0, blocks // 2, project)
    for k in range(PIECES):
        if_needed(k, spreads[k].relay_first)
    out_spread = Spread(wide_weight, 0, 128, spread_send.at[2 + PIECES], spread_recv.at[2 + PIECES])
    out_spread.own()
    here.relay_rest()
    here.finish()
    prepare(0, blocks)

    def complete(k):
        spreads[k].finish()
        prepare(firsts[k], per_piece)

    for k in range(PIECES + 1):
        if k < PIECES:
            if_needed(k, spreads[k].relay_rest)
        if k > 0:
            if_needed(k - 1, functools.partial(complete, k - 1))
    token_spread.drain()

    def heads_copy(to, b, slot):
        return remote(staged.at[b, to], heads.at[slot, b], heads_send, heads_recv.at[lax.div(b, HALF)], "tp", to)

    sides, heads_here = 2, up.shape[0]
    span = GROUP * BLOCK
    weights = full.reshape(sides, heads_here, -1, width)

    def weigh(b, side, g):
        picked = jnp.concatenate([keys[places[b, g * GROUP + i]] for i in range(GROUP)], axis=0)
        scores = lax.dot_general(
            picked, queries[b], (((1,), (1,)), ((), ())), preferred_element_type=jnp.float32
        )
        diagonal = jnp.exp2(scores[:BLOCK] + bias[jnp.minimum(g, 1)]).astype(jnp.bfloat16)
        others = jnp.exp2(scores[BLOCK:]).astype(jnp.bfloat16)
        for h in range(heads_here):
            cols = slice(h * BLOCK, (h + 1) * BLOCK)
            weights[side, h, :BLOCK, :] = diagonal[:, cols]
            weights[side, h, BLOCK:span, :] = others[:, cols]

    def add_up(b, side, g):
        held = jnp.concatenate([values[places[b, g * GROUP + i]] for i in range(GROUP)], axis=1)
        right = jnp.concatenate([weights[side, h, :span, :] for h in range(heads_here)], axis=1)
        return jnp.dot(held, right, preferred_element_type=jnp.float32)

    def hand_over(b, ended):
        shares = []
        for total in ended:
            shares.append((total[:BLOCK] / total[BLOCK : BLOCK + 1]).astype(jnp.bfloat16))
        turned, flipped = [], []
        for side in range(sides):
            for h in range(heads_here):
                share = shares[side][:, h * BLOCK : (h + 1) * BLOCK]
                turned.append(jnp.dot(up[h], share, preferred_element_type=jnp.float32))
        for side in range(sides):
            both = jnp.concatenate(turned[side * heads_here : (side + 1) * heads_here], axis=0)
            flipped.append(jnp.transpose(both).astype(jnp.bfloat16).reshape(peers, group, width))
        for side in range(sides):
            staged[b + side] = flipped[side]

    def start(i):
        for side in range(sides):
            weigh(sides * i + side, side, 0)

    groups = lax.div(jnp.minimum(picks, blocks + PER_OWNER * kv) + GROUP - 1, GROUP)

    def attend(i, following):
        first = sides * i
        for side in range(sides):
            totals[side] = jnp.zeros(totals.shape[1:], jnp.float32)

        def both(g):
            for side in range(sides):
                totals[side] = totals[side] + add_up(first + side, side, g - 1)
            for side in range(sides):
                weigh(first + side, side, g)

        each(1, groups, both)
        if not following:
            out_spread.relay_rest()
        ended = [totals[side] + add_up(first + side, side, groups - 1) for side in range(sides)]
        if following:
            start(i + 1)
        hand_over(first, ended)
        for side in range(sides):
            each(1, peers, lambda j: heads_copy(peer(j), first + side, tp).start())

    def part(half):
        return (0, HALF) if half == 0 else (HALF, blocks - HALF)

    def out_copy(to, half, slot):
        lower = pl.ds(*part(half))
        return remote(rows.at[to, lower], out.at[lower, slot], out_send, out_recv, "tp", to)

    @functools.partial(jax.jit, static_argnums=0)
    def mix(half):
        lower, count = pl.ds(*part(half)), part(half)[1]
        features = jnp.concatenate([heads[p, lower].reshape(count * group, width) for p in range(peers)], axis=1)
        summed = jnp.dot(
            features, wide_weight[...].reshape(peers * 128, peers * 128), preferred_element_type=jnp.float32
        )
        mixed = unit(summed, out_gain[...])
        for t in range(peers):
            rows[t, lower] = mixed[:, t * 128 : (t + 1) * 128].reshape(count, group, 128)

    def conclude(half):
        first, count = part(half)
        lower = pl.ds(first, count)
        wait_bytes(heads.at[pl.ds(0, peers - 1), lower], heads_recv.at[half])
        for b in range(first, first + count):
            heads[tp, b] = staged[b, tp]
        mix(half)
        each(1, peers, lambda i: out_copy(peer(i), half, tp).start())
        out[lower, tp] = rows[tp, lower]

    def turn(i):
        attend(i, True)

        @pl.when(i == 0)
        def _():
            out_spread.relay_first()

    last = blocks // sides - 1
    each(0, 1, start)
    each(0, last, turn)
    each(last, last + 1, lambda i: attend(i, False))
    out_spread.finish()
    conclude(0)
    conclude(1)

    wait_bytes(asks.at[pl.ds(0, others)], ask_send)
    wait_bytes(served.at[pl.ds(0, others)], serve_send)
    for spread in (here, out_spread):
        spread.drain()
    for k in range(PIECES):
        if_needed(k, spreads[k].drain)
    wait_bytes(staged.at[:, pl.ds(0, peers - 1)], heads_send)
    wait_bytes(rows.at[pl.ds(0, peers - 1)], out_send)
    wait_bytes(out.at[:, pl.ds(0, peers - 1)], out_recv)


def shards(
    tokens, query_weight, latent_weight, query_gain, key_gain, value_up, out_weight, out_gain, chosen
):
    peers, owners = lax.axis_size("tp"), lax.axis_size("kv")
    blocks, picks = chosen.shape
    rows, width = tokens.shape
    group = BLOCK // peers
    slots = blocks + owners * PER_OWNER
    heads = value_up.shape[0]
    vmem = pl.BlockSpec(memory_space=pltpu.VMEM)
    anywhere = pl.BlockSpec(memory_space=pl.ANY)
    dma = pltpu.SemaphoreType.DMA
    bf16 = jnp.bfloat16
    mixed = pl.pallas_call(
        kernel,
        out_shape=pltpu.VMEM((blocks, peers, group, width), bf16),
        in_specs=[anywhere] * 9,
        out_specs=vmem,
        scratch_shapes=[
            pltpu.SMEM((blocks, picks), jnp.int32),
            pltpu.VMEM((1, width), jnp.float32),
            pltpu.VMEM((1, width), jnp.float32),
            pltpu.VMEM((heads, value_up.shape[2], width), bf16),
            pltpu.VMEM((1, out_gain.shape[0]), jnp.float32),
            pltpu.VMEM((peers, blocks, peers, group, width), bf16),
            pltpu.VMEM((peers, slots, group, width), bf16),
            pltpu.VMEM((peers, *out_weight.shape), bf16),
            pltpu.VMEM(latent_weight.shape, bf16),
            pltpu.VMEM(query_weight.shape, bf16),
            pltpu.VMEM((peers, blocks, group, width), bf16),
            pltpu.VMEM((owners, PER_OWNER, 128), jnp.float32),
            pltpu.VMEM((owners, PER_OWNER, 128), jnp.float32),
            pltpu.VMEM((owners, PER_OWNER, group, width), bf16),
            pltpu.VMEM((blocks, 128), jnp.int32),
            pltpu.SMEM((blocks, 128), jnp.int32),
            pltpu.VMEM((blocks, heads * BLOCK, width), bf16),
            pltpu.VMEM((slots + 1, BLOCK, width), bf16),
            pltpu.VMEM((slots + 1, BLOCK + ONES, BLOCK), bf16),
            pltpu.VMEM((2, BLOCK + ONES, heads * BLOCK), jnp.float32),
            pltpu.VMEM((2, BLOCK, heads * BLOCK), jnp.float32),
            pltpu.SMEM((blocks, picks), jnp.int32),
            pltpu.VMEM((blocks, peers, group, width), bf16),
            pltpu.VMEM((peers, blocks, group, width), bf16),
            dma((10,)),
            dma, dma,
            dma, dma,
            dma, dma((PIECES,)),
            dma, dma((2,)),
            dma, dma,
            dma((3 + PIECES,)), dma((3 + PIECES, 3)),
        ],
        compiler_params=pltpu.CompilerParams(collective_id=0, has_side_effects=True),
    )(
        chosen,
        tokens.reshape(blocks, peers, group, width),
        latent_weight,
        query_weight,
        out_weight,
        query_gain.reshape(1, width),
        key_gain.reshape(1, width),
        jnp.swapaxes(value_up, 1, 2),
        out_gain.reshape(1, out_gain.shape[0]),
    )
    return mixed.reshape(rows, width)


def solution(mesh):
    in_specs = (
        P("kv", "tp"),
        P(None, "tp"),
        P(),
        P(),
        P(),
        P("tp", None, None),
        P("tp", None),
        P(),
        P("kv", None),
    )
    return jax.shard_map(shards, mesh=mesh, in_specs=in_specs, out_specs=P("kv", "tp"), check_vma=False)
```

```python
import functools

import jax
import jax.numpy as jnp
from jax import lax
from jax.experimental import pallas as pl
from jax.experimental.pallas import tpu as pltpu
from jax.sharding import PartitionSpec as P

BLOCK = 128
PER_OWNER = 2
MESH = pl.DeviceIdType.MESH
GROUP = 8
PIECES = 4
ONES = 16
HALF = 6
LOG2E = 1.4426950408889634


epsilon = 1e-06
masked_score = -1e30


def neighbours(tp):
    side = lax.rem(tp, 2)
    right = lax.rem(tp + 2, 8)
    left = lax.rem(tp + 6, 8)
    far = lax.rem(tp + 4, 8)
    return right, left, far, tp + 1 - 2 * side


class Spread:
    def __init__(self, full, first, size, send_sem, recv_sem):
        self.full, self.send_sem, self.recv_sem = full, send_sem, recv_sem
        half = size // 2
        self.ranges = ((first, half), (first + half, size - half))
        self.tp = lax.axis_index("tp")
        self.right, self.left, self.far, self.other = neighbours(self.tp)

    def sends(self):
        me, right, left, far, other = self.tp, self.right, self.left, self.far, self.other
        return (
            (me, 0, right, 0), (me, 1, left, 0), (me, 1, right, 1), (me, 0, left, 1), (me, 0, other, 2), (me, 1, other, 2),
            (left, 0, right, 1), (right, 1, left, 1), (left, 0, other, 2), (right, 1, other, 2), (left, 1, other, 2),
            (right, 0, other, 2), (far, 0, other, 2), (far, 1, other, 2),
        )

    def start(self, *kinds):
        every = self.sends()
        for kind in kinds:
            slot, part, dest, arrival = every[kind]
            first, size = self.ranges[part]
            piece = self.full.at[slot, pl.ds(first, size)]
            remote(piece, piece, self.send_sem, self.recv_sem.at[arrival], "tp", dest).start()

    def slices(self, count, sem):
        wait_bytes(self.full.at[pl.ds(0, count), pl.ds(self.ranges[0][0], sum(size for _, size in self.ranges))], sem)

    def own(self):
        self.start(0, 1, 2, 3, 4, 5)

    def relay_first(self):
        self.slices(1, self.recv_sem.at[0])
        self.start(6, 7, 8, 9)

    def relay_rest(self):
        self.slices(2, self.recv_sem.at[1])
        self.start(10, 11, 12, 13)

    def finish(self):
        self.slices(4, self.recv_sem.at[2])

    def drain(self):
        self.slices(7, self.send_sem)


def wait_bytes(region, sem):
    pltpu.make_async_copy(region, region, sem).wait()


def each(low, high, act):
    def step(i, carry):
        act(i)
        return carry

    lax.fori_loop(low, high, step, 0)


def remote(source, target, send_sem, recv_sem, axis, to):
    return pltpu.make_async_remote_copy(
        src_ref=source,
        dst_ref=target,
        send_sem=send_sem,
        recv_sem=recv_sem,
        device_id={axis: to},
        device_id_type=MESH,
    )


def unit(values, gain_row):
    mean_sq = jnp.mean(values * values, axis=-1, keepdims=True)
    return (values * lax.rsqrt(mean_sq + epsilon) * gain_row).astype(jnp.bfloat16)


def kernel(
    chosen_in, tokens, latent_weight, query_weight, out_weight, query_gain_in, key_gain_in, up_in, out_gain_in,
    out,
    chosen, query_gain, key_gain, up, out_gain,
    full, pool, wide_weight, weight, projection, rows, asked, asks, served, listed, table,
    queries, keys, values, totals, bias, places, staged, heads,
    local_sem, rows_send, rows_recv, ask_send, ask_recv, serve_send, serve_recv,
    heads_send, heads_recv, out_send, out_recv, spread_send, spread_recv,
):
    kv, tp = lax.axis_index("kv"), lax.axis_index("tp")
    owners, peers = asked.shape[0], full.shape[0]
    blocks, group, width = rows.shape[1:]
    picks = chosen.shape[1]
    slots = pool.shape[1]
    lines = blocks * group

    own_tokens = pltpu.make_async_copy(tokens, full.at[tp], local_sem.at[0])
    own_latent = pltpu.make_async_copy(latent_weight, weight, local_sem.at[1])
    own_query = pltpu.make_async_copy(query_weight, projection, local_sem.at[2])
    own_out = pltpu.make_async_copy(out_weight, wide_weight.at[tp], local_sem.at[3])
    small = [
        pltpu.make_async_copy(source, target, local_sem.at[5 + i])
        for i, (source, target) in enumerate(
            (
                (chosen_in, chosen), (query_gain_in, query_gain), (key_gain_in, key_gain), (up_in, up), (out_gain_in, out_gain)
            )
        )
    ]
    barrier = pltpu.get_barrier_semaphore()

    def greet(axis, index, size):
        def signal(step):
            pl.semaphore_signal(barrier, inc=1, device_id={axis: lax.rem(index + step, size)}, device_id_type=MESH)

        each(1, size, signal)

    greet("kv", kv, owners)
    greet("tp", tp, peers)

    for copy in (own_tokens, *small, own_latent, own_query, own_out):
        copy.start()
    own_tokens.wait()
    pl.semaphore_wait(barrier, owners + peers - 2)

    share = owners // PIECES

    def rows_copy(to, slot):
        return remote(full.at[tp, :, to], rows.at[slot], rows_send, rows_recv, "tp", to)

    def ask_copy(to, slot):
        return remote(asks.at[to], asked.at[slot], ask_send, ask_recv, "kv", to)

    def serve_target(slot):
        return pool.at[tp, pl.ds(blocks + slot * PER_OWNER, PER_OWNER)]

    def serve_copy(to, slot):
        return remote(served.at[to], serve_target(slot), serve_send, serve_recv.at[lax.div(slot, share)], "kv", to)

    def peer(i):
        return lax.rem(tp + i, peers)

    each(1, peers, lambda i: rows_copy(peer(i), tp).start())
    token_spread = Spread(
        full.reshape(peers, blocks * peers, group, width), 0, blocks * peers, spread_send.at[0], spread_recv.at[0]
    )
    token_spread.own()

    tile = (blocks, 128)
    lane = lax.broadcasted_iota(jnp.int32, tile, 1)
    sub = lax.broadcasted_iota(jnp.int32, tile, 0)
    ids = lane * blocks + sub

    small[0].wait()

    def mark(b, needed):
        for c in range(picks):
            needed = jnp.where(ids == chosen[b, c], 1, needed)
        return needed

    needed = lax.fori_loop(0, blocks, mark, jnp.zeros(tile, jnp.int32))
    first = jnp.full((1, 128), -1, jnp.int32)
    second = first
    for j in reversed(range(blocks)):
        hit = needed[j : j + 1, :] > 0
        second = jnp.where(hit, first, second)
        first = jnp.where(hit, j, first)
    both = jnp.where(sub == 0, first, jnp.where(sub == 1, second, 0))
    listed[...] = both
    to_scalars = pltpu.make_async_copy(listed, table, local_sem.at[4])
    to_scalars.start()
    both = both.astype(jnp.float32)

    for o in range(owners):
        spread_out = jnp.sum(jnp.where(lane == o, both, 0.0), axis=1, keepdims=True)
        asks[o] = jnp.broadcast_to(spread_out, tile)[:PER_OWNER]
    others = owners - 1

    def stay(source, target, sem):
        pltpu.make_async_copy(source, target, sem).start()

    each(0, kv, lambda o: ask_copy(o, kv).start())
    each(0, kv, lambda o: stay(asks.at[kv], asked.at[o], ask_recv))
    each(kv + 1, owners, lambda o: stay(asks.at[kv], asks.at[o], ask_send))

    ones = jnp.ones((ONES, BLOCK), jnp.bfloat16)

    def fill(slot):
        values[slot, BLOCK:, :] = ones

    each(0, slots, fill)
    key = lax.broadcasted_iota(jnp.int32, bias.shape[1:], 0)
    query = lax.rem(lax.broadcasted_iota(jnp.int32, bias.shape[1:], 1), BLOCK)
    bias[0] = jnp.where(key <= query, 0.0, masked_score)
    bias[1] = jnp.zeros(bias.shape[1:], jnp.float32)
    keys[slots] = jnp.zeros((BLOCK, width), jnp.bfloat16)
    values[slots] = jnp.zeros((BLOCK + ONES, BLOCK), jnp.bfloat16)
    def place(b):
        for c in range(picks):
            block = chosen[b, c]
            held = jnp.maximum(block, 0)
            owner = lax.div(held, blocks)
            inside = held - owner * blocks
            away = blocks + owner * PER_OWNER + jnp.where(table[1, owner] == inside, 1, 0)
            places[b, c] = jnp.where(block < 0, slots, jnp.where(owner == kv, inside, away))

    to_scalars.wait()
    each(0, blocks, place)
    for copy in small[1:]:
        copy.wait()
    rows[tp] = full[tp, :, tp]
    own_latent.wait()
    wait_bytes(rows.at[pl.ds(0, peers - 1)], rows_recv)

    @jax.jit
    def compress():
        features = jnp.concatenate([rows[p].reshape(lines, width) for p in range(peers)], axis=1)
        latent = jnp.dot(features, weight[...], preferred_element_type=jnp.float32)
        return latent.astype(jnp.bfloat16).reshape(blocks, group, 128)

    latent = compress()
    pool[tp, 0:blocks] = latent
    latent = latent.astype(jnp.float32)

    def serve(i):
        r = others - i
        for k in range(PER_OWNER):
            want = asked[r, k : k + 1, :]
            picked = jnp.zeros((group, 128), jnp.float32)
            for j in range(blocks):
                picked = jnp.where(want == float(j), latent[j], picked)
            served[r, k] = picked.astype(jnp.bfloat16)
        serve_copy(r, kv).start()

    wait_bytes(asked.at[pl.ds(0, others)], ask_recv)
    each(0, others - kv, serve)
    low = pool.at[tp, pl.ds(0, PER_OWNER)]
    each(0, kv, lambda o: stay(low, served.at[o], serve_send))
    full_share = lax.div(kv + share - 1, share) * share
    each(kv, full_share, lambda o: stay(low, serve_target(o), serve_recv.at[lax.div(o, share)]))
    here = Spread(pool, 0, blocks, spread_send.at[1], spread_recv.at[1])
    here.own()

    per_piece = share * PER_OWNER
    pieces = [lax.rem(lax.div(kv, share) + step, PIECES) for step in (0, 3, 1, 2)]
    firsts = [blocks + piece * per_piece for piece in pieces]
    spreads = [
        Spread(pool, first, per_piece, spread_send.at[2 + k], spread_recv.at[2 + k]) for k, first in enumerate(firsts)
    ]

    def if_needed(k, act):
        pl.when(pieces[k] * share < kv)(act)

    def gathered(k):
        wait_bytes(pool.at[tp, pl.ds(firsts[k], per_piece)], serve_recv.at[pieces[k]])
        spreads[k].start(0, 1)

    scale = width ** (-0.5) * LOG2E
    query_row = query_gain[...] * scale

    def project(j):
        features = jnp.concatenate(
            [full[p, pl.ds(2 * j, 2)].reshape(2 * BLOCK, width) for p in range(peers)], axis=1
        )
        projected = jnp.dot(features, projection[...], preferred_element_type=jnp.float32)
        projected = projected.astype(jnp.bfloat16).astype(jnp.float32)
        for i in range(2):
            for h in range(up.shape[0]):
                head = projected[i * BLOCK : (i + 1) * BLOCK, h * 128 : (h + 1) * 128]
                queries[2 * j + i, h * BLOCK : (h + 1) * BLOCK, :] = unit(head, query_row)

    eye_shape = (BLOCK, BLOCK)
    same = lax.broadcasted_iota(jnp.int32, eye_shape, 0) == lax.broadcasted_iota(jnp.int32, eye_shape, 1)
    eye = jnp.where(same, 1.0, 0.0).astype(jnp.bfloat16)

    def prepare(low, count):
        def several(j):
            first = low + 8 * j
            picked = [pool[:, first + i].reshape(BLOCK, width) for i in range(8)]
            turned = lax.dot_general(
                eye, jnp.concatenate(picked, axis=0), (((1,), (1,)), ((), ())), preferred_element_type=jnp.float32
            ).astype(jnp.bfloat16)
            for i in range(8):
                keys[first + i] = unit(picked[i].astype(jnp.float32), key_gain[...])
                values[first + i, :BLOCK, :] = turned[:, i * BLOCK : (i + 1) * BLOCK]

        each(0, count // 8, several)

    wait_bytes(rows.at[pl.ds(0, peers - 1)], rows_send)
    token_spread.relay_first()
    here.relay_first()
    near = kv >= owners - share

    def far_pieces():
        for k in range(1, PIECES):
            if_needed(k, functools.partial(gathered, k))
        for k in range(1, PIECES):
            if_needed(k, functools.partial(spreads[k].start, 2, 3, 4, 5))

    if_needed(0, functools.partial(gathered, 0))
    if_needed(0, functools.partial(spreads[0].start, 2, 3, 4, 5))
    pl.when(near)(far_pieces)
    token_spread.relay_rest()
    token_spread.finish()
    own_query.wait()
    own_out.wait()
    each(0, blocks // 2, project)
    pl.when(jnp.logical_not(near))(far_pieces)
    for k in range(PIECES):
        if_needed(k, spreads[k].relay_first)
    out_spread = Spread(wide_weight, 0, 128, spread_send.at[2 + PIECES], spread_recv.at[2 + PIECES])
    out_spread.own()
    here.relay_rest()
    here.finish()
    prepare(0, blocks)

    def complete(k):
        spreads[k].finish()
        prepare(firsts[k], per_piece)

    for k in range(PIECES + 1):
        if k < PIECES:
            if_needed(k, spreads[k].relay_rest)
        if k > 0:
            if_needed(k - 1, functools.partial(complete, k - 1))
    token_spread.drain()

    def heads_copy(to, b, slot):
        return remote(staged.at[b, to], heads.at[slot, b], heads_send, heads_recv.at[lax.div(b, HALF)], "tp", to)

    sides, heads_here = 2, up.shape[0]
    span = GROUP * BLOCK
    weights = full.reshape(sides, heads_here, -1, width)

    def weigh(b, side, g):
        picked = jnp.concatenate([keys[places[b, g * GROUP + i]] for i in range(GROUP)], axis=0)
        scores = lax.dot_general(
            picked, queries[b], (((1,), (1,)), ((), ())), preferred_element_type=jnp.float32
        )
        diagonal = jnp.exp2(scores[:BLOCK] + bias[jnp.minimum(g, 1)]).astype(jnp.bfloat16)
        others = jnp.exp2(scores[BLOCK:]).astype(jnp.bfloat16)
        for h in range(heads_here):
            cols = slice(h * BLOCK, (h + 1) * BLOCK)
            weights[side, h, :BLOCK, :] = diagonal[:, cols]
            weights[side, h, BLOCK:span, :] = others[:, cols]

    def add_up(b, side, g):
        held = jnp.concatenate([values[places[b, g * GROUP + i]] for i in range(GROUP)], axis=1)
        right = jnp.concatenate([weights[side, h, :span, :] for h in range(heads_here)], axis=1)
        return jnp.dot(held, right, preferred_element_type=jnp.float32)

    def hand_over(b, ended):
        shares = []
        for total in ended:
            shares.append((total[:BLOCK] / total[BLOCK : BLOCK + 1]).astype(jnp.bfloat16))
        turned, flipped = [], []
        for side in range(sides):
            for h in range(heads_here):
                share = shares[side][:, h * BLOCK : (h + 1) * BLOCK]
                turned.append(jnp.dot(up[h], share, preferred_element_type=jnp.float32))
        for side in range(sides):
            both = jnp.concatenate(turned[side * heads_here : (side + 1) * heads_here], axis=0)
            flipped.append(jnp.transpose(both).astype(jnp.bfloat16).reshape(peers, group, width))
        for side in range(sides):
            staged[b + side] = flipped[side]

    def start(i):
        for side in range(sides):
            weigh(sides * i + side, side, 0)

    groups = lax.div(jnp.minimum(picks, blocks + PER_OWNER * kv) + GROUP - 1, GROUP)

    def attend(i, following):
        first = sides * i
        for side in range(sides):
            totals[side] = jnp.zeros(totals.shape[1:], jnp.float32)

        def both(g):
            for side in range(sides):
                totals[side] = totals[side] + add_up(first + side, side, g - 1)
            for side in range(sides):
                weigh(first + side, side, g)

        each(1, groups, both)
        if not following:
            out_spread.relay_rest()
        ended = [totals[side] + add_up(first + side, side, groups - 1) for side in range(sides)]
        if following:
            start(i + 1)
        hand_over(first, ended)
        for side in range(sides):
            each(1, peers, lambda j: heads_copy(peer(j), first + side, tp).start())

    def part(half):
        return (0, HALF) if half == 0 else (HALF, blocks - HALF)

    def out_copy(to, half, slot):
        lower = pl.ds(*part(half))
        return remote(rows.at[to, lower], out.at[lower, slot], out_send, out_recv, "tp", to)

    @functools.partial(jax.jit, static_argnums=0)
    def mix(half):
        lower, count = pl.ds(*part(half)), part(half)[1]
        features = jnp.concatenate([heads[p, lower].reshape(count * group, width) for p in range(peers)], axis=1)
        summed = jnp.dot(
            features, wide_weight[...].reshape(peers * 128, peers * 128), preferred_element_type=jnp.float32
        )
        mixed = unit(summed, out_gain[...])
        for t in range(peers):
            rows[t, lower] = mixed[:, t * 128 : (t + 1) * 128].reshape(count, group, 128)

    def conclude(half):
        first, count = part(half)
        lower = pl.ds(first, count)
        wait_bytes(heads.at[pl.ds(0, peers - 1), lower], heads_recv.at[half])
        for b in range(first, first + count):
            heads[tp, b] = staged[b, tp]
        mix(half)
        each(1, peers, lambda i: out_copy(peer(i), half, tp).start())
        out[lower, tp] = rows[tp, lower]

    def turn(i):
        attend(i, True)

        @pl.when(i == 0)
        def _():
            out_spread.relay_first()

    last = blocks // sides - 1
    each(0, 1, start)
    each(0, last, turn)
    each(last, last + 1, lambda i: attend(i, False))
    out_spread.finish()
    conclude(0)
    conclude(1)

    wait_bytes(asks.at[pl.ds(0, others)], ask_send)
    wait_bytes(served.at[pl.ds(0, others)], serve_send)
    for spread in (here, out_spread):
        spread.drain()
    for k in range(PIECES):
        if_needed(k, spreads[k].drain)
    wait_bytes(staged.at[:, pl.ds(0, peers - 1)], heads_send)
    wait_bytes(rows.at[pl.ds(0, peers - 1)], out_send)
    wait_bytes(out.at[:, pl.ds(0, peers - 1)], out_recv)


def shards(
    tokens, query_weight, latent_weight, query_gain, key_gain, value_up, out_weight, out_gain, chosen
):
    peers, owners = lax.axis_size("tp"), lax.axis_size("kv")
    blocks, picks = chosen.shape
    rows, width = tokens.shape
    group = BLOCK // peers
    slots = blocks + owners * PER_OWNER
    heads = value_up.shape[0]
    vmem = pl.BlockSpec(memory_space=pltpu.VMEM)
    anywhere = pl.BlockSpec(memory_space=pl.ANY)
    dma = pltpu.SemaphoreType.DMA
    bf16 = jnp.bfloat16
    mixed = pl.pallas_call(
        kernel,
        out_shape=pltpu.VMEM((blocks, peers, group, width), bf16),
        in_specs=[anywhere] * 9,
        out_specs=vmem,
        scratch_shapes=[
            pltpu.SMEM((blocks, picks), jnp.int32),
            pltpu.VMEM((1, width), jnp.float32),
            pltpu.VMEM((1, width), jnp.float32),
            pltpu.VMEM((heads, value_up.shape[2], width), bf16),
            pltpu.VMEM((1, out_gain.shape[0]), jnp.float32),
            pltpu.VMEM((peers, blocks, peers, group, width), bf16),
            pltpu.VMEM((peers, slots, group, width), bf16),
            pltpu.VMEM((peers, *out_weight.shape), bf16),
            pltpu.VMEM(latent_weight.shape, bf16),
            pltpu.VMEM(query_weight.shape, bf16),
            pltpu.VMEM((peers, blocks, group, width), bf16),
            pltpu.VMEM((owners, PER_OWNER, 128), jnp.float32),
            pltpu.VMEM((owners, PER_OWNER, 128), jnp.float32),
            pltpu.VMEM((owners, PER_OWNER, group, width), bf16),
            pltpu.VMEM((blocks, 128), jnp.int32),
            pltpu.SMEM((blocks, 128), jnp.int32),
            pltpu.VMEM((blocks, heads * BLOCK, width), bf16),
            pltpu.VMEM((slots + 1, BLOCK, width), bf16),
            pltpu.VMEM((slots + 1, BLOCK + ONES, BLOCK), bf16),
            pltpu.VMEM((2, BLOCK + ONES, heads * BLOCK), jnp.float32),
            pltpu.VMEM((2, BLOCK, heads * BLOCK), jnp.float32),
            pltpu.SMEM((blocks, picks), jnp.int32),
            pltpu.VMEM((blocks, peers, group, width), bf16),
            pltpu.VMEM((peers, blocks, group, width), bf16),
            dma((10,)),
            dma, dma,
            dma, dma,
            dma, dma((PIECES,)),
            dma, dma((2,)),
            dma, dma,
            dma((3 + PIECES,)), dma((3 + PIECES, 3)),
        ],
        compiler_params=pltpu.CompilerParams(collective_id=0, has_side_effects=True),
    )(
        chosen,
        tokens.reshape(blocks, peers, group, width),
        latent_weight,
        query_weight,
        out_weight,
        query_gain.reshape(1, width),
        key_gain.reshape(1, width),
        jnp.swapaxes(value_up, 1, 2),
        out_gain.reshape(1, out_gain.shape[0]),
    )
    return mixed.reshape(rows, width)


def solution(mesh):
    in_specs = (
        P("kv", "tp"),
        P(None, "tp"),
        P(),
        P(),
        P(),
        P("tp", None, None),
        P("tp", None),
        P(),
        P("kv", None),
    )
    return jax.shard_map(shards, mesh=mesh, in_specs=in_specs, out_specs=P("kv", "tp"), check_vma=False)
```

```python
import functools

import jax
import jax.numpy as jnp
from jax import lax
from jax.experimental import pallas as pl
from jax.experimental.pallas import tpu as pltpu
from jax.sharding import PartitionSpec as P

BLOCK = 128
PER_OWNER = 2
MESH = pl.DeviceIdType.MESH
GROUP = 8
PIECES = 4
ONES = 16
HALF = 6
LOG2E = 1.4426950408889634


epsilon = 1e-06
masked_score = -1e30


def neighbours(tp):
    side = lax.rem(tp, 2)
    right = lax.rem(tp + 2, 8)
    left = lax.rem(tp + 6, 8)
    far = lax.rem(tp + 4, 8)
    return right, left, far, tp + 1 - 2 * side


class Spread:
    def __init__(self, full, first, size, send_sem, recv_sem):
        self.full, self.send_sem, self.recv_sem = full, send_sem, recv_sem
        half = size // 2
        self.ranges = ((first, half), (first + half, size - half))
        self.tp = lax.axis_index("tp")
        self.right, self.left, self.far, self.other = neighbours(self.tp)

    def sends(self):
        me, right, left, far, other = self.tp, self.right, self.left, self.far, self.other
        return (
            (me, 0, right, 0), (me, 1, left, 0), (me, 1, right, 1), (me, 0, left, 1), (me, 0, other, 2), (me, 1, other, 2),
            (left, 0, right, 1), (right, 1, left, 1), (left, 0, other, 2), (right, 1, other, 2), (left, 1, other, 2),
            (right, 0, other, 2), (far, 0, other, 2), (far, 1, other, 2),
        )

    def start(self, *kinds):
        every = self.sends()
        for kind in kinds:
            slot, part, dest, arrival = every[kind]
            first, size = self.ranges[part]
            piece = self.full.at[slot, pl.ds(first, size)]
            remote(piece, piece, self.send_sem, self.recv_sem.at[arrival], "tp", dest).start()

    def slices(self, count, sem):
        wait_bytes(self.full.at[pl.ds(0, count), pl.ds(self.ranges[0][0], sum(size for _, size in self.ranges))], sem)

    def own(self):
        self.start(0, 1, 2, 3, 4, 5)

    def relay_first(self):
        self.slices(1, self.recv_sem.at[0])
        self.start(6, 7, 8, 9)

    def relay_rest(self):
        self.slices(2, self.recv_sem.at[1])
        self.start(10, 11, 12, 13)

    def finish(self):
        self.slices(4, self.recv_sem.at[2])

    def drain(self):
        self.slices(7, self.send_sem)


def wait_bytes(region, sem):
    pltpu.make_async_copy(region, region, sem).wait()


def each(low, high, act):
    def step(i, carry):
        act(i)
        return carry

    lax.fori_loop(low, high, step, 0)


def remote(source, target, send_sem, recv_sem, axis, to):
    return pltpu.make_async_remote_copy(
        src_ref=source,
        dst_ref=target,
        send_sem=send_sem,
        recv_sem=recv_sem,
        device_id={axis: to},
        device_id_type=MESH,
    )


def unit(values, gain_row):
    mean_sq = jnp.mean(values * values, axis=-1, keepdims=True)
    return (values * lax.rsqrt(mean_sq + epsilon) * gain_row).astype(jnp.bfloat16)


def kernel(
    chosen_in, tokens, latent_weight, query_weight, out_weight, query_gain_in, key_gain_in, up_in, out_gain_in,
    out,
    chosen, query_gain, key_gain, up, out_gain,
    full, pool, wide_weight, weight, projection, rows, asked, asks, served, listed, table,
    queries, keys, values, totals, bias, places, staged, heads,
    local_sem, rows_send, rows_recv, ask_send, ask_recv, serve_send, serve_recv,
    heads_send, heads_recv, out_send, out_recv, spread_send, spread_recv,
):
    kv, tp = lax.axis_index("kv"), lax.axis_index("tp")
    owners, peers = asked.shape[0], full.shape[0]
    blocks, group, width = rows.shape[1:]
    picks = chosen.shape[1]
    slots = pool.shape[1]
    lines = blocks * group

    own_tokens = pltpu.make_async_copy(tokens, full.at[tp], local_sem.at[0])
    own_latent = pltpu.make_async_copy(latent_weight, weight, local_sem.at[1])
    own_query = pltpu.make_async_copy(query_weight, projection, local_sem.at[2])
    own_out = pltpu.make_async_copy(out_weight, wide_weight.at[tp], local_sem.at[3])
    small = [
        pltpu.make_async_copy(source, target, local_sem.at[5 + i])
        for i, (source, target) in enumerate(
            (
                (chosen_in, chosen), (query_gain_in, query_gain), (key_gain_in, key_gain), (up_in, up), (out_gain_in, out_gain)
            )
        )
    ]
    barrier = pltpu.get_barrier_semaphore()

    def greet(axis, index, size):
        def signal(step):
            pl.semaphore_signal(barrier, inc=1, device_id={axis: lax.rem(index + step, size)}, device_id_type=MESH)

        each(1, size, signal)

    greet("kv", kv, owners)
    greet("tp", tp, peers)

    for copy in (own_tokens, *small, own_latent, own_query, own_out):
        copy.start()
    own_tokens.wait()
    pl.semaphore_wait(barrier, owners + peers - 2)

    share = owners // PIECES

    def rows_copy(to, slot):
        return remote(full.at[tp, :, to], rows.at[slot], rows_send, rows_recv, "tp", to)

    def ask_copy(to, slot):
        return remote(asks.at[to], asked.at[slot], ask_send, ask_recv, "kv", to)

    def serve_target(slot):
        return pool.at[tp, pl.ds(blocks + slot * PER_OWNER, PER_OWNER)]

    def serve_copy(to, slot):
        return remote(served.at[to], serve_target(slot), serve_send, serve_recv.at[lax.div(slot, share)], "kv", to)

    def peer(i):
        return lax.rem(tp + i, peers)

    each(1, peers, lambda i: rows_copy(peer(i), tp).start())
    token_spread = Spread(
        full.reshape(peers, blocks * peers, group, width), 0, blocks * peers, spread_send.at[0], spread_recv.at[0]
    )
    token_spread.own()

    tile = (blocks, 128)
    lane = lax.broadcasted_iota(jnp.int32, tile, 1)
    sub = lax.broadcasted_iota(jnp.int32, tile, 0)
    ids = lane * blocks + sub

    small[0].wait()

    def mark(b, needed):
        for c in range(picks):
            needed = jnp.where(ids == chosen[b, c], 1, needed)
        return needed

    needed = lax.fori_loop(0, blocks, mark, jnp.zeros(tile, jnp.int32))
    first = jnp.full((1, 128), -1, jnp.int32)
    second = first
    for j in reversed(range(blocks)):
        hit = needed[j : j + 1, :] > 0
        second = jnp.where(hit, first, second)
        first = jnp.where(hit, j, first)
    both = jnp.where(sub == 0, first, jnp.where(sub == 1, second, 0))
    listed[...] = both
    to_scalars = pltpu.make_async_copy(listed, table, local_sem.at[4])
    to_scalars.start()
    both = both.astype(jnp.float32)

    for o in range(owners):
        spread_out = jnp.sum(jnp.where(lane == o, both, 0.0), axis=1, keepdims=True)
        asks[o] = jnp.broadcast_to(spread_out, tile)[:PER_OWNER]
    others = owners - 1

    def stay(source, target, sem):
        pltpu.make_async_copy(source, target, sem).start()

    each(0, kv, lambda o: ask_copy(o, kv).start())
    each(0, kv, lambda o: stay(asks.at[kv], asked.at[o], ask_recv))
    each(kv + 1, owners, lambda o: stay(asks.at[kv], asks.at[o], ask_send))

    ones = jnp.ones((ONES, BLOCK), jnp.bfloat16)

    def fill(slot):
        values[slot, BLOCK:, :] = ones

    each(0, slots, fill)
    key = lax.broadcasted_iota(jnp.int32, bias.shape[1:], 0)
    query = lax.rem(lax.broadcasted_iota(jnp.int32, bias.shape[1:], 1), BLOCK)
    bias[0] = jnp.where(key <= query, 0.0, masked_score)
    bias[1] = jnp.zeros(bias.shape[1:], jnp.float32)
    keys[slots] = jnp.zeros((BLOCK, width), jnp.bfloat16)
    values[slots] = jnp.zeros((BLOCK + ONES, BLOCK), jnp.bfloat16)
    def place(b):
        for c in range(picks):
            block = chosen[b, c]
            held = jnp.maximum(block, 0)
            owner = lax.div(held, blocks)
            inside = held - owner * blocks
            away = blocks + owner * PER_OWNER + jnp.where(table[1, owner] == inside, 1, 0)
            places[b, c] = jnp.where(block < 0, slots, jnp.where(owner == kv, inside, away))

    to_scalars.wait()
    each(0, blocks, place)
    for copy in small[1:]:
        copy.wait()
    rows[tp] = full[tp, :, tp]
    own_latent.wait()
    wait_bytes(rows.at[pl.ds(0, peers - 1)], rows_recv)

    @jax.jit
    def compress():
        features = jnp.concatenate([rows[p].reshape(lines, width) for p in range(peers)], axis=1)
        latent = jnp.dot(features, weight[...], preferred_element_type=jnp.float32)
        return latent.astype(jnp.bfloat16).reshape(blocks, group, 128)

    latent = compress()
    pool[tp, 0:blocks] = latent
    latent = latent.astype(jnp.float32)

    def serve(i):
        r = others - i
        for k in range(PER_OWNER):
            want = asked[r, k : k + 1, :]
            picked = jnp.zeros((group, 128), jnp.float32)
            for j in range(blocks):
                picked = jnp.where(want == float(j), latent[j], picked)
            served[r, k] = picked.astype(jnp.bfloat16)
        serve_copy(r, kv).start()

    wait_bytes(asked.at[pl.ds(0, others)], ask_recv)
    each(0, others - kv, serve)
    low = pool.at[tp, pl.ds(0, PER_OWNER)]
    each(0, kv, lambda o: stay(low, served.at[o], serve_send))
    full_share = lax.div(kv + share - 1, share) * share
    each(kv, full_share, lambda o: stay(low, serve_target(o), serve_recv.at[lax.div(o, share)]))
    here = Spread(pool, 0, blocks, spread_send.at[1], spread_recv.at[1])
    here.own()

    per_piece = share * PER_OWNER
    pieces = [lax.rem(lax.div(kv, share) + step, PIECES) for step in (0, 3, 1, 2)]
    firsts = [blocks + piece * per_piece for piece in pieces]
    spreads = [
        Spread(pool, first, per_piece, spread_send.at[2 + k], spread_recv.at[2 + k]) for k, first in enumerate(firsts)
    ]

    def if_needed(k, act):
        pl.when(pieces[k] * share < kv)(act)

    def gathered(k):
        wait_bytes(pool.at[tp, pl.ds(firsts[k], per_piece)], serve_recv.at[pieces[k]])
        spreads[k].start(0, 1)

    scale = width ** (-0.5) * LOG2E
    query_row = query_gain[...] * scale

    def project(j):
        features = jnp.concatenate(
            [full[p, pl.ds(2 * j, 2)].reshape(2 * BLOCK, width) for p in range(peers)], axis=1
        )
        projected = jnp.dot(features, projection[...], preferred_element_type=jnp.float32)
        projected = projected.astype(jnp.bfloat16).astype(jnp.float32)
        for i in range(2):
            for h in range(up.shape[0]):
                head = projected[i * BLOCK : (i + 1) * BLOCK, h * 128 : (h + 1) * 128]
                queries[2 * j + i, h * BLOCK : (h + 1) * BLOCK, :] = unit(head, query_row)

    eye_shape = (BLOCK, BLOCK)
    same = lax.broadcasted_iota(jnp.int32, eye_shape, 0) == lax.broadcasted_iota(jnp.int32, eye_shape, 1)
    eye = jnp.where(same, 1.0, 0.0).astype(jnp.bfloat16)

    def prepare(low, count):
        def several(j):
            first = low + 8 * j
            picked = [pool[:, first + i].reshape(BLOCK, width) for i in range(8)]
            turned = lax.dot_general(
                eye, jnp.concatenate(picked, axis=0), (((1,), (1,)), ((), ())), preferred_element_type=jnp.float32
            ).astype(jnp.bfloat16)
            for i in range(8):
                keys[first + i] = unit(picked[i].astype(jnp.float32), key_gain[...])
                values[first + i, :BLOCK, :] = turned[:, i * BLOCK : (i + 1) * BLOCK]

        each(0, count // 8, several)

    wait_bytes(rows.at[pl.ds(0, peers - 1)], rows_send)
    token_spread.relay_first()
    here.relay_first()
    near = jnp.logical_or(kv >= owners - share, kv < owners // 2)

    def far_pieces():
        for k in range(1, PIECES):
            if_needed(k, functools.partial(gathered, k))
        for k in range(1, PIECES):
            if_needed(k, functools.partial(spreads[k].start, 2, 3, 4, 5))

    if_needed(0, functools.partial(gathered, 0))
    if_needed(0, functools.partial(spreads[0].start, 2, 3, 4, 5))
    pl.when(near)(far_pieces)
    token_spread.relay_rest()
    token_spread.finish()
    own_query.wait()
    own_out.wait()
    each(0, blocks // 2, project)
    here.relay_rest()
    pl.when(jnp.logical_not(near))(far_pieces)
    for k in range(PIECES):
        if_needed(k, spreads[k].relay_first)
    out_spread = Spread(wide_weight, 0, 128, spread_send.at[2 + PIECES], spread_recv.at[2 + PIECES])
    out_spread.own()
    here.finish()
    prepare(0, blocks)

    def complete(k):
        spreads[k].finish()
        prepare(firsts[k], per_piece)

    for k in range(PIECES + 1):
        if k < PIECES:
            if_needed(k, spreads[k].relay_rest)
        if k > 0:
            if_needed(k - 1, functools.partial(complete, k - 1))
    token_spread.drain()

    def heads_copy(to, b, slot):
        return remote(staged.at[b, to], heads.at[slot, b], heads_send, heads_recv.at[lax.div(b, HALF)], "tp", to)

    sides, heads_here = 2, up.shape[0]
    span = GROUP * BLOCK
    weights = full.reshape(sides, heads_here, -1, width)

    def weigh(b, side, g):
        picked = jnp.concatenate([keys[places[b, g * GROUP + i]] for i in range(GROUP)], axis=0)
        scores = lax.dot_general(
            picked, queries[b], (((1,), (1,)), ((), ())), preferred_element_type=jnp.float32
        )
        diagonal = jnp.exp2(scores[:BLOCK] + bias[jnp.minimum(g, 1)]).astype(jnp.bfloat16)
        others = jnp.exp2(scores[BLOCK:]).astype(jnp.bfloat16)
        for h in range(heads_here):
            cols = slice(h * BLOCK, (h + 1) * BLOCK)
            weights[side, h, :BLOCK, :] = diagonal[:, cols]
            weights[side, h, BLOCK:span, :] = others[:, cols]

    def add_up(b, side, g):
        held = jnp.concatenate([values[places[b, g * GROUP + i]] for i in range(GROUP)], axis=1)
        right = jnp.concatenate([weights[side, h, :span, :] for h in range(heads_here)], axis=1)
        return jnp.dot(held, right, preferred_element_type=jnp.float32)

    def hand_over(b, ended):
        shares = []
        for total in ended:
            shares.append((total[:BLOCK] / total[BLOCK : BLOCK + 1]).astype(jnp.bfloat16))
        turned, flipped = [], []
        for side in range(sides):
            for h in range(heads_here):
                share = shares[side][:, h * BLOCK : (h + 1) * BLOCK]
                turned.append(jnp.dot(up[h], share, preferred_element_type=jnp.float32))
        for side in range(sides):
            both = jnp.concatenate(turned[side * heads_here : (side + 1) * heads_here], axis=0)
            flipped.append(jnp.transpose(both).astype(jnp.bfloat16).reshape(peers, group, width))
        for side in range(sides):
            staged[b + side] = flipped[side]

    def start(i):
        for side in range(sides):
            weigh(sides * i + side, side, 0)

    groups = lax.div(jnp.minimum(picks, blocks + PER_OWNER * kv) + GROUP - 1, GROUP)

    def attend(i, following):
        first = sides * i
        for side in range(sides):
            totals[side] = jnp.zeros(totals.shape[1:], jnp.float32)

        def both(g):
            for side in range(sides):
                totals[side] = totals[side] + add_up(first + side, side, g - 1)
            for side in range(sides):
                weigh(first + side, side, g)

        each(1, groups, both)
        if not following:
            out_spread.relay_rest()
        ended = [totals[side] + add_up(first + side, side, groups - 1) for side in range(sides)]
        if following:
            start(i + 1)
        hand_over(first, ended)
        for side in range(sides):
            each(1, peers, lambda j: heads_copy(peer(j), first + side, tp).start())

    def part(half):
        return (0, HALF) if half == 0 else (HALF, blocks - HALF)

    def out_copy(to, half, slot):
        lower = pl.ds(*part(half))
        return remote(rows.at[to, lower], out.at[lower, slot], out_send, out_recv, "tp", to)

    @functools.partial(jax.jit, static_argnums=0)
    def mix(half):
        lower, count = pl.ds(*part(half)), part(half)[1]
        features = jnp.concatenate([heads[p, lower].reshape(count * group, width) for p in range(peers)], axis=1)
        summed = jnp.dot(
            features, wide_weight[...].reshape(peers * 128, peers * 128), preferred_element_type=jnp.float32
        )
        mixed = unit(summed, out_gain[...])
        for t in range(peers):
            rows[t, lower] = mixed[:, t * 128 : (t + 1) * 128].reshape(count, group, 128)

    def conclude(half):
        first, count = part(half)
        lower = pl.ds(first, count)
        wait_bytes(heads.at[pl.ds(0, peers - 1), lower], heads_recv.at[half])
        for b in range(first, first + count):
            heads[tp, b] = staged[b, tp]
        mix(half)
        each(1, peers, lambda i: out_copy(peer(i), half, tp).start())
        out[lower, tp] = rows[tp, lower]

    def turn(i):
        attend(i, True)

        @pl.when(i == 0)
        def _():
            out_spread.relay_first()

    last = blocks // sides - 1
    each(0, 1, start)
    each(0, last, turn)
    each(last, last + 1, lambda i: attend(i, False))
    out_spread.finish()
    conclude(0)
    conclude(1)

    wait_bytes(asks.at[pl.ds(0, others)], ask_send)
    wait_bytes(served.at[pl.ds(0, others)], serve_send)
    for spread in (here, out_spread):
        spread.drain()
    for k in range(PIECES):
        if_needed(k, spreads[k].drain)
    wait_bytes(staged.at[:, pl.ds(0, peers - 1)], heads_send)
    wait_bytes(rows.at[pl.ds(0, peers - 1)], out_send)
    wait_bytes(out.at[:, pl.ds(0, peers - 1)], out_recv)


def shards(
    tokens, query_weight, latent_weight, query_gain, key_gain, value_up, out_weight, out_gain, chosen
):
    peers, owners = lax.axis_size("tp"), lax.axis_size("kv")
    blocks, picks = chosen.shape
    rows, width = tokens.shape
    group = BLOCK // peers
    slots = blocks + owners * PER_OWNER
    heads = value_up.shape[0]
    vmem = pl.BlockSpec(memory_space=pltpu.VMEM)
    anywhere = pl.BlockSpec(memory_space=pl.ANY)
    dma = pltpu.SemaphoreType.DMA
    bf16 = jnp.bfloat16
    mixed = pl.pallas_call(
        kernel,
        out_shape=pltpu.VMEM((blocks, peers, group, width), bf16),
        in_specs=[anywhere] * 9,
        out_specs=vmem,
        scratch_shapes=[
            pltpu.SMEM((blocks, picks), jnp.int32),
            pltpu.VMEM((1, width), jnp.float32),
            pltpu.VMEM((1, width), jnp.float32),
            pltpu.VMEM((heads, value_up.shape[2], width), bf16),
            pltpu.VMEM((1, out_gain.shape[0]), jnp.float32),
            pltpu.VMEM((peers, blocks, peers, group, width), bf16),
            pltpu.VMEM((peers, slots, group, width), bf16),
            pltpu.VMEM((peers, *out_weight.shape), bf16),
            pltpu.VMEM(latent_weight.shape, bf16),
            pltpu.VMEM(query_weight.shape, bf16),
            pltpu.VMEM((peers, blocks, group, width), bf16),
            pltpu.VMEM((owners, PER_OWNER, 128), jnp.float32),
            pltpu.VMEM((owners, PER_OWNER, 128), jnp.float32),
            pltpu.VMEM((owners, PER_OWNER, group, width), bf16),
            pltpu.VMEM((blocks, 128), jnp.int32),
            pltpu.SMEM((blocks, 128), jnp.int32),
            pltpu.VMEM((blocks, heads * BLOCK, width), bf16),
            pltpu.VMEM((slots + 1, BLOCK, width), bf16),
            pltpu.VMEM((slots + 1, BLOCK + ONES, BLOCK), bf16),
            pltpu.VMEM((2, BLOCK + ONES, heads * BLOCK), jnp.float32),
            pltpu.VMEM((2, BLOCK, heads * BLOCK), jnp.float32),
            pltpu.SMEM((blocks, picks), jnp.int32),
            pltpu.VMEM((blocks, peers, group, width), bf16),
            pltpu.VMEM((peers, blocks, group, width), bf16),
            dma((10,)),
            dma, dma,
            dma, dma,
            dma, dma((PIECES,)),
            dma, dma((2,)),
            dma, dma,
            dma((3 + PIECES,)), dma((3 + PIECES, 3)),
        ],
        compiler_params=pltpu.CompilerParams(collective_id=0, has_side_effects=True),
    )(
        chosen,
        tokens.reshape(blocks, peers, group, width),
        latent_weight,
        query_weight,
        out_weight,
        query_gain.reshape(1, width),
        key_gain.reshape(1, width),
        jnp.swapaxes(value_up, 1, 2),
        out_gain.reshape(1, out_gain.shape[0]),
    )
    return mixed.reshape(rows, width)


def solution(mesh):
    in_specs = (
        P("kv", "tp"),
        P(None, "tp"),
        P(),
        P(),
        P(),
        P("tp", None, None),
        P("tp", None),
        P(),
        P("kv", None),
    )
    return jax.shard_map(shards, mesh=mesh, in_specs=in_specs, out_specs=P("kv", "tp"), check_vma=False)
```

```python
import functools

import jax
import jax.numpy as jnp
from jax import lax
from jax.experimental import pallas as pl
from jax.experimental.pallas import tpu as pltpu
from jax.sharding import PartitionSpec as P

BLOCK = 128
PER_OWNER = 2
MESH = pl.DeviceIdType.MESH
GROUP = 8
PIECES = 4
ONES = 16
HALF = 6
LOG2E = 1.4426950408889634


epsilon = 1e-06
masked_score = -1e30


def neighbours(tp):
    side = lax.rem(tp, 2)
    right = lax.rem(tp + 2, 8)
    left = lax.rem(tp + 6, 8)
    far = lax.rem(tp + 4, 8)
    return right, left, far, tp + 1 - 2 * side


class Spread:
    def __init__(self, full, first, size, send_sem, recv_sem):
        self.full, self.send_sem, self.recv_sem = full, send_sem, recv_sem
        half = size // 2
        self.ranges = ((first, half), (first + half, size - half))
        self.tp = lax.axis_index("tp")
        self.right, self.left, self.far, self.other = neighbours(self.tp)

    def sends(self):
        me, right, left, far, other = self.tp, self.right, self.left, self.far, self.other
        return (
            (me, 0, right, 0), (me, 1, left, 0), (me, 1, right, 1), (me, 0, left, 1), (me, 0, other, 2), (me, 1, other, 2),
            (left, 0, right, 1), (right, 1, left, 1), (left, 0, other, 2), (right, 1, other, 2), (left, 1, other, 2),
            (right, 0, other, 2), (far, 0, other, 2), (far, 1, other, 2),
        )

    def start(self, *kinds):
        every = self.sends()
        for kind in kinds:
            slot, part, dest, arrival = every[kind]
            first, size = self.ranges[part]
            piece = self.full.at[slot, pl.ds(first, size)]
            remote(piece, piece, self.send_sem, self.recv_sem.at[arrival], "tp", dest).start()

    def slices(self, count, sem):
        wait_bytes(self.full.at[pl.ds(0, count), pl.ds(self.ranges[0][0], sum(size for _, size in self.ranges))], sem)

    def own(self):
        self.start(0, 1, 2, 3, 4, 5)

    def relay_first(self):
        self.slices(1, self.recv_sem.at[0])
        self.start(6, 7, 8, 9)

    def relay_rest(self):
        self.slices(2, self.recv_sem.at[1])
        self.start(10, 11, 12, 13)

    def finish(self):
        self.slices(4, self.recv_sem.at[2])

    def drain(self):
        self.slices(7, self.send_sem)


def wait_bytes(region, sem):
    pltpu.make_async_copy(region, region, sem).wait()


def each(low, high, act):
    def step(i, carry):
        act(i)
        return carry

    lax.fori_loop(low, high, step, 0)


def remote(source, target, send_sem, recv_sem, axis, to):
    return pltpu.make_async_remote_copy(
        src_ref=source,
        dst_ref=target,
        send_sem=send_sem,
        recv_sem=recv_sem,
        device_id={axis: to},
        device_id_type=MESH,
    )


def unit(values, gain_row):
    mean_sq = jnp.mean(values * values, axis=-1, keepdims=True)
    return (values * lax.rsqrt(mean_sq + epsilon) * gain_row).astype(jnp.bfloat16)


def kernel(
    chosen_in, tokens, latent_weight, query_weight, out_weight, query_gain_in, key_gain_in, up_in, out_gain_in,
    out,
    chosen, query_gain, key_gain, up, out_gain,
    full, pool, wide_weight, weight, projection, rows, asked, asks, served, listed, table,
    queries, keys, values, totals, bias, places, staged, heads,
    local_sem, rows_send, rows_recv, ask_send, ask_recv, serve_send, serve_recv,
    heads_send, heads_recv, out_send, out_recv, spread_send, spread_recv,
):
    kv, tp = lax.axis_index("kv"), lax.axis_index("tp")
    owners, peers = asked.shape[0], full.shape[0]
    blocks, group, width = rows.shape[1:]
    picks = chosen.shape[1]
    slots = pool.shape[1]
    lines = blocks * group

    own_tokens = pltpu.make_async_copy(tokens, full.at[tp], local_sem.at[0])
    own_latent = pltpu.make_async_copy(latent_weight, weight, local_sem.at[1])
    own_query = pltpu.make_async_copy(query_weight, projection, local_sem.at[2])
    own_out = pltpu.make_async_copy(out_weight, wide_weight.at[tp], local_sem.at[3])
    small = [
        pltpu.make_async_copy(source, target, local_sem.at[5 + i])
        for i, (source, target) in enumerate(
            (
                (chosen_in, chosen), (query_gain_in, query_gain), (key_gain_in, key_gain), (up_in, up), (out_gain_in, out_gain)
            )
        )
    ]
    barrier = pltpu.get_barrier_semaphore()

    def greet(axis, index, size):
        def signal(step):
            pl.semaphore_signal(barrier, inc=1, device_id={axis: lax.rem(index + step, size)}, device_id_type=MESH)

        each(1, size, signal)

    greet("kv", kv, owners)
    greet("tp", tp, peers)

    for copy in (own_tokens, *small, own_latent, own_query, own_out):
        copy.start()
    own_tokens.wait()
    pl.semaphore_wait(barrier, owners + peers - 2)

    share = owners // PIECES

    def rows_copy(to, slot):
        return remote(full.at[tp, :, to], rows.at[slot], rows_send, rows_recv, "tp", to)

    def ask_copy(to, slot):
        return remote(asks.at[to], asked.at[slot], ask_send, ask_recv, "kv", to)

    def serve_target(slot):
        return pool.at[tp, pl.ds(blocks + slot * PER_OWNER, PER_OWNER)]

    def serve_copy(to, slot):
        return remote(served.at[to], serve_target(slot), serve_send, serve_recv.at[lax.div(slot, share)], "kv", to)

    def peer(i):
        return lax.rem(tp + i, peers)

    each(1, peers, lambda i: rows_copy(peer(i), tp).start())
    token_spread = Spread(
        full.reshape(peers, blocks * peers, group, width), 0, blocks * peers, spread_send.at[0], spread_recv.at[0]
    )
    token_spread.own()

    tile = (blocks, 128)
    lane = lax.broadcasted_iota(jnp.int32, tile, 1)
    sub = lax.broadcasted_iota(jnp.int32, tile, 0)
    ids = lane * blocks + sub

    small[0].wait()

    def mark(b, needed):
        for c in range(picks):
            needed = jnp.where(ids == chosen[b, c], 1, needed)
        return needed

    needed = lax.fori_loop(0, blocks, mark, jnp.zeros(tile, jnp.int32))
    first = jnp.full((1, 128), -1, jnp.int32)
    second = first
    for j in reversed(range(blocks)):
        hit = needed[j : j + 1, :] > 0
        second = jnp.where(hit, first, second)
        first = jnp.where(hit, j, first)
    both = jnp.where(sub == 0, first, jnp.where(sub == 1, second, 0))
    listed[...] = both
    to_scalars = pltpu.make_async_copy(listed, table, local_sem.at[4])
    to_scalars.start()
    both = both.astype(jnp.float32)

    for o in range(owners):
        spread_out = jnp.sum(jnp.where(lane == o, both, 0.0), axis=1, keepdims=True)
        asks[o] = jnp.broadcast_to(spread_out, tile)[:PER_OWNER]
    others = owners - 1

    def stay(source, target, sem):
        pltpu.make_async_copy(source, target, sem).start()

    each(0, kv, lambda o: ask_copy(o, kv).start())
    each(0, kv, lambda o: stay(asks.at[kv], asked.at[o], ask_recv))
    each(kv + 1, owners, lambda o: stay(asks.at[kv], asks.at[o], ask_send))

    ones = jnp.ones((ONES, BLOCK), jnp.bfloat16)

    def fill(slot):
        values[slot, BLOCK:, :] = ones

    each(0, slots, fill)
    key = lax.broadcasted_iota(jnp.int32, bias.shape[1:], 0)
    query = lax.rem(lax.broadcasted_iota(jnp.int32, bias.shape[1:], 1), BLOCK)
    bias[0] = jnp.where(key <= query, 0.0, masked_score)
    bias[1] = jnp.zeros(bias.shape[1:], jnp.float32)
    keys[slots] = jnp.zeros((BLOCK, width), jnp.bfloat16)
    values[slots] = jnp.zeros((BLOCK + ONES, BLOCK), jnp.bfloat16)
    def place(b):
        for c in range(picks):
            block = chosen[b, c]
            held = jnp.maximum(block, 0)
            owner = lax.div(held, blocks)
            inside = held - owner * blocks
            away = blocks + owner * PER_OWNER + jnp.where(table[1, owner] == inside, 1, 0)
            places[b, c] = jnp.where(block < 0, slots, jnp.where(owner == kv, inside, away))

    to_scalars.wait()
    each(0, blocks, place)
    for copy in small[1:]:
        copy.wait()
    rows[tp] = full[tp, :, tp]
    own_latent.wait()
    wait_bytes(rows.at[pl.ds(0, peers - 1)], rows_recv)

    @jax.jit
    def compress():
        features = jnp.concatenate([rows[p].reshape(lines, width) for p in range(peers)], axis=1)
        latent = jnp.dot(features, weight[...], preferred_element_type=jnp.float32)
        return latent.astype(jnp.bfloat16).reshape(blocks, group, 128)

    latent = compress()
    pool[tp, 0:blocks] = latent
    latent = latent.astype(jnp.float32)

    def serve(i):
        r = others - i
        for k in range(PER_OWNER):
            want = asked[r, k : k + 1, :]
            picked = jnp.zeros((group, 128), jnp.float32)
            for j in range(blocks):
                picked = jnp.where(want == float(j), latent[j], picked)
            served[r, k] = picked.astype(jnp.bfloat16)
        serve_copy(r, kv).start()

    wait_bytes(asked.at[pl.ds(0, others)], ask_recv)
    each(0, others - kv, serve)
    low = pool.at[tp, pl.ds(0, PER_OWNER)]
    each(0, kv, lambda o: stay(low, served.at[o], serve_send))
    full_share = lax.div(kv + share - 1, share) * share
    each(kv, full_share, lambda o: stay(low, serve_target(o), serve_recv.at[lax.div(o, share)]))
    here = Spread(pool, 0, blocks, spread_send.at[1], spread_recv.at[1])
    here.own()

    per_piece = share * PER_OWNER
    pieces = [lax.rem(lax.div(kv, share) + step, PIECES) for step in (0, 3, 1, 2)]
    firsts = [blocks + piece * per_piece for piece in pieces]
    spreads = [
        Spread(pool, first, per_piece, spread_send.at[2 + k], spread_recv.at[2 + k]) for k, first in enumerate(firsts)
    ]

    def if_needed(k, act):
        pl.when(pieces[k] * share < kv)(act)

    def gathered(k):
        wait_bytes(pool.at[tp, pl.ds(firsts[k], per_piece)], serve_recv.at[pieces[k]])
        spreads[k].start(0, 1)

    scale = width ** (-0.5) * LOG2E
    query_row = query_gain[...] * scale

    def project(j):
        features = jnp.concatenate(
            [full[p, pl.ds(2 * j, 2)].reshape(2 * BLOCK, width) for p in range(peers)], axis=1
        )
        projected = jnp.dot(features, projection[...], preferred_element_type=jnp.float32)
        projected = projected.astype(jnp.bfloat16).astype(jnp.float32)
        for i in range(2):
            for h in range(up.shape[0]):
                head = projected[i * BLOCK : (i + 1) * BLOCK, h * 128 : (h + 1) * 128]
                queries[2 * j + i, h * BLOCK : (h + 1) * BLOCK, :] = unit(head, query_row)

    eye_shape = (BLOCK, BLOCK)
    same = lax.broadcasted_iota(jnp.int32, eye_shape, 0) == lax.broadcasted_iota(jnp.int32, eye_shape, 1)
    eye = jnp.where(same, 1.0, 0.0).astype(jnp.bfloat16)

    def prepare(low, count):
        def several(j):
            first = low + 8 * j
            picked = [pool[:, first + i].reshape(BLOCK, width) for i in range(8)]
            turned = lax.dot_general(
                eye, jnp.concatenate(picked, axis=0), (((1,), (1,)), ((), ())), preferred_element_type=jnp.float32
            ).astype(jnp.bfloat16)
            for i in range(8):
                keys[first + i] = unit(picked[i].astype(jnp.float32), key_gain[...])
                values[first + i, :BLOCK, :] = turned[:, i * BLOCK : (i + 1) * BLOCK]

        each(0, count // 8, several)

    wait_bytes(rows.at[pl.ds(0, peers - 1)], rows_send)
    token_spread.relay_first()
    here.relay_first()
    near = jnp.logical_or(kv >= owners - share, kv < owners // 2)

    def far_pieces():
        for k in range(1, PIECES):
            if_needed(k, functools.partial(gathered, k))
        for k in range(1, PIECES):
            if_needed(k, functools.partial(spreads[k].start, 2, 3, 4, 5))

    if_needed(0, functools.partial(gathered, 0))
    if_needed(0, functools.partial(spreads[0].start, 2, 3, 4, 5))
    pl.when(near)(far_pieces)
    token_spread.relay_rest()
    token_spread.finish()
    own_query.wait()
    own_out.wait()
    each(0, blocks // 2, project)
    here.relay_rest()
    pl.when(jnp.logical_not(near))(far_pieces)
    for k in range(PIECES):
        if_needed(k, spreads[k].relay_first)
    out_spread = Spread(wide_weight, 0, 128, spread_send.at[2 + PIECES], spread_recv.at[2 + PIECES])
    out_spread.own()
    here.finish()
    prepare(0, blocks)

    def complete(k):
        spreads[k].finish()
        prepare(firsts[k], per_piece)

    for k in range(PIECES + 1):
        if k < PIECES:
            if_needed(k, spreads[k].relay_rest)
        if k > 0:
            if_needed(k - 1, functools.partial(complete, k - 1))
    token_spread.drain()

    def heads_copy(to, b, slot):
        return remote(staged.at[b, to], heads.at[slot, b], heads_send, heads_recv.at[lax.div(b, HALF)], "tp", to)

    sides, heads_here = 2, up.shape[0]
    span = GROUP * BLOCK
    weights = full.reshape(sides, heads_here, -1, width)

    def weigh(b, side, g):
        picked = jnp.concatenate([keys[places[b, g * GROUP + i]] for i in range(GROUP)], axis=0)
        scores = lax.dot_general(
            picked, queries[b], (((1,), (1,)), ((), ())), preferred_element_type=jnp.float32
        )
        diagonal = jnp.exp2(scores[:BLOCK] + bias[jnp.minimum(g, 1)]).astype(jnp.bfloat16)
        others = jnp.exp2(scores[BLOCK:]).astype(jnp.bfloat16)
        for h in range(heads_here):
            cols = slice(h * BLOCK, (h + 1) * BLOCK)
            weights[side, h, :BLOCK, :] = diagonal[:, cols]
            weights[side, h, BLOCK:span, :] = others[:, cols]

    def add_up(b, side, g):
        held = jnp.concatenate([values[places[b, g * GROUP + i]] for i in range(GROUP)], axis=1)
        right = jnp.concatenate([weights[side, h, :span, :] for h in range(heads_here)], axis=1)
        return jnp.dot(held, right, preferred_element_type=jnp.float32)

    def hand_over(b, ended):
        shares = []
        for total in ended:
            shares.append((total[:BLOCK] / total[BLOCK : BLOCK + 1]).astype(jnp.bfloat16))
        turned, flipped = [], []
        for side in range(sides):
            for h in range(heads_here):
                share = shares[side][:, h * BLOCK : (h + 1) * BLOCK]
                turned.append(jnp.dot(up[h], share, preferred_element_type=jnp.float32))
        for side in range(sides):
            both = jnp.concatenate(turned[side * heads_here : (side + 1) * heads_here], axis=0)
            flipped.append(jnp.transpose(both).astype(jnp.bfloat16).reshape(peers, group, width))
        for side in range(sides):
            staged[b + side] = flipped[side]

    def start(i):
        for side in range(sides):
            weigh(sides * i + side, side, 0)

    groups = lax.div(jnp.minimum(picks, blocks + PER_OWNER * kv) + GROUP - 1, GROUP)

    def attend(i, following):
        first = sides * i
        for side in range(sides):
            totals[side] = jnp.zeros(totals.shape[1:], jnp.float32)

        def both(g):
            for side in range(sides):
                totals[side] = totals[side] + add_up(first + side, side, g - 1)
            for side in range(sides):
                weigh(first + side, side, g)

        if following:
            each(1, groups, both)
        else:
            each(1, jnp.minimum(groups, 2), both)
            out_spread.relay_rest()
            each(2, groups, both)
        ended = [totals[side] + add_up(first + side, side, groups - 1) for side in range(sides)]
        if following:
            start(i + 1)
        hand_over(first, ended)
        for side in range(sides):
            each(1, peers, lambda j: heads_copy(peer(j), first + side, tp).start())

    def part(half):
        return (0, HALF) if half == 0 else (HALF, blocks - HALF)

    def out_copy(to, half, slot):
        lower = pl.ds(*part(half))
        return remote(rows.at[to, lower], out.at[lower, slot], out_send, out_recv, "tp", to)

    @functools.partial(jax.jit, static_argnums=0)
    def mix(half):
        lower, count = pl.ds(*part(half)), part(half)[1]
        features = jnp.concatenate([heads[p, lower].reshape(count * group, width) for p in range(peers)], axis=1)
        summed = jnp.dot(
            features, wide_weight[...].reshape(peers * 128, peers * 128), preferred_element_type=jnp.float32
        )
        mixed = unit(summed, out_gain[...])
        for t in range(peers):
            rows[t, lower] = mixed[:, t * 128 : (t + 1) * 128].reshape(count, group, 128)

    def conclude(half):
        first, count = part(half)
        lower = pl.ds(first, count)
        wait_bytes(heads.at[pl.ds(0, peers - 1), lower], heads_recv.at[half])
        for b in range(first, first + count):
            heads[tp, b] = staged[b, tp]
        mix(half)
        each(1, peers, lambda i: out_copy(peer(i), half, tp).start())
        out[lower, tp] = rows[tp, lower]

    def turn(i):
        attend(i, True)

        @pl.when(i == 0)
        def _():
            out_spread.relay_first()

    last = blocks // sides - 1
    each(0, 1, start)
    each(0, last, turn)
    each(last, last + 1, lambda i: attend(i, False))
    out_spread.finish()
    conclude(0)
    conclude(1)

    wait_bytes(asks.at[pl.ds(0, others)], ask_send)
    wait_bytes(served.at[pl.ds(0, others)], serve_send)
    for spread in (here, out_spread):
        spread.drain()
    for k in range(PIECES):
        if_needed(k, spreads[k].drain)
    wait_bytes(staged.at[:, pl.ds(0, peers - 1)], heads_send)
    wait_bytes(rows.at[pl.ds(0, peers - 1)], out_send)
    wait_bytes(out.at[:, pl.ds(0, peers - 1)], out_recv)


def shards(
    tokens, query_weight, latent_weight, query_gain, key_gain, value_up, out_weight, out_gain, chosen
):
    peers, owners = lax.axis_size("tp"), lax.axis_size("kv")
    blocks, picks = chosen.shape
    rows, width = tokens.shape
    group = BLOCK // peers
    slots = blocks + owners * PER_OWNER
    heads = value_up.shape[0]
    vmem = pl.BlockSpec(memory_space=pltpu.VMEM)
    anywhere = pl.BlockSpec(memory_space=pl.ANY)
    dma = pltpu.SemaphoreType.DMA
    bf16 = jnp.bfloat16
    mixed = pl.pallas_call(
        kernel,
        out_shape=pltpu.VMEM((blocks, peers, group, width), bf16),
        in_specs=[anywhere] * 9,
        out_specs=vmem,
        scratch_shapes=[
            pltpu.SMEM((blocks, picks), jnp.int32),
            pltpu.VMEM((1, width), jnp.float32),
            pltpu.VMEM((1, width), jnp.float32),
            pltpu.VMEM((heads, value_up.shape[2], width), bf16),
            pltpu.VMEM((1, out_gain.shape[0]), jnp.float32),
            pltpu.VMEM((peers, blocks, peers, group, width), bf16),
            pltpu.VMEM((peers, slots, group, width), bf16),
            pltpu.VMEM((peers, *out_weight.shape), bf16),
            pltpu.VMEM(latent_weight.shape, bf16),
            pltpu.VMEM(query_weight.shape, bf16),
            pltpu.VMEM((peers, blocks, group, width), bf16),
            pltpu.VMEM((owners, PER_OWNER, 128), jnp.float32),
            pltpu.VMEM((owners, PER_OWNER, 128), jnp.float32),
            pltpu.VMEM((owners, PER_OWNER, group, width), bf16),
            pltpu.VMEM((blocks, 128), jnp.int32),
            pltpu.SMEM((blocks, 128), jnp.int32),
            pltpu.VMEM((blocks, heads * BLOCK, width), bf16),
            pltpu.VMEM((slots + 1, BLOCK, width), bf16),
            pltpu.VMEM((slots + 1, BLOCK + ONES, BLOCK), bf16),
            pltpu.VMEM((2, BLOCK + ONES, heads * BLOCK), jnp.float32),
            pltpu.VMEM((2, BLOCK, heads * BLOCK), jnp.float32),
            pltpu.SMEM((blocks, picks), jnp.int32),
            pltpu.VMEM((blocks, peers, group, width), bf16),
            pltpu.VMEM((peers, blocks, group, width), bf16),
            dma((10,)),
            dma, dma,
            dma, dma,
            dma, dma((PIECES,)),
            dma, dma((2,)),
            dma, dma,
            dma((3 + PIECES,)), dma((3 + PIECES, 3)),
        ],
        compiler_params=pltpu.CompilerParams(collective_id=0, has_side_effects=True),
    )(
        chosen,
        tokens.reshape(blocks, peers, group, width),
        latent_weight,
        query_weight,
        out_weight,
        query_gain.reshape(1, width),
        key_gain.reshape(1, width),
        jnp.swapaxes(value_up, 1, 2),
        out_gain.reshape(1, out_gain.shape[0]),
    )
    return mixed.reshape(rows, width)


def solution(mesh):
    in_specs = (
        P("kv", "tp"),
        P(None, "tp"),
        P(),
        P(),
        P(),
        P("tp", None, None),
        P("tp", None),
        P(),
        P("kv", None),
    )
    return jax.shard_map(shards, mesh=mesh, in_specs=in_specs, out_specs=P("kv", "tp"), check_vma=False)
```

```python
import functools

import jax
import jax.numpy as jnp
from jax import lax
from jax.experimental import pallas as pl
from jax.experimental.pallas import tpu as pltpu
from jax.sharding import PartitionSpec as P

BLOCK = 128
PER_OWNER = 2
MESH = pl.DeviceIdType.MESH
GROUP = 8
PIECES = 4
ONES = 16
HALF = 6
GROUPS_EARLY = 3
LOG2E = 1.4426950408889634


epsilon = 1e-06
masked_score = -1e30


def neighbours(tp):
    side = lax.rem(tp, 2)
    right = lax.rem(tp + 2, 8)
    left = lax.rem(tp + 6, 8)
    far = lax.rem(tp + 4, 8)
    return right, left, far, tp + 1 - 2 * side


class Spread:
    def __init__(self, full, first, size, send_sem, recv_sem):
        self.full, self.send_sem, self.recv_sem = full, send_sem, recv_sem
        half = size // 2
        self.ranges = ((first, half), (first + half, size - half))
        self.tp = lax.axis_index("tp")
        self.right, self.left, self.far, self.other = neighbours(self.tp)

    def sends(self):
        me, right, left, far, other = self.tp, self.right, self.left, self.far, self.other
        return (
            (me, 0, right, 0), (me, 1, left, 0), (me, 1, right, 1), (me, 0, left, 1), (me, 0, other, 2), (me, 1, other, 2),
            (left, 0, right, 1), (right, 1, left, 1), (left, 0, other, 2), (right, 1, other, 2), (left, 1, other, 2),
            (right, 0, other, 2), (far, 0, other, 2), (far, 1, other, 2),
        )

    def start(self, *kinds):
        every = self.sends()
        for kind in kinds:
            slot, part, dest, arrival = every[kind]
            first, size = self.ranges[part]
            piece = self.full.at[slot, pl.ds(first, size)]
            remote(piece, piece, self.send_sem, self.recv_sem.at[arrival], "tp", dest).start()

    def slices(self, count, sem):
        wait_bytes(self.full.at[pl.ds(0, count), pl.ds(self.ranges[0][0], sum(size for _, size in self.ranges))], sem)

    def own(self):
        self.start(0, 1, 2, 3, 4, 5)

    def relay_first(self):
        self.slices(1, self.recv_sem.at[0])
        self.start(6, 7, 8, 9)

    def relay_rest(self):
        self.slices(2, self.recv_sem.at[1])
        self.start(10, 11, 12, 13)

    def finish(self):
        self.slices(4, self.recv_sem.at[2])

    def drain(self):
        self.slices(7, self.send_sem)


def wait_bytes(region, sem):
    pltpu.make_async_copy(region, region, sem).wait()


def each(low, high, act):
    def step(i, carry):
        act(i)
        return carry

    lax.fori_loop(low, high, step, 0)


def remote(source, target, send_sem, recv_sem, axis, to):
    return pltpu.make_async_remote_copy(
        src_ref=source,
        dst_ref=target,
        send_sem=send_sem,
        recv_sem=recv_sem,
        device_id={axis: to},
        device_id_type=MESH,
    )


def unit(values, gain_row):
    mean_sq = jnp.mean(values * values, axis=-1, keepdims=True)
    return (values * lax.rsqrt(mean_sq + epsilon) * gain_row).astype(jnp.bfloat16)


def kernel(
    chosen_in, tokens, latent_weight, query_weight, out_weight, query_gain_in, key_gain_in, up_in, out_gain_in,
    out,
    chosen, query_gain, key_gain, up, out_gain,
    full, pool, wide_weight, weight, projection, rows, asked, asks, served, listed, table,
    queries, keys, values, totals, bias, places, staged, heads,
    local_sem, rows_send, rows_recv, ask_send, ask_recv, serve_send, serve_recv,
    heads_send, heads_recv, out_send, out_recv, spread_send, spread_recv,
):
    kv, tp = lax.axis_index("kv"), lax.axis_index("tp")
    owners, peers = asked.shape[0], full.shape[0]
    blocks, group, width = rows.shape[1:]
    picks = chosen.shape[1]
    slots = pool.shape[1]
    lines = blocks * group

    own_tokens = pltpu.make_async_copy(tokens, full.at[tp], local_sem.at[0])
    own_latent = pltpu.make_async_copy(latent_weight, weight, local_sem.at[1])
    own_query = pltpu.make_async_copy(query_weight, projection, local_sem.at[2])
    own_out = pltpu.make_async_copy(out_weight, wide_weight.at[tp], local_sem.at[3])
    small = [
        pltpu.make_async_copy(source, target, local_sem.at[5 + i])
        for i, (source, target) in enumerate(
            (
                (chosen_in, chosen), (query_gain_in, query_gain), (key_gain_in, key_gain), (up_in, up), (out_gain_in, out_gain)
            )
        )
    ]
    barrier = pltpu.get_barrier_semaphore()

    def greet(axis, index, size):
        def signal(step):
            pl.semaphore_signal(barrier, inc=1, device_id={axis: lax.rem(index + step, size)}, device_id_type=MESH)

        each(1, size, signal)

    greet("kv", kv, owners)
    greet("tp", tp, peers)

    for copy in (own_tokens, *small, own_latent, own_query, own_out):
        copy.start()
    own_tokens.wait()
    pl.semaphore_wait(barrier, owners + peers - 2)

    share = owners // PIECES

    def rows_copy(to, slot):
        return remote(full.at[tp, :, to], rows.at[slot], rows_send, rows_recv, "tp", to)

    def ask_copy(to, slot):
        return remote(asks.at[to], asked.at[slot], ask_send, ask_recv, "kv", to)

    def serve_target(slot):
        return pool.at[tp, pl.ds(blocks + slot * PER_OWNER, PER_OWNER)]

    def serve_copy(to, slot):
        return remote(served.at[to], serve_target(slot), serve_send, serve_recv.at[lax.div(slot, share)], "kv", to)

    def peer(i):
        return lax.rem(tp + i, peers)

    each(1, peers, lambda i: rows_copy(peer(i), tp).start())
    token_spread = Spread(
        full.reshape(peers, blocks * peers, group, width), 0, blocks * peers, spread_send.at[0], spread_recv.at[0]
    )
    token_spread.own()

    tile = (blocks, 128)
    lane = lax.broadcasted_iota(jnp.int32, tile, 1)
    sub = lax.broadcasted_iota(jnp.int32, tile, 0)
    ids = lane * blocks + sub

    small[0].wait()

    def mark(b, needed):
        for c in range(picks):
            needed = jnp.where(ids == chosen[b, c], 1, needed)
        return needed

    needed = lax.fori_loop(0, blocks, mark, jnp.zeros(tile, jnp.int32))
    first = jnp.full((1, 128), -1, jnp.int32)
    second = first
    for j in reversed(range(blocks)):
        hit = needed[j : j + 1, :] > 0
        second = jnp.where(hit, first, second)
        first = jnp.where(hit, j, first)
    both = jnp.where(sub == 0, first, jnp.where(sub == 1, second, 0))
    listed[...] = both
    to_scalars = pltpu.make_async_copy(listed, table, local_sem.at[4])
    to_scalars.start()
    both = both.astype(jnp.float32)

    for o in range(owners):
        spread_out = jnp.sum(jnp.where(lane == o, both, 0.0), axis=1, keepdims=True)
        asks[o] = jnp.broadcast_to(spread_out, tile)[:PER_OWNER]
    others = owners - 1

    def stay(source, target, sem):
        pltpu.make_async_copy(source, target, sem).start()

    each(0, kv, lambda o: ask_copy(o, kv).start())
    each(0, kv, lambda o: stay(asks.at[kv], asked.at[o], ask_recv))
    each(kv + 1, owners, lambda o: stay(asks.at[kv], asks.at[o], ask_send))

    ones = jnp.ones((ONES, BLOCK), jnp.bfloat16)

    def fill(slot):
        values[slot, BLOCK:, :] = ones

    each(0, slots, fill)
    key = lax.broadcasted_iota(jnp.int32, bias.shape[1:], 0)
    query = lax.rem(lax.broadcasted_iota(jnp.int32, bias.shape[1:], 1), BLOCK)
    bias[0] = jnp.where(key <= query, 0.0, masked_score)
    bias[1] = jnp.zeros(bias.shape[1:], jnp.float32)
    keys[slots] = jnp.zeros((BLOCK, width), jnp.bfloat16)
    values[slots] = jnp.zeros((BLOCK + ONES, BLOCK), jnp.bfloat16)
    def place(b):
        for c in range(picks):
            block = chosen[b, c]
            held = jnp.maximum(block, 0)
            owner = lax.div(held, blocks)
            inside = held - owner * blocks
            away = blocks + owner * PER_OWNER + jnp.where(table[1, owner] == inside, 1, 0)
            places[b, c] = jnp.where(block < 0, slots, jnp.where(owner == kv, inside, away))

    to_scalars.wait()
    each(0, blocks, place)
    for copy in small[1:]:
        copy.wait()
    rows[tp] = full[tp, :, tp]
    own_latent.wait()
    wait_bytes(rows.at[pl.ds(0, peers - 1)], rows_recv)

    @jax.jit
    def compress():
        features = jnp.concatenate([rows[p].reshape(lines, width) for p in range(peers)], axis=1)
        latent = jnp.dot(features, weight[...], preferred_element_type=jnp.float32)
        return latent.astype(jnp.bfloat16).reshape(blocks, group, 128)

    latent = compress()
    pool[tp, 0:blocks] = latent
    latent = latent.astype(jnp.float32)

    def serve(i):
        r = others - i
        for k in range(PER_OWNER):
            want = asked[r, k : k + 1, :]
            picked = jnp.zeros((group, 128), jnp.float32)
            for j in range(blocks):
                picked = jnp.where(want == float(j), latent[j], picked)
            served[r, k] = picked.astype(jnp.bfloat16)
        serve_copy(r, kv).start()

    wait_bytes(asked.at[pl.ds(0, others)], ask_recv)
    each(0, others - kv, serve)
    low = pool.at[tp, pl.ds(0, PER_OWNER)]
    each(0, kv, lambda o: stay(low, served.at[o], serve_send))
    full_share = lax.div(kv + share - 1, share) * share
    each(kv, full_share, lambda o: stay(low, serve_target(o), serve_recv.at[lax.div(o, share)]))
    here = Spread(pool, 0, blocks, spread_send.at[1], spread_recv.at[1])
    here.own()

    per_piece = share * PER_OWNER
    pieces = [lax.rem(lax.div(kv, share) + step, PIECES) for step in (0, 3, 1, 2)]
    firsts = [blocks + piece * per_piece for piece in pieces]
    spreads = [
        Spread(pool, first, per_piece, spread_send.at[2 + k], spread_recv.at[2 + k]) for k, first in enumerate(firsts)
    ]

    def if_needed(k, act):
        pl.when(pieces[k] * share < kv)(act)

    def gathered(k):
        wait_bytes(pool.at[tp, pl.ds(firsts[k], per_piece)], serve_recv.at[pieces[k]])
        spreads[k].start(0, 1)

    scale = width ** (-0.5) * LOG2E
    query_row = query_gain[...] * scale

    def project(j):
        features = jnp.concatenate(
            [full[p, pl.ds(2 * j, 2)].reshape(2 * BLOCK, width) for p in range(peers)], axis=1
        )
        projected = jnp.dot(features, projection[...], preferred_element_type=jnp.float32)
        projected = projected.astype(jnp.bfloat16).astype(jnp.float32)
        for i in range(2):
            for h in range(up.shape[0]):
                head = projected[i * BLOCK : (i + 1) * BLOCK, h * 128 : (h + 1) * 128]
                queries[2 * j + i, h * BLOCK : (h + 1) * BLOCK, :] = unit(head, query_row)

    eye_shape = (BLOCK, BLOCK)
    same = lax.broadcasted_iota(jnp.int32, eye_shape, 0) == lax.broadcasted_iota(jnp.int32, eye_shape, 1)
    eye = jnp.where(same, 1.0, 0.0).astype(jnp.bfloat16)

    def prepare(low, count):
        def several(j):
            first = low + 8 * j
            picked = [pool[:, first + i].reshape(BLOCK, width) for i in range(8)]
            turned = lax.dot_general(
                eye, jnp.concatenate(picked, axis=0), (((1,), (1,)), ((), ())), preferred_element_type=jnp.float32
            ).astype(jnp.bfloat16)
            for i in range(8):
                keys[first + i] = unit(picked[i].astype(jnp.float32), key_gain[...])
                values[first + i, :BLOCK, :] = turned[:, i * BLOCK : (i + 1) * BLOCK]

        each(0, count // 8, several)

    wait_bytes(rows.at[pl.ds(0, peers - 1)], rows_send)
    token_spread.relay_first()
    here.relay_first()
    near = jnp.logical_or(kv >= owners - share, kv < owners // 2)

    def far_pieces():
        for k in range(1, PIECES):
            if_needed(k, functools.partial(gathered, k))
        for k in range(1, PIECES):
            if_needed(k, functools.partial(spreads[k].start, 2, 3, 4, 5))

    if_needed(0, functools.partial(gathered, 0))
    if_needed(0, functools.partial(spreads[0].start, 2, 3, 4, 5))
    pl.when(near)(far_pieces)
    token_spread.relay_rest()
    token_spread.finish()
    own_query.wait()
    own_out.wait()
    each(0, blocks // 2, project)
    here.relay_rest()
    pl.when(jnp.logical_not(near))(far_pieces)
    for k in range(PIECES):
        if_needed(k, spreads[k].relay_first)
    out_spread = Spread(wide_weight, 0, 128, spread_send.at[2 + PIECES], spread_recv.at[2 + PIECES])
    out_spread.own()
    here.finish()
    prepare(0, blocks)

    def complete(k):
        spreads[k].finish()
        prepare(firsts[k], per_piece)

    for k in range(PIECES + 1):
        if k < PIECES:
            if_needed(k, spreads[k].relay_rest)
        if k > 0:
            if_needed(k - 1, functools.partial(complete, k - 1))
    token_spread.drain()

    def heads_copy(to, b, slot):
        return remote(staged.at[b, to], heads.at[slot, b], heads_send, heads_recv.at[lax.div(b, HALF)], "tp", to)

    sides, heads_here = 2, up.shape[0]
    span = GROUP * BLOCK
    weights = full.reshape(sides, heads_here, -1, width)

    def weigh(b, side, g):
        picked = jnp.concatenate([keys[places[b, g * GROUP + i]] for i in range(GROUP)], axis=0)
        scores = lax.dot_general(
            picked, queries[b], (((1,), (1,)), ((), ())), preferred_element_type=jnp.float32
        )
        diagonal = jnp.exp2(scores[:BLOCK] + bias[jnp.minimum(g, 1)]).astype(jnp.bfloat16)
        others = jnp.exp2(scores[BLOCK:]).astype(jnp.bfloat16)
        for h in range(heads_here):
            cols = slice(h * BLOCK, (h + 1) * BLOCK)
            weights[side, h, :BLOCK, :] = diagonal[:, cols]
            weights[side, h, BLOCK:span, :] = others[:, cols]

    def add_up(b, side, g):
        held = jnp.concatenate([values[places[b, g * GROUP + i]] for i in range(GROUP)], axis=1)
        right = jnp.concatenate([weights[side, h, :span, :] for h in range(heads_here)], axis=1)
        return jnp.dot(held, right, preferred_element_type=jnp.float32)

    def hand_over(b, ended):
        shares = []
        for total in ended:
            shares.append((total[:BLOCK] / total[BLOCK : BLOCK + 1]).astype(jnp.bfloat16))
        turned, flipped = [], []
        for side in range(sides):
            for h in range(heads_here):
                share = shares[side][:, h * BLOCK : (h + 1) * BLOCK]
                turned.append(jnp.dot(up[h], share, preferred_element_type=jnp.float32))
        for side in range(sides):
            both = jnp.concatenate(turned[side * heads_here : (side + 1) * heads_here], axis=0)
            flipped.append(jnp.transpose(both).astype(jnp.bfloat16).reshape(peers, group, width))
        for side in range(sides):
            staged[b + side] = flipped[side]

    def start(i):
        for side in range(sides):
            weigh(sides * i + side, side, 0)

    groups = lax.div(jnp.minimum(picks, blocks + PER_OWNER * kv) + GROUP - 1, GROUP)

    def attend(i, following):
        first = sides * i
        for side in range(sides):
            totals[side] = jnp.zeros(totals.shape[1:], jnp.float32)

        def both(g):
            for side in range(sides):
                totals[side] = totals[side] + add_up(first + side, side, g - 1)
            for side in range(sides):
                weigh(first + side, side, g)

        early = jnp.minimum(groups, GROUPS_EARLY)
        each(1, early, both)
        if following:
            pl.when(i == 0)(out_spread.relay_first)
        else:
            out_spread.relay_rest()
        each(early, groups, both)
        ended = [totals[side] + add_up(first + side, side, groups - 1) for side in range(sides)]
        if following:
            start(i + 1)
        hand_over(first, ended)
        for side in range(sides):
            each(1, peers, lambda j: heads_copy(peer(j), first + side, tp).start())

    def part(half):
        return (0, HALF) if half == 0 else (HALF, blocks - HALF)

    def out_copy(to, half, slot):
        lower = pl.ds(*part(half))
        return remote(rows.at[to, lower], out.at[lower, slot], out_send, out_recv, "tp", to)

    @functools.partial(jax.jit, static_argnums=0)
    def mix(half):
        lower, count = pl.ds(*part(half)), part(half)[1]
        features = jnp.concatenate([heads[p, lower].reshape(count * group, width) for p in range(peers)], axis=1)
        summed = jnp.dot(
            features, wide_weight[...].reshape(peers * 128, peers * 128), preferred_element_type=jnp.float32
        )
        mixed = unit(summed, out_gain[...])
        for t in range(peers):
            rows[t, lower] = mixed[:, t * 128 : (t + 1) * 128].reshape(count, group, 128)

    def conclude(half):
        first, count = part(half)
        lower = pl.ds(first, count)
        wait_bytes(heads.at[pl.ds(0, peers - 1), lower], heads_recv.at[half])
        for b in range(first, first + count):
            heads[tp, b] = staged[b, tp]
        mix(half)
        each(1, peers, lambda i: out_copy(peer(i), half, tp).start())
        out[lower, tp] = rows[tp, lower]

    def turn(i):
        attend(i, True)

    last = blocks // sides - 1
    each(0, 1, start)
    each(0, last, turn)
    each(last, last + 1, lambda i: attend(i, False))
    out_spread.finish()
    conclude(0)
    conclude(1)

    wait_bytes(asks.at[pl.ds(0, others)], ask_send)
    wait_bytes(served.at[pl.ds(0, others)], serve_send)
    for spread in (here, out_spread):
        spread.drain()
    for k in range(PIECES):
        if_needed(k, spreads[k].drain)
    wait_bytes(staged.at[:, pl.ds(0, peers - 1)], heads_send)
    wait_bytes(rows.at[pl.ds(0, peers - 1)], out_send)
    wait_bytes(out.at[:, pl.ds(0, peers - 1)], out_recv)


def shards(
    tokens, query_weight, latent_weight, query_gain, key_gain, value_up, out_weight, out_gain, chosen
):
    peers, owners = lax.axis_size("tp"), lax.axis_size("kv")
    blocks, picks = chosen.shape
    rows, width = tokens.shape
    group = BLOCK // peers
    slots = blocks + owners * PER_OWNER
    heads = value_up.shape[0]
    vmem = pl.BlockSpec(memory_space=pltpu.VMEM)
    anywhere = pl.BlockSpec(memory_space=pl.ANY)
    dma = pltpu.SemaphoreType.DMA
    bf16 = jnp.bfloat16
    mixed = pl.pallas_call(
        kernel,
        out_shape=pltpu.VMEM((blocks, peers, group, width), bf16),
        in_specs=[anywhere] * 9,
        out_specs=vmem,
        scratch_shapes=[
            pltpu.SMEM((blocks, picks), jnp.int32),
            pltpu.VMEM((1, width), jnp.float32),
            pltpu.VMEM((1, width), jnp.float32),
            pltpu.VMEM((heads, value_up.shape[2], width), bf16),
            pltpu.VMEM((1, out_gain.shape[0]), jnp.float32),
            pltpu.VMEM((peers, blocks, peers, group, width), bf16),
            pltpu.VMEM((peers, slots, group, width), bf16),
            pltpu.VMEM((peers, *out_weight.shape), bf16),
            pltpu.VMEM(latent_weight.shape, bf16),
            pltpu.VMEM(query_weight.shape, bf16),
            pltpu.VMEM((peers, blocks, group, width), bf16),
            pltpu.VMEM((owners, PER_OWNER, 128), jnp.float32),
            pltpu.VMEM((owners, PER_OWNER, 128), jnp.float32),
            pltpu.VMEM((owners, PER_OWNER, group, width), bf16),
            pltpu.VMEM((blocks, 128), jnp.int32),
            pltpu.SMEM((blocks, 128), jnp.int32),
            pltpu.VMEM((blocks, heads * BLOCK, width), bf16),
            pltpu.VMEM((slots + 1, BLOCK, width), bf16),
            pltpu.VMEM((slots + 1, BLOCK + ONES, BLOCK), bf16),
            pltpu.VMEM((2, BLOCK + ONES, heads * BLOCK), jnp.float32),
            pltpu.VMEM((2, BLOCK, heads * BLOCK), jnp.float32),
            pltpu.SMEM((blocks, picks), jnp.int32),
            pltpu.VMEM((blocks, peers, group, width), bf16),
            pltpu.VMEM((peers, blocks, group, width), bf16),
            dma((10,)),
            dma, dma,
            dma, dma,
            dma, dma((PIECES,)),
            dma, dma((2,)),
            dma, dma,
            dma((3 + PIECES,)), dma((3 + PIECES, 3)),
        ],
        compiler_params=pltpu.CompilerParams(collective_id=0, has_side_effects=True),
    )(
        chosen,
        tokens.reshape(blocks, peers, group, width),
        latent_weight,
        query_weight,
        out_weight,
        query_gain.reshape(1, width),
        key_gain.reshape(1, width),
        jnp.swapaxes(value_up, 1, 2),
        out_gain.reshape(1, out_gain.shape[0]),
    )
    return mixed.reshape(rows, width)


def solution(mesh):
    in_specs = (
        P("kv", "tp"),
        P(None, "tp"),
        P(),
        P(),
        P(),
        P("tp", None, None),
        P("tp", None),
        P(),
        P("kv", None),
    )
    return jax.shard_map(shards, mesh=mesh, in_specs=in_specs, out_specs=P("kv", "tp"), check_vma=False)
```

```python
import functools

import jax
import jax.numpy as jnp
from jax import lax
from jax.experimental import pallas as pl
from jax.experimental.pallas import tpu as pltpu
from jax.sharding import PartitionSpec as P

BLOCK = 128
PER_OWNER = 2
MESH = pl.DeviceIdType.MESH
GROUP = 8
PIECES = 4
ONES = 16
HALF = 6
LAYERS = 8
GROUPS_EARLY = 3
LOG2E = 1.4426950408889634


epsilon = 1e-06
masked_score = -1e30


def neighbours(tp):
    side = lax.rem(tp, 2)
    right = lax.rem(tp + 2, 8)
    left = lax.rem(tp + 6, 8)
    far = lax.rem(tp + 4, 8)
    return right, left, far, tp + 1 - 2 * side


class Spread:
    def __init__(self, full, first, size, send_sem, recv_sem):
        self.full, self.send_sem, self.recv_sem = full, send_sem, recv_sem
        half = size // 2
        self.ranges = ((first, half), (first + half, size - half))
        self.tp = lax.axis_index("tp")
        self.right, self.left, self.far, self.other = neighbours(self.tp)

    def sends(self):
        me, right, left, far, other = self.tp, self.right, self.left, self.far, self.other
        return (
            (me, 0, right, 0), (me, 1, left, 0), (me, 1, right, 1), (me, 0, left, 1), (me, 0, other, 2), (me, 1, other, 2),
            (left, 0, right, 1), (right, 1, left, 1), (left, 0, other, 2), (right, 1, other, 2), (left, 1, other, 2),
            (right, 0, other, 2), (far, 0, other, 2), (far, 1, other, 2),
        )

    def start(self, *kinds):
        every = self.sends()
        for kind in kinds:
            slot, part, dest, arrival = every[kind]
            first, size = self.ranges[part]
            piece = self.full.at[slot, pl.ds(first, size)]
            remote(piece, piece, self.send_sem, self.recv_sem.at[arrival], "tp", dest).start()

    def slices(self, count, sem):
        wait_bytes(self.full.at[pl.ds(0, count), pl.ds(self.ranges[0][0], sum(size for _, size in self.ranges))], sem)

    def own(self):
        self.start(0, 1, 2, 3, 4, 5)

    def relay_first(self):
        self.slices(1, self.recv_sem.at[0])
        self.start(6, 7, 8, 9)

    def relay_rest(self):
        self.slices(2, self.recv_sem.at[1])
        self.start(10, 11, 12, 13)

    def finish(self):
        self.slices(4, self.recv_sem.at[2])

    def drain(self):
        self.slices(7, self.send_sem)


def wait_bytes(region, sem):
    pltpu.make_async_copy(region, region, sem).wait()


def each(low, high, act):
    def step(i, carry):
        act(i)
        return carry

    lax.fori_loop(low, high, step, 0)


def remote(source, target, send_sem, recv_sem, axis, to):
    return pltpu.make_async_remote_copy(
        src_ref=source,
        dst_ref=target,
        send_sem=send_sem,
        recv_sem=recv_sem,
        device_id={axis: to},
        device_id_type=MESH,
    )


def unit(values, gain_row):
    mean_sq = jnp.mean(values * values, axis=-1, keepdims=True)
    return (values * lax.rsqrt(mean_sq + epsilon) * gain_row).astype(jnp.bfloat16)


def kernel(
    chosen_in, tokens, latent_weight, query_weight, out_weight, query_gain_in, key_gain_in, up_in, out_gain_in,
    out,
    chosen, query_gain, key_gain, up, out_gain,
    full, pool, wide_weight, weight, projection, rows, asked, asks, served, listed, table,
    queries, keys, values, totals, bias, places, staged, heads,
    local_sem, rows_send, rows_recv, ask_send, ask_recv, serve_send, serve_recv,
    heads_send, heads_recv, out_send, out_recv, spread_send, spread_recv,
):
    kv, tp = lax.axis_index("kv"), lax.axis_index("tp")
    owners, peers = asked.shape[0], full.shape[0]
    blocks, group, width = rows.shape[1:]
    picks = chosen.shape[1]
    slots = pool.shape[1]
    lines = blocks * group

    own_tokens = pltpu.make_async_copy(tokens, full.at[tp], local_sem.at[0])
    own_latent = pltpu.make_async_copy(latent_weight, weight, local_sem.at[1])
    own_query = pltpu.make_async_copy(query_weight, projection, local_sem.at[2])
    own_out = pltpu.make_async_copy(out_weight, wide_weight.at[tp], local_sem.at[3])
    small = [
        pltpu.make_async_copy(source, target, local_sem.at[5 + i])
        for i, (source, target) in enumerate(
            (
                (chosen_in, chosen), (query_gain_in, query_gain), (key_gain_in, key_gain), (up_in, up), (out_gain_in, out_gain)
            )
        )
    ]
    barrier = pltpu.get_barrier_semaphore()

    def greet(axis, index, size):
        def signal(step):
            pl.semaphore_signal(barrier, inc=1, device_id={axis: lax.rem(index + step, size)}, device_id_type=MESH)

        each(1, size, signal)

    greet("kv", kv, owners)
    greet("tp", tp, peers)

    for copy in (own_tokens, *small, own_latent, own_query, own_out):
        copy.start()
    own_tokens.wait()
    pl.semaphore_wait(barrier, owners + peers - 2)

    share = owners // PIECES

    def rows_copy(to, slot):
        return remote(full.at[tp, :, to], rows.at[slot], rows_send, rows_recv, "tp", to)

    def ask_copy(to, slot):
        return remote(asks.at[to], asked.at[slot], ask_send, ask_recv, "kv", to)

    def serve_target(slot):
        return pool.at[tp, pl.ds(blocks + slot * PER_OWNER, PER_OWNER)]

    def serve_copy(to, slot):
        return remote(served.at[to], serve_target(slot), serve_send, serve_recv.at[lax.div(slot, share)], "kv", to)

    def peer(i):
        return lax.rem(tp + i, peers)

    each(1, peers, lambda i: rows_copy(peer(i), tp).start())
    token_spread = Spread(
        full.reshape(peers, blocks * peers, group, width), 0, blocks * peers, spread_send.at[0], spread_recv.at[0]
    )
    token_spread.own()

    tile = (blocks, 128)
    lane = lax.broadcasted_iota(jnp.int32, tile, 1)
    sub = lax.broadcasted_iota(jnp.int32, tile, 0)
    ids = lane * blocks + sub

    small[0].wait()

    def mark(b, needed):
        for c in range(picks):
            needed = jnp.where(ids == chosen[b, c], 1, needed)
        return needed

    needed = lax.fori_loop(0, blocks, mark, jnp.zeros(tile, jnp.int32))
    first = jnp.full((1, 128), -1, jnp.int32)
    second = first
    for j in reversed(range(blocks)):
        hit = needed[j : j + 1, :] > 0
        second = jnp.where(hit, first, second)
        first = jnp.where(hit, j, first)
    both = jnp.where(sub == 0, first, jnp.where(sub == 1, second, 0))
    listed[...] = both
    to_scalars = pltpu.make_async_copy(listed, table, local_sem.at[4])
    to_scalars.start()
    both = both.astype(jnp.float32)

    for o in range(owners):
        spread_out = jnp.sum(jnp.where(lane == o, both, 0.0), axis=1, keepdims=True)
        asks[o] = jnp.broadcast_to(spread_out, tile)[:PER_OWNER]
    others = owners - 1

    def stay(source, target, sem):
        pltpu.make_async_copy(source, target, sem).start()

    each(0, kv, lambda o: ask_copy(o, kv).start())
    each(0, kv, lambda o: stay(asks.at[kv], asked.at[o], ask_recv))
    each(kv + 1, owners, lambda o: stay(asks.at[kv], asks.at[o], ask_send))

    ones = jnp.ones((ONES, BLOCK), jnp.bfloat16)

    def fill(slot):
        values[slot, BLOCK:, :] = ones

    each(0, slots, fill)
    key = lax.broadcasted_iota(jnp.int32, bias.shape[1:], 0)
    query = lax.rem(lax.broadcasted_iota(jnp.int32, bias.shape[1:], 1), BLOCK)
    bias[0] = jnp.where(key <= query, 0.0, masked_score)
    bias[1] = jnp.zeros(bias.shape[1:], jnp.float32)
    keys[slots] = jnp.zeros((BLOCK, width), jnp.bfloat16)
    values[slots] = jnp.zeros((BLOCK + ONES, BLOCK), jnp.bfloat16)
    def place(b):
        for c in range(picks):
            block = chosen[b, c]
            held = jnp.maximum(block, 0)
            owner = lax.div(held, blocks)
            inside = held - owner * blocks
            away = blocks + owner * PER_OWNER + jnp.where(table[1, owner] == inside, 1, 0)
            places[b, c] = jnp.where(block < 0, slots, jnp.where(owner == kv, inside, away))

    to_scalars.wait()
    each(0, blocks, place)
    for copy in small[1:]:
        copy.wait()
    rows[tp] = full[tp, :, tp]
    own_latent.wait()
    wait_bytes(rows.at[pl.ds(0, peers - 1)], rows_recv)

    @jax.jit
    def compress():
        features = jnp.concatenate([rows[p].reshape(lines, width) for p in range(peers)], axis=1)
        latent = jnp.dot(features, weight[...], preferred_element_type=jnp.float32)
        return latent.astype(jnp.bfloat16).reshape(blocks, group, 128)

    latent = compress()
    pool[tp, 0:blocks] = latent
    latent = latent.astype(jnp.float32)

    def serve(r):
        for k in range(PER_OWNER):
            want = asked[r, k : k + 1, :]
            picked = jnp.zeros((group, 128), jnp.float32)
            for j in range(blocks):
                picked = jnp.where(want == float(j), latent[j], picked)
            served[r, k] = picked.astype(jnp.bfloat16)
        serve_copy(r, kv).start()

    def serve_in_turn(n):
        turn = lax.rem(n, LAYERS)
        away = lax.div(turn + 1, 2) * (2 * lax.rem(turn, 2) - 1)
        r = lax.rem(LAYERS // 2 + away, LAYERS) * (owners // LAYERS) + lax.div(n, LAYERS)
        pl.when(r > kv)(lambda: serve(r))

    wait_bytes(asked.at[pl.ds(0, others)], ask_recv)
    each(0, owners, serve_in_turn)
    low = pool.at[tp, pl.ds(0, PER_OWNER)]
    each(0, kv, lambda o: stay(low, served.at[o], serve_send))
    full_share = lax.div(kv + share - 1, share) * share
    each(kv, full_share, lambda o: stay(low, serve_target(o), serve_recv.at[lax.div(o, share)]))
    here = Spread(pool, 0, blocks, spread_send.at[1], spread_recv.at[1])
    here.own()

    per_piece = share * PER_OWNER
    pieces = [lax.rem(lax.div(kv, share) + step, PIECES) for step in (0, 3, 1, 2)]
    firsts = [blocks + piece * per_piece for piece in pieces]
    spreads = [
        Spread(pool, first, per_piece, spread_send.at[2 + k], spread_recv.at[2 + k]) for k, first in enumerate(firsts)
    ]

    def if_needed(k, act):
        pl.when(pieces[k] * share < kv)(act)

    def gathered(k):
        wait_bytes(pool.at[tp, pl.ds(firsts[k], per_piece)], serve_recv.at[pieces[k]])
        spreads[k].start(0, 1)

    scale = width ** (-0.5) * LOG2E
    query_row = query_gain[...] * scale

    def project(j):
        features = jnp.concatenate(
            [full[p, pl.ds(2 * j, 2)].reshape(2 * BLOCK, width) for p in range(peers)], axis=1
        )
        projected = jnp.dot(features, projection[...], preferred_element_type=jnp.float32)
        projected = projected.astype(jnp.bfloat16).astype(jnp.float32)
        for i in range(2):
            for h in range(up.shape[0]):
                head = projected[i * BLOCK : (i + 1) * BLOCK, h * 128 : (h + 1) * 128]
                queries[2 * j + i, h * BLOCK : (h + 1) * BLOCK, :] = unit(head, query_row)

    eye_shape = (BLOCK, BLOCK)
    same = lax.broadcasted_iota(jnp.int32, eye_shape, 0) == lax.broadcasted_iota(jnp.int32, eye_shape, 1)
    eye = jnp.where(same, 1.0, 0.0).astype(jnp.bfloat16)

    def prepare(low, count):
        def several(j):
            first = low + 8 * j
            picked = [pool[:, first + i].reshape(BLOCK, width) for i in range(8)]
            turned = lax.dot_general(
                eye, jnp.concatenate(picked, axis=0), (((1,), (1,)), ((), ())), preferred_element_type=jnp.float32
            ).astype(jnp.bfloat16)
            for i in range(8):
                keys[first + i] = unit(picked[i].astype(jnp.float32), key_gain[...])
                values[first + i, :BLOCK, :] = turned[:, i * BLOCK : (i + 1) * BLOCK]

        each(0, count // 8, several)

    wait_bytes(rows.at[pl.ds(0, peers - 1)], rows_send)
    token_spread.relay_first()
    here.relay_first()
    near = jnp.logical_or(kv >= owners - share, kv < owners // 2)

    def far_pieces():
        for k in range(1, PIECES):
            if_needed(k, functools.partial(gathered, k))
        for k in range(1, PIECES):
            if_needed(k, functools.partial(spreads[k].start, 2, 3, 4, 5))

    if_needed(0, functools.partial(gathered, 0))
    if_needed(0, functools.partial(spreads[0].start, 2, 3, 4, 5))
    pl.when(near)(far_pieces)
    token_spread.relay_rest()
    token_spread.finish()
    own_query.wait()
    own_out.wait()
    each(0, blocks // 2, project)
    here.relay_rest()
    pl.when(jnp.logical_not(near))(far_pieces)
    for k in range(PIECES):
        if_needed(k, spreads[k].relay_first)
    out_spread = Spread(wide_weight, 0, 128, spread_send.at[2 + PIECES], spread_recv.at[2 + PIECES])
    out_spread.own()
    here.finish()
    prepare(0, blocks)

    def complete(k):
        spreads[k].finish()
        prepare(firsts[k], per_piece)

    for k in range(PIECES + 1):
        if k < PIECES:
            if_needed(k, spreads[k].relay_rest)
        if k > 0:
            if_needed(k - 1, functools.partial(complete, k - 1))
    token_spread.drain()

    def heads_copy(to, b, slot):
        return remote(staged.at[b, to], heads.at[slot, b], heads_send, heads_recv.at[lax.div(b, HALF)], "tp", to)

    sides, heads_here = 2, up.shape[0]
    span = GROUP * BLOCK
    weights = full.reshape(sides, heads_here, -1, width)

    def weigh(b, side, g):
        picked = jnp.concatenate([keys[places[b, g * GROUP + i]] for i in range(GROUP)], axis=0)
        scores = lax.dot_general(
            picked, queries[b], (((1,), (1,)), ((), ())), preferred_element_type=jnp.float32
        )
        diagonal = jnp.exp2(scores[:BLOCK] + bias[jnp.minimum(g, 1)]).astype(jnp.bfloat16)
        others = jnp.exp2(scores[BLOCK:]).astype(jnp.bfloat16)
        for h in range(heads_here):
            cols = slice(h * BLOCK, (h + 1) * BLOCK)
            weights[side, h, :BLOCK, :] = diagonal[:, cols]
            weights[side, h, BLOCK:span, :] = others[:, cols]

    def add_up(b, side, g):
        held = jnp.concatenate([values[places[b, g * GROUP + i]] for i in range(GROUP)], axis=1)
        right = jnp.concatenate([weights[side, h, :span, :] for h in range(heads_here)], axis=1)
        return jnp.dot(held, right, preferred_element_type=jnp.float32)

    def hand_over(b, ended):
        shares = []
        for total in ended:
            shares.append((total[:BLOCK] / total[BLOCK : BLOCK + 1]).astype(jnp.bfloat16))
        turned, flipped = [], []
        for side in range(sides):
            for h in range(heads_here):
                share = shares[side][:, h * BLOCK : (h + 1) * BLOCK]
                turned.append(jnp.dot(up[h], share, preferred_element_type=jnp.float32))
        for side in range(sides):
            both = jnp.concatenate(turned[side * heads_here : (side + 1) * heads_here], axis=0)
            flipped.append(jnp.transpose(both).astype(jnp.bfloat16).reshape(peers, group, width))
        for side in range(sides):
            staged[b + side] = flipped[side]

    def start(i):
        for side in range(sides):
            weigh(sides * i + side, side, 0)

    groups = lax.div(jnp.minimum(picks, blocks + PER_OWNER * kv) + GROUP - 1, GROUP)

    def attend(i, following):
        first = sides * i
        for side in range(sides):
            totals[side] = jnp.zeros(totals.shape[1:], jnp.float32)

        def both(g):
            for side in range(sides):
                totals[side] = totals[side] + add_up(first + side, side, g - 1)
            for side in range(sides):
                weigh(first + side, side, g)

        early = jnp.minimum(groups, GROUPS_EARLY)
        each(1, early, both)
        if following:
            pl.when(i == 0)(out_spread.relay_first)
        else:
            out_spread.relay_rest()
        each(early, groups, both)
        ended = [totals[side] + add_up(first + side, side, groups - 1) for side in range(sides)]
        if following:
            start(i + 1)
        hand_over(first, ended)
        for side in range(sides):
            each(1, peers, lambda j: heads_copy(peer(j), first + side, tp).start())

    def part(half):
        return (0, HALF) if half == 0 else (HALF, blocks - HALF)

    def out_copy(to, half, slot):
        lower = pl.ds(*part(half))
        return remote(rows.at[to, lower], out.at[lower, slot], out_send, out_recv, "tp", to)

    @functools.partial(jax.jit, static_argnums=0)
    def mix(half):
        lower, count = pl.ds(*part(half)), part(half)[1]
        features = jnp.concatenate([heads[p, lower].reshape(count * group, width) for p in range(peers)], axis=1)
        summed = jnp.dot(
            features, wide_weight[...].reshape(peers * 128, peers * 128), preferred_element_type=jnp.float32
        )
        mixed = unit(summed, out_gain[...])
        for t in range(peers):
            rows[t, lower] = mixed[:, t * 128 : (t + 1) * 128].reshape(count, group, 128)

    def conclude(half):
        first, count = part(half)
        lower = pl.ds(first, count)
        wait_bytes(heads.at[pl.ds(0, peers - 1), lower], heads_recv.at[half])
        for b in range(first, first + count):
            heads[tp, b] = staged[b, tp]
        mix(half)
        each(1, peers, lambda i: out_copy(peer(i), half, tp).start())
        out[lower, tp] = rows[tp, lower]

    def turn(i):
        attend(i, True)

    last = blocks // sides - 1
    each(0, 1, start)
    each(0, last, turn)
    each(last, last + 1, lambda i: attend(i, False))
    out_spread.finish()
    conclude(0)
    conclude(1)

    wait_bytes(asks.at[pl.ds(0, others)], ask_send)
    wait_bytes(served.at[pl.ds(0, others)], serve_send)
    for spread in (here, out_spread):
        spread.drain()
    for k in range(PIECES):
        if_needed(k, spreads[k].drain)
    wait_bytes(staged.at[:, pl.ds(0, peers - 1)], heads_send)
    wait_bytes(rows.at[pl.ds(0, peers - 1)], out_send)
    wait_bytes(out.at[:, pl.ds(0, peers - 1)], out_recv)


def shards(
    tokens, query_weight, latent_weight, query_gain, key_gain, value_up, out_weight, out_gain, chosen
):
    peers, owners = lax.axis_size("tp"), lax.axis_size("kv")
    blocks, picks = chosen.shape
    rows, width = tokens.shape
    group = BLOCK // peers
    slots = blocks + owners * PER_OWNER
    heads = value_up.shape[0]
    vmem = pl.BlockSpec(memory_space=pltpu.VMEM)
    anywhere = pl.BlockSpec(memory_space=pl.ANY)
    dma = pltpu.SemaphoreType.DMA
    bf16 = jnp.bfloat16
    mixed = pl.pallas_call(
        kernel,
        out_shape=pltpu.VMEM((blocks, peers, group, width), bf16),
        in_specs=[anywhere] * 9,
        out_specs=vmem,
        scratch_shapes=[
            pltpu.SMEM((blocks, picks), jnp.int32),
            pltpu.VMEM((1, width), jnp.float32),
            pltpu.VMEM((1, width), jnp.float32),
            pltpu.VMEM((heads, value_up.shape[2], width), bf16),
            pltpu.VMEM((1, out_gain.shape[0]), jnp.float32),
            pltpu.VMEM((peers, blocks, peers, group, width), bf16),
            pltpu.VMEM((peers, slots, group, width), bf16),
            pltpu.VMEM((peers, *out_weight.shape), bf16),
            pltpu.VMEM(latent_weight.shape, bf16),
            pltpu.VMEM(query_weight.shape, bf16),
            pltpu.VMEM((peers, blocks, group, width), bf16),
            pltpu.VMEM((owners, PER_OWNER, 128), jnp.float32),
            pltpu.VMEM((owners, PER_OWNER, 128), jnp.float32),
            pltpu.VMEM((owners, PER_OWNER, group, width), bf16),
            pltpu.VMEM((blocks, 128), jnp.int32),
            pltpu.SMEM((blocks, 128), jnp.int32),
            pltpu.VMEM((blocks, heads * BLOCK, width), bf16),
            pltpu.VMEM((slots + 1, BLOCK, width), bf16),
            pltpu.VMEM((slots + 1, BLOCK + ONES, BLOCK), bf16),
            pltpu.VMEM((2, BLOCK + ONES, heads * BLOCK), jnp.float32),
            pltpu.VMEM((2, BLOCK, heads * BLOCK), jnp.float32),
            pltpu.SMEM((blocks, picks), jnp.int32),
            pltpu.VMEM((blocks, peers, group, width), bf16),
            pltpu.VMEM((peers, blocks, group, width), bf16),
            dma((10,)),
            dma, dma,
            dma, dma,
            dma, dma((PIECES,)),
            dma, dma((2,)),
            dma, dma,
            dma((3 + PIECES,)), dma((3 + PIECES, 3)),
        ],
        compiler_params=pltpu.CompilerParams(collective_id=0, has_side_effects=True),
    )(
        chosen,
        tokens.reshape(blocks, peers, group, width),
        latent_weight,
        query_weight,
        out_weight,
        query_gain.reshape(1, width),
        key_gain.reshape(1, width),
        jnp.swapaxes(value_up, 1, 2),
        out_gain.reshape(1, out_gain.shape[0]),
    )
    return mixed.reshape(rows, width)


def solution(mesh):
    in_specs = (
        P("kv", "tp"),
        P(None, "tp"),
        P(),
        P(),
        P(),
        P("tp", None, None),
        P("tp", None),
        P(),
        P("kv", None),
    )
    return jax.shard_map(shards, mesh=mesh, in_specs=in_specs, out_specs=P("kv", "tp"), check_vma=False)
```

```python
import functools

import jax
import jax.numpy as jnp
from jax import lax
from jax.experimental import pallas as pl
from jax.experimental.pallas import tpu as pltpu
from jax.sharding import PartitionSpec as P

BLOCK = 128
PER_OWNER = 2
MESH = pl.DeviceIdType.MESH
GROUP = 8
PIECES = 4
ONES = 16
HALF = 6
LAYERS = 8
GROUPS_EARLY = 3
LOG2E = 1.4426950408889634


epsilon = 1e-06
masked_score = -1e30


def neighbours(tp):
    side = lax.rem(tp, 2)
    right = lax.rem(tp + 2, 8)
    left = lax.rem(tp + 6, 8)
    far = lax.rem(tp + 4, 8)
    return right, left, far, tp + 1 - 2 * side


class Spread:
    def __init__(self, full, first, size, send_sem, recv_sem):
        self.full, self.send_sem, self.recv_sem = full, send_sem, recv_sem
        half = size // 2
        self.ranges = ((first, half), (first + half, size - half))
        self.tp = lax.axis_index("tp")
        self.right, self.left, self.far, self.other = neighbours(self.tp)

    def sends(self):
        me, right, left, far, other = self.tp, self.right, self.left, self.far, self.other
        return (
            (me, 0, right, 0), (me, 1, left, 0), (me, 1, right, 1), (me, 0, left, 1), (me, 0, other, 2), (me, 1, other, 2),
            (left, 0, right, 1), (right, 1, left, 1), (left, 0, other, 2), (right, 1, other, 2), (left, 1, other, 2),
            (right, 0, other, 2), (far, 0, other, 2), (far, 1, other, 2),
        )

    def start(self, *kinds):
        every = self.sends()
        for kind in kinds:
            slot, part, dest, arrival = every[kind]
            first, size = self.ranges[part]
            piece = self.full.at[slot, pl.ds(first, size)]
            remote(piece, piece, self.send_sem, self.recv_sem.at[arrival], "tp", dest).start()

    def slices(self, count, sem):
        wait_bytes(self.full.at[pl.ds(0, count), pl.ds(self.ranges[0][0], sum(size for _, size in self.ranges))], sem)

    def own(self):
        self.start(0, 1, 2, 3, 4, 5)

    def relay_first(self):
        self.slices(1, self.recv_sem.at[0])
        self.start(6, 7, 8, 9)

    def relay_rest(self):
        self.slices(2, self.recv_sem.at[1])
        self.start(10, 11, 12, 13)

    def finish(self):
        self.slices(4, self.recv_sem.at[2])

    def drain(self):
        self.slices(7, self.send_sem)


def wait_bytes(region, sem):
    pltpu.make_async_copy(region, region, sem).wait()


def each(low, high, act):
    def step(i, carry):
        act(i)
        return carry

    lax.fori_loop(low, high, step, 0)


def remote(source, target, send_sem, recv_sem, axis, to):
    return pltpu.make_async_remote_copy(
        src_ref=source,
        dst_ref=target,
        send_sem=send_sem,
        recv_sem=recv_sem,
        device_id={axis: to},
        device_id_type=MESH,
    )


def unit(values, gain_row):
    mean_sq = jnp.mean(values * values, axis=-1, keepdims=True)
    return (values * lax.rsqrt(mean_sq + epsilon) * gain_row).astype(jnp.bfloat16)


def kernel(
    chosen_in, tokens, latent_weight, query_weight, out_weight, query_gain_in, key_gain_in, up_in, out_gain_in,
    out,
    chosen, query_gain, key_gain, up, out_gain,
    full, pool, wide_weight, weight, projection, rows, asked, asks, served, listed, table,
    queries, keys, values, totals, bias, places, staged, heads,
    local_sem, rows_send, rows_recv, ask_send, ask_recv, serve_send, serve_recv,
    heads_send, heads_recv, out_send, out_recv, spread_send, spread_recv,
):
    kv, tp = lax.axis_index("kv"), lax.axis_index("tp")
    owners, peers = asked.shape[0], full.shape[0]
    blocks, group, width = rows.shape[1:]
    picks = chosen.shape[1]
    slots = pool.shape[1]
    lines = blocks * group

    own_tokens = pltpu.make_async_copy(tokens, full.at[tp], local_sem.at[0])
    own_latent = pltpu.make_async_copy(latent_weight, weight, local_sem.at[1])
    own_query = pltpu.make_async_copy(query_weight, projection, local_sem.at[2])
    own_out = pltpu.make_async_copy(out_weight, wide_weight.at[tp], local_sem.at[3])
    small = [
        pltpu.make_async_copy(source, target, local_sem.at[5 + i])
        for i, (source, target) in enumerate(
            (
                (chosen_in, chosen), (query_gain_in, query_gain), (key_gain_in, key_gain), (up_in, up), (out_gain_in, out_gain)
            )
        )
    ]
    barrier = pltpu.get_barrier_semaphore()

    def greet(axis, index, size):
        def signal(step):
            pl.semaphore_signal(barrier, inc=1, device_id={axis: lax.rem(index + step, size)}, device_id_type=MESH)

        each(1, size, signal)

    greet("kv", kv, owners)
    greet("tp", tp, peers)

    for copy in (own_tokens, *small, own_latent, own_query, own_out):
        copy.start()
    own_tokens.wait()
    pl.semaphore_wait(barrier, owners + peers - 2)

    share = owners // PIECES

    def rows_copy(to, slot):
        return remote(full.at[tp, :, to], rows.at[slot], rows_send, rows_recv, "tp", to)

    def ask_copy(to, slot):
        return remote(asks.at[to], asked.at[slot], ask_send, ask_recv, "kv", to)

    def serve_target(slot):
        return pool.at[tp, pl.ds(blocks + slot * PER_OWNER, PER_OWNER)]

    def serve_copy(to, slot):
        return remote(served.at[to], serve_target(slot), serve_send, serve_recv.at[lax.div(slot, share)], "kv", to)

    def peer(i):
        return lax.rem(tp + i, peers)

    each(1, peers, lambda i: rows_copy(peer(i), tp).start())
    token_spread = Spread(
        full.reshape(peers, blocks * peers, group, width), 0, blocks * peers, spread_send.at[0], spread_recv.at[0]
    )
    token_spread.own()

    tile = (blocks, 128)
    lane = lax.broadcasted_iota(jnp.int32, tile, 1)
    sub = lax.broadcasted_iota(jnp.int32, tile, 0)
    ids = lane * blocks + sub

    small[0].wait()

    def mark(b, needed):
        for c in range(picks):
            needed = jnp.where(ids == chosen[b, c], 1, needed)
        return needed

    needed = lax.fori_loop(0, blocks, mark, jnp.zeros(tile, jnp.int32))
    first = jnp.full((1, 128), -1, jnp.int32)
    second = first
    for j in reversed(range(blocks)):
        hit = needed[j : j + 1, :] > 0
        second = jnp.where(hit, first, second)
        first = jnp.where(hit, j, first)
    both = jnp.where(sub == 0, first, jnp.where(sub == 1, second, 0))
    listed[...] = both
    to_scalars = pltpu.make_async_copy(listed, table, local_sem.at[4])
    to_scalars.start()
    both = both.astype(jnp.float32)

    for o in range(owners):
        spread_out = jnp.sum(jnp.where(lane == o, both, 0.0), axis=1, keepdims=True)
        asks[o] = jnp.broadcast_to(spread_out, tile)[:PER_OWNER]
    others = owners - 1

    def stay(source, target, sem):
        pltpu.make_async_copy(source, target, sem).start()

    each(0, kv, lambda o: ask_copy(o, kv).start())
    each(0, kv, lambda o: stay(asks.at[kv], asked.at[o], ask_recv))
    each(kv + 1, owners, lambda o: stay(asks.at[kv], asks.at[o], ask_send))

    ones = jnp.ones((ONES, BLOCK), jnp.bfloat16)

    def fill(slot):
        values[slot, BLOCK:, :] = ones

    each(0, slots, fill)
    key = lax.broadcasted_iota(jnp.int32, bias.shape[1:], 0)
    query = lax.rem(lax.broadcasted_iota(jnp.int32, bias.shape[1:], 1), BLOCK)
    bias[0] = jnp.where(key <= query, 0.0, masked_score)
    bias[1] = jnp.zeros(bias.shape[1:], jnp.float32)
    keys[slots] = jnp.zeros((BLOCK, width), jnp.bfloat16)
    values[slots] = jnp.zeros((BLOCK + ONES, BLOCK), jnp.bfloat16)
    def place(b):
        for c in range(picks):
            block = chosen[b, c]
            held = jnp.maximum(block, 0)
            owner = lax.div(held, blocks)
            inside = held - owner * blocks
            away = blocks + owner * PER_OWNER + jnp.where(table[1, owner] == inside, 1, 0)
            places[b, c] = jnp.where(block < 0, slots, jnp.where(owner == kv, inside, away))

    to_scalars.wait()
    each(0, blocks, place)
    for copy in small[1:]:
        copy.wait()
    rows[tp] = full[tp, :, tp]
    own_latent.wait()
    wait_bytes(rows.at[pl.ds(0, peers - 1)], rows_recv)

    @jax.jit
    def compress():
        features = jnp.concatenate([rows[p].reshape(lines, width) for p in range(peers)], axis=1)
        latent = jnp.dot(features, weight[...], preferred_element_type=jnp.float32)
        return latent.astype(jnp.bfloat16).reshape(blocks, group, 128)

    latent = compress()
    pool[tp, 0:blocks] = latent
    latent = latent.astype(jnp.float32)

    def serve(r):
        for k in range(PER_OWNER):
            want = asked[r, k : k + 1, :]
            picked = jnp.zeros((group, 128), jnp.float32)
            for j in range(blocks):
                picked = jnp.where(want == float(j), latent[j], picked)
            served[r, k] = picked.astype(jnp.bfloat16)
        serve_copy(r, kv).start()

    def serve_in_turn(n):
        turn = lax.rem(n, LAYERS)
        away = lax.div(turn + 1, 2) * (2 * lax.rem(turn, 2) - 1)
        r = lax.rem(LAYERS // 2 + away, LAYERS) * (owners // LAYERS) + lax.div(n, LAYERS)
        pl.when(r > kv)(lambda: serve(r))

    wait_bytes(asked.at[pl.ds(0, others)], ask_recv)
    each(0, owners, serve_in_turn)
    low = pool.at[tp, pl.ds(0, PER_OWNER)]
    each(0, kv, lambda o: stay(low, served.at[o], serve_send))
    full_share = lax.div(kv + share - 1, share) * share
    each(kv, full_share, lambda o: stay(low, serve_target(o), serve_recv.at[lax.div(o, share)]))
    here = Spread(pool, 0, blocks, spread_send.at[1], spread_recv.at[1])
    here.own()

    per_piece = share * PER_OWNER
    pieces = [lax.rem(lax.div(kv, share) + step, PIECES) for step in (0, 3, 1, 2)]
    firsts = [blocks + piece * per_piece for piece in pieces]
    spreads = [
        Spread(pool, first, per_piece, spread_send.at[2 + k], spread_recv.at[2 + k]) for k, first in enumerate(firsts)
    ]

    def if_needed(k, act):
        pl.when(pieces[k] * share < kv)(act)

    def gathered(k):
        wait_bytes(pool.at[tp, pl.ds(firsts[k], per_piece)], serve_recv.at[pieces[k]])
        spreads[k].start(0, 1)

    scale = width ** (-0.5) * LOG2E
    query_row = query_gain[...] * scale

    def project(j):
        features = jnp.concatenate(
            [full[p, pl.ds(2 * j, 2)].reshape(2 * BLOCK, width) for p in range(peers)], axis=1
        )
        projected = jnp.dot(features, projection[...], preferred_element_type=jnp.float32)
        projected = projected.astype(jnp.bfloat16).astype(jnp.float32)
        for i in range(2):
            for h in range(up.shape[0]):
                head = projected[i * BLOCK : (i + 1) * BLOCK, h * 128 : (h + 1) * 128]
                queries[2 * j + i, h * BLOCK : (h + 1) * BLOCK, :] = unit(head, query_row)

    eye_shape = (BLOCK, BLOCK)
    same = lax.broadcasted_iota(jnp.int32, eye_shape, 0) == lax.broadcasted_iota(jnp.int32, eye_shape, 1)
    eye = jnp.where(same, 1.0, 0.0).astype(jnp.bfloat16)

    def prepare(low, count):
        def several(j):
            first = low + 8 * j
            picked = [pool[:, first + i].reshape(BLOCK, width) for i in range(8)]
            turned = lax.dot_general(
                eye, jnp.concatenate(picked, axis=0), (((1,), (1,)), ((), ())), preferred_element_type=jnp.float32
            ).astype(jnp.bfloat16)
            for i in range(8):
                keys[first + i] = unit(picked[i].astype(jnp.float32), key_gain[...])
                values[first + i, :BLOCK, :] = turned[:, i * BLOCK : (i + 1) * BLOCK]

        each(0, count // 8, several)

    wait_bytes(rows.at[pl.ds(0, peers - 1)], rows_send)
    token_spread.relay_first()
    here.relay_first()
    def far_pieces():
        for k in range(1, PIECES):
            if_needed(k, functools.partial(gathered, k))
        for k in range(1, PIECES):
            if_needed(k, functools.partial(spreads[k].start, 2, 3, 4, 5))

    if_needed(0, functools.partial(gathered, 0))
    if_needed(0, functools.partial(spreads[0].start, 2, 3, 4, 5))
    far_pieces()
    token_spread.relay_rest()
    token_spread.finish()
    own_query.wait()
    own_out.wait()
    each(0, blocks // 2, project)
    here.relay_rest()
    for k in range(PIECES):
        if_needed(k, spreads[k].relay_first)
    out_spread = Spread(wide_weight, 0, 128, spread_send.at[2 + PIECES], spread_recv.at[2 + PIECES])
    out_spread.own()
    here.finish()
    prepare(0, blocks)

    def complete(k):
        spreads[k].finish()
        prepare(firsts[k], per_piece)

    for k in range(PIECES + 1):
        if k < PIECES:
            if_needed(k, spreads[k].relay_rest)
        if k > 0:
            if_needed(k - 1, functools.partial(complete, k - 1))
    token_spread.drain()

    def heads_copy(to, b, slot):
        return remote(staged.at[b, to], heads.at[slot, b], heads_send, heads_recv.at[lax.div(b, HALF)], "tp", to)

    sides, heads_here = 2, up.shape[0]
    span = GROUP * BLOCK
    weights = full.reshape(sides, heads_here, -1, width)

    def weigh(b, side, g):
        picked = jnp.concatenate([keys[places[b, g * GROUP + i]] for i in range(GROUP)], axis=0)
        scores = lax.dot_general(
            picked, queries[b], (((1,), (1,)), ((), ())), preferred_element_type=jnp.float32
        )
        diagonal = jnp.exp2(scores[:BLOCK] + bias[jnp.minimum(g, 1)]).astype(jnp.bfloat16)
        others = jnp.exp2(scores[BLOCK:]).astype(jnp.bfloat16)
        for h in range(heads_here):
            cols = slice(h * BLOCK, (h + 1) * BLOCK)
            weights[side, h, :BLOCK, :] = diagonal[:, cols]
            weights[side, h, BLOCK:span, :] = others[:, cols]

    def add_up(b, side, g):
        held = jnp.concatenate([values[places[b, g * GROUP + i]] for i in range(GROUP)], axis=1)
        right = jnp.concatenate([weights[side, h, :span, :] for h in range(heads_here)], axis=1)
        return jnp.dot(held, right, preferred_element_type=jnp.float32)

    def hand_over(b, ended):
        shares = []
        for total in ended:
            shares.append((total[:BLOCK] / total[BLOCK : BLOCK + 1]).astype(jnp.bfloat16))
        turned, flipped = [], []
        for side in range(sides):
            for h in range(heads_here):
                share = shares[side][:, h * BLOCK : (h + 1) * BLOCK]
                turned.append(jnp.dot(up[h], share, preferred_element_type=jnp.float32))
        for side in range(sides):
            both = jnp.concatenate(turned[side * heads_here : (side + 1) * heads_here], axis=0)
            flipped.append(jnp.transpose(both).astype(jnp.bfloat16).reshape(peers, group, width))
        for side in range(sides):
            staged[b + side] = flipped[side]

    def start(i):
        for side in range(sides):
            weigh(sides * i + side, side, 0)

    groups = lax.div(jnp.minimum(picks, blocks + PER_OWNER * kv) + GROUP - 1, GROUP)

    def attend(i, following):
        first = sides * i
        for side in range(sides):
            totals[side] = jnp.zeros(totals.shape[1:], jnp.float32)

        def both(g):
            for side in range(sides):
                totals[side] = totals[side] + add_up(first + side, side, g - 1)
            for side in range(sides):
                weigh(first + side, side, g)

        early = jnp.minimum(groups, GROUPS_EARLY)
        each(1, early, both)
        if following:
            pl.when(i == 0)(out_spread.relay_first)
        else:
            out_spread.relay_rest()
        each(early, groups, both)
        ended = [totals[side] + add_up(first + side, side, groups - 1) for side in range(sides)]
        if following:
            start(i + 1)
        hand_over(first, ended)
        for side in range(sides):
            each(1, peers, lambda j: heads_copy(peer(j), first + side, tp).start())

    def part(half):
        return (0, HALF) if half == 0 else (HALF, blocks - HALF)

    def out_copy(to, half, slot):
        lower = pl.ds(*part(half))
        return remote(rows.at[to, lower], out.at[lower, slot], out_send, out_recv, "tp", to)

    @functools.partial(jax.jit, static_argnums=0)
    def mix(half):
        lower, count = pl.ds(*part(half)), part(half)[1]
        features = jnp.concatenate([heads[p, lower].reshape(count * group, width) for p in range(peers)], axis=1)
        summed = jnp.dot(
            features, wide_weight[...].reshape(peers * 128, peers * 128), preferred_element_type=jnp.float32
        )
        mixed = unit(summed, out_gain[...])
        for t in range(peers):
            rows[t, lower] = mixed[:, t * 128 : (t + 1) * 128].reshape(count, group, 128)

    def conclude(half):
        first, count = part(half)
        lower = pl.ds(first, count)
        wait_bytes(heads.at[pl.ds(0, peers - 1), lower], heads_recv.at[half])
        for b in range(first, first + count):
            heads[tp, b] = staged[b, tp]
        mix(half)
        each(1, peers, lambda i: out_copy(peer(i), half, tp).start())
        out[lower, tp] = rows[tp, lower]

    def turn(i):
        attend(i, True)

    last = blocks // sides - 1
    each(0, 1, start)
    each(0, last, turn)
    each(last, last + 1, lambda i: attend(i, False))
    out_spread.finish()
    conclude(0)
    conclude(1)

    wait_bytes(asks.at[pl.ds(0, others)], ask_send)
    wait_bytes(served.at[pl.ds(0, others)], serve_send)
    for spread in (here, out_spread):
        spread.drain()
    for k in range(PIECES):
        if_needed(k, spreads[k].drain)
    wait_bytes(staged.at[:, pl.ds(0, peers - 1)], heads_send)
    wait_bytes(rows.at[pl.ds(0, peers - 1)], out_send)
    wait_bytes(out.at[:, pl.ds(0, peers - 1)], out_recv)


def shards(
    tokens, query_weight, latent_weight, query_gain, key_gain, value_up, out_weight, out_gain, chosen
):
    peers, owners = lax.axis_size("tp"), lax.axis_size("kv")
    blocks, picks = chosen.shape
    rows, width = tokens.shape
    group = BLOCK // peers
    slots = blocks + owners * PER_OWNER
    heads = value_up.shape[0]
    vmem = pl.BlockSpec(memory_space=pltpu.VMEM)
    anywhere = pl.BlockSpec(memory_space=pl.ANY)
    dma = pltpu.SemaphoreType.DMA
    bf16 = jnp.bfloat16
    mixed = pl.pallas_call(
        kernel,
        out_shape=pltpu.VMEM((blocks, peers, group, width), bf16),
        in_specs=[anywhere] * 9,
        out_specs=vmem,
        scratch_shapes=[
            pltpu.SMEM((blocks, picks), jnp.int32),
            pltpu.VMEM((1, width), jnp.float32),
            pltpu.VMEM((1, width), jnp.float32),
            pltpu.VMEM((heads, value_up.shape[2], width), bf16),
            pltpu.VMEM((1, out_gain.shape[0]), jnp.float32),
            pltpu.VMEM((peers, blocks, peers, group, width), bf16),
            pltpu.VMEM((peers, slots, group, width), bf16),
            pltpu.VMEM((peers, *out_weight.shape), bf16),
            pltpu.VMEM(latent_weight.shape, bf16),
            pltpu.VMEM(query_weight.shape, bf16),
            pltpu.VMEM((peers, blocks, group, width), bf16),
            pltpu.VMEM((owners, PER_OWNER, 128), jnp.float32),
            pltpu.VMEM((owners, PER_OWNER, 128), jnp.float32),
            pltpu.VMEM((owners, PER_OWNER, group, width), bf16),
            pltpu.VMEM((blocks, 128), jnp.int32),
            pltpu.SMEM((blocks, 128), jnp.int32),
            pltpu.VMEM((blocks, heads * BLOCK, width), bf16),
            pltpu.VMEM((slots + 1, BLOCK, width), bf16),
            pltpu.VMEM((slots + 1, BLOCK + ONES, BLOCK), bf16),
            pltpu.VMEM((2, BLOCK + ONES, heads * BLOCK), jnp.float32),
            pltpu.VMEM((2, BLOCK, heads * BLOCK), jnp.float32),
            pltpu.SMEM((blocks, picks), jnp.int32),
            pltpu.VMEM((blocks, peers, group, width), bf16),
            pltpu.VMEM((peers, blocks, group, width), bf16),
            dma((10,)),
            dma, dma,
            dma, dma,
            dma, dma((PIECES,)),
            dma, dma((2,)),
            dma, dma,
            dma((3 + PIECES,)), dma((3 + PIECES, 3)),
        ],
        compiler_params=pltpu.CompilerParams(collective_id=0, has_side_effects=True),
    )(
        chosen,
        tokens.reshape(blocks, peers, group, width),
        latent_weight,
        query_weight,
        out_weight,
        query_gain.reshape(1, width),
        key_gain.reshape(1, width),
        jnp.swapaxes(value_up, 1, 2),
        out_gain.reshape(1, out_gain.shape[0]),
    )
    return mixed.reshape(rows, width)


def solution(mesh):
    in_specs = (
        P("kv", "tp"),
        P(None, "tp"),
        P(),
        P(),
        P(),
        P("tp", None, None),
        P("tp", None),
        P(),
        P("kv", None),
    )
    return jax.shard_map(shards, mesh=mesh, in_specs=in_specs, out_specs=P("kv", "tp"), check_vma=False)
```

```python
import functools

import jax
import jax.numpy as jnp
from jax import lax
from jax.experimental import pallas as pl
from jax.experimental.pallas import tpu as pltpu
from jax.sharding import PartitionSpec as P

BLOCK = 128
PER_OWNER = 2
MESH = pl.DeviceIdType.MESH
GROUP = 8
PIECES = 4
ONES = 16
HALF = 6
LAYERS = 8
GROUPS_EARLY = 3
LOG2E = 1.4426950408889634


epsilon = 1e-06
masked_score = -1e30


def neighbours(tp):
    side = lax.rem(tp, 2)
    right = lax.rem(tp + 2, 8)
    left = lax.rem(tp + 6, 8)
    far = lax.rem(tp + 4, 8)
    return right, left, far, tp + 1 - 2 * side


class Spread:
    def __init__(self, full, first, size, send_sem, recv_sem):
        self.full, self.send_sem, self.recv_sem = full, send_sem, recv_sem
        half = size // 2
        self.ranges = ((first, half), (first + half, size - half))
        self.tp = lax.axis_index("tp")
        self.right, self.left, self.far, self.other = neighbours(self.tp)

    def sends(self):
        me, right, left, far, other = self.tp, self.right, self.left, self.far, self.other
        return (
            (me, 0, right, 0), (me, 1, left, 0), (me, 1, right, 1), (me, 0, left, 1), (me, 0, other, 2), (me, 1, other, 2),
            (left, 0, right, 3), (right, 1, left, 3), (left, 0, other, 2), (right, 1, other, 2), (left, 1, other, 2),
            (right, 0, other, 2), (far, 0, other, 2), (far, 1, other, 2),
        )

    def start(self, *kinds):
        every = self.sends()
        for kind in kinds:
            slot, part, dest, arrival = every[kind]
            first, size = self.ranges[part]
            piece = self.full.at[slot, pl.ds(first, size)]
            remote(piece, piece, self.send_sem, self.recv_sem.at[arrival], "tp", dest).start()

    def slices(self, count, sem):
        wait_bytes(self.full.at[pl.ds(0, count), pl.ds(self.ranges[0][0], sum(size for _, size in self.ranges))], sem)

    def own(self):
        self.start(0, 1, 2, 3, 4, 5)

    def relay_first(self):
        self.slices(1, self.recv_sem.at[0])
        self.start(6, 7, 8, 9)

    def relay_near(self):
        self.slices(1, self.recv_sem.at[1])
        self.start(10, 11)

    def relay_far(self):
        self.slices(1, self.recv_sem.at[3])
        self.start(12, 13)

    def relay_rest(self):
        self.relay_near()
        self.relay_far()

    def finish(self):
        self.slices(4, self.recv_sem.at[2])

    def drain(self):
        self.slices(7, self.send_sem)


def wait_bytes(region, sem):
    pltpu.make_async_copy(region, region, sem).wait()


def each(low, high, act):
    def step(i, carry):
        act(i)
        return carry

    lax.fori_loop(low, high, step, 0)


def remote(source, target, send_sem, recv_sem, axis, to):
    return pltpu.make_async_remote_copy(
        src_ref=source,
        dst_ref=target,
        send_sem=send_sem,
        recv_sem=recv_sem,
        device_id={axis: to},
        device_id_type=MESH,
    )


def unit(values, gain_row):
    mean_sq = jnp.mean(values * values, axis=-1, keepdims=True)
    return (values * lax.rsqrt(mean_sq + epsilon) * gain_row).astype(jnp.bfloat16)


def kernel(
    chosen_in, tokens, latent_weight, query_weight, out_weight, query_gain_in, key_gain_in, up_in, out_gain_in,
    out,
    chosen, query_gain, key_gain, up, out_gain,
    full, pool, wide_weight, weight, projection, rows, asked, asks, served, listed, table,
    queries, keys, values, totals, bias, places, staged, heads,
    local_sem, rows_send, rows_recv, ask_send, ask_recv, serve_send, serve_recv,
    heads_send, heads_recv, out_send, out_recv, spread_send, spread_recv,
):
    kv, tp = lax.axis_index("kv"), lax.axis_index("tp")
    owners, peers = asked.shape[0], full.shape[0]
    blocks, group, width = rows.shape[1:]
    picks = chosen.shape[1]
    slots = pool.shape[1]
    lines = blocks * group

    own_tokens = pltpu.make_async_copy(tokens, full.at[tp], local_sem.at[0])
    own_latent = pltpu.make_async_copy(latent_weight, weight, local_sem.at[1])
    own_query = pltpu.make_async_copy(query_weight, projection, local_sem.at[2])
    own_out = pltpu.make_async_copy(out_weight, wide_weight.at[tp], local_sem.at[3])
    small = [
        pltpu.make_async_copy(source, target, local_sem.at[5 + i])
        for i, (source, target) in enumerate(
            (
                (chosen_in, chosen), (query_gain_in, query_gain), (key_gain_in, key_gain), (up_in, up), (out_gain_in, out_gain)
            )
        )
    ]
    barrier = pltpu.get_barrier_semaphore()

    def greet(axis, index, size):
        def signal(step):
            pl.semaphore_signal(barrier, inc=1, device_id={axis: lax.rem(index + step, size)}, device_id_type=MESH)

        each(1, size, signal)

    greet("kv", kv, owners)
    greet("tp", tp, peers)

    for copy in (own_tokens, *small, own_latent, own_query, own_out):
        copy.start()
    own_tokens.wait()
    pl.semaphore_wait(barrier, owners + peers - 2)

    share = owners // PIECES

    def rows_copy(to, slot):
        return remote(full.at[tp, :, to], rows.at[slot], rows_send, rows_recv, "tp", to)

    def ask_copy(to, slot):
        return remote(asks.at[to], asked.at[slot], ask_send, ask_recv, "kv", to)

    def serve_target(slot):
        return pool.at[tp, pl.ds(blocks + slot * PER_OWNER, PER_OWNER)]

    def serve_copy(to, slot):
        return remote(served.at[to], serve_target(slot), serve_send, serve_recv.at[lax.div(slot, share)], "kv", to)

    def peer(i):
        return lax.rem(tp + i, peers)

    each(1, peers, lambda i: rows_copy(peer(i), tp).start())
    token_spread = Spread(
        full.reshape(peers, blocks * peers, group, width), 0, blocks * peers, spread_send.at[0], spread_recv.at[0]
    )
    token_spread.own()

    tile = (blocks, 128)
    lane = lax.broadcasted_iota(jnp.int32, tile, 1)
    sub = lax.broadcasted_iota(jnp.int32, tile, 0)
    ids = lane * blocks + sub

    small[0].wait()

    def mark(b, needed):
        for c in range(picks):
            needed = jnp.where(ids == chosen[b, c], 1, needed)
        return needed

    needed = lax.fori_loop(0, blocks, mark, jnp.zeros(tile, jnp.int32))
    first = jnp.full((1, 128), -1, jnp.int32)
    second = first
    for j in reversed(range(blocks)):
        hit = needed[j : j + 1, :] > 0
        second = jnp.where(hit, first, second)
        first = jnp.where(hit, j, first)
    both = jnp.where(sub == 0, first, jnp.where(sub == 1, second, 0))
    listed[...] = both
    to_scalars = pltpu.make_async_copy(listed, table, local_sem.at[4])
    to_scalars.start()
    both = both.astype(jnp.float32)

    for o in range(owners):
        spread_out = jnp.sum(jnp.where(lane == o, both, 0.0), axis=1, keepdims=True)
        asks[o] = jnp.broadcast_to(spread_out, tile)[:PER_OWNER]
    others = owners - 1

    def stay(source, target, sem):
        pltpu.make_async_copy(source, target, sem).start()

    each(0, kv, lambda o: ask_copy(o, kv).start())
    each(0, kv, lambda o: stay(asks.at[kv], asked.at[o], ask_recv))
    each(kv + 1, owners, lambda o: stay(asks.at[kv], asks.at[o], ask_send))

    ones = jnp.ones((ONES, BLOCK), jnp.bfloat16)

    def fill(slot):
        values[slot, BLOCK:, :] = ones

    each(0, slots, fill)
    key = lax.broadcasted_iota(jnp.int32, bias.shape[1:], 0)
    query = lax.rem(lax.broadcasted_iota(jnp.int32, bias.shape[1:], 1), BLOCK)
    bias[0] = jnp.where(key <= query, 0.0, masked_score)
    bias[1] = jnp.zeros(bias.shape[1:], jnp.float32)
    keys[slots] = jnp.zeros((BLOCK, width), jnp.bfloat16)
    values[slots] = jnp.zeros((BLOCK + ONES, BLOCK), jnp.bfloat16)
    def place(b):
        for c in range(picks):
            block = chosen[b, c]
            held = jnp.maximum(block, 0)
            owner = lax.div(held, blocks)
            inside = held - owner * blocks
            away = blocks + owner * PER_OWNER + jnp.where(table[1, owner] == inside, 1, 0)
            places[b, c] = jnp.where(block < 0, slots, jnp.where(owner == kv, inside, away))

    to_scalars.wait()
    each(0, blocks, place)
    for copy in small[1:]:
        copy.wait()
    rows[tp] = full[tp, :, tp]
    own_latent.wait()
    wait_bytes(rows.at[pl.ds(0, peers - 1)], rows_recv)

    @jax.jit
    def compress():
        features = jnp.concatenate([rows[p].reshape(lines, width) for p in range(peers)], axis=1)
        latent = jnp.dot(features, weight[...], preferred_element_type=jnp.float32)
        return latent.astype(jnp.bfloat16).reshape(blocks, group, 128)

    latent = compress()
    pool[tp, 0:blocks] = latent
    latent = latent.astype(jnp.float32)

    def serve(r):
        for k in range(PER_OWNER):
            want = asked[r, k : k + 1, :]
            picked = jnp.zeros((group, 128), jnp.float32)
            for j in range(blocks):
                picked = jnp.where(want == float(j), latent[j], picked)
            served[r, k] = picked.astype(jnp.bfloat16)
        serve_copy(r, kv).start()

    def serve_in_turn(n):
        turn = lax.rem(n, LAYERS)
        away = lax.div(turn + 1, 2) * (2 * lax.rem(turn, 2) - 1)
        r = lax.rem(LAYERS // 2 + away, LAYERS) * (owners // LAYERS) + lax.div(n, LAYERS)
        pl.when(r > kv)(lambda: serve(r))

    wait_bytes(asked.at[pl.ds(0, others)], ask_recv)
    each(0, owners, serve_in_turn)
    low = pool.at[tp, pl.ds(0, PER_OWNER)]
    each(0, kv, lambda o: stay(low, served.at[o], serve_send))
    full_share = lax.div(kv + share - 1, share) * share
    each(kv, full_share, lambda o: stay(low, serve_target(o), serve_recv.at[lax.div(o, share)]))
    here = Spread(pool, 0, blocks, spread_send.at[1], spread_recv.at[1])
    here.own()

    per_piece = share * PER_OWNER
    pieces = [lax.rem(lax.div(kv, share) + step, PIECES) for step in (0, 3, 1, 2)]
    firsts = [blocks + piece * per_piece for piece in pieces]
    spreads = [
        Spread(pool, first, per_piece, spread_send.at[2 + k], spread_recv.at[2 + k]) for k, first in enumerate(firsts)
    ]

    def if_needed(k, act):
        pl.when(pieces[k] * share < kv)(act)

    def gathered(k):
        wait_bytes(pool.at[tp, pl.ds(firsts[k], per_piece)], serve_recv.at[pieces[k]])
        spreads[k].start(0, 1)

    scale = width ** (-0.5) * LOG2E
    query_row = query_gain[...] * scale

    def project(j):
        features = jnp.concatenate(
            [full[p, pl.ds(2 * j, 2)].reshape(2 * BLOCK, width) for p in range(peers)], axis=1
        )
        projected = jnp.dot(features, projection[...], preferred_element_type=jnp.float32)
        projected = projected.astype(jnp.bfloat16).astype(jnp.float32)
        for i in range(2):
            for h in range(up.shape[0]):
                head = projected[i * BLOCK : (i + 1) * BLOCK, h * 128 : (h + 1) * 128]
                queries[2 * j + i, h * BLOCK : (h + 1) * BLOCK, :] = unit(head, query_row)

    eye_shape = (BLOCK, BLOCK)
    same = lax.broadcasted_iota(jnp.int32, eye_shape, 0) == lax.broadcasted_iota(jnp.int32, eye_shape, 1)
    eye = jnp.where(same, 1.0, 0.0).astype(jnp.bfloat16)

    def prepare(low, count):
        def several(j):
            first = low + 8 * j
            picked = [pool[:, first + i].reshape(BLOCK, width) for i in range(8)]
            turned = lax.dot_general(
                eye, jnp.concatenate(picked, axis=0), (((1,), (1,)), ((), ())), preferred_element_type=jnp.float32
            ).astype(jnp.bfloat16)
            for i in range(8):
                keys[first + i] = unit(picked[i].astype(jnp.float32), key_gain[...])
                values[first + i, :BLOCK, :] = turned[:, i * BLOCK : (i + 1) * BLOCK]

        each(0, count // 8, several)

    wait_bytes(rows.at[pl.ds(0, peers - 1)], rows_send)
    token_spread.relay_first()
    token_spread.relay_near()
    here.relay_first()
    near = jnp.logical_or(kv >= owners - share, kv < owners // 2)

    def far_pieces():
        for k in range(1, PIECES):
            if_needed(k, functools.partial(gathered, k))
        for k in range(1, PIECES):
            if_needed(k, functools.partial(spreads[k].start, 2, 3, 4, 5))

    if_needed(0, functools.partial(gathered, 0))
    if_needed(0, functools.partial(spreads[0].start, 2, 3, 4, 5))
    pl.when(near)(far_pieces)
    token_spread.relay_far()
    token_spread.finish()
    own_query.wait()
    own_out.wait()
    each(0, blocks // 2, project)
    here.relay_rest()
    pl.when(jnp.logical_not(near))(far_pieces)
    for k in range(PIECES):
        if_needed(k, spreads[k].relay_first)
    out_spread = Spread(wide_weight, 0, 128, spread_send.at[2 + PIECES], spread_recv.at[2 + PIECES])
    out_spread.own()
    here.finish()
    prepare(0, blocks)

    def complete(k):
        spreads[k].finish()
        prepare(firsts[k], per_piece)

    for k in range(PIECES + 1):
        if k < PIECES:
            if_needed(k, spreads[k].relay_rest)
        if k > 0:
            if_needed(k - 1, functools.partial(complete, k - 1))
    token_spread.drain()

    def heads_copy(to, b, slot):
        return remote(staged.at[b, to], heads.at[slot, b], heads_send, heads_recv.at[lax.div(b, HALF)], "tp", to)

    sides, heads_here = 2, up.shape[0]
    span = GROUP * BLOCK
    weights = full.reshape(sides, heads_here, -1, width)

    def weigh(b, side, g):
        picked = jnp.concatenate([keys[places[b, g * GROUP + i]] for i in range(GROUP)], axis=0)
        scores = lax.dot_general(
            picked, queries[b], (((1,), (1,)), ((), ())), preferred_element_type=jnp.float32
        )
        diagonal = jnp.exp2(scores[:BLOCK] + bias[jnp.minimum(g, 1)]).astype(jnp.bfloat16)
        others = jnp.exp2(scores[BLOCK:]).astype(jnp.bfloat16)
        for h in range(heads_here):
            cols = slice(h * BLOCK, (h + 1) * BLOCK)
            weights[side, h, :BLOCK, :] = diagonal[:, cols]
            weights[side, h, BLOCK:span, :] = others[:, cols]

    def add_up(b, side, g):
        held = jnp.concatenate([values[places[b, g * GROUP + i]] for i in range(GROUP)], axis=1)
        right = jnp.concatenate([weights[side, h, :span, :] for h in range(heads_here)], axis=1)
        return jnp.dot(held, right, preferred_element_type=jnp.float32)

    def hand_over(b, ended):
        shares = []
        for total in ended:
            shares.append((total[:BLOCK] / total[BLOCK : BLOCK + 1]).astype(jnp.bfloat16))
        turned, flipped = [], []
        for side in range(sides):
            for h in range(heads_here):
                share = shares[side][:, h * BLOCK : (h + 1) * BLOCK]
                turned.append(jnp.dot(up[h], share, preferred_element_type=jnp.float32))
        for side in range(sides):
            both = jnp.concatenate(turned[side * heads_here : (side + 1) * heads_here], axis=0)
            flipped.append(jnp.transpose(both).astype(jnp.bfloat16).reshape(peers, group, width))
        for side in range(sides):
            staged[b + side] = flipped[side]

    def start(i):
        for side in range(sides):
            weigh(sides * i + side, side, 0)

    groups = lax.div(jnp.minimum(picks, blocks + PER_OWNER * kv) + GROUP - 1, GROUP)

    def attend(i, following):
        first = sides * i
        for side in range(sides):
            totals[side] = jnp.zeros(totals.shape[1:], jnp.float32)

        def both(g):
            for side in range(sides):
                totals[side] = totals[side] + add_up(first + side, side, g - 1)
            for side in range(sides):
                weigh(first + side, side, g)

        early = jnp.minimum(groups, GROUPS_EARLY)
        each(1, early, both)
        if following:
            pl.when(i == 0)(out_spread.relay_first)
        else:
            out_spread.relay_rest()
        each(early, groups, both)
        ended = [totals[side] + add_up(first + side, side, groups - 1) for side in range(sides)]
        if following:
            start(i + 1)
        hand_over(first, ended)
        for side in range(sides):
            each(1, peers, lambda j: heads_copy(peer(j), first + side, tp).start())

    def part(half):
        return (0, HALF) if half == 0 else (HALF, blocks - HALF)

    def out_copy(to, half, slot):
        lower = pl.ds(*part(half))
        return remote(rows.at[to, lower], out.at[lower, slot], out_send, out_recv, "tp", to)

    @functools.partial(jax.jit, static_argnums=0)
    def mix(half):
        lower, count = pl.ds(*part(half)), part(half)[1]
        features = jnp.concatenate([heads[p, lower].reshape(count * group, width) for p in range(peers)], axis=1)
        summed = jnp.dot(
            features, wide_weight[...].reshape(peers * 128, peers * 128), preferred_element_type=jnp.float32
        )
        mixed = unit(summed, out_gain[...])
        for t in range(peers):
            rows[t, lower] = mixed[:, t * 128 : (t + 1) * 128].reshape(count, group, 128)

    def conclude(half):
        first, count = part(half)
        lower = pl.ds(first, count)
        wait_bytes(heads.at[pl.ds(0, peers - 1), lower], heads_recv.at[half])
        for b in range(first, first + count):
            heads[tp, b] = staged[b, tp]
        mix(half)
        each(1, peers, lambda i: out_copy(peer(i), half, tp).start())
        out[lower, tp] = rows[tp, lower]

    def turn(i):
        attend(i, True)

    last = blocks // sides - 1
    each(0, 1, start)
    each(0, last, turn)
    each(last, last + 1, lambda i: attend(i, False))
    out_spread.finish()
    conclude(0)
    conclude(1)

    wait_bytes(asks.at[pl.ds(0, others)], ask_send)
    wait_bytes(served.at[pl.ds(0, others)], serve_send)
    for spread in (here, out_spread):
        spread.drain()
    for k in range(PIECES):
        if_needed(k, spreads[k].drain)
    wait_bytes(staged.at[:, pl.ds(0, peers - 1)], heads_send)
    wait_bytes(rows.at[pl.ds(0, peers - 1)], out_send)
    wait_bytes(out.at[:, pl.ds(0, peers - 1)], out_recv)


def shards(
    tokens, query_weight, latent_weight, query_gain, key_gain, value_up, out_weight, out_gain, chosen
):
    peers, owners = lax.axis_size("tp"), lax.axis_size("kv")
    blocks, picks = chosen.shape
    rows, width = tokens.shape
    group = BLOCK // peers
    slots = blocks + owners * PER_OWNER
    heads = value_up.shape[0]
    vmem = pl.BlockSpec(memory_space=pltpu.VMEM)
    anywhere = pl.BlockSpec(memory_space=pl.ANY)
    dma = pltpu.SemaphoreType.DMA
    bf16 = jnp.bfloat16
    mixed = pl.pallas_call(
        kernel,
        out_shape=pltpu.VMEM((blocks, peers, group, width), bf16),
        in_specs=[anywhere] * 9,
        out_specs=vmem,
        scratch_shapes=[
            pltpu.SMEM((blocks, picks), jnp.int32),
            pltpu.VMEM((1, width), jnp.float32),
            pltpu.VMEM((1, width), jnp.float32),
            pltpu.VMEM((heads, value_up.shape[2], width), bf16),
            pltpu.VMEM((1, out_gain.shape[0]), jnp.float32),
            pltpu.VMEM((peers, blocks, peers, group, width), bf16),
            pltpu.VMEM((peers, slots, group, width), bf16),
            pltpu.VMEM((peers, *out_weight.shape), bf16),
            pltpu.VMEM(latent_weight.shape, bf16),
            pltpu.VMEM(query_weight.shape, bf16),
            pltpu.VMEM((peers, blocks, group, width), bf16),
            pltpu.VMEM((owners, PER_OWNER, 128), jnp.float32),
            pltpu.VMEM((owners, PER_OWNER, 128), jnp.float32),
            pltpu.VMEM((owners, PER_OWNER, group, width), bf16),
            pltpu.VMEM((blocks, 128), jnp.int32),
            pltpu.SMEM((blocks, 128), jnp.int32),
            pltpu.VMEM((blocks, heads * BLOCK, width), bf16),
            pltpu.VMEM((slots + 1, BLOCK, width), bf16),
            pltpu.VMEM((slots + 1, BLOCK + ONES, BLOCK), bf16),
            pltpu.VMEM((2, BLOCK + ONES, heads * BLOCK), jnp.float32),
            pltpu.VMEM((2, BLOCK, heads * BLOCK), jnp.float32),
            pltpu.SMEM((blocks, picks), jnp.int32),
            pltpu.VMEM((blocks, peers, group, width), bf16),
            pltpu.VMEM((peers, blocks, group, width), bf16),
            dma((10,)),
            dma, dma,
            dma, dma,
            dma, dma((PIECES,)),
            dma, dma((2,)),
            dma, dma,
            dma((3 + PIECES,)), dma((3 + PIECES, 4)),
        ],
        compiler_params=pltpu.CompilerParams(collective_id=0, has_side_effects=True),
    )(
        chosen,
        tokens.reshape(blocks, peers, group, width),
        latent_weight,
        query_weight,
        out_weight,
        query_gain.reshape(1, width),
        key_gain.reshape(1, width),
        jnp.swapaxes(value_up, 1, 2),
        out_gain.reshape(1, out_gain.shape[0]),
    )
    return mixed.reshape(rows, width)


def solution(mesh):
    in_specs = (
        P("kv", "tp"),
        P(None, "tp"),
        P(),
        P(),
        P(),
        P("tp", None, None),
        P("tp", None),
        P(),
        P("kv", None),
    )
    return jax.shard_map(shards, mesh=mesh, in_specs=in_specs, out_specs=P("kv", "tp"), check_vma=False)
```

```python
import functools

import jax
import jax.numpy as jnp
from jax import lax
from jax.experimental import pallas as pl
from jax.experimental.pallas import tpu as pltpu
from jax.sharding import PartitionSpec as P

BLOCK = 128
PER_OWNER = 2
MESH = pl.DeviceIdType.MESH
GROUP = 8
PIECES = 4
ONES = 16
HALF = 6
LAYERS = 8
GROUPS_EARLY = 3
LOG2E = 1.4426950408889634


epsilon = 1e-06
masked_score = -1e30


def neighbours(tp):
    side = lax.rem(tp, 2)
    right = lax.rem(tp + 2, 8)
    left = lax.rem(tp + 6, 8)
    far = lax.rem(tp + 4, 8)
    return right, left, far, tp + 1 - 2 * side


class Spread:
    def __init__(self, full, first, size, send_sem, recv_sem):
        self.full, self.send_sem, self.recv_sem = full, send_sem, recv_sem
        half = size // 2
        self.ranges = ((first, half), (first + half, size - half))
        self.tp = lax.axis_index("tp")
        self.right, self.left, self.far, self.other = neighbours(self.tp)

    def sends(self):
        me, right, left, far, other = self.tp, self.right, self.left, self.far, self.other
        return (
            (me, 0, right, 0), (me, 1, left, 0), (me, 1, right, 1), (me, 0, left, 1), (me, 0, other, 2), (me, 1, other, 2),
            (left, 0, right, 3), (right, 1, left, 3), (left, 0, other, 2), (right, 1, other, 2), (left, 1, other, 2),
            (right, 0, other, 2), (far, 0, other, 2), (far, 1, other, 2),
        )

    def start(self, *kinds):
        every = self.sends()
        for kind in kinds:
            slot, part, dest, arrival = every[kind]
            first, size = self.ranges[part]
            piece = self.full.at[slot, pl.ds(first, size)]
            remote(piece, piece, self.send_sem, self.recv_sem.at[arrival], "tp", dest).start()

    def slices(self, count, sem):
        wait_bytes(self.full.at[pl.ds(0, count), pl.ds(self.ranges[0][0], sum(size for _, size in self.ranges))], sem)

    def own(self):
        self.start(0, 1, 2, 3, 4, 5)

    def relay_first(self):
        self.slices(1, self.recv_sem.at[0])
        self.start(6, 7, 8, 9)

    def relay_near(self):
        self.slices(1, self.recv_sem.at[1])
        self.start(10, 11)

    def relay_far(self):
        self.slices(1, self.recv_sem.at[3])
        self.start(12, 13)

    def relay_rest(self):
        self.relay_near()
        self.relay_far()

    def finish(self):
        self.slices(4, self.recv_sem.at[2])

    def drain(self):
        self.slices(7, self.send_sem)


def wait_bytes(region, sem):
    pltpu.make_async_copy(region, region, sem).wait()


def each(low, high, act):
    def step(i, carry):
        act(i)
        return carry

    lax.fori_loop(low, high, step, 0)


def remote(source, target, send_sem, recv_sem, axis, to):
    return pltpu.make_async_remote_copy(
        src_ref=source,
        dst_ref=target,
        send_sem=send_sem,
        recv_sem=recv_sem,
        device_id={axis: to},
        device_id_type=MESH,
    )


def unit(values, gain_row):
    mean_sq = jnp.mean(values * values, axis=-1, keepdims=True)
    return (values * lax.rsqrt(mean_sq + epsilon) * gain_row).astype(jnp.bfloat16)


def kernel(
    chosen_in, tokens, latent_weight, query_weight, out_weight, query_gain_in, key_gain_in, up_in, out_gain_in,
    out,
    chosen, query_gain, key_gain, up, out_gain,
    full, pool, wide_weight, weight, projection, rows, asked, asks, served, listed, table,
    queries, keys, values, totals, bias, places, staged, heads,
    local_sem, rows_send, rows_recv, ask_send, ask_recv, serve_send, serve_recv,
    heads_send, heads_recv, out_send, out_recv, spread_send, spread_recv,
):
    kv, tp = lax.axis_index("kv"), lax.axis_index("tp")
    owners, peers = asked.shape[0], full.shape[0]
    blocks, group, width = rows.shape[1:]
    picks = chosen.shape[1]
    slots = pool.shape[1]
    lines = blocks * group

    own_tokens = pltpu.make_async_copy(tokens, full.at[tp], local_sem.at[0])
    own_latent = pltpu.make_async_copy(latent_weight, weight, local_sem.at[1])
    own_query = pltpu.make_async_copy(query_weight, projection, local_sem.at[2])
    own_out = pltpu.make_async_copy(out_weight, wide_weight.at[tp], local_sem.at[3])
    small = [
        pltpu.make_async_copy(source, target, local_sem.at[5 + i])
        for i, (source, target) in enumerate(
            (
                (chosen_in, chosen), (query_gain_in, query_gain), (key_gain_in, key_gain), (up_in, up), (out_gain_in, out_gain)
            )
        )
    ]
    barrier = pltpu.get_barrier_semaphore()

    def greet(axis, index, size):
        def signal(step):
            pl.semaphore_signal(barrier, inc=1, device_id={axis: lax.rem(index + step, size)}, device_id_type=MESH)

        each(1, size, signal)

    greet("kv", kv, owners)
    greet("tp", tp, peers)

    for copy in (own_tokens, *small, own_latent, own_query, own_out):
        copy.start()
    own_tokens.wait()
    pl.semaphore_wait(barrier, owners + peers - 2)

    share = owners // PIECES

    def rows_copy(to, slot):
        return remote(full.at[tp, :, to], rows.at[slot], rows_send, rows_recv, "tp", to)

    def ask_copy(to, slot):
        return remote(asks.at[to], asked.at[slot], ask_send, ask_recv, "kv", to)

    def serve_target(slot):
        return pool.at[tp, pl.ds(blocks + slot * PER_OWNER, PER_OWNER)]

    def serve_copy(to, slot):
        return remote(served.at[to], serve_target(slot), serve_send, serve_recv.at[lax.div(slot, share)], "kv", to)

    def peer(i):
        away = lax.div(i, 2) * (1 - 2 * lax.rem(i, 2))
        return lax.rem(tp + peers // 2 + away, peers)

    each(1, peers, lambda i: rows_copy(peer(i), tp).start())
    token_spread = Spread(
        full.reshape(peers, blocks * peers, group, width), 0, blocks * peers, spread_send.at[0], spread_recv.at[0]
    )
    token_spread.own()

    tile = (blocks, 128)
    lane = lax.broadcasted_iota(jnp.int32, tile, 1)
    sub = lax.broadcasted_iota(jnp.int32, tile, 0)
    ids = lane * blocks + sub

    small[0].wait()

    def mark(b, needed):
        for c in range(picks):
            needed = jnp.where(ids == chosen[b, c], 1, needed)
        return needed

    needed = lax.fori_loop(0, blocks, mark, jnp.zeros(tile, jnp.int32))
    first = jnp.full((1, 128), -1, jnp.int32)
    second = first
    for j in reversed(range(blocks)):
        hit = needed[j : j + 1, :] > 0
        second = jnp.where(hit, first, second)
        first = jnp.where(hit, j, first)
    both = jnp.where(sub == 0, first, jnp.where(sub == 1, second, 0))
    listed[...] = both
    to_scalars = pltpu.make_async_copy(listed, table, local_sem.at[4])
    to_scalars.start()
    both = both.astype(jnp.float32)

    for o in range(owners):
        spread_out = jnp.sum(jnp.where(lane == o, both, 0.0), axis=1, keepdims=True)
        asks[o] = jnp.broadcast_to(spread_out, tile)[:PER_OWNER]
    others = owners - 1

    def stay(source, target, sem):
        pltpu.make_async_copy(source, target, sem).start()

    each(0, kv, lambda o: ask_copy(o, kv).start())
    each(0, kv, lambda o: stay(asks.at[kv], asked.at[o], ask_recv))
    each(kv + 1, owners, lambda o: stay(asks.at[kv], asks.at[o], ask_send))

    ones = jnp.ones((ONES, BLOCK), jnp.bfloat16)

    def fill(slot):
        values[slot, BLOCK:, :] = ones

    each(0, slots, fill)
    key = lax.broadcasted_iota(jnp.int32, bias.shape[1:], 0)
    query = lax.rem(lax.broadcasted_iota(jnp.int32, bias.shape[1:], 1), BLOCK)
    bias[0] = jnp.where(key <= query, 0.0, masked_score)
    bias[1] = jnp.zeros(bias.shape[1:], jnp.float32)
    keys[slots] = jnp.zeros((BLOCK, width), jnp.bfloat16)
    values[slots] = jnp.zeros((BLOCK + ONES, BLOCK), jnp.bfloat16)
    def place(b):
        for c in range(picks):
            block = chosen[b, c]
            held = jnp.maximum(block, 0)
            owner = lax.div(held, blocks)
            inside = held - owner * blocks
            away = blocks + owner * PER_OWNER + jnp.where(table[1, owner] == inside, 1, 0)
            places[b, c] = jnp.where(block < 0, slots, jnp.where(owner == kv, inside, away))

    to_scalars.wait()
    each(0, blocks, place)
    for copy in small[1:]:
        copy.wait()
    rows[tp] = full[tp, :, tp]
    own_latent.wait()
    wait_bytes(rows.at[pl.ds(0, peers - 1)], rows_recv)

    @jax.jit
    def compress():
        features = jnp.concatenate([rows[p].reshape(lines, width) for p in range(peers)], axis=1)
        latent = jnp.dot(features, weight[...], preferred_element_type=jnp.float32)
        return latent.astype(jnp.bfloat16).reshape(blocks, group, 128)

    latent = compress()
    pool[tp, 0:blocks] = latent
    latent = latent.astype(jnp.float32)

    def serve(r):
        for k in range(PER_OWNER):
            want = asked[r, k : k + 1, :]
            picked = jnp.zeros((group, 128), jnp.float32)
            for j in range(blocks):
                picked = jnp.where(want == float(j), latent[j], picked)
            served[r, k] = picked.astype(jnp.bfloat16)
        serve_copy(r, kv).start()

    def serve_in_turn(n):
        turn = lax.rem(n, LAYERS)
        away = lax.div(turn + 1, 2) * (2 * lax.rem(turn, 2) - 1)
        r = lax.rem(LAYERS // 2 + away, LAYERS) * (owners // LAYERS) + lax.div(n, LAYERS)
        pl.when(r > kv)(lambda: serve(r))

    wait_bytes(asked.at[pl.ds(0, others)], ask_recv)
    each(0, owners, serve_in_turn)
    low = pool.at[tp, pl.ds(0, PER_OWNER)]
    each(0, kv, lambda o: stay(low, served.at[o], serve_send))
    full_share = lax.div(kv + share - 1, share) * share
    each(kv, full_share, lambda o: stay(low, serve_target(o), serve_recv.at[lax.div(o, share)]))
    here = Spread(pool, 0, blocks, spread_send.at[1], spread_recv.at[1])
    here.own()

    per_piece = share * PER_OWNER
    pieces = [lax.rem(lax.div(kv, share) + step, PIECES) for step in (0, 3, 1, 2)]
    firsts = [blocks + piece * per_piece for piece in pieces]
    spreads = [
        Spread(pool, first, per_piece, spread_send.at[2 + k], spread_recv.at[2 + k]) for k, first in enumerate(firsts)
    ]

    def if_needed(k, act):
        pl.when(pieces[k] * share < kv)(act)

    def gathered(k):
        wait_bytes(pool.at[tp, pl.ds(firsts[k], per_piece)], serve_recv.at[pieces[k]])
        spreads[k].start(0, 1)

    scale = width ** (-0.5) * LOG2E
    query_row = query_gain[...] * scale

    def project(j):
        features = jnp.concatenate(
            [full[p, pl.ds(2 * j, 2)].reshape(2 * BLOCK, width) for p in range(peers)], axis=1
        )
        projected = jnp.dot(features, projection[...], preferred_element_type=jnp.float32)
        projected = projected.astype(jnp.bfloat16).astype(jnp.float32)
        for i in range(2):
            for h in range(up.shape[0]):
                head = projected[i * BLOCK : (i + 1) * BLOCK, h * 128 : (h + 1) * 128]
                queries[2 * j + i, h * BLOCK : (h + 1) * BLOCK, :] = unit(head, query_row)

    eye_shape = (BLOCK, BLOCK)
    same = lax.broadcasted_iota(jnp.int32, eye_shape, 0) == lax.broadcasted_iota(jnp.int32, eye_shape, 1)
    eye = jnp.where(same, 1.0, 0.0).astype(jnp.bfloat16)

    def prepare(low, count):
        def several(j):
            first = low + 8 * j
            picked = [pool[:, first + i].reshape(BLOCK, width) for i in range(8)]
            turned = lax.dot_general(
                eye, jnp.concatenate(picked, axis=0), (((1,), (1,)), ((), ())), preferred_element_type=jnp.float32
            ).astype(jnp.bfloat16)
            for i in range(8):
                keys[first + i] = unit(picked[i].astype(jnp.float32), key_gain[...])
                values[first + i, :BLOCK, :] = turned[:, i * BLOCK : (i + 1) * BLOCK]

        each(0, count // 8, several)

    wait_bytes(rows.at[pl.ds(0, peers - 1)], rows_send)
    token_spread.relay_first()
    token_spread.relay_near()
    here.relay_first()
    near = jnp.logical_or(kv >= owners - share, kv < owners // 2)

    def far_pieces():
        for k in range(1, PIECES):
            if_needed(k, functools.partial(gathered, k))
        for k in range(1, PIECES):
            if_needed(k, functools.partial(spreads[k].start, 2, 3, 4, 5))

    if_needed(0, functools.partial(gathered, 0))
    if_needed(0, functools.partial(spreads[0].start, 2, 3, 4, 5))
    pl.when(near)(far_pieces)
    token_spread.relay_far()
    token_spread.finish()
    own_query.wait()
    own_out.wait()
    each(0, blocks // 2, project)
    here.relay_rest()
    pl.when(jnp.logical_not(near))(far_pieces)
    for k in range(PIECES):
        if_needed(k, spreads[k].relay_first)
    out_spread = Spread(wide_weight, 0, 128, spread_send.at[2 + PIECES], spread_recv.at[2 + PIECES])
    out_spread.own()
    here.finish()
    prepare(0, blocks)

    def complete(k):
        spreads[k].finish()
        prepare(firsts[k], per_piece)

    for k in range(PIECES + 1):
        if k < PIECES:
            if_needed(k, spreads[k].relay_rest)
        if k > 0:
            if_needed(k - 1, functools.partial(complete, k - 1))
    token_spread.drain()

    def heads_copy(to, b, slot):
        return remote(staged.at[b, to], heads.at[slot, b], heads_send, heads_recv.at[lax.div(b, HALF)], "tp", to)

    sides, heads_here = 2, up.shape[0]
    span = GROUP * BLOCK
    weights = full.reshape(sides, heads_here, -1, width)

    def weigh(b, side, g):
        picked = jnp.concatenate([keys[places[b, g * GROUP + i]] for i in range(GROUP)], axis=0)
        scores = lax.dot_general(
            picked, queries[b], (((1,), (1,)), ((), ())), preferred_element_type=jnp.float32
        )
        diagonal = jnp.exp2(scores[:BLOCK] + bias[jnp.minimum(g, 1)]).astype(jnp.bfloat16)
        others = jnp.exp2(scores[BLOCK:]).astype(jnp.bfloat16)
        for h in range(heads_here):
            cols = slice(h * BLOCK, (h + 1) * BLOCK)
            weights[side, h, :BLOCK, :] = diagonal[:, cols]
            weights[side, h, BLOCK:span, :] = others[:, cols]

    def add_up(b, side, g):
        held = jnp.concatenate([values[places[b, g * GROUP + i]] for i in range(GROUP)], axis=1)
        right = jnp.concatenate([weights[side, h, :span, :] for h in range(heads_here)], axis=1)
        return jnp.dot(held, right, preferred_element_type=jnp.float32)

    def hand_over(b, ended):
        shares = []
        for total in ended:
            shares.append((total[:BLOCK] / total[BLOCK : BLOCK + 1]).astype(jnp.bfloat16))
        turned, flipped = [], []
        for side in range(sides):
            for h in range(heads_here):
                share = shares[side][:, h * BLOCK : (h + 1) * BLOCK]
                turned.append(jnp.dot(up[h], share, preferred_element_type=jnp.float32))
        for side in range(sides):
            both = jnp.concatenate(turned[side * heads_here : (side + 1) * heads_here], axis=0)
            flipped.append(jnp.transpose(both).astype(jnp.bfloat16).reshape(peers, group, width))
        for side in range(sides):
            staged[b + side] = flipped[side]

    def start(i):
        for side in range(sides):
            weigh(sides * i + side, side, 0)

    groups = lax.div(jnp.minimum(picks, blocks + PER_OWNER * kv) + GROUP - 1, GROUP)

    def attend(i, following):
        first = sides * i
        for side in range(sides):
            totals[side] = jnp.zeros(totals.shape[1:], jnp.float32)

        def both(g):
            for side in range(sides):
                totals[side] = totals[side] + add_up(first + side, side, g - 1)
            for side in range(sides):
                weigh(first + side, side, g)

        early = jnp.minimum(groups, GROUPS_EARLY)
        each(1, early, both)
        if following:
            pl.when(i == 0)(out_spread.relay_first)
        else:
            out_spread.relay_rest()
        each(early, groups, both)
        ended = [totals[side] + add_up(first + side, side, groups - 1) for side in range(sides)]
        if following:
            start(i + 1)
        hand_over(first, ended)
        for side in range(sides):
            each(1, peers, lambda j: heads_copy(peer(j), first + side, tp).start())

    def part(half):
        return (0, HALF) if half == 0 else (HALF, blocks - HALF)

    def out_copy(to, half, slot):
        lower = pl.ds(*part(half))
        return remote(rows.at[to, lower], out.at[lower, slot], out_send, out_recv, "tp", to)

    @functools.partial(jax.jit, static_argnums=0)
    def mix(half):
        lower, count = pl.ds(*part(half)), part(half)[1]
        features = jnp.concatenate([heads[p, lower].reshape(count * group, width) for p in range(peers)], axis=1)
        summed = jnp.dot(
            features, wide_weight[...].reshape(peers * 128, peers * 128), preferred_element_type=jnp.float32
        )
        mixed = unit(summed, out_gain[...])
        for t in range(peers):
            rows[t, lower] = mixed[:, t * 128 : (t + 1) * 128].reshape(count, group, 128)

    def conclude(half):
        first, count = part(half)
        lower = pl.ds(first, count)
        wait_bytes(heads.at[pl.ds(0, peers - 1), lower], heads_recv.at[half])
        for b in range(first, first + count):
            heads[tp, b] = staged[b, tp]
        mix(half)
        each(1, peers, lambda i: out_copy(peer(i), half, tp).start())
        out[lower, tp] = rows[tp, lower]

    def turn(i):
        attend(i, True)

    last = blocks // sides - 1
    each(0, 1, start)
    each(0, last, turn)
    each(last, last + 1, lambda i: attend(i, False))
    out_spread.finish()
    conclude(0)
    conclude(1)

    wait_bytes(asks.at[pl.ds(0, others)], ask_send)
    wait_bytes(served.at[pl.ds(0, others)], serve_send)
    for spread in (here, out_spread):
        spread.drain()
    for k in range(PIECES):
        if_needed(k, spreads[k].drain)
    wait_bytes(staged.at[:, pl.ds(0, peers - 1)], heads_send)
    wait_bytes(rows.at[pl.ds(0, peers - 1)], out_send)
    wait_bytes(out.at[:, pl.ds(0, peers - 1)], out_recv)


def shards(
    tokens, query_weight, latent_weight, query_gain, key_gain, value_up, out_weight, out_gain, chosen
):
    peers, owners = lax.axis_size("tp"), lax.axis_size("kv")
    blocks, picks = chosen.shape
    rows, width = tokens.shape
    group = BLOCK // peers
    slots = blocks + owners * PER_OWNER
    heads = value_up.shape[0]
    vmem = pl.BlockSpec(memory_space=pltpu.VMEM)
    anywhere = pl.BlockSpec(memory_space=pl.ANY)
    dma = pltpu.SemaphoreType.DMA
    bf16 = jnp.bfloat16
    mixed = pl.pallas_call(
        kernel,
        out_shape=pltpu.VMEM((blocks, peers, group, width), bf16),
        in_specs=[anywhere] * 9,
        out_specs=vmem,
        scratch_shapes=[
            pltpu.SMEM((blocks, picks), jnp.int32),
            pltpu.VMEM((1, width), jnp.float32),
            pltpu.VMEM((1, width), jnp.float32),
            pltpu.VMEM((heads, value_up.shape[2], width), bf16),
            pltpu.VMEM((1, out_gain.shape[0]), jnp.float32),
            pltpu.VMEM((peers, blocks, peers, group, width), bf16),
            pltpu.VMEM((peers, slots, group, width), bf16),
            pltpu.VMEM((peers, *out_weight.shape), bf16),
            pltpu.VMEM(latent_weight.shape, bf16),
            pltpu.VMEM(query_weight.shape, bf16),
            pltpu.VMEM((peers, blocks, group, width), bf16),
            pltpu.VMEM((owners, PER_OWNER, 128), jnp.float32),
            pltpu.VMEM((owners, PER_OWNER, 128), jnp.float32),
            pltpu.VMEM((owners, PER_OWNER, group, width), bf16),
            pltpu.VMEM((blocks, 128), jnp.int32),
            pltpu.SMEM((blocks, 128), jnp.int32),
            pltpu.VMEM((blocks, heads * BLOCK, width), bf16),
            pltpu.VMEM((slots + 1, BLOCK, width), bf16),
            pltpu.VMEM((slots + 1, BLOCK + ONES, BLOCK), bf16),
            pltpu.VMEM((2, BLOCK + ONES, heads * BLOCK), jnp.float32),
            pltpu.VMEM((2, BLOCK, heads * BLOCK), jnp.float32),
            pltpu.SMEM((blocks, picks), jnp.int32),
            pltpu.VMEM((blocks, peers, group, width), bf16),
            pltpu.VMEM((peers, blocks, group, width), bf16),
            dma((10,)),
            dma, dma,
            dma, dma,
            dma, dma((PIECES,)),
            dma, dma((2,)),
            dma, dma,
            dma((3 + PIECES,)), dma((3 + PIECES, 4)),
        ],
        compiler_params=pltpu.CompilerParams(collective_id=0, has_side_effects=True),
    )(
        chosen,
        tokens.reshape(blocks, peers, group, width),
        latent_weight,
        query_weight,
        out_weight,
        query_gain.reshape(1, width),
        key_gain.reshape(1, width),
        jnp.swapaxes(value_up, 1, 2),
        out_gain.reshape(1, out_gain.shape[0]),
    )
    return mixed.reshape(rows, width)


def solution(mesh):
    in_specs = (
        P("kv", "tp"),
        P(None, "tp"),
        P(),
        P(),
        P(),
        P("tp", None, None),
        P("tp", None),
        P(),
        P("kv", None),
    )
    return jax.shard_map(shards, mesh=mesh, in_specs=in_specs, out_specs=P("kv", "tp"), check_vma=False)
```
